256 devices in a mesh: sp: 128 (over z, y, x), tp: 2 (over core).
Axes of the slice: x: 4, y: 4, z: 8, core: 2. Of those that a mesh axis runs over, the one named last changes fastest.
Arguments:
- block_input: bfloat16 [16384, 2048], P('sp'), may hold values from -6 to 6
- value_weight: bfloat16 [2048, 384], P(None, 'tp'), may hold values from -0.125 to 0.125
- query_pre: bfloat16 [16384, 384], P('sp', 'tp'), may hold values from -6 to 6
- forget_pre: bfloat16 [16384, 384], P('sp', 'tp'), may hold values from -5.5 to 5.5
- lower_bound: float32 [384], P('tp'), may hold values from 0.94 to 1, as said below
- out_grad: bfloat16 [16384, 384], P('sp', 'tp'), may hold values from -6 to 6
Outputs:
- grad_query_pre: bfloat16 [16384, 384], P('sp', 'tp')
- grad_forget_pre: bfloat16 [16384, 384], P('sp', 'tp')
- grad_block_input: bfloat16 [16384, 2048], P(('sp', 'tp'))
- grad_value_weight: float32 [2048, 384], P('sp', 'tp')
The draws below stay inside these ranges and needn't reach their ends.
Inputs may be any that keep to these rules, and one draw needn't show every extreme that they name: `lower_bound`: each channel's floor is below 1 and at least 0.94.
All inputs are finite; a program needn't handle non-finite values.
Results may differ from the reference program's by a relative error of at most 0.009.
Values may be sent and summed in bfloat16 or wider, within the bound.
A program may use at most 64 MiB of HBM per device.

```python
import math
import jax
import jax.numpy as jnp
from jax import lax

D = 2048
HEADS = 6
HEAD = 64
BLOCK = 64
TOK_DEV = 128
WIDTH = 384
TOKENS = 16384
N_TP = 2


def draw_lower_bound(key, part):
    pick_key, fast_key, slow_key = jax.random.split(jax.random.fold_in(key, 11), 3)
    fast_share = 0.5
    head_fast = jax.random.uniform(pick_key, (HEADS,), jnp.float32) < fast_share
    channel_fast = jnp.repeat(head_fast, HEAD)
    fast_gap = jnp.exp(jax.random.uniform(fast_key, (WIDTH,), jnp.float32, math.log(0.02), math.log(0.06)))
    slow_gap = 2.0 / TOKENS * jnp.exp(jax.random.uniform(slow_key, (WIDTH,), jnp.float32, math.log(0.5), math.log(2.0)))
    return (1.0 - jnp.where(channel_fast, fast_gap, slow_gap)).astype(jnp.float32)


def draw_forget_pre(key, part):
    noise_key, shift_key = jax.random.split(jax.random.fold_in(key, 23), 2)
    noise = jnp.clip(jax.random.normal(noise_key, (TOKENS, WIDTH), jnp.float32), -4.0, 4.0)
    shifts = jax.random.uniform(shift_key, (TOKENS // TOK_DEV, WIDTH), jnp.float32, -1.5, 1.5)
    return (noise + jnp.repeat(shifts, TOK_DEV, axis=0)).astype(jnp.bfloat16)


def steps_of(stream_key, shape, shards, low, top_value):
    factor_of, own = 1.0, jax.random.fold_in(stream_key, 6)
    for axis_at, shards_of in shards:
        draws = jnp.exp(jax.random.uniform(jax.random.fold_in(own, axis_at), (shards_of,), jnp.float32, low / len(shards), top_value / len(shards)))
        factor_of = factor_of * jnp.repeat(draws, shape[axis_at] // shards_of).reshape([-1 if axis == axis_at else 1 for axis in range(len(shape))])
    return factor_of


def gaussian(own_key, shape, spread, bound, cuts=(), held_as=jnp.bfloat16):
    loudness = steps_of(own_key, shape, cuts, -0.22, 0.18) if cuts else 1.0
    values = jax.random.normal(own_key, shape, jnp.float32) * spread * loudness
    return jnp.minimum(jnp.maximum(values, -bound), bound).astype(held_as)


def setup_inputs(seed: int = 0) -> dict:
    key_list = jax.random.split(jax.random.key(seed), 7)
    return {
        "block_input": gaussian(key_list[0], (TOKENS, D), 1.0, 6.0, ((0, 128),)),
        "value_weight": gaussian(key_list[1], (D, WIDTH), D ** -0.5, 0.125, ((1, 2),)),
        "query_pre": gaussian(key_list[2], (TOKENS, WIDTH), 1.0, 6.0, ((0, 128), (1, 2))),
        "forget_pre": draw_forget_pre(jax.random.fold_in(key_list[6], 71), 0),
        "lower_bound": draw_lower_bound(jax.random.fold_in(key_list[6], 71), 0),
        "out_grad": gaussian(key_list[5], (TOKENS, WIDTH), 1.0, 6.0, ((0, 128), (1, 2))),
    }


highest = lax.Precision.HIGHEST

def blocked(array, head_count, block_count):
    return jnp.transpose(array.reshape(block_count, BLOCK, head_count, HEAD), (0, 2, 1, 3))

def recurrence(query, key_rate, value_rows, decay_log):
    tokens_all, width_all = query.shape
    head_count = width_all // HEAD
    block_count = tokens_all // BLOCK
    causal = (jnp.arange(BLOCK)[:, None] >= jnp.arange(BLOCK)[None, :]).astype(query.dtype)

    def advance(carried, pieces):
        query_b, key_b, value_b, decay_b = pieces
        cumulative = jnp.cumsum(decay_b, axis=1)
        closing = cumulative[:, -1:, :]
        query_dec = query_b * jnp.exp(cumulative)
        key_dec = key_b * jnp.exp(-cumulative)
        mixing = jnp.einsum('htd,hsd->hts', query_dec, key_dec, precision=highest) * causal
        output = jnp.einsum('hts,hsv->htv', mixing, value_b, precision=highest)
        output = output + jnp.einsum('htd,hdv->htv', query_dec, carried, precision=highest)
        renewed = jnp.exp(closing[:, 0, :])[:, :, None] * carried
        renewed = renewed + jnp.einsum('hsd,hsv->hdv', key_b * jnp.exp(closing - cumulative), value_b, precision=highest)
        return (renewed, output)
    initial = jnp.zeros((head_count, HEAD, HEAD), query.dtype)
    pieces = tuple((blocked(array, head_count, block_count) for array in (query, key_rate, value_rows, decay_log)))
    _, outputs = lax.scan(advance, initial, pieces)
    return jnp.transpose(outputs, (0, 2, 1, 3)).reshape(tokens_all, width_all)

def reference(block_input, value_weight, query_pre, forget_pre, lower_bound, out_grad):
    value_rows = jnp.dot(block_input, value_weight, preferred_element_type=jnp.float32).astype(jnp.bfloat16)

    def forward(query_f, forget_f, value_f):
        query = jax.nn.silu(query_f)
        key_rate = (1.0 - lower_bound) * jax.nn.sigmoid(-forget_f)
        decay_log = jnp.log1p(-key_rate)
        return recurrence(query, key_rate, value_f, decay_log)
    _, pullback = jax.vjp(forward, query_pre.astype(jnp.float32), forget_pre.astype(jnp.float32), value_rows.astype(jnp.float32))
    grad_query, grad_forget, grad_value = pullback(out_grad.astype(jnp.float32))
    value_grad = grad_value.astype(jnp.bfloat16)
    weight_grad = lax.dot_general(block_input, value_grad, (((0,), (0,)), ((), ())), preferred_element_type=jnp.float32)
    group_width = WIDTH // N_TP
    summed = jnp.zeros((block_input.shape[0], D), jnp.float32)
    for member in range(N_TP):
        lo_col = member * group_width
        partial_value = lax.dot_general(value_grad[:, lo_col:lo_col + group_width], value_weight[:, lo_col:lo_col + group_width], (((1,), (1,)), ((), ())), preferred_element_type=jnp.float32)
        partial_value = lax.optimization_barrier(partial_value.astype(jnp.bfloat16))
        summed = summed + partial_value.astype(jnp.float32)
    return (grad_query.astype(jnp.bfloat16), grad_forget.astype(jnp.bfloat16), summed.astype(jnp.bfloat16), weight_grad)
```

```python
import functools

import jax
import jax.numpy as jnp
from jax import lax
from jax.experimental import pallas as pl
from jax.experimental.pallas import tpu as pltpu
from jax.sharding import Mesh
from jax.sharding import PartitionSpec as P

HEAD = 64
SP = ("sp_0", "sp_1", "sp_2")
SP_TP = ("sp_0", "sp_1", "sp_2", "tp")
F32, BF16 = jnp.float32, jnp.bfloat16
LOGICAL = pl.DeviceIdType.MESH


def nn(a, b):
    return lax.dot_general(a, b, (((1,), (0,)), ((), ())), preferred_element_type=F32)


def nt(a, b):
    return lax.dot_general(a, b, (((1,), (1,)), ((), ())), preferred_element_type=F32)


def tn(a, b):
    return lax.dot_general(a, b, (((0,), (0,)), ((), ())), preferred_element_type=F32)


def exact_sum(ones, values):
    high = values.astype(BF16)
    low = (values - high.astype(F32)).astype(BF16)
    return nn(ones, high) + nn(ones, low)


def rcopy(src, dst, send, recv, device):
    return pltpu.make_async_remote_copy(
        src_ref=src, dst_ref=dst, send_sem=send, recv_sem=recv, device_id=device, device_id_type=LOGICAL
    )


def kernel(
    nz, ny, nx,
    x_hbm, w_hbm, q_hbm, f_hbm, go_hbm, lb_ref,
    gq_out, gf_out, gx_out, gw_out,
    x_v, w_v, q_v, f_v, go_v,
    s_send, e_send, s_buf, e_buf, l_buf, fl_buf, t_send, ft_send, t_buf, ft_buf, o_send, p_buf,
    xt, xtl, vg_v, vgl, ig, ig_recv, gx_v, acc, y_send, y_recv, w2, z_send, z_recv,
    gq_v, gf_v, gw_v,
    lsem, s_ss, s_rs, e_ss, e_rs, t_ss, t_rs, ft_ss, ft_rs, p_ss, p_rs,
    xt_ss, xt_rs, vg_ss, vg_rs, y_ss, y_rs, z_ss, z_rs, ig_ss, ig_rs,
):
    pln = ny * nx
    tok, d_model = x_v.shape
    ch = w_v.shape[1]
    heads = ch // HEAD
    z, y, x, c = (lax.axis_index(a) for a in SP_TP)
    me = y * nx + x
    back = (me * 2) // pln

    def plane(i):
        return (z, i // nx, lax.rem(i, nx), c)

    loads = [
        pltpu.make_async_copy(src, dst, lsem.at[k])
        for k, (src, dst) in enumerate(
            ((f_hbm, f_v), (q_hbm, q_v), (go_hbm, go_v), (x_hbm, x_v), (w_hbm, w_v))
        )
    ]
    for copy in loads:
        copy.start()

    barrier = pltpu.get_barrier_semaphore()
    for k in range(1, pln):
        pl.semaphore_signal(barrier, inc=1, device_id=plane(lax.rem(me + k, pln)), device_id_type=LOGICAL)
    for k in range(1, nz):
        pl.semaphore_signal(barrier, inc=1, device_id=(lax.rem(z + k, nz), y, x, c), device_id_type=LOGICAL)
    pl.semaphore_signal(barrier, inc=1, device_id=(z, y, x, 1 - c), device_id_type=LOGICAL)

    lane = lax.broadcasted_iota(jnp.int32, (1, ch), 1)
    mf = [jnp.where((lane >= HEAD * h) & (lane < HEAD * (h + 1)), 1.0, 0.0).astype(F32) for h in range(heads)]
    mb = [m.astype(BF16) for m in mf]
    row = lax.broadcasted_iota(jnp.int32, (tok, tok), 0)
    col = lax.broadcasted_iota(jnp.int32, (tok, tok), 1)
    lower, upper = row >= col, col >= row
    lower_ones = jnp.where(lower, 1.0, 0.0).astype(BF16)
    upper_ones = jnp.where(upper, 1.0, 0.0).astype(BF16)

    def stacked(a):
        return jnp.concatenate([a * m for m in mb], axis=0)

    def folded(full):
        out = full[:HEAD] * mf[0]
        for h in range(1, heads):
            out = out + full[HEAD * h : HEAD * (h + 1)] * mf[h]
        return out

    loads[0].wait()
    f = f_v[...].astype(F32)
    f_neg = 1.0 / (1.0 + jnp.exp(f))
    f_sig = 1.0 / (1.0 + jnp.exp(-f))
    k_rate = (1.0 - lb_ref[...]) * f_neg
    cum = exact_sum(lower_ones, jnp.log1p(-k_rate))
    closing = cum[tok - 1 : tok, :]
    growth = jnp.exp(cum)
    shrink = jnp.exp(-cum)
    remain = jnp.exp(closing - cum)
    total = jnp.exp(closing)
    e_send[...] = total
    k_dec = (k_rate * shrink).astype(BF16)
    k_end = (k_rate * remain).astype(BF16)
    loads[1].wait()
    q = q_v[...].astype(F32)
    q_sig = 1.0 / (1.0 + jnp.exp(-q))
    query = q * q_sig
    q_dec = (query * growth).astype(BF16)
    loads[2].wait()
    go = go_v[...]
    reach = folded(tn(go, q_dec))
    loads[3].wait()
    loads[4].wait()
    v = nn(x_v[...], w_v[...]).astype(BF16)
    update = folded(tn(v, k_end))
    s_send[...] = jnp.concatenate([update, reach], axis=0).reshape(s_send.shape)

    pl.semaphore_wait(barrier, pln + nz - 1)
    sends = []
    for k in range(1, pln):
        to = lax.rem(me + k, pln)
        sends.append(rcopy(e_send, e_buf.at[me], e_ss.at[k], e_rs.at[me], plane(to)))
        sends.append(rcopy(s_send.at[to], s_buf.at[me], s_ss.at[k], s_rs.at[me], plane(to)))
        sends[-2].start()
        sends[-1].start()
    s_buf[me] = s_send[me]
    e_buf[me] = e_send[...]

    rows = d_model // (nz * ny * nx)
    per = tok // rows
    for b in range(d_model // tok):
        turned = x_v[:, tok * b : tok * (b + 1)].T
        for g in range(per):
            at = b * per + g
            zz, yy, xx = at // pln, (at // nx) % ny, at % nx
            xt[xx, pl.ds((yy * nz + zz) * rows, rows), :] = turned[rows * g : rows * (g + 1)]
    for k in range(1, nx):
        to = lax.rem(x + k, nx)
        copy = rcopy(xt.at[to], xtl.at[x], xt_ss.at[k], xt_rs.at[x], (z, y, to, c))
        copy.start()
        sends.append(copy)

    go_st, v_st, qd_st, kd_st = stacked(go), stacked(v), stacked(q_dec), stacked(k_dec)

    def beside(full, keep):
        return jnp.concatenate(
            [jnp.where(keep, full[tok * h : tok * (h + 1)], 0.0).astype(BF16) for h in range(heads)], axis=1
        )

    gv_own = nn(beside(nt(kd_st, q_dec), upper), go_st)

    for k in range(1, pln):
        frm = lax.rem(me + k, pln)
        rcopy(e_send, e_buf.at[frm], e_ss.at[k], e_rs.at[frm], plane(frm)).wait_recv()
        rcopy(s_send.at[0], s_buf.at[frm], s_ss.at[k], s_rs.at[frm], plane(frm)).wait_recv()
    held = jnp.zeros(t_send.shape, F32)
    factor = jnp.ones((1, ch), F32)
    for o in range(pln):
        it = o + back * (pln - 1 - 2 * o)
        l_buf[it] = held
        fl_buf[it] = factor
        decay = e_buf[it]
        held = decay * held + s_buf[it]
        factor = decay * factor
    t_send[...] = held
    ft_send[...] = factor

    z_order = z + back * (nz - 1 - 2 * z)

    def z_sends(k):
        at = z_order + k
        to = at + back * (nz - 1 - 2 * at)
        return (
            rcopy(ft_send, ft_buf.at[z], ft_ss.at[k], ft_rs.at[z], (to, y, x, c)),
            rcopy(t_send, t_buf.at[z], t_ss.at[k], t_rs.at[z], (to, y, x, c)),
        )

    for k in range(1, nz):

        @pl.when(z_order + k < nz)
        def _():
            for copy in z_sends(k):
                copy.start()

    gq_own = nn(beside(nt(go_st, v), lower), kd_st)
    gk_own = nn(beside(nt(v_st, go), upper), qd_st)

    def arriving(o, carried):
        frm = o + back * (nz - 1 - 2 * o)
        rcopy(ft_send, ft_buf.at[frm], ft_ss.at[0], ft_rs.at[frm], (z, y, x, c)).wait_recv()
        rcopy(t_send, t_buf.at[frm], t_ss.at[0], t_rs.at[frm], (z, y, x, c)).wait_recv()
        return ft_buf[frm] * carried + t_buf[frm]

    carried = lax.fori_loop(0, z_order, arriving, jnp.zeros(t_send.shape, F32))

    o_send[...] = l_buf[...] + fl_buf[...] * carried[None]
    for k in range(1, pln):
        to = lax.rem(me + k, pln)
        copy = rcopy(o_send.at[to], p_buf.at[me], p_ss.at[k], p_rs.at[me], plane(to))
        copy.start()
        sends.append(copy)
    p_buf[me] = o_send[me]
    for k in range(1, pln):
        frm = lax.rem(me + k, pln)
        rcopy(o_send.at[0], p_buf.at[frm], p_ss.at[k], p_rs.at[frm], plane(frm)).wait_recv()
    carries = p_buf[...].reshape(2 * HEAD, ch)
    state, grad = carries[:HEAD], carries[HEAD:]
    bd_state = jnp.concatenate([(state * m).astype(BF16) for m in mf], axis=0)
    bd_grad = jnp.concatenate([(grad * m).astype(BF16) for m in mf], axis=0)

    value_grad = (gv_own + nt(k_end, bd_grad)).astype(BF16)
    vg_v[...] = value_grad
    for k in range(1, nx):
        to = lax.rem(x + k, nx)
        copy = rcopy(vg_v, vgl.at[x], vg_ss.at[k], vg_rs.at[x], (z, y, to, c))
        copy.start()
        sends.append(copy)

    width = 512 if d_model % 512 == 0 else d_model
    for j in range(d_model // width):
        cols = pl.ds(j * width, width)
        ig[:, :, cols] = nt(value_grad, w_v[cols, :]).astype(BF16).reshape(2, tok // 2, width)
    ig_copy = rcopy(ig.at[1 - c], ig_recv, ig_ss, ig_rs, (z, y, x, 1 - c))
    ig_copy.start()

    total_w = nn(xt[x], value_grad)
    for k in range(1, nx):
        frm = lax.rem(x + k, nx)
        rcopy(xt.at[0], xtl.at[frm], xt_ss.at[k], xt_rs.at[frm], (z, y, frm, c)).wait_recv()
        rcopy(vg_v, vgl.at[frm], vg_ss.at[k], vg_rs.at[frm], (z, y, frm, c)).wait_recv()
        total_w = total_w + nn(xtl[frm], vgl[frm])
    acc[...] = total_w.reshape(acc.shape)
    y_send[...] = total_w.astype(BF16).reshape(y_send.shape)
    for k in range(1, ny):
        to = lax.rem(y + k, ny)
        copy = rcopy(y_send.at[to], y_recv.at[y], y_ss.at[k], y_rs.at[y], (z, to, x, c))
        copy.start()
        sends.append(copy)

    g_query = growth * (gq_own + nn(go, bd_state))
    g_key = shrink * gk_own + remain * nn(v, bd_grad)
    gq_v[...] = (g_query * (q_sig * (1.0 + q * (1.0 - q_sig)))).astype(BF16)
    out_q = pltpu.make_async_copy(gq_v, gq_out, lsem.at[0])
    out_q.start()
    boundary = jnp.sum(grad * (total * state + update), axis=0, keepdims=True)
    g_decay = exact_sum(upper_ones, query * g_query - k_rate * g_key) + boundary
    gf_v[...] = ((g_decay / (1.0 - k_rate) - g_key) * k_rate * f_sig).astype(BF16)
    out_f = pltpu.make_async_copy(gf_v, gf_out, lsem.at[1])
    out_f.start()

    w_sum = acc[y]
    for k in range(1, ny):
        frm = lax.rem(y + k, ny)
        rcopy(y_send.at[0], y_recv.at[frm], y_ss.at[k], y_rs.at[frm], (z, frm, x, c)).wait_recv()
        w_sum = w_sum + y_recv[frm].astype(F32)
    w2[...] = w_sum.reshape(w2.shape)
    z_send[...] = w_sum.astype(BF16).reshape(z_send.shape)
    for k in range(1, nz):
        to = lax.rem(z + k, nz)
        copy = rcopy(z_send.at[to], z_recv.at[z], z_ss.at[k], z_rs.at[z], (to, y, x, c))
        copy.start()
        sends.append(copy)

    ig_copy.wait_recv()
    gx_v[...] = (ig[c].astype(F32) + ig_recv[...].astype(F32)).astype(BF16)
    out_x = pltpu.make_async_copy(gx_v, gx_out, lsem.at[2])
    out_x.start()

    w_last = w2[z]
    for k in range(1, nz):
        frm = lax.rem(z + k, nz)
        rcopy(z_send.at[0], z_recv.at[frm], z_ss.at[k], z_rs.at[frm], (frm, y, x, c)).wait_recv()
        w_last = w_last + z_recv[frm].astype(F32)
    gw_v[...] = w_last
    out_w = pltpu.make_async_copy(gw_v, gw_out, lsem.at[3])
    out_w.start()

    for copy in sends:
        copy.wait_send()
    ig_copy.wait_send()
    for k in range(1, nz):

        @pl.when(z_order + k < nz)
        def _():
            for copy in z_sends(k):
                copy.wait_send()

    for copy in (out_q, out_f, out_x, out_w):
        copy.wait()


def on_device(nz, ny, nx, block_input, value_weight, query_pre, forget_pre, lower_bound, out_grad):
    tok, d_model = block_input.shape
    ch = value_weight.shape[1]
    pln = ny * nx
    piece = 2 * HEAD // pln
    rows = d_model // (nz * pln)
    vm, dma = pltpu.VMEM, pltpu.SemaphoreType.DMA
    scratch = [
        vm((tok, d_model), BF16), vm((d_model, ch), BF16),
        vm((tok, ch), BF16), vm((tok, ch), BF16), vm((tok, ch), BF16),
        vm((pln, piece, ch), F32), vm((1, ch), F32),
        vm((pln, piece, ch), F32), vm((pln, 1, ch), F32),
        vm((pln, piece, ch), F32), vm((pln, 1, ch), F32),
        vm((piece, ch), F32), vm((1, ch), F32),
        vm((nz, piece, ch), F32), vm((nz, 1, ch), F32),
        vm((pln, piece, ch), F32), vm((pln, piece, ch), F32),
        vm((nx, d_model // nx, tok), BF16), vm((nx, d_model // nx, tok), BF16),
        vm((tok, ch), BF16), vm((nx, tok, ch), BF16),
        vm((2, tok // 2, d_model), BF16), vm((tok // 2, d_model), BF16), vm((tok // 2, d_model), BF16),
        vm((ny, nz * rows, ch), F32), vm((ny, nz * rows, ch), BF16), vm((ny, nz * rows, ch), BF16),
        vm((nz, rows, ch), F32), vm((nz, rows, ch), BF16), vm((nz, rows, ch), BF16),
        vm((tok, ch), BF16), vm((tok, ch), BF16), vm((rows, ch), F32),
        dma((5,)),
        dma((pln,)), dma((pln,)), dma((pln,)), dma((pln,)),
        dma((nz,)), dma((nz,)), dma((nz,)), dma((nz,)),
        dma((pln,)), dma((pln,)),
        dma((nx,)), dma((nx,)), dma((nx,)), dma((nx,)),
        dma((ny,)), dma((ny,)), dma((nz,)), dma((nz,)),
        dma, dma,
    ]
    hbm = pl.BlockSpec(memory_space=pl.ANY)
    return pl.pallas_call(
        functools.partial(kernel, nz, ny, nx),
        out_shape=(
            jax.ShapeDtypeStruct((tok, ch), BF16),
            jax.ShapeDtypeStruct((tok, ch), BF16),
            jax.ShapeDtypeStruct((tok // 2, d_model), BF16),
            jax.ShapeDtypeStruct((rows, ch), F32),
        ),
        in_specs=[hbm] * 5 + [pl.BlockSpec(memory_space=pltpu.VMEM)],
        out_specs=(hbm,) * 4,
        scratch_shapes=scratch,
        compiler_params=pltpu.CompilerParams(collective_id=0, has_side_effects=True),
    )(block_input, value_weight, query_pre, forget_pre, out_grad, lower_bound.reshape(1, ch))


def on_mesh(devices):
    nz, ny, nx = devices.shape[:3]
    split = Mesh(devices, SP_TP)
    in_specs = (P(SP, None), P(None, "tp"), P(SP, "tp"), P(SP, "tp"), P("tp"), P(SP, "tp"))
    out_specs = (P(SP, "tp"), P(SP, "tp"), P(SP_TP, None), P(SP, "tp"))
    return jax.shard_map(
        functools.partial(on_device, nz, ny, nx), mesh=split, in_specs=in_specs, out_specs=out_specs, check_vma=False
    )


def solution(mesh):
    return on_mesh(mesh.devices.reshape(8, 4, 4, mesh.shape["tp"]))
```

```python
import functools

import jax
import jax.numpy as jnp
from jax import lax
from jax.experimental import pallas as pl
from jax.experimental.pallas import tpu as pltpu
from jax.sharding import Mesh
from jax.sharding import PartitionSpec as P

HEAD = 64
SP = ("sp_0", "sp_1", "sp_2")
SP_TP = ("sp_0", "sp_1", "sp_2", "tp")
F32, BF16 = jnp.float32, jnp.bfloat16
LOGICAL = pl.DeviceIdType.MESH


def nn(a, b):
    return lax.dot_general(a, b, (((1,), (0,)), ((), ())), preferred_element_type=F32)


def nt(a, b):
    return lax.dot_general(a, b, (((1,), (1,)), ((), ())), preferred_element_type=F32)


def tn(a, b):
    return lax.dot_general(a, b, (((0,), (0,)), ((), ())), preferred_element_type=F32)


def rcopy(src, dst, send, recv, device):
    return pltpu.make_async_remote_copy(
        src_ref=src, dst_ref=dst, send_sem=send, recv_sem=recv, device_id=device, device_id_type=LOGICAL
    )


def kernel(
    nz, ny, nx,
    x_hbm, w_hbm, q_hbm, f_hbm, go_hbm, lb_ref,
    gq_out, gf_out, gx_out, gw_out,
    x_v, w_v, q_v, f_v, go_v,
    s_send, e_send, s_buf, e_buf, l_buf, fl_buf, t_send, ft_send, t_buf, ft_buf, o_send, p_buf,
    xt, xtl, vg_v, vgl, ig, ig_recv, acc, y_send, y_recv, w2, z_send, z_recv,
    lsem, s_ss, s_rs, e_ss, e_rs, t_ss, t_rs, ft_ss, ft_rs, p_ss, p_rs,
    xt_ss, xt_rs, vg_ss, vg_rs, y_ss, y_rs, z_ss, z_rs, ig_ss, ig_rs,
):
    pln = ny * nx
    tok, d_model = x_v.shape
    ch = w_v.shape[0]
    heads = ch // HEAD
    z, y, x, c = (lax.axis_index(a) for a in SP_TP)
    me = y * nx + x
    back = (me * 2) // pln

    def plane(i):
        return (z, i // nx, lax.rem(i, nx), c)

    def head_of(a, h):
        return a[HEAD * h : HEAD * (h + 1)]

    def by_head(parts):
        return jnp.concatenate(list(parts), axis=0)

    scope = jax.named_scope
    with scope("loads_barrier"):
        loads = [
            pltpu.make_async_copy(src, dst, lsem.at[k])
            for k, (src, dst) in enumerate(
                ((f_hbm, f_v), (q_hbm, q_v), (go_hbm, go_v), (x_hbm, x_v), (w_hbm, w_v))
            )
        ]
        for copy in loads:
            copy.start()
        barrier = pltpu.get_barrier_semaphore()
        for k in range(1, pln):
            pl.semaphore_signal(barrier, inc=1, device_id=plane(lax.rem(me + k, pln)), device_id_type=LOGICAL)
        for k in range(1, nz):
            pl.semaphore_signal(barrier, inc=1, device_id=(lax.rem(z + k, nz), y, x, c), device_id_type=LOGICAL)
        pl.semaphore_signal(barrier, inc=1, device_id=(z, y, x, 1 - c), device_id_type=LOGICAL)

    lane = lax.broadcasted_iota(jnp.int32, (1, ch), 1)
    mf = [jnp.where((lane >= HEAD * h) & (lane < HEAD * (h + 1)), 1.0, 0.0).astype(F32) for h in range(heads)]
    row = lax.broadcasted_iota(jnp.int32, (tok, tok), 0)
    col = lax.broadcasted_iota(jnp.int32, (tok, tok), 1)
    lower, upper = row >= col, col >= row
    lower_ones = jnp.where(lower, 1.0, 0.0).astype(BF16)
    upper_ones = jnp.where(upper, 1.0, 0.0).astype(BF16)

    def folded(full):
        out = full[:HEAD] * mf[0]
        for h in range(1, heads):
            out = out + head_of(full, h) * mf[h]
        return out

    with scope("gates"):
        gap = jnp.broadcast_to(1.0 - lb_ref[...], (tok, ch)).T
        loads[0].wait()
        f = f_v[...].astype(F32)
        f_neg = 1.0 / (1.0 + jnp.exp(f))
        f_sig = 1.0 / (1.0 + jnp.exp(-f))
        k_rate = gap * f_neg
        logs = jnp.log1p(-k_rate)
        high = logs.astype(BF16)
        low = (logs - high.astype(F32)).astype(BF16)
        cum = nn(high, upper_ones) + nn(low, upper_ones)
        row_ones = jnp.ones((8, tok), BF16)
        total = jnp.exp((nt(row_ones, high) + nt(row_ones, low))[:1])
        closing = cum[:, tok - 1 : tok]
        growth = jnp.exp(cum)
        shrink = jnp.exp(-cum)
        remain = jnp.exp(closing - cum)
        e_send[...] = total
        k_dec = (k_rate * shrink).astype(BF16)
        k_end = (k_rate * remain).astype(BF16)
        loads[1].wait()
        q = q_v[...].astype(F32)
        q_sig = 1.0 / (1.0 + jnp.exp(-q))
        query = q * q_sig
        q_dec = (query * growth).astype(BF16)
        loads[2].wait()
        go = go_v[...]
        reach = folded(nt(go, q_dec))
    with scope("values"):
        loads[3].wait()
        loads[4].wait()
        v = nt(w_v[...], x_v[...]).astype(BF16)
        update = folded(nt(v, k_end))
        s_send[...] = jnp.concatenate([update, reach], axis=0).reshape(s_send.shape).astype(BF16)

    with scope("barrier_wait"):
        pl.semaphore_wait(barrier, pln + nz - 1)
    with scope("send1"):
        sends = []
        for k in range(1, pln):
            to = lax.rem(me + k, pln)
            sends.append(rcopy(e_send, e_buf.at[me], e_ss.at[k], e_rs.at[me], plane(to)))
            sends.append(rcopy(s_send.at[to], s_buf.at[me], s_ss.at[k], s_rs.at[me], plane(to)))
            sends[-2].start()
            sends[-1].start()
        s_buf[me] = s_send[me]
        e_buf[me] = e_send[...]

    with scope("turn"):
        rows = d_model // (nz * ny * nx)
        per = tok // rows
        for b in range(d_model // tok):
            turned = x_v[:, tok * b : tok * (b + 1)].T
            for g in range(per):
                at = b * per + g
                zz, yy, xx = at // pln, (at // nx) % ny, at % nx
                xt[xx, pl.ds((yy * nz + zz) * rows, rows), :] = turned[rows * g : rows * (g + 1)]
        for k in range(1, nx):
            to = lax.rem(x + k, nx)
            copy = rcopy(xt.at[to], xtl.at[x], xt_ss.at[k], xt_rs.at[x], (z, y, to, c))
            copy.start()
            sends.append(copy)

    with scope("pairs_value"):
        mixing = [jnp.where(lower, tn(head_of(q_dec, h), head_of(k_dec, h)), 0.0).astype(BF16) for h in range(heads)]
        gv_own = by_head(nn(head_of(go, h), mixing[h]) for h in range(heads))

    with scope("wait1"):
        for k in range(1, pln):
            frm = lax.rem(me + k, pln)
            rcopy(e_send, e_buf.at[frm], e_ss.at[k], e_rs.at[frm], plane(frm)).wait_recv()
            rcopy(s_send.at[0], s_buf.at[frm], s_ss.at[k], s_rs.at[frm], plane(frm)).wait_recv()
    with scope("scan1"):
        held = jnp.zeros(t_send.shape, F32)
        factor = jnp.ones((1, ch), F32)
        for o in range(pln):
            it = o + back * (pln - 1 - 2 * o)
            l_buf[it] = held
            fl_buf[it] = factor
            decay = e_buf[it]
            held = decay * held + s_buf[it].astype(F32)
            factor = decay * factor
        t_send[...] = held.astype(BF16)
        ft_send[...] = factor

    z_order = z + back * (nz - 1 - 2 * z)

    def z_sends(k):
        at = z_order + k
        to = at + back * (nz - 1 - 2 * at)
        return (
            rcopy(ft_send, ft_buf.at[z], ft_ss.at[k], ft_rs.at[z], (to, y, x, c)),
            rcopy(t_send, t_buf.at[z], t_ss.at[k], t_rs.at[z], (to, y, x, c)),
        )

    with scope("send2"):
        for k in range(1, nz):

            @pl.when(z_order + k < nz)
            def _():
                for copy in z_sends(k):
                    copy.start()

    with scope("pairs_query"):
        pairing = [jnp.where(upper, tn(head_of(v, h), head_of(go, h)), 0.0).astype(BF16) for h in range(heads)]
        gq_own = by_head(nn(head_of(k_dec, h), pairing[h]) for h in range(heads))
        gk_own = by_head(nt(head_of(q_dec, h), pairing[h]) for h in range(heads))

    def arriving(o, carried):
        frm = o + back * (nz - 1 - 2 * o)
        rcopy(ft_send, ft_buf.at[frm], ft_ss.at[0], ft_rs.at[frm], (z, y, x, c)).wait_recv()
        rcopy(t_send, t_buf.at[frm], t_ss.at[0], t_rs.at[frm], (z, y, x, c)).wait_recv()
        return ft_buf[frm] * carried + t_buf[frm].astype(F32)

    with scope("wait2"):
        carried = lax.fori_loop(0, z_order, arriving, jnp.zeros(t_send.shape, F32))

    with scope("send3"):
        o_send[...] = (l_buf[...] + fl_buf[...] * carried[None]).astype(BF16)
        for k in range(1, pln):
            to = lax.rem(me + k, pln)
            copy = rcopy(o_send.at[to], p_buf.at[me], p_ss.at[k], p_rs.at[me], plane(to))
            copy.start()
            sends.append(copy)
        p_buf[me] = o_send[me]
    with scope("wait3"):
        for k in range(1, pln):
            frm = lax.rem(me + k, pln)
            rcopy(o_send.at[0], p_buf.at[frm], p_ss.at[k], p_rs.at[frm], plane(frm)).wait_recv()
    with scope("value_grad"):
        carries = p_buf[...].astype(F32).reshape(2 * HEAD, ch)
        state, grad = carries[:HEAD], carries[HEAD:]
        bd_state = by_head((state * m).astype(BF16) for m in mf)
        bd_grad = by_head((grad * m).astype(BF16) for m in mf)
        value_grad = (gv_own + nn(bd_grad, k_end)).astype(BF16)
        vg_v[...] = value_grad
        for k in range(1, nx):
            to = lax.rem(x + k, nx)
            copy = rcopy(vg_v, vgl.at[x], vg_ss.at[k], vg_rs.at[x], (z, y, to, c))
            copy.start()
            sends.append(copy)

    with scope("input_grad"):
        width = 512 if d_model % 512 == 0 else d_model
        turned = value_grad.T
        for j in range(d_model // width):
            cols = pl.ds(j * width, width)
            ig[:, :, cols] = nn(turned, w_v[:, cols]).astype(BF16).reshape(2, tok // 2, width)
        ig_copy = rcopy(ig.at[1 - c], ig_recv, ig_ss, ig_rs, (z, y, x, 1 - c))
        ig_copy.start()

    with scope("weight_own"):
        total_w = nt(xt[x], value_grad)
    for k in range(1, nx):
        frm = lax.rem(x + k, nx)
        with scope(f"wait_vg{k}"):
            rcopy(xt.at[0], xtl.at[frm], xt_ss.at[k], xt_rs.at[frm], (z, y, frm, c)).wait_recv()
            rcopy(vg_v, vgl.at[frm], vg_ss.at[k], vg_rs.at[frm], (z, y, frm, c)).wait_recv()
        total_w = total_w + nt(xtl[frm], vgl[frm])
    with scope("send_y"):
        acc[...] = total_w.reshape(acc.shape)
        y_send[...] = total_w.astype(BF16).reshape(y_send.shape)
        for k in range(1, ny):
            to = lax.rem(y + k, ny)
            copy = rcopy(y_send.at[to], y_recv.at[y], y_ss.at[k], y_rs.at[y], (z, to, x, c))
            copy.start()
            sends.append(copy)

    with scope("query_forget"):
        g_query = growth * (gq_own + tn(bd_state, go))
        g_key = shrink * gk_own + remain * tn(bd_grad, v)
        gq_out[...] = (g_query * (q_sig * (1.0 + q * (1.0 - q_sig)))).astype(BF16)
        ends = grad * (total * state + update)
        ends_high = ends.astype(BF16)
        ends_low = (ends - ends_high.astype(F32)).astype(BF16)
        tall_ones = jnp.ones((HEAD, tok), BF16)
        boundary = tn(ends_high, tall_ones) + tn(ends_low, tall_ones)
        flow = query * g_query - k_rate * g_key
        flow_high = flow.astype(BF16)
        flow_low = (flow - flow_high.astype(F32)).astype(BF16)
        g_decay = nn(flow_high, lower_ones) + nn(flow_low, lower_ones) + boundary
        gf_out[...] = ((g_decay / (1.0 - k_rate) - g_key) * k_rate * f_sig).astype(BF16)

    w_sum = acc[y]
    with scope("wait_y"):
        for k in range(1, ny):
            frm = lax.rem(y + k, ny)
            rcopy(y_send.at[0], y_recv.at[frm], y_ss.at[k], y_rs.at[frm], (z, frm, x, c)).wait_recv()
            w_sum = w_sum + y_recv[frm].astype(F32)
    with scope("send_z"):
        w2[...] = w_sum.reshape(w2.shape)
        z_send[...] = w_sum.astype(BF16).reshape(z_send.shape)
        for k in range(1, nz):
            to = lax.rem(z + k, nz)
            copy = rcopy(z_send.at[to], z_recv.at[z], z_ss.at[k], z_rs.at[z], (to, y, x, c))
            copy.start()
            sends.append(copy)
    with scope("input_sum"):
        ig_copy.wait_recv()
        gx_out[...] = (ig[c].astype(F32) + ig_recv[...].astype(F32)).astype(BF16)

    w_last = w2[z]
    with scope("wait_z"):
        for k in range(1, nz):
            frm = lax.rem(z + k, nz)
            rcopy(z_send.at[0], z_recv.at[frm], z_ss.at[k], z_rs.at[frm], (frm, y, x, c)).wait_recv()
            w_last = w_last + z_recv[frm].astype(F32)
        gw_out[...] = w_last

    with scope("drain"):
        for copy in sends:
            copy.wait_send()
        ig_copy.wait_send()
        for k in range(1, nz):

            @pl.when(z_order + k < nz)
            def _():
                for copy in z_sends(k):
                    copy.wait_send()


def on_device(nz, ny, nx, block_input, value_weight, query_pre, forget_pre, lower_bound, out_grad):
    tok, d_model = block_input.shape
    ch = value_weight.shape[1]
    pln = ny * nx
    piece = 2 * HEAD // pln
    rows = d_model // (nz * pln)
    vm, dma = pltpu.VMEM, pltpu.SemaphoreType.DMA
    scratch = [
        vm((tok, d_model), BF16), vm((ch, d_model), BF16),
        vm((ch, tok), BF16), vm((ch, tok), BF16), vm((ch, tok), BF16),
        vm((pln, piece, ch), BF16), vm((1, ch), F32),
        vm((pln, piece, ch), BF16), vm((pln, 1, ch), F32),
        vm((pln, piece, ch), F32), vm((pln, 1, ch), F32),
        vm((piece, ch), BF16), vm((1, ch), F32),
        vm((nz, piece, ch), BF16), vm((nz, 1, ch), F32),
        vm((pln, piece, ch), BF16), vm((pln, piece, ch), BF16),
        vm((nx, d_model // nx, tok), BF16), vm((nx, d_model // nx, tok), BF16),
        vm((ch, tok), BF16), vm((nx, ch, tok), BF16),
        vm((2, tok // 2, d_model), BF16), vm((tok // 2, d_model), BF16),
        vm((ny, nz * rows, ch), F32), vm((ny, nz * rows, ch), BF16), vm((ny, nz * rows, ch), BF16),
        vm((nz, rows, ch), F32), vm((nz, rows, ch), BF16), vm((nz, rows, ch), BF16),
        dma((5,)),
        dma((pln,)), dma((pln,)), dma((pln,)), dma((pln,)),
        dma((nz,)), dma((nz,)), dma((nz,)), dma((nz,)),
        dma((pln,)), dma((pln,)),
        dma((nx,)), dma((nx,)), dma((nx,)), dma((nx,)),
        dma((ny,)), dma((ny,)), dma((nz,)), dma((nz,)),
        dma, dma,
    ]
    hbm, near = pl.BlockSpec(memory_space=pl.ANY), pl.BlockSpec(memory_space=pltpu.VMEM)
    g_query, g_forget, g_input, g_weight = pl.pallas_call(
        functools.partial(kernel, nz, ny, nx),
        out_shape=(
            vm((ch, tok), BF16),
            vm((ch, tok), BF16),
            vm((tok // 2, d_model), BF16),
            vm((rows, ch), F32),
        ),
        in_specs=[hbm] * 5 + [near],
        out_specs=(near,) * 4,
        scratch_shapes=scratch,
        compiler_params=pltpu.CompilerParams(collective_id=0, has_side_effects=True),
    )(block_input, value_weight.T, query_pre.T, forget_pre.T, out_grad.T, lower_bound.reshape(1, ch))
    return g_query.T, g_forget.T, g_input, g_weight


def on_mesh(devices):
    nz, ny, nx = devices.shape[:3]
    split = Mesh(devices, SP_TP)
    in_specs = (P(SP, None), P(None, "tp"), P(SP, "tp"), P(SP, "tp"), P("tp"), P(SP, "tp"))
    out_specs = (P(SP, "tp"), P(SP, "tp"), P(SP_TP, None), P(SP, "tp"))
    return jax.shard_map(
        functools.partial(on_device, nz, ny, nx), mesh=split, in_specs=in_specs, out_specs=out_specs, check_vma=False
    )


def solution(mesh):
    return on_mesh(mesh.devices.reshape(8, 4, 4, mesh.shape["tp"]))
```

```python
import functools

import jax
import jax.numpy as jnp
from jax import lax
from jax.experimental import pallas as pl
from jax.experimental.pallas import tpu as pltpu
from jax.sharding import Mesh
from jax.sharding import PartitionSpec as P

HEAD = 64
SP = ("sp_0", "sp_1", "sp_2")
SP_TP = ("sp_0", "sp_1", "sp_2", "tp")
F32, BF16 = jnp.float32, jnp.bfloat16
LOGICAL = pl.DeviceIdType.MESH


def nn(a, b):
    return lax.dot_general(a, b, (((1,), (0,)), ((), ())), preferred_element_type=F32)


def nt(a, b):
    return lax.dot_general(a, b, (((1,), (1,)), ((), ())), preferred_element_type=F32)


def tn(a, b):
    return lax.dot_general(a, b, (((0,), (0,)), ((), ())), preferred_element_type=F32)


def rcopy(src, dst, send, recv, device):
    return pltpu.make_async_remote_copy(
        src_ref=src, dst_ref=dst, send_sem=send, recv_sem=recv, device_id=device, device_id_type=LOGICAL
    )


def kernel(
    nz, ny, nx,
    x_hbm, w_hbm, q_hbm, f_hbm, go_hbm, lb_hbm,
    gq_out, gf_out, gx_out, gw_out,
    x_v, w_v, q_v, f_v, go_v, lb_v,
    s_send, e_send, s_buf, e_buf, l_buf, fl_buf, t_send, ft_send, t_buf, ft_buf, o_send, p_buf,
    xt, xtl, vg_v, vgl, ig, ig_recv, acc, y_send, y_recv, w2, z_send, z_recv,
    lsem, s_ss, s_rs, e_ss, e_rs, t_ss, t_rs, ft_ss, ft_rs, p_ss, p_rs,
    xt_ss, xt_rs, vg_ss, vg_rs, y_ss, y_rs, z_ss, z_rs, ig_ss, ig_rs,
):
    pln = ny * nx
    tok, d_model = x_v.shape
    ch = w_v.shape[0]
    heads = ch // HEAD
    z, y, x, c = (lax.axis_index(a) for a in SP_TP)
    me = y * nx + x
    back = (me * 2) // pln

    def plane(i):
        return (z, i // nx, lax.rem(i, nx), c)

    def head_of(a, h):
        return a[HEAD * h : HEAD * (h + 1)]

    def by_head(parts):
        return jnp.concatenate(list(parts), axis=0)

    scope = jax.named_scope
    with scope("loads_barrier"):
        loads = [
            pltpu.make_async_copy(src, dst, lsem.at[k])
            for k, (src, dst) in enumerate(
                ((f_hbm, f_v), (q_hbm, q_v), (go_hbm, go_v), (x_hbm, x_v), (w_hbm, w_v), (lb_hbm, lb_v))
            )
        ]
        for copy in loads:
            copy.start()
        barrier = pltpu.get_barrier_semaphore()
        for k in range(1, pln):
            pl.semaphore_signal(barrier, inc=1, device_id=plane(lax.rem(me + k, pln)), device_id_type=LOGICAL)
        for k in range(1, nz):
            pl.semaphore_signal(barrier, inc=1, device_id=(lax.rem(z + k, nz), y, x, c), device_id_type=LOGICAL)
        pl.semaphore_signal(barrier, inc=1, device_id=(z, y, x, 1 - c), device_id_type=LOGICAL)

    lane = lax.broadcasted_iota(jnp.int32, (1, ch), 1)
    mf = [jnp.where((lane >= HEAD * h) & (lane < HEAD * (h + 1)), 1.0, 0.0).astype(F32) for h in range(heads)]
    row = lax.broadcasted_iota(jnp.int32, (tok, tok), 0)
    col = lax.broadcasted_iota(jnp.int32, (tok, tok), 1)
    lower, upper = row >= col, col >= row
    lower_ones = jnp.where(lower, 1.0, 0.0).astype(BF16)
    upper_ones = jnp.where(upper, 1.0, 0.0).astype(BF16)

    def folded(full):
        out = full[:HEAD] * mf[0]
        for h in range(1, heads):
            out = out + head_of(full, h) * mf[h]
        return out

    with scope("gates"):
        loads[5].wait()
        gap = jnp.broadcast_to(1.0 - lb_v[...], (tok, ch)).T
        loads[0].wait()
        f = f_v[...].astype(F32)
        f_neg = 1.0 / (1.0 + jnp.exp(f))
        f_sig = 1.0 / (1.0 + jnp.exp(-f))
        k_rate = gap * f_neg
        logs = jnp.log1p(-k_rate)
        high = logs.astype(BF16)
        low = (logs - high.astype(F32)).astype(BF16)
        cum = nn(high, upper_ones) + nn(low, upper_ones)
        row_ones = jnp.ones((8, tok), BF16)
        total = jnp.exp((nt(row_ones, high) + nt(row_ones, low))[:1])
        closing = cum[:, tok - 1 : tok]
        growth = jnp.exp(cum)
        shrink = jnp.exp(-cum)
        remain = jnp.exp(closing - cum)
        e_send[...] = total
        k_dec = (k_rate * shrink).astype(BF16)
        k_end = (k_rate * remain).astype(BF16)
        loads[1].wait()
        q = q_v[...].astype(F32)
        q_sig = 1.0 / (1.0 + jnp.exp(-q))
        query = q * q_sig
        q_dec = (query * growth).astype(BF16)
        loads[2].wait()
        go = go_v[...]
        reach = folded(nt(go, q_dec))
    with scope("values"):
        loads[3].wait()
        loads[4].wait()
        v = nt(w_v[...], x_v[...]).astype(BF16)
        update = folded(nt(v, k_end))
        s_send[...] = jnp.concatenate([update, reach], axis=0).reshape(s_send.shape).astype(BF16)

    with scope("barrier_wait"):
        pl.semaphore_wait(barrier, pln + nz - 1)
    with scope("send1"):
        sends = []
        for k in range(1, pln):
            to = lax.rem(me + k, pln)
            sends.append(rcopy(e_send, e_buf.at[me], e_ss.at[k], e_rs.at[me], plane(to)))
            sends.append(rcopy(s_send.at[to], s_buf.at[me], s_ss.at[k], s_rs.at[me], plane(to)))
            sends[-2].start()
            sends[-1].start()
        s_buf[me] = s_send[me]
        e_buf[me] = e_send[...]

    with scope("turn"):
        rows = d_model // (nz * ny * nx)
        per = tok // rows
        for b in range(d_model // tok):
            turned = x_v[:, tok * b : tok * (b + 1)].T
            for g in range(per):
                at = b * per + g
                zz, yy, xx = at // pln, (at // nx) % ny, at % nx
                xt[xx, pl.ds((yy * nz + zz) * rows, rows), :] = turned[rows * g : rows * (g + 1)]
        for k in range(1, nx):
            to = lax.rem(x + k, nx)
            copy = rcopy(xt.at[to], xtl.at[x], xt_ss.at[k], xt_rs.at[x], (z, y, to, c))
            copy.start()
            sends.append(copy)

    with scope("pairs_value"):
        mixing = [jnp.where(lower, tn(head_of(q_dec, h), head_of(k_dec, h)), 0.0).astype(BF16) for h in range(heads)]
        gv_own = by_head(nn(head_of(go, h), mixing[h]) for h in range(heads))

    with scope("wait1"):
        for k in range(1, pln):
            frm = lax.rem(me + k, pln)
            rcopy(e_send, e_buf.at[frm], e_ss.at[k], e_rs.at[frm], plane(frm)).wait_recv()
            rcopy(s_send.at[0], s_buf.at[frm], s_ss.at[k], s_rs.at[frm], plane(frm)).wait_recv()
    with scope("scan1"):
        held = jnp.zeros(t_send.shape, F32)
        factor = jnp.ones((1, ch), F32)
        for o in range(pln):
            it = o + back * (pln - 1 - 2 * o)
            l_buf[it] = held
            fl_buf[it] = factor
            decay = e_buf[it]
            held = decay * held + s_buf[it].astype(F32)
            factor = decay * factor
        t_send[...] = held.astype(BF16)
        ft_send[...] = factor

    z_order = z + back * (nz - 1 - 2 * z)

    def z_sends(k):
        at = z_order + k
        to = at + back * (nz - 1 - 2 * at)
        return (
            rcopy(ft_send, ft_buf.at[z], ft_ss.at[k], ft_rs.at[z], (to, y, x, c)),
            rcopy(t_send, t_buf.at[z], t_ss.at[k], t_rs.at[z], (to, y, x, c)),
        )

    with scope("send2"):
        for k in range(1, nz):

            @pl.when(z_order + k < nz)
            def _():
                for copy in z_sends(k):
                    copy.start()

    with scope("pairs_query"):
        pairing = [jnp.where(upper, tn(head_of(v, h), head_of(go, h)), 0.0).astype(BF16) for h in range(heads)]
        gq_own = by_head(nn(head_of(k_dec, h), pairing[h]) for h in range(heads))
        gk_own = by_head(nt(head_of(q_dec, h), pairing[h]) for h in range(heads))

    def arriving(o, carried):
        frm = o + back * (nz - 1 - 2 * o)
        rcopy(ft_send, ft_buf.at[frm], ft_ss.at[0], ft_rs.at[frm], (z, y, x, c)).wait_recv()
        rcopy(t_send, t_buf.at[frm], t_ss.at[0], t_rs.at[frm], (z, y, x, c)).wait_recv()
        return ft_buf[frm] * carried + t_buf[frm].astype(F32)

    with scope("wait2"):
        carried = lax.fori_loop(0, z_order, arriving, jnp.zeros(t_send.shape, F32))

    with scope("send3"):
        o_send[...] = (l_buf[...] + fl_buf[...] * carried[None]).astype(BF16)
        for k in range(1, pln):
            to = lax.rem(me + k, pln)
            copy = rcopy(o_send.at[to], p_buf.at[me], p_ss.at[k], p_rs.at[me], plane(to))
            copy.start()
            sends.append(copy)
        p_buf[me] = o_send[me]
    with scope("wait3"):
        for k in range(1, pln):
            frm = lax.rem(me + k, pln)
            rcopy(o_send.at[0], p_buf.at[frm], p_ss.at[k], p_rs.at[frm], plane(frm)).wait_recv()
    with scope("value_grad"):
        carries = p_buf[...].astype(F32).reshape(2 * HEAD, ch)
        state, grad = carries[:HEAD], carries[HEAD:]
        bd_state = by_head((state * m).astype(BF16) for m in mf)
        bd_grad = by_head((grad * m).astype(BF16) for m in mf)
        value_grad = (gv_own + nn(bd_grad, k_end)).astype(BF16)
        vg_v[...] = value_grad
        for k in range(1, nx):
            to = lax.rem(x + k, nx)
            copy = rcopy(vg_v, vgl.at[x], vg_ss.at[k], vg_rs.at[x], (z, y, to, c))
            copy.start()
            sends.append(copy)

    with scope("input_grad"):
        width = 512 if d_model % 512 == 0 else d_model
        turned = value_grad.T
        for j in range(d_model // width):
            cols = pl.ds(j * width, width)
            ig[:, :, cols] = nn(turned, w_v[:, cols]).astype(BF16).reshape(2, tok // 2, width)
        ig_copy = rcopy(ig.at[1 - c], ig_recv, ig_ss, ig_rs, (z, y, x, 1 - c))
        ig_copy.start()

    with scope("weight_own"):
        total_w = nt(xt[x], value_grad)
    for k in range(1, nx):
        frm = lax.rem(x + k, nx)
        with scope(f"wait_vg{k}"):
            rcopy(xt.at[0], xtl.at[frm], xt_ss.at[k], xt_rs.at[frm], (z, y, frm, c)).wait_recv()
            rcopy(vg_v, vgl.at[frm], vg_ss.at[k], vg_rs.at[frm], (z, y, frm, c)).wait_recv()
        total_w = total_w + nt(xtl[frm], vgl[frm])
    with scope("send_y"):
        acc[...] = total_w.reshape(acc.shape)
        y_send[...] = total_w.astype(BF16).reshape(y_send.shape)
        for k in range(1, ny):
            to = lax.rem(y + k, ny)
            copy = rcopy(y_send.at[to], y_recv.at[y], y_ss.at[k], y_rs.at[y], (z, to, x, c))
            copy.start()
            sends.append(copy)

    with scope("query_forget"):
        g_query = growth * (gq_own + tn(bd_state, go))
        g_key = shrink * gk_own + remain * tn(bd_grad, v)
        gq_out[...] = (g_query * (q_sig * (1.0 + q * (1.0 - q_sig)))).astype(BF16)
        ends = grad * (total * state + update)
        ends_high = ends.astype(BF16)
        ends_low = (ends - ends_high.astype(F32)).astype(BF16)
        tall_ones = jnp.ones((HEAD, tok), BF16)
        boundary = tn(ends_high, tall_ones) + tn(ends_low, tall_ones)
        flow = query * g_query - k_rate * g_key
        flow_high = flow.astype(BF16)
        flow_low = (flow - flow_high.astype(F32)).astype(BF16)
        g_decay = nn(flow_high, lower_ones) + nn(flow_low, lower_ones) + boundary
        gf_out[...] = ((g_decay / (1.0 - k_rate) - g_key) * k_rate * f_sig).astype(BF16)

    w_sum = acc[y]
    with scope("wait_y"):
        for k in range(1, ny):
            frm = lax.rem(y + k, ny)
            rcopy(y_send.at[0], y_recv.at[frm], y_ss.at[k], y_rs.at[frm], (z, frm, x, c)).wait_recv()
            w_sum = w_sum + y_recv[frm].astype(F32)
    with scope("send_z"):
        w2[...] = w_sum.reshape(w2.shape)
        z_send[...] = w_sum.astype(BF16).reshape(z_send.shape)
        for k in range(1, nz):
            to = lax.rem(z + k, nz)
            copy = rcopy(z_send.at[to], z_recv.at[z], z_ss.at[k], z_rs.at[z], (to, y, x, c))
            copy.start()
            sends.append(copy)
    with scope("input_sum"):
        ig_copy.wait_recv()
        gx_out[...] = (ig[c].astype(F32) + ig_recv[...].astype(F32)).astype(BF16)

    w_last = w2[z]
    with scope("wait_z"):
        for k in range(1, nz):
            frm = lax.rem(z + k, nz)
            rcopy(z_send.at[0], z_recv.at[frm], z_ss.at[k], z_rs.at[frm], (frm, y, x, c)).wait_recv()
            w_last = w_last + z_recv[frm].astype(F32)
        gw_out[...] = w_last

    with scope("drain"):
        for copy in sends:
            copy.wait_send()
        ig_copy.wait_send()
        for k in range(1, nz):

            @pl.when(z_order + k < nz)
            def _():
                for copy in z_sends(k):
                    copy.wait_send()


def write_out(*refs):
    copies = [pltpu.make_async_copy(refs[k], refs[4 + k], refs[8].at[k]) for k in range(4)]
    for copy in copies:
        copy.start()
    for copy in copies:
        copy.wait()


def on_device(nz, ny, nx, block_input, value_weight, query_pre, forget_pre, lower_bound, out_grad):
    tok, d_model = block_input.shape
    ch = value_weight.shape[1]
    pln = ny * nx
    piece = 2 * HEAD // pln
    rows = d_model // (nz * pln)
    vm, dma = pltpu.VMEM, pltpu.SemaphoreType.DMA
    scratch = [
        vm((tok, d_model), BF16), vm((ch, d_model), BF16),
        vm((ch, tok), BF16), vm((ch, tok), BF16), vm((ch, tok), BF16), vm((1, ch), F32),
        vm((pln, piece, ch), BF16), vm((1, ch), F32),
        vm((pln, piece, ch), BF16), vm((pln, 1, ch), F32),
        vm((pln, piece, ch), F32), vm((pln, 1, ch), F32),
        vm((piece, ch), BF16), vm((1, ch), F32),
        vm((nz, piece, ch), BF16), vm((nz, 1, ch), F32),
        vm((pln, piece, ch), BF16), vm((pln, piece, ch), BF16),
        vm((nx, d_model // nx, tok), BF16), vm((nx, d_model // nx, tok), BF16),
        vm((ch, tok), BF16), vm((nx, ch, tok), BF16),
        vm((2, tok // 2, d_model), BF16), vm((tok // 2, d_model), BF16),
        vm((ny, nz * rows, ch), F32), vm((ny, nz * rows, ch), BF16), vm((ny, nz * rows, ch), BF16),
        vm((nz, rows, ch), F32), vm((nz, rows, ch), BF16), vm((nz, rows, ch), BF16),
        dma((6,)),
        dma((pln,)), dma((pln,)), dma((pln,)), dma((pln,)),
        dma((nz,)), dma((nz,)), dma((nz,)), dma((nz,)),
        dma((pln,)), dma((pln,)),
        dma((nx,)), dma((nx,)), dma((nx,)), dma((nx,)),
        dma((ny,)), dma((ny,)), dma((nz,)), dma((nz,)),
        dma, dma,
    ]
    hbm, near = pl.BlockSpec(memory_space=pl.ANY), pl.BlockSpec(memory_space=pltpu.VMEM)
    results = pl.pallas_call(
        functools.partial(kernel, nz, ny, nx),
        out_shape=(
            vm((ch, tok), BF16),
            vm((ch, tok), BF16),
            vm((tok // 2, d_model), BF16),
            vm((rows, ch), F32),
        ),
        in_specs=[hbm] * 6,
        out_specs=(near,) * 4,
        scratch_shapes=scratch,
        compiler_params=pltpu.CompilerParams(collective_id=0, has_side_effects=True),
    )(block_input, value_weight.T, query_pre.T, forget_pre.T, out_grad.T, lower_bound.reshape(1, ch))
    g_query, g_forget, g_input, g_weight = pl.pallas_call(
        write_out,
        out_shape=tuple(jax.ShapeDtypeStruct(a.shape, a.dtype) for a in results),
        in_specs=[near] * 4,
        out_specs=(hbm,) * 4,
        scratch_shapes=[dma((4,))],
    )(*(pltpu.with_memory_space_constraint(a, pltpu.VMEM) for a in results))
    return g_query.T, g_forget.T, g_input, g_weight


def on_mesh(devices):
    nz, ny, nx = devices.shape[:3]
    split = Mesh(devices, SP_TP)
    in_specs = (P(SP, None), P(None, "tp"), P(SP, "tp"), P(SP, "tp"), P("tp"), P(SP, "tp"))
    out_specs = (P(SP, "tp"), P(SP, "tp"), P(SP_TP, None), P(SP, "tp"))
    return jax.shard_map(
        functools.partial(on_device, nz, ny, nx), mesh=split, in_specs=in_specs, out_specs=out_specs, check_vma=False
    )


def solution(mesh):
    return on_mesh(mesh.devices.reshape(8, 4, 4, mesh.shape["tp"]))
```

```python
import functools

import jax
import jax.numpy as jnp
from jax import lax
from jax.experimental import pallas as pl
from jax.experimental.pallas import tpu as pltpu
from jax.sharding import Mesh
from jax.sharding import PartitionSpec as P

HEAD = 64
SP = ("sp_0", "sp_1", "sp_2")
SP_TP = ("sp_0", "sp_1", "sp_2", "tp")
F32, BF16 = jnp.float32, jnp.bfloat16
LOGICAL = pl.DeviceIdType.MESH


def nn(a, b):
    return lax.dot_general(a, b, (((1,), (0,)), ((), ())), preferred_element_type=F32)


def nt(a, b):
    return lax.dot_general(a, b, (((1,), (1,)), ((), ())), preferred_element_type=F32)


def tn(a, b):
    return lax.dot_general(a, b, (((0,), (0,)), ((), ())), preferred_element_type=F32)


def rcopy(src, dst, send, recv, device):
    return pltpu.make_async_remote_copy(
        src_ref=src, dst_ref=dst, send_sem=send, recv_sem=recv, device_id=device, device_id_type=LOGICAL
    )


def kernel(
    nz, ny, nx,
    x_hbm, w_hbm, q_hbm, f_hbm, go_hbm, lb_hbm,
    gq_out, gf_out, gx_out, gw_out,
    x_v, w_v, q_v, f_v, go_v, lb_v,
    s_send, e_send, s_buf, e_buf, l_buf, l_send, q_buf, t_send, ft_send, t_buf, ft_buf, o_send, p_buf,
    xt, xtl, r_send, rl, k_send, kl, own_send, ownl, ig, ig_recv,
    m_send, m_recv, aacc, a_send, a_recv, w2, z_send, z_recv,
    lsem, s_ss, s_rs, e_ss, e_rs, q_ss, q_rs, t_ss, t_rs, ft_ss, ft_rs, p_ss, p_rs,
    xt_ss, xt_rs, xd_ss, xd_rs, r_ss, r_rs, k_ss, k_rs, own_ss, own_rs,
    m_ss, m_rs, a_ss, a_rs, z_ss, z_rs, ig_ss, ig_rs,
):
    pln = ny * nx
    tok, d_model = x_v.shape
    ch = w_v.shape[0]
    heads = ch // HEAD
    z, y, x, c = (lax.axis_index(a) for a in SP_TP)
    me = y * nx + x
    back = (me * 2) // pln

    def plane(i):
        return (z, i // nx, lax.rem(i, nx), c)

    def head_of(a, h):
        return a[HEAD * h : HEAD * (h + 1)]

    def by_head(parts):
        return jnp.concatenate(list(parts), axis=0)

    scope = jax.named_scope
    with scope("loads_barrier"):
        loads = [
            pltpu.make_async_copy(src, dst, lsem.at[k])
            for k, (src, dst) in enumerate(
                ((f_hbm, f_v), (q_hbm, q_v), (go_hbm, go_v), (x_hbm, x_v), (w_hbm, w_v), (lb_hbm, lb_v))
            )
        ]
        for copy in loads:
            copy.start()
        barrier = pltpu.get_barrier_semaphore()
        for k in range(1, pln):
            pl.semaphore_signal(barrier, inc=1, device_id=plane(lax.rem(me + k, pln)), device_id_type=LOGICAL)
        for k in range(1, nz):
            pl.semaphore_signal(barrier, inc=1, device_id=(lax.rem(z + k, nz), y, x, c), device_id_type=LOGICAL)
        pl.semaphore_signal(barrier, inc=1, device_id=(z, y, x, 1 - c), device_id_type=LOGICAL)

    lane = lax.broadcasted_iota(jnp.int32, (1, ch), 1)
    mf = [jnp.where((lane >= HEAD * h) & (lane < HEAD * (h + 1)), 1.0, 0.0).astype(F32) for h in range(heads)]
    row = lax.broadcasted_iota(jnp.int32, (tok, tok), 0)
    col = lax.broadcasted_iota(jnp.int32, (tok, tok), 1)
    lower, upper = row >= col, col >= row
    lower_ones = jnp.where(lower, 1.0, 0.0).astype(BF16)
    upper_ones = jnp.where(upper, 1.0, 0.0).astype(BF16)

    def folded(full):
        out = full[:HEAD] * mf[0]
        for h in range(1, heads):
            out = out + head_of(full, h) * mf[h]
        return out

    with scope("gates"):
        loads[5].wait()
        gap = jnp.broadcast_to(1.0 - lb_v[...], (tok, ch)).T
        loads[0].wait()
        f = f_v[...].astype(F32)
        f_neg = 1.0 / (1.0 + jnp.exp(f))
        f_sig = 1.0 / (1.0 + jnp.exp(-f))
        k_rate = gap * f_neg
        logs = jnp.log1p(-k_rate)
        high = logs.astype(BF16)
        low = (logs - high.astype(F32)).astype(BF16)
        cum = nn(high, upper_ones) + nn(low, upper_ones)
        row_ones = jnp.ones((8, tok), BF16)
        total = jnp.exp((nt(row_ones, high) + nt(row_ones, low))[:1])
        closing = cum[:, tok - 1 : tok]
        growth = jnp.exp(cum)
        shrink = jnp.exp(-cum)
        remain = jnp.exp(closing - cum)
        e_send[...] = total
        k_dec = (k_rate * shrink).astype(BF16)
        k_end = (k_rate * remain).astype(BF16)
        loads[1].wait()
        q = q_v[...].astype(F32)
        q_sig = 1.0 / (1.0 + jnp.exp(-q))
        query = q * q_sig
        q_dec = (query * growth).astype(BF16)
        loads[2].wait()
        go = go_v[...]
        reach = folded(nt(go, q_dec))
    with scope("values"):
        loads[3].wait()
        loads[4].wait()
        v = nt(w_v[...], x_v[...]).astype(BF16)
        update = folded(nt(v, k_end))
        s_send[...] = jnp.concatenate([update, reach], axis=0).reshape(s_send.shape).astype(BF16)
        r_send[...] = reach.astype(BF16)
        k_send[...] = k_end

    with scope("turn"):
        rows = d_model // (nz * ny * nx)
        per = tok // rows
        half = xt.shape[2]
        for b in range(d_model // tok):
            turned = x_v[:, tok * b : tok * (b + 1)].T
            for g in range(per):
                at = b * per + g
                zz, yy, xx = at // pln, (at // nx) % ny, at % nx
                into = (yy * nz + zz) * rows
                xt[xx, into // half, pl.ds(into % half, rows), :] = turned[rows * g : rows * (g + 1)]

    with scope("barrier_wait"):
        pl.semaphore_wait(barrier, pln + nz - 1)

    sends = []

    def start(copy):
        copy.start()
        sends.append(copy)

    def to_line(source, target, send_sem, recv_sem):
        for k in range(1, nx):
            start(rcopy(source, target.at[x], send_sem.at[k], recv_sem.at[x], (z, y, lax.rem(x + k, nx), c)))

    def from_line(source, target, send_sem, recv_sem):
        for k in range(1, nx):
            frm = lax.rem(x + k, nx)
            rcopy(source, target.at[frm], send_sem.at[k], recv_sem.at[frm], (z, y, frm, c)).wait_recv()

    def to_column(source, target, send_sem, recv_sem):
        for k in range(1, ny):
            to = lax.rem(y + k, ny)
            start(rcopy(source.at[to], target.at[y], send_sem.at[k], recv_sem.at[y], (z, to, x, c)))

    def from_column(own, source, target, send_sem, recv_sem):
        out = own[...].astype(F32)
        for k in range(1, ny):
            frm = lax.rem(y + k, ny)
            rcopy(source.at[0], target.at[frm], send_sem.at[k], recv_sem.at[frm], (z, frm, x, c)).wait_recv()
            out = out + target[frm].astype(F32)
        return out

    with scope("send1"):
        for k in range(1, pln):
            to = lax.rem(me + k, pln)
            start(rcopy(e_send, e_buf.at[me], e_ss.at[k], e_rs.at[me], plane(to)))
            start(rcopy(s_send.at[to], s_buf.at[me], s_ss.at[k], s_rs.at[me], plane(to)))
        for k in range(1, nx):
            to = lax.rem(x + k, nx)
            start(rcopy(xt.at[to, c], xtl.at[x, c], xt_ss.at[k], xt_rs.at[x], (z, y, to, c)))
        to_line(k_send, kl, k_ss, k_rs)
        to_line(r_send, rl, r_ss, r_rs)
        s_buf[me] = s_send[me]
        e_buf[me] = e_send[...]
        xtl[x] = xt[x]
        kl[x] = k_end
        rl[x] = r_send[...]

    with scope("pairs_value"):
        mixing = [jnp.where(lower, tn(head_of(q_dec, h), head_of(k_dec, h)), 0.0).astype(BF16) for h in range(heads)]
        gv_own = by_head(nn(head_of(go, h), mixing[h]) for h in range(heads))
        own_send[...] = gv_own.astype(BF16)
        ownl[x] = own_send[...]

    with scope("wait1"):
        for k in range(1, pln):
            frm = lax.rem(me + k, pln)
            rcopy(e_send, e_buf.at[frm], e_ss.at[k], e_rs.at[frm], plane(frm)).wait_recv()
            rcopy(s_send.at[0], s_buf.at[frm], s_ss.at[k], s_rs.at[frm], plane(frm)).wait_recv()
    with scope("scan1"):
        held = jnp.zeros(t_send.shape, F32)
        factor = jnp.ones((1, ch), F32)
        for o in range(pln):
            it = o + back * (pln - 1 - 2 * o)
            l_buf[it] = held
            decay = e_buf[it]
            held = decay * held + s_buf[it].astype(F32)
            factor = decay * factor
        t_send[...] = held.astype(BF16)
        ft_send[...] = factor

    z_order = z + back * (nz - 1 - 2 * z)

    def z_sends(k):
        at = z_order + k
        to = at + back * (nz - 1 - 2 * at)
        return (
            rcopy(ft_send, ft_buf.at[z], ft_ss.at[k], ft_rs.at[z], (to, y, x, c)),
            rcopy(t_send, t_buf.at[z], t_ss.at[k], t_rs.at[z], (to, y, x, c)),
        )

    with scope("send2"):
        for k in range(1, nz):

            @pl.when(z_order + k < nz)
            def _():
                for copy in z_sends(k):
                    copy.start()

        l_send[...] = l_buf[...].astype(BF16)

        def within(i):
            return i + back * ((i // nx) * nx + nx - 1 - i)

        for k in range(1, pln):
            to = lax.rem(me + k, pln)
            start(rcopy(l_send.at[within(to)], q_buf.at[me], q_ss.at[k], q_rs.at[me], plane(to)))
        q_buf[me] = l_send[within(me)]
        to_line(own_send, ownl, own_ss, own_rs)

    with scope("pairs_query"):
        pairing = [jnp.where(upper, tn(head_of(v, h), head_of(go, h)), 0.0).astype(BF16) for h in range(heads)]
        gq_own = by_head(nn(head_of(k_dec, h), pairing[h]) for h in range(heads))
        gk_own = by_head(nt(head_of(q_dec, h), pairing[h]) for h in range(heads))

    def swaps(k, part):
        frm = lax.rem(x + k, nx)
        return rcopy(xtl.at[frm, part], xtl.at[frm, part], xd_ss.at[k], xd_rs.at[frm], (z, y, x, 1 - c))

    with scope("swap"):
        for k in range(1, nx):
            frm = lax.rem(x + k, nx)
            rcopy(xt.at[0, c], xtl.at[frm, c], xt_ss.at[k], xt_rs.at[frm], (z, y, frm, c)).wait_recv()
            start(swaps(k, c))

    def arriving(o, carried):
        frm = o + back * (nz - 1 - 2 * o)
        rcopy(ft_send, ft_buf.at[frm], ft_ss.at[0], ft_rs.at[frm], (z, y, x, c)).wait_recv()
        rcopy(t_send, t_buf.at[frm], t_ss.at[0], t_rs.at[frm], (z, y, x, c)).wait_recv()
        return ft_buf[frm] * carried + t_buf[frm].astype(F32)

    with scope("wait2"):
        carried = lax.fori_loop(0, z_order, arriving, jnp.zeros(t_send.shape, F32))

    with scope("send3"):
        o_send[...] = carried.astype(BF16)
        for k in range(1, pln):
            start(rcopy(o_send, p_buf.at[me], p_ss.at[k], p_rs.at[me], plane(lax.rem(me + k, pln))))
        p_buf[me] = o_send[...]

    with scope("decays"):
        ones_row = jnp.ones((1, ch), F32)
        line_after, line_before = ones_row, ones_row
        for i in range(pln):
            line_after = line_after * jnp.where(i // nx > y, e_buf[i], 1.0)
            line_before = line_before * jnp.where(i < me, e_buf[i], 1.0)
        line_decay = [e_buf[y * nx + i] for i in range(nx)]
        after = [line_after] * nx
        for i in range(nx - 2, -1, -1):
            after[i] = after[i + 1] * line_decay[i + 1]

    with scope("wait_swap"):
        from_line(k_send, kl, k_ss, k_rs)
        for k in range(1, nx):
            swaps(k, 1 - c).wait_recv()
    with scope("line_m"):
        all_rows = d_model // nx
        turned_of = [xtl[i].reshape(all_rows, tok) for i in range(nx)]
        m_sum = nt(turned_of[0], kl[0]) * after[0]
        for i in range(1, nx):
            m_sum = m_sum + nt(turned_of[i], kl[i]) * after[i]
        m_sum = m_sum.reshape(ny, nz * rows, ch)
        m_send[...] = m_sum.astype(BF16)
        to_column(m_send, m_recv, m_ss, m_rs)

    with scope("wait_1b"):
        from_line(r_send, rl, r_ss, r_rs)
        for k in range(1, pln):
            frm = lax.rem(me + k, pln)
            rcopy(l_send.at[0], q_buf.at[frm], q_ss.at[k], q_rs.at[frm], plane(frm)).wait_recv()
        from_line(own_send, ownl, own_ss, own_rs)
    with scope("line_a"):
        inner = q_buf[...].astype(F32).reshape(2 * HEAD, ch)
        state_in, grad_at = inner[:HEAD], inner[HEAD:]
        grad_in = grad_at
        a_sum = None
        for i in range(nx - 1, -1, -1):
            if i < nx - 1:
                grad_at = line_decay[i + 1] * grad_at + rl[i + 1].astype(F32)
            grad_in = jnp.where(x == i, grad_at, grad_in)
            bd_in = by_head((grad_at * m).astype(BF16) for m in mf)
            part = (ownl[i].astype(F32) + nn(bd_in, kl[i])).astype(BF16)
            term = nt(turned_of[i], part)
            a_sum = term if a_sum is None else a_sum + term
        aacc[...] = a_sum.reshape(aacc.shape)
        a_send[...] = a_sum.astype(BF16).reshape(a_send.shape)
        to_column(a_send, a_recv, a_ss, a_rs)

    with scope("wait_m"):
        m_plane = from_column(m_send.at[y], m_send, m_recv, m_ss, m_rs).astype(BF16)
    with scope("wait3"):
        for k in range(1, pln):
            frm = lax.rem(me + k, pln)
            rcopy(o_send, p_buf.at[frm], p_ss.at[k], p_rs.at[frm], plane(frm)).wait_recv()
    with scope("wait_a"):
        a_plane = from_column(aacc.at[y], a_send, a_recv, a_ss, a_rs)
    with scope("send_z"):
        outer = p_buf[...].astype(F32).reshape(2 * HEAD, ch)
        state_out, grad_out = outer[:HEAD], outer[HEAD:]
        bd_out = by_head((grad_out * m).astype(BF16) for m in mf)
        w_sum = a_plane + nt(m_plane, bd_out)
        w2[...] = w_sum.reshape(w2.shape)
        z_send[...] = w_sum.astype(BF16).reshape(z_send.shape)
        for k in range(1, nz):
            to = lax.rem(z + k, nz)
            start(rcopy(z_send.at[to], z_recv.at[z], z_ss.at[k], z_rs.at[z], (to, y, x, c)))

    with scope("value_grad"):
        own_after = after[nx - 1]
        for i in range(nx - 1):
            own_after = jnp.where(x == i, after[i], own_after)
        state = state_in + line_before * state_out
        grad = grad_in + own_after * grad_out
        bd_state = by_head((state * m).astype(BF16) for m in mf)
        bd_grad = by_head((grad * m).astype(BF16) for m in mf)
        value_grad = (gv_own + nn(bd_grad, k_end)).astype(BF16)

    with scope("input_grad"):
        width = 512 if d_model % 512 == 0 else d_model
        turned = value_grad.T
        for j in range(d_model // width):
            cols = pl.ds(j * width, width)
            ig[:, :, cols] = nn(turned, w_v[:, cols]).astype(BF16).reshape(2, tok // 2, width)
        ig_copy = rcopy(ig.at[1 - c], ig_recv, ig_ss, ig_rs, (z, y, x, 1 - c))
        ig_copy.start()

    with scope("query_forget"):
        g_query = growth * (gq_own + tn(bd_state, go))
        g_key = shrink * gk_own + remain * tn(bd_grad, v)
        gq_out[...] = (g_query * (q_sig * (1.0 + q * (1.0 - q_sig)))).astype(BF16)
        ends = grad * (total * state + update)
        ends_high = ends.astype(BF16)
        ends_low = (ends - ends_high.astype(F32)).astype(BF16)
        tall_ones = jnp.ones((HEAD, tok), BF16)
        boundary = tn(ends_high, tall_ones) + tn(ends_low, tall_ones)
        flow = query * g_query - k_rate * g_key
        flow_high = flow.astype(BF16)
        flow_low = (flow - flow_high.astype(F32)).astype(BF16)
        g_decay = nn(flow_high, lower_ones) + nn(flow_low, lower_ones) + boundary
        gf_out[...] = ((g_decay / (1.0 - k_rate) - g_key) * k_rate * f_sig).astype(BF16)

    with scope("input_sum"):
        ig_copy.wait_recv()
        gx_out[...] = (ig[c].astype(F32) + ig_recv[...].astype(F32)).astype(BF16)

    with scope("wait_z"):
        w_last = w2[z]
        for k in range(1, nz):
            frm = lax.rem(z + k, nz)
            rcopy(z_send.at[0], z_recv.at[frm], z_ss.at[k], z_rs.at[frm], (frm, y, x, c)).wait_recv()
            w_last = w_last + z_recv[frm].astype(F32)
        gw_out[...] = w_last

    with scope("drain"):
        for copy in sends:
            copy.wait_send()
        ig_copy.wait_send()
        for k in range(1, nz):

            @pl.when(z_order + k < nz)
            def _():
                for copy in z_sends(k):
                    copy.wait_send()


def write_out(*refs):
    copies = [pltpu.make_async_copy(refs[k], refs[4 + k], refs[8].at[k]) for k in range(4)]
    for copy in copies:
        copy.start()
    for copy in copies:
        copy.wait()


def on_device(nz, ny, nx, block_input, value_weight, query_pre, forget_pre, lower_bound, out_grad):
    tok, d_model = block_input.shape
    ch = value_weight.shape[1]
    pln = ny * nx
    piece = 2 * HEAD // pln
    rows = d_model // (nz * pln)
    vm, dma = pltpu.VMEM, pltpu.SemaphoreType.DMA
    scratch = [
        vm((tok, d_model), BF16), vm((ch, d_model), BF16),
        vm((ch, tok), BF16), vm((ch, tok), BF16), vm((ch, tok), BF16), vm((1, ch), F32),
        vm((pln, piece, ch), BF16), vm((1, ch), F32),
        vm((pln, piece, ch), BF16), vm((pln, 1, ch), F32),
        vm((pln, piece, ch), F32), vm((pln, piece, ch), BF16), vm((pln, piece, ch), BF16),
        vm((piece, ch), BF16), vm((1, ch), F32),
        vm((nz, piece, ch), BF16), vm((nz, 1, ch), F32),
        vm((piece, ch), BF16), vm((pln, piece, ch), BF16),
        vm((nx, 2, d_model // nx // 2, tok), BF16), vm((nx, 2, d_model // nx // 2, tok), BF16),
        vm((HEAD, ch), BF16), vm((nx, HEAD, ch), BF16),
        vm((ch, tok), BF16), vm((nx, ch, tok), BF16),
        vm((ch, tok), BF16), vm((nx, ch, tok), BF16),
        vm((2, tok // 2, d_model), BF16), vm((tok // 2, d_model), BF16),
        vm((ny, nz * rows, ch), BF16), vm((ny, nz * rows, ch), BF16),
        vm((ny, nz * rows, ch), F32), vm((ny, nz * rows, ch), BF16), vm((ny, nz * rows, ch), BF16),
        vm((nz, rows, ch), F32), vm((nz, rows, ch), BF16), vm((nz, rows, ch), BF16),
        dma((6,)),
        dma((pln,)), dma((pln,)), dma((pln,)), dma((pln,)), dma((pln,)), dma((pln,)),
        dma((nz,)), dma((nz,)), dma((nz,)), dma((nz,)),
        dma((pln,)), dma((pln,)),
        *(dma((nx,)) for _ in range(10)),
        *(dma((ny,)) for _ in range(4)),
        dma((nz,)), dma((nz,)),
        dma, dma,
    ]
    hbm, near = pl.BlockSpec(memory_space=pl.ANY), pl.BlockSpec(memory_space=pltpu.VMEM)
    results = pl.pallas_call(
        functools.partial(kernel, nz, ny, nx),
        out_shape=(
            vm((ch, tok), BF16),
            vm((ch, tok), BF16),
            vm((tok // 2, d_model), BF16),
            vm((rows, ch), F32),
        ),
        in_specs=[hbm] * 6,
        out_specs=(near,) * 4,
        scratch_shapes=scratch,
        compiler_params=pltpu.CompilerParams(collective_id=0, has_side_effects=True),
    )(block_input, value_weight.T, query_pre.T, forget_pre.T, out_grad.T, lower_bound.reshape(1, ch))
    g_query, g_forget, g_input, g_weight = pl.pallas_call(
        write_out,
        out_shape=tuple(jax.ShapeDtypeStruct(a.shape, a.dtype) for a in results),
        in_specs=[near] * 4,
        out_specs=(hbm,) * 4,
        scratch_shapes=[dma((4,))],
    )(*(pltpu.with_memory_space_constraint(a, pltpu.VMEM) for a in results))
    return g_query.T, g_forget.T, g_input, g_weight


def on_mesh(devices):
    nz, ny, nx = devices.shape[:3]
    split = Mesh(devices, SP_TP)
    in_specs = (P(SP, None), P(None, "tp"), P(SP, "tp"), P(SP, "tp"), P("tp"), P(SP, "tp"))
    out_specs = (P(SP, "tp"), P(SP, "tp"), P(SP_TP, None), P(SP, "tp"))
    return jax.shard_map(
        functools.partial(on_device, nz, ny, nx), mesh=split, in_specs=in_specs, out_specs=out_specs, check_vma=False
    )


def solution(mesh):
    return on_mesh(mesh.devices.reshape(8, 4, 4, mesh.shape["tp"]))
```

```python
import functools

import jax
import jax.numpy as jnp
from jax import lax
from jax.experimental import pallas as pl
from jax.experimental.pallas import tpu as pltpu
from jax.sharding import Mesh
from jax.sharding import PartitionSpec as P

HEAD = 64
SP = ("sp_0", "sp_1", "sp_2")
SP_TP = ("sp_0", "sp_1", "sp_2", "tp")
F32, BF16 = jnp.float32, jnp.bfloat16
LOGICAL = pl.DeviceIdType.MESH


def nn(a, b):
    return lax.dot_general(a, b, (((1,), (0,)), ((), ())), preferred_element_type=F32)


def nt(a, b):
    return lax.dot_general(a, b, (((1,), (1,)), ((), ())), preferred_element_type=F32)


def tn(a, b):
    return lax.dot_general(a, b, (((0,), (0,)), ((), ())), preferred_element_type=F32)


def rcopy(src, dst, send, recv, device):
    return pltpu.make_async_remote_copy(
        src_ref=src, dst_ref=dst, send_sem=send, recv_sem=recv, device_id=device, device_id_type=LOGICAL
    )


def kernel(
    nz, ny, nx,
    x_hbm, w_hbm, q_hbm, f_hbm, go_hbm, lb_hbm,
    gq_out, gf_out, gx_out, gw_out,
    x_v, w_v, q_v, f_v, go_v, lb_v,
    s_send, e_send, s_buf, e_buf, l_send, q_state, q_grad, t_send, ft_send, t_buf, ft_buf, o_send, p_buf,
    xt, xtl, k_send, kl, own_send, ownl, ig, ig_recv,
    m_send, m_recv, aacc, a_send, a_recv, w2, z_send, z_recv,
    lsem, s_ss, s_rs, e_ss, e_rs, q_ss, q_rs, t_ss, t_rs, ft_ss, ft_rs, p_ss, p_rs,
    xt_ss, xt_rs, k_ss, k_rs, own_ss, own_rs,
    m_ss, m_rs, a_ss, a_rs, z_ss, z_rs, ig_ss, ig_rs,
):
    pln = ny * nx
    tok, d_model = x_v.shape
    ch = w_v.shape[0]
    heads = ch // HEAD
    z, y, x, c = (lax.axis_index(a) for a in SP_TP)
    me = y * nx + x
    back = lax.rem(me, 2)
    at_line, at_col = x * (1 - c) + y * c, y * (1 - c) + x * c

    def line(i):
        return (z, y * (1 - c) + i * c, i * (1 - c) + x * c, c)

    def column(i):
        return (z, i * (1 - c) + y * c, x * (1 - c) + i * c, c)

    def by_lines(i):
        return i * (1 - c) + (lax.rem(i, nx) * ny + i // nx) * c

    def piece_of(i):
        return i // 2 + lax.rem(i, 2) * (pln // 2)

    def plane(i):
        return (z, i // nx, lax.rem(i, nx), c)

    def head_of(a, h):
        return a[HEAD * h : HEAD * (h + 1)]

    def by_head(parts):
        return jnp.concatenate(list(parts), axis=0)

    scope = jax.named_scope
    with scope("loads_barrier"):
        loads = [
            pltpu.make_async_copy(src, dst, lsem.at[k])
            for k, (src, dst) in enumerate(
                ((f_hbm, f_v), (q_hbm, q_v), (go_hbm, go_v), (x_hbm, x_v), (w_hbm, w_v), (lb_hbm, lb_v))
            )
        ]
        for copy in loads:
            copy.start()
        barrier = pltpu.get_barrier_semaphore()
        for k in range(1, pln):
            pl.semaphore_signal(barrier, inc=1, device_id=plane(lax.rem(me + k, pln)), device_id_type=LOGICAL)
        for k in range(1, nz):
            pl.semaphore_signal(barrier, inc=1, device_id=(lax.rem(z + k, nz), y, x, c), device_id_type=LOGICAL)
        pl.semaphore_signal(barrier, inc=1, device_id=(z, y, x, 1 - c), device_id_type=LOGICAL)

    lane = lax.broadcasted_iota(jnp.int32, (1, ch), 1)
    mf = [jnp.where((lane >= HEAD * h) & (lane < HEAD * (h + 1)), 1.0, 0.0).astype(F32) for h in range(heads)]
    row = lax.broadcasted_iota(jnp.int32, (tok, tok), 0)
    col = lax.broadcasted_iota(jnp.int32, (tok, tok), 1)
    lower, upper = row >= col, col >= row
    lower_ones = jnp.where(lower, 1.0, 0.0).astype(BF16)
    upper_ones = jnp.where(upper, 1.0, 0.0).astype(BF16)

    def folded(full):
        out = full[:HEAD] * mf[0]
        for h in range(1, heads):
            out = out + head_of(full, h) * mf[h]
        return out

    with scope("gates"):
        loads[5].wait()
        gap = jnp.broadcast_to(1.0 - lb_v[...], (tok, ch)).T
        loads[0].wait()
        f = f_v[...].astype(F32)
        f_neg = 1.0 / (1.0 + jnp.exp(f))
        f_sig = 1.0 / (1.0 + jnp.exp(-f))
        k_rate = gap * f_neg
        logs = jnp.log1p(-k_rate)
        high = logs.astype(BF16)
        low = (logs - high.astype(F32)).astype(BF16)
        cum = nn(high, upper_ones) + nn(low, upper_ones)
        row_ones = jnp.ones((8, tok), BF16)
        total = jnp.exp((nt(row_ones, high) + nt(row_ones, low))[:1])
        closing = cum[:, tok - 1 : tok]
        growth = jnp.exp(cum)
        shrink = jnp.exp(-cum)
        remain = jnp.exp(closing - cum)
        e_send[...] = total
        k_dec = (k_rate * shrink).astype(BF16)
        k_end = (k_rate * remain).astype(BF16)
        loads[1].wait()
        q = q_v[...].astype(F32)
        q_sig = 1.0 / (1.0 + jnp.exp(-q))
        query = q * q_sig
        q_dec = (query * growth).astype(BF16)
        loads[2].wait()
        go = go_v[...]
        reach = folded(nt(go, q_dec))
    with scope("values"):
        loads[3].wait()
        loads[4].wait()
        v = nt(w_v[...], x_v[...]).astype(BF16)
        update = folded(nt(v, k_end))
        s_send[...] = jnp.concatenate([update, reach], axis=0).reshape(s_send.shape).astype(BF16)
        k_send[...] = k_end

    with scope("turn"):
        rows = d_model // (nz * ny * nx)
        per = tok // rows
        for b in range(d_model // tok):
            turned = x_v[:, tok * b : tok * (b + 1)].T
            for g in range(per):
                at = b * per + g
                zz, yy, xx = at // pln, (at // nx) % ny, at % nx
                group, into = xx * (1 - c) + yy * c, yy * (1 - c) + xx * c
                xt[group, into, zz] = turned[rows * g : rows * (g + 1)]

    with scope("barrier_wait"):
        pl.semaphore_wait(barrier, pln + nz - 1)

    sends = []

    def start(copy):
        copy.start()
        sends.append(copy)

    def to_line(source, target, send_sem, recv_sem):
        for k in range(1, nx):
            start(rcopy(source, target.at[at_line], send_sem.at[k], recv_sem.at[at_line], line(lax.rem(at_line + k, nx))))

    def from_line(source, target, send_sem, recv_sem):
        for k in range(1, nx):
            frm = lax.rem(at_line + k, nx)
            rcopy(source, target.at[frm], send_sem.at[k], recv_sem.at[frm], line(frm)).wait_recv()

    def to_column(source, target, send_sem, recv_sem):
        for k in range(1, ny):
            to = lax.rem(at_col + k, ny)
            start(rcopy(source.at[to], target.at[at_col], send_sem.at[k], recv_sem.at[at_col], column(to)))

    def from_column(own, source, target, send_sem, recv_sem):
        out = own[...].astype(F32)
        for k in range(1, ny):
            frm = lax.rem(at_col + k, ny)
            rcopy(source.at[0], target.at[frm], send_sem.at[k], recv_sem.at[frm], column(frm)).wait_recv()
            out = out + target[frm].astype(F32)
        return out

    with scope("send1"):
        for k in range(1, pln):
            to = lax.rem(me + k, pln)
            start(rcopy(e_send, e_buf.at[me], e_ss.at[k], e_rs.at[me], plane(to)))
            start(rcopy(s_send.at[piece_of(to)], s_buf.at[me], s_ss.at[k], s_rs.at[me], plane(to)))
        for k in range(1, nx):
            to = lax.rem(at_line + k, nx)
            start(rcopy(xt.at[to], xtl.at[at_line], xt_ss.at[k], xt_rs.at[at_line], line(to)))
        to_line(k_send, kl, k_ss, k_rs)
        s_buf[me] = s_send[piece_of(me)]
        e_buf[me] = e_send[...]
        xtl[at_line] = xt[at_line]
        kl[at_line] = k_end

    with scope("pairs_value"):
        mixing = [jnp.where(lower, tn(head_of(q_dec, h), head_of(k_dec, h)), 0.0).astype(BF16) for h in range(heads)]
        gv_own = by_head(nn(head_of(go, h), mixing[h]) for h in range(heads))
        own_send[...] = gv_own.astype(BF16)
        ownl[at_line] = own_send[...]

    with scope("wait1"):
        for k in range(1, pln):
            frm = lax.rem(me + k, pln)
            rcopy(e_send, e_buf.at[frm], e_ss.at[k], e_rs.at[frm], plane(frm)).wait_recv()
            rcopy(s_send.at[0], s_buf.at[frm], s_ss.at[k], s_rs.at[frm], plane(frm)).wait_recv()
    with scope("scan1"):
        held = jnp.zeros(t_send.shape, F32)
        factor = jnp.ones((1, ch), F32)
        for o in range(pln):
            it = o + back * (pln - 1 - 2 * o)
            l_send[by_lines(it)] = held.astype(BF16)
            decay = e_buf[it]
            held = decay * held + s_buf[it].astype(F32)
            factor = decay * factor
        t_send[...] = held.astype(BF16)
        ft_send[...] = factor

    z_order = z + back * (nz - 1 - 2 * z)

    def z_sends(k):
        at = z_order + k
        to = at + back * (nz - 1 - 2 * at)
        return (
            rcopy(ft_send, ft_buf.at[z], ft_ss.at[k], ft_rs.at[z], (to, y, x, c)),
            rcopy(t_send, t_buf.at[z], t_ss.at[k], t_rs.at[z], (to, y, x, c)),
        )

    def state_sends(k, to):
        return rcopy(l_send.at[by_lines(to)], q_state.at[me // 2], q_ss.at[k], q_rs.at[me], plane(to))

    def grad_sends(k, to):
        first = by_lines(to) // nx * nx
        return rcopy(l_send.at[pl.ds(first, nx)], q_grad.at[me // 2], q_ss.at[k], q_rs.at[me], plane(to))

    with scope("send2"):
        for k in range(1, nz):

            @pl.when(z_order + k < nz)
            def _():
                for copy in z_sends(k):
                    copy.start()

        for k in range(1, pln):
            to = lax.rem(me + k, pln)

            @pl.when(back == 0)
            def _():
                state_sends(k, to).start()

            @pl.when(back == 1)
            def _():
                grad_sends(k, to).start()

        @pl.when(back == 0)
        def _():
            q_state[me // 2] = l_send[by_lines(me)]

        @pl.when(back == 1)
        def _():
            q_grad[me // 2] = l_send[pl.ds(at_col * nx, nx)]

        to_line(own_send, ownl, own_ss, own_rs)

    with scope("pairs_query"):
        pairing = [jnp.where(upper, tn(head_of(v, h), head_of(go, h)), 0.0).astype(BF16) for h in range(heads)]
        gq_own = by_head(nn(head_of(k_dec, h), pairing[h]) for h in range(heads))
        gk_own = by_head(nt(head_of(q_dec, h), pairing[h]) for h in range(heads))

    with scope("decays"):
        before, after = jnp.ones((1, ch), F32), [jnp.ones((1, ch), F32)] * nx
        ids = [line(i)[1] * nx + line(i)[2] for i in range(nx)]
        for i in range(pln):
            before = before * jnp.where(i < me, e_buf[i], 1.0)
            after = [a * jnp.where(i > n, e_buf[i], 1.0) for a, n in zip(after, ids)]

    with scope("wait_line"):
        for k in range(1, nx):
            frm = lax.rem(at_line + k, nx)
            rcopy(xt.at[0], xtl.at[frm], xt_ss.at[k], xt_rs.at[frm], line(frm)).wait_recv()
        from_line(k_send, kl, k_ss, k_rs)
    with scope("line_m"):
        all_rows = d_model // nx
        turned_of = [xtl[i].reshape(all_rows, tok) for i in range(nx)]
        m_sum = nt(turned_of[0], kl[0]) * after[0]
        for i in range(1, nx):
            m_sum = m_sum + nt(turned_of[i], kl[i]) * after[i]
        m_send[...] = m_sum.reshape(ny, nz * rows, ch).astype(BF16)
        to_column(m_send, m_recv, m_ss, m_rs)

    def arriving(o, carried):
        frm = o + back * (nz - 1 - 2 * o)
        rcopy(ft_send, ft_buf.at[frm], ft_ss.at[0], ft_rs.at[frm], (z, y, x, c)).wait_recv()
        rcopy(t_send, t_buf.at[frm], t_ss.at[0], t_rs.at[frm], (z, y, x, c)).wait_recv()
        return ft_buf[frm] * carried + t_buf[frm].astype(F32)

    with scope("wait2"):
        carried = lax.fori_loop(0, z_order, arriving, jnp.zeros(t_send.shape, F32))

    with scope("send3"):
        o_send[...] = carried.astype(BF16)
        mine = piece_of(me)
        for k in range(1, pln):
            start(rcopy(o_send, p_buf.at[mine], p_ss.at[k], p_rs.at[mine], plane(lax.rem(me + k, pln))))
        p_buf[mine] = o_send[...]

    with scope("wait_1b"):
        for j in range(pln // 2):

            @pl.when(me != 2 * j)
            def _():
                rcopy(l_send.at[0], q_state.at[j], q_ss.at[0], q_rs.at[2 * j], plane(2 * j)).wait_recv()

            @pl.when(me != 2 * j + 1)
            def _():
                rcopy(
                    l_send.at[pl.ds(0, nx)], q_grad.at[j], q_ss.at[0], q_rs.at[2 * j + 1], plane(2 * j + 1)
                ).wait_recv()

        from_line(own_send, ownl, own_ss, own_rs)
    with scope("line_a"):
        state_in = q_state[...].astype(F32).reshape(HEAD, ch)
        a_sum, grad_in = None, None
        for i in range(nx):
            grad_at = q_grad[:, i].astype(F32).reshape(HEAD, ch)
            grad_in = grad_at if i == 0 else jnp.where(at_line == i, grad_at, grad_in)
            bd_in = by_head((grad_at * m).astype(BF16) for m in mf)
            part = (ownl[i].astype(F32) + nn(bd_in, kl[i])).astype(BF16)
            term = nt(turned_of[i], part)
            a_sum = term if a_sum is None else a_sum + term
        aacc[...] = a_sum.reshape(aacc.shape)
        a_send[...] = a_sum.astype(BF16).reshape(a_send.shape)
        to_column(a_send, a_recv, a_ss, a_rs)

    with scope("wait_m"):
        m_plane = from_column(m_send.at[at_col], m_send, m_recv, m_ss, m_rs).astype(BF16)
    with scope("wait3"):
        for k in range(1, pln):
            frm = lax.rem(me + k, pln)
            part = piece_of(frm)
            rcopy(o_send, p_buf.at[part], p_ss.at[k], p_rs.at[part], plane(frm)).wait_recv()
    with scope("wait_a"):
        a_plane = from_column(aacc.at[at_col], a_send, a_recv, a_ss, a_rs)
    with scope("send_z"):
        outer = p_buf[...].astype(F32).reshape(2 * HEAD, ch)
        state_out, grad_out = outer[:HEAD], outer[HEAD:]
        bd_out = by_head((grad_out * m).astype(BF16) for m in mf)
        w_sum = a_plane + nt(m_plane, bd_out)
        w2[...] = w_sum.reshape(w2.shape)
        z_send[...] = w_sum.astype(BF16).reshape(z_send.shape)
        for k in range(1, nz):
            to = lax.rem(z + k, nz)
            start(rcopy(z_send.at[to], z_recv.at[z], z_ss.at[k], z_rs.at[z], (to, y, x, c)))

    with scope("value_grad"):
        own_after = after[nx - 1]
        for i in range(nx - 1):
            own_after = jnp.where(at_line == i, after[i], own_after)
        state = state_in + before * state_out
        grad = grad_in + own_after * grad_out
        bd_state = by_head((state * m).astype(BF16) for m in mf)
        bd_grad = by_head((grad * m).astype(BF16) for m in mf)
        value_grad = (gv_own + nn(bd_grad, k_end)).astype(BF16)

    with scope("input_grad"):
        width = 512 if d_model % 512 == 0 else d_model
        turned = value_grad.T
        for j in range(d_model // width):
            cols = pl.ds(j * width, width)
            ig[:, :, cols] = nn(turned, w_v[:, cols]).astype(BF16).reshape(2, tok // 2, width)
        ig_copy = rcopy(ig.at[1 - c], ig_recv, ig_ss, ig_rs, (z, y, x, 1 - c))
        ig_copy.start()

    with scope("query_forget"):
        g_query = growth * (gq_own + tn(bd_state, go))
        g_key = shrink * gk_own + remain * tn(bd_grad, v)
        gq_out[...] = (g_query * (q_sig * (1.0 + q * (1.0 - q_sig)))).astype(BF16)
        ends = grad * (total * state + update)
        ends_high = ends.astype(BF16)
        ends_low = (ends - ends_high.astype(F32)).astype(BF16)
        tall_ones = jnp.ones((HEAD, tok), BF16)
        boundary = tn(ends_high, tall_ones) + tn(ends_low, tall_ones)
        flow = query * g_query - k_rate * g_key
        flow_high = flow.astype(BF16)
        flow_low = (flow - flow_high.astype(F32)).astype(BF16)
        g_decay = nn(flow_high, lower_ones) + nn(flow_low, lower_ones) + boundary
        gf_out[...] = ((g_decay / (1.0 - k_rate) - g_key) * k_rate * f_sig).astype(BF16)

    with scope("input_sum"):
        ig_copy.wait_recv()
        gx_out[...] = (ig[c].astype(F32) + ig_recv[...].astype(F32)).astype(BF16)

    with scope("wait_z"):
        w_last = w2[z]
        for k in range(1, nz):
            frm = lax.rem(z + k, nz)
            rcopy(z_send.at[0], z_recv.at[frm], z_ss.at[k], z_rs.at[frm], (frm, y, x, c)).wait_recv()
            w_last = w_last + z_recv[frm].astype(F32)
        gw_out[...] = w_last

    with scope("drain"):
        for copy in sends:
            copy.wait_send()
        ig_copy.wait_send()
        for k in range(1, pln):
            to = lax.rem(me + k, pln)

            @pl.when(back == 0)
            def _():
                state_sends(k, to).wait_send()

            @pl.when(back == 1)
            def _():
                grad_sends(k, to).wait_send()

        for k in range(1, nz):

            @pl.when(z_order + k < nz)
            def _():
                for copy in z_sends(k):
                    copy.wait_send()


def write_out(*refs):
    copies = [pltpu.make_async_copy(refs[k], refs[4 + k], refs[8].at[k]) for k in range(4)]
    for copy in copies:
        copy.start()
    for copy in copies:
        copy.wait()


def on_device(nz, ny, nx, block_input, value_weight, query_pre, forget_pre, lower_bound, out_grad):
    tok, d_model = block_input.shape
    ch = value_weight.shape[1]
    pln = ny * nx
    piece = 2 * HEAD // pln
    rows = d_model // (nz * pln)
    vm, dma = pltpu.VMEM, pltpu.SemaphoreType.DMA
    scratch = [
        vm((tok, d_model), BF16), vm((ch, d_model), BF16),
        vm((ch, tok), BF16), vm((ch, tok), BF16), vm((ch, tok), BF16), vm((1, ch), F32),
        vm((pln, piece, ch), BF16), vm((1, ch), F32),
        vm((pln, piece, ch), BF16), vm((pln, 1, ch), F32),
        vm((pln, piece, ch), BF16), vm((pln // 2, piece, ch), BF16), vm((pln // 2, nx, piece, ch), BF16),
        vm((piece, ch), BF16), vm((1, ch), F32),
        vm((nz, piece, ch), BF16), vm((nz, 1, ch), F32),
        vm((piece, ch), BF16), vm((pln, piece, ch), BF16),
        vm((nx, ny, nz, rows, tok), BF16), vm((nx, ny, nz, rows, tok), BF16),
        vm((ch, tok), BF16), vm((nx, ch, tok), BF16),
        vm((ch, tok), BF16), vm((nx, ch, tok), BF16),
        vm((2, tok // 2, d_model), BF16), vm((tok // 2, d_model), BF16),
        vm((ny, nz * rows, ch), BF16), vm((ny, nz * rows, ch), BF16),
        vm((ny, nz * rows, ch), F32), vm((ny, nz * rows, ch), BF16), vm((ny, nz * rows, ch), BF16),
        vm((nz, rows, ch), F32), vm((nz, rows, ch), BF16), vm((nz, rows, ch), BF16),
        dma((6,)),
        dma((pln,)), dma((pln,)), dma((pln,)), dma((pln,)), dma((pln,)), dma((pln,)),
        dma((nz,)), dma((nz,)), dma((nz,)), dma((nz,)),
        dma((pln,)), dma((pln,)),
        *(dma((nx,)) for _ in range(6)),
        *(dma((ny,)) for _ in range(4)),
        dma((nz,)), dma((nz,)),
        dma, dma,
    ]
    hbm, near = pl.BlockSpec(memory_space=pl.ANY), pl.BlockSpec(memory_space=pltpu.VMEM)
    results = pl.pallas_call(
        functools.partial(kernel, nz, ny, nx),
        out_shape=(
            vm((ch, tok), BF16),
            vm((ch, tok), BF16),
            vm((tok // 2, d_model), BF16),
            vm((rows, ch), F32),
        ),
        in_specs=[hbm] * 6,
        out_specs=(near,) * 4,
        scratch_shapes=scratch,
        compiler_params=pltpu.CompilerParams(collective_id=0, has_side_effects=True),
    )(block_input, value_weight.T, query_pre.T, forget_pre.T, out_grad.T, lower_bound.reshape(1, ch))
    g_query, g_forget, g_input, g_weight = pl.pallas_call(
        write_out,
        out_shape=tuple(jax.ShapeDtypeStruct(a.shape, a.dtype) for a in results),
        in_specs=[near] * 4,
        out_specs=(hbm,) * 4,
        scratch_shapes=[dma((4,))],
    )(*(pltpu.with_memory_space_constraint(a, pltpu.VMEM) for a in results))
    return g_query.T, g_forget.T, g_input, g_weight


def on_mesh(devices):
    nz, ny, nx = devices.shape[:3]
    split = Mesh(devices, SP_TP)
    in_specs = (P(SP, None), P(None, "tp"), P(SP, "tp"), P(SP, "tp"), P("tp"), P(SP, "tp"))
    out_specs = (P(SP, "tp"), P(SP, "tp"), P(SP_TP, None), P(SP, "tp"))
    return jax.shard_map(
        functools.partial(on_device, nz, ny, nx), mesh=split, in_specs=in_specs, out_specs=out_specs, check_vma=False
    )


def solution(mesh):
    return on_mesh(mesh.devices.reshape(8, 4, 4, mesh.shape["tp"]))
```

```python
import functools

import jax
import jax.numpy as jnp
from jax import lax
from jax.experimental import pallas as pl
from jax.experimental.pallas import tpu as pltpu
from jax.sharding import Mesh
from jax.sharding import PartitionSpec as P

HEAD = 64
SP = ("sp_0", "sp_1", "sp_2")
SP_TP = ("sp_0", "sp_1", "sp_2", "tp")
F32, BF16 = jnp.float32, jnp.bfloat16
LOGICAL = pl.DeviceIdType.MESH


def nn(a, b):
    return lax.dot_general(a, b, (((1,), (0,)), ((), ())), preferred_element_type=F32)


def nt(a, b):
    return lax.dot_general(a, b, (((1,), (1,)), ((), ())), preferred_element_type=F32)


def tn(a, b):
    return lax.dot_general(a, b, (((0,), (0,)), ((), ())), preferred_element_type=F32)


def rcopy(src, dst, send, recv, device):
    return pltpu.make_async_remote_copy(
        src_ref=src, dst_ref=dst, send_sem=send, recv_sem=recv, device_id=device, device_id_type=LOGICAL
    )


def kernel(
    nz, ny, nx,
    x_hbm, w_hbm, q_hbm, f_hbm, go_hbm, lb_hbm,
    gq_out, gf_out, gx_out, gw_out,
    x_v, w_v, q_v, f_v, go_v, lb_v,
    s_send, e_send, s_buf, e_buf, l_send, q_state, q_grad, q_line, t_send, ft_send, t_buf, ft_buf, o_send, p_buf,
    xt, xtl, r_send, rl, k_send, kl, own_send, ownl, g_all, ig, ig_recv,
    m_send, m_recv, aacc, a_send, a_recv, w2, z_send, z_recv,
    lsem, s_ss, s_rs, e_ss, e_rs, q_ss, q_rs, t_ss, t_rs, ft_ss, ft_rs, p_ss, p_rs,
    xt_ss, xt_rs, r_ss, r_rs, k_ss, k_rs, own_ss, own_rs,
    m_ss, m_rs, a_ss, a_rs, z_ss, z_rs, ig_ss, ig_rs,
):
    pln = ny * nx
    tok, d_model = x_v.shape
    ch = w_v.shape[0]
    heads = ch // HEAD
    z, y, x, c = (lax.axis_index(a) for a in SP_TP)
    me = y * nx + x
    back = lax.rem(me, 2)
    at_line, at_col = x * (1 - c) + y * c, y * (1 - c) + x * c

    def line(i):
        return (z, y * (1 - c) + i * c, i * (1 - c) + x * c, c)

    def column(i):
        return (z, i * (1 - c) + y * c, x * (1 - c) + i * c, c)

    def by_lines(i):
        return i * (1 - c) + (lax.rem(i, nx) * ny + i // nx) * c

    def piece_of(i):
        return i // 2 + lax.rem(i, 2) * (pln // 2)

    def plane(i):
        return (z, i // nx, lax.rem(i, nx), c)

    def head_of(a, h):
        return a[HEAD * h : HEAD * (h + 1)]

    def by_head(parts):
        return jnp.concatenate(list(parts), axis=0)

    scope = jax.named_scope
    with scope("loads_barrier"):
        loads = [
            pltpu.make_async_copy(src, dst, lsem.at[k])
            for k, (src, dst) in enumerate(
                ((f_hbm, f_v), (q_hbm, q_v), (go_hbm, go_v), (x_hbm, x_v), (w_hbm, w_v), (lb_hbm, lb_v))
            )
        ]
        for copy in loads:
            copy.start()
        barrier = pltpu.get_barrier_semaphore()
        for k in range(1, pln):
            pl.semaphore_signal(barrier, inc=1, device_id=plane(lax.rem(me + k, pln)), device_id_type=LOGICAL)
        for k in range(1, nz):
            pl.semaphore_signal(barrier, inc=1, device_id=(lax.rem(z + k, nz), y, x, c), device_id_type=LOGICAL)
        pl.semaphore_signal(barrier, inc=1, device_id=(z, y, x, 1 - c), device_id_type=LOGICAL)

    lane = lax.broadcasted_iota(jnp.int32, (1, ch), 1)
    mf = [jnp.where((lane >= HEAD * h) & (lane < HEAD * (h + 1)), 1.0, 0.0).astype(F32) for h in range(heads)]
    row = lax.broadcasted_iota(jnp.int32, (tok, tok), 0)
    col = lax.broadcasted_iota(jnp.int32, (tok, tok), 1)
    lower, upper = row >= col, col >= row
    lower_ones = jnp.where(lower, 1.0, 0.0).astype(BF16)
    upper_ones = jnp.where(upper, 1.0, 0.0).astype(BF16)

    def folded(full):
        out = full[:HEAD] * mf[0]
        for h in range(1, heads):
            out = out + head_of(full, h) * mf[h]
        return out

    with scope("gates"):
        loads[5].wait()
        gap = jnp.broadcast_to(1.0 - lb_v[...], (tok, ch)).T
        loads[0].wait()
        f = f_v[...].astype(F32)
        f_neg = 1.0 / (1.0 + jnp.exp(f))
        f_sig = 1.0 / (1.0 + jnp.exp(-f))
        k_rate = gap * f_neg
        logs = jnp.log1p(-k_rate)
        high = logs.astype(BF16)
        low = (logs - high.astype(F32)).astype(BF16)
        cum = nn(high, upper_ones) + nn(low, upper_ones)
        row_ones = jnp.ones((8, tok), BF16)
        total = jnp.exp((nt(row_ones, high) + nt(row_ones, low))[:1])
        closing = cum[:, tok - 1 : tok]
        growth = jnp.exp(cum)
        shrink = jnp.exp(-cum)
        remain = jnp.exp(closing - cum)
        e_send[...] = total
        k_dec = (k_rate * shrink).astype(BF16)
        k_end = (k_rate * remain).astype(BF16)
        loads[1].wait()
        q = q_v[...].astype(F32)
        q_sig = 1.0 / (1.0 + jnp.exp(-q))
        query = q * q_sig
        q_dec = (query * growth).astype(BF16)
        loads[2].wait()
        go = go_v[...]
        reach = folded(nt(go, q_dec))
    with scope("values"):
        loads[3].wait()
        loads[4].wait()
        v = nt(w_v[...], x_v[...]).astype(BF16)
        update = folded(nt(v, k_end))
        s_send[...] = jnp.concatenate([update, reach], axis=0).reshape(s_send.shape).astype(BF16)
        r_send[...] = reach.astype(BF16)
        k_send[...] = k_end

    with scope("turn"):
        rows = d_model // (nz * ny * nx)
        per = tok // rows
        for b in range(d_model // tok):
            turned = x_v[:, tok * b : tok * (b + 1)].T
            for g in range(per):
                at = b * per + g
                zz, yy, xx = at // pln, (at // nx) % ny, at % nx
                group, into = xx * (1 - c) + yy * c, yy * (1 - c) + xx * c
                xt[group, into, zz] = turned[rows * g : rows * (g + 1)]

    with scope("barrier_wait"):
        pl.semaphore_wait(barrier, pln + nz - 1)

    sends = []

    def start(copy):
        copy.start()
        sends.append(copy)

    def to_line(source, target, send_sem, recv_sem):
        for k in range(1, nx):
            start(rcopy(source, target.at[at_line], send_sem.at[k], recv_sem.at[at_line], line(lax.rem(at_line + k, nx))))

    def from_line(source, target, send_sem, recv_sem):
        for k in range(1, nx):
            frm = lax.rem(at_line + k, nx)
            rcopy(source, target.at[frm], send_sem.at[k], recv_sem.at[frm], line(frm)).wait_recv()

    def to_column(source, target, send_sem, recv_sem):
        for k in range(1, ny):
            to = lax.rem(at_col + k, ny)
            start(rcopy(source.at[to], target.at[at_col], send_sem.at[k], recv_sem.at[at_col], column(to)))

    def from_column(own, source, target, send_sem, recv_sem):
        out = own[...].astype(F32)
        for k in range(1, ny):
            frm = lax.rem(at_col + k, ny)
            rcopy(source.at[0], target.at[frm], send_sem.at[k], recv_sem.at[frm], column(frm)).wait_recv()
            out = out + target[frm].astype(F32)
        return out

    def reach_sends(k):
        to = lax.rem(at_line + k, nx)
        return rcopy(r_send, rl.at[at_line], r_ss.at[k], r_rs.at[at_line], line(to))

    with scope("send1"):
        for k in range(1, pln):
            to = lax.rem(me + k, pln)
            start(rcopy(e_send, e_buf.at[me], e_ss.at[k], e_rs.at[me], plane(to)))
            start(rcopy(s_send.at[piece_of(to)], s_buf.at[me], s_ss.at[k], s_rs.at[me], plane(to)))
        for k in range(1, nx):
            to = lax.rem(at_line + k, nx)
            start(rcopy(xt.at[to], xtl.at[at_line], xt_ss.at[k], xt_rs.at[at_line], line(to)))
        to_line(k_send, kl, k_ss, k_rs)

        @pl.when(c == 0)
        def _():
            for k in range(1, nx):
                reach_sends(k).start()

        s_buf[me] = s_send[piece_of(me)]
        e_buf[me] = e_send[...]
        xtl[at_line] = xt[at_line]
        kl[at_line] = k_end
        rl[at_line] = r_send[...]

    with scope("pairs_value"):
        mixing = [jnp.where(lower, tn(head_of(q_dec, h), head_of(k_dec, h)), 0.0).astype(BF16) for h in range(heads)]
        gv_own = by_head(nn(head_of(go, h), mixing[h]) for h in range(heads))
        own_send[...] = gv_own.astype(BF16)
        ownl[at_line] = own_send[...]

    with scope("wait1"):
        for k in range(1, pln):
            frm = lax.rem(me + k, pln)
            rcopy(e_send, e_buf.at[frm], e_ss.at[k], e_rs.at[frm], plane(frm)).wait_recv()
            rcopy(s_send.at[0], s_buf.at[frm], s_ss.at[k], s_rs.at[frm], plane(frm)).wait_recv()
    with scope("scan1"):
        held = jnp.zeros(t_send.shape, F32)
        factor = jnp.ones((1, ch), F32)
        for o in range(pln):
            it = o + back * (pln - 1 - 2 * o)
            l_send[by_lines(it)] = held.astype(BF16)
            decay = e_buf[it]
            held = decay * held + s_buf[it].astype(F32)
            factor = decay * factor
        t_send[...] = held.astype(BF16)
        ft_send[...] = factor

    z_order = z + back * (nz - 1 - 2 * z)

    def z_sends(k):
        at = z_order + k
        to = at + back * (nz - 1 - 2 * at)
        return (
            rcopy(ft_send, ft_buf.at[z], ft_ss.at[k], ft_rs.at[z], (to, y, x, c)),
            rcopy(t_send, t_buf.at[z], t_ss.at[k], t_rs.at[z], (to, y, x, c)),
        )

    def state_sends(k, to):
        return rcopy(l_send.at[by_lines(to)], q_state.at[me // 2], q_ss.at[k], q_rs.at[me], plane(to))

    def line_sends(k, to):
        last = to // nx * nx + nx - 1
        return rcopy(l_send.at[last], q_line.at[me // 2], q_ss.at[k], q_rs.at[me], plane(to))

    def grad_sends(k, to):
        first = by_lines(to) // nx * nx
        return rcopy(l_send.at[pl.ds(first, nx)], q_grad.at[me // 2], q_ss.at[k], q_rs.at[me], plane(to))

    with scope("send2"):
        for k in range(1, nz):

            @pl.when(z_order + k < nz)
            def _():
                for copy in z_sends(k):
                    copy.start()

        for k in range(1, pln):
            to = lax.rem(me + k, pln)

            @pl.when(back == 0)
            def _():
                state_sends(k, to).start()

            @pl.when((back == 1) & (c == 0))
            def _():
                line_sends(k, to).start()

            @pl.when((back == 1) & (c == 1))
            def _():
                grad_sends(k, to).start()

        @pl.when(back == 0)
        def _():
            q_state[me // 2] = l_send[by_lines(me)]

        @pl.when(back == 1)
        def _():
            q_grad[me // 2] = l_send[pl.ds(at_col * nx, nx)]
            q_line[me // 2] = l_send[at_col * nx + nx - 1]

        to_line(own_send, ownl, own_ss, own_rs)

    with scope("pairs_query"):
        pairing = [jnp.where(upper, tn(head_of(v, h), head_of(go, h)), 0.0).astype(BF16) for h in range(heads)]
        gq_own = by_head(nn(head_of(k_dec, h), pairing[h]) for h in range(heads))
        gk_own = by_head(nt(head_of(q_dec, h), pairing[h]) for h in range(heads))

    with scope("decays"):
        before, after = jnp.ones((1, ch), F32), [jnp.ones((1, ch), F32)] * nx
        ids = [line(i)[1] * nx + line(i)[2] for i in range(nx)]
        for i in range(pln):
            before = before * jnp.where(i < me, e_buf[i], 1.0)
            after = [a * jnp.where(i > n, e_buf[i], 1.0) for a, n in zip(after, ids)]

    with scope("wait_line"):
        for k in range(1, nx):
            frm = lax.rem(at_line + k, nx)
            rcopy(xt.at[0], xtl.at[frm], xt_ss.at[k], xt_rs.at[frm], line(frm)).wait_recv()
        from_line(k_send, kl, k_ss, k_rs)
    def pairs(parts):
        return [jnp.concatenate(parts[i : i + 2], axis=1) for i in range(0, nx, 2)]

    def to_chunks(ref, total):
        for i in range(ny):
            ref[i] = total[:, i * nz * rows : (i + 1) * nz * rows].astype(ref.dtype)

    with scope("line_m"):
        turned_of = pairs([xtl[i].reshape(d_model // nx, tok) for i in range(nx)])
        tall_after = jnp.concatenate(after + [jnp.ones((8 - nx, ch), F32)], axis=0).T
        scaled = pairs([(kl[i].astype(F32) * tall_after[:, i : i + 1]).astype(BF16) for i in range(nx)])
        m_sum = nt(scaled[0], turned_of[0])
        for a, b in zip(scaled[1:], turned_of[1:]):
            m_sum = m_sum + nt(a, b)
        to_chunks(m_send, m_sum)

    def arriving(o, carried):
        frm = o + back * (nz - 1 - 2 * o)
        rcopy(ft_send, ft_buf.at[frm], ft_ss.at[0], ft_rs.at[frm], (z, y, x, c)).wait_recv()
        rcopy(t_send, t_buf.at[frm], t_ss.at[0], t_rs.at[frm], (z, y, x, c)).wait_recv()
        return ft_buf[frm] * carried + t_buf[frm].astype(F32)

    with scope("wait2"):
        carried = lax.fori_loop(0, z_order, arriving, jnp.zeros(t_send.shape, F32))

    with scope("send3"):
        o_send[...] = carried.astype(BF16)
        mine = piece_of(me)
        for k in range(1, pln):
            start(rcopy(o_send, p_buf.at[mine], p_ss.at[k], p_rs.at[mine], plane(lax.rem(me + k, pln))))
        p_buf[mine] = o_send[...]
        to_column(m_send, m_recv, m_ss, m_rs)

    with scope("wait_1b"):
        for j in range(pln // 2):

            @pl.when(me != 2 * j)
            def _():
                rcopy(l_send.at[0], q_state.at[j], q_ss.at[0], q_rs.at[2 * j], plane(2 * j)).wait_recv()

            @pl.when((me != 2 * j + 1) & (c == 0))
            def _():
                rcopy(
                    l_send.at[0], q_line.at[j], q_ss.at[0], q_rs.at[2 * j + 1], plane(2 * j + 1)
                ).wait_recv()

            @pl.when((me != 2 * j + 1) & (c == 1))
            def _():
                rcopy(
                    l_send.at[pl.ds(0, nx)], q_grad.at[j], q_ss.at[0], q_rs.at[2 * j + 1], plane(2 * j + 1)
                ).wait_recv()

        @pl.when(c == 0)
        def _():
            from_line(r_send, rl, r_ss, r_rs)

    with scope("wait_own"):
        from_line(own_send, ownl, own_ss, own_rs)
    with scope("line_a"):
        state_in = q_state[...].astype(F32).reshape(HEAD, ch)

        @pl.when(c == 0)
        def _():
            grad_at = q_line[...].astype(F32).reshape(HEAD, ch)
            g_all[nx - 1] = grad_at
            for i in range(nx - 2, -1, -1):
                grad_at = e_buf[y * nx + i + 1] * grad_at + rl[i + 1].astype(F32)
                g_all[i] = grad_at

        @pl.when(c == 1)
        def _():
            for i in range(nx):
                g_all[i] = q_grad[:, i].astype(F32).reshape(HEAD, ch)

        parts = []
        for i in range(nx):
            grad_at = g_all[i]
            bd_in = by_head((grad_at * m).astype(BF16) for m in mf)
            parts.append((ownl[i].astype(F32) + nn(bd_in, kl[i])).astype(BF16))
        parts = pairs(parts)
        a_sum = nt(parts[0], turned_of[0])
        for a, b in zip(parts[1:], turned_of[1:]):
            a_sum = a_sum + nt(a, b)
        to_chunks(aacc, a_sum)
        to_chunks(a_send, a_sum)
        to_column(a_send, a_recv, a_ss, a_rs)

    with scope("wait_m"):
        m_plane = from_column(m_send.at[at_col], m_send, m_recv, m_ss, m_rs).T.astype(BF16)
    with scope("wait3"):
        for k in range(1, pln):
            frm = lax.rem(me + k, pln)
            part = piece_of(frm)
            rcopy(o_send, p_buf.at[part], p_ss.at[k], p_rs.at[part], plane(frm)).wait_recv()
    with scope("wait_a"):
        a_plane = from_column(aacc.at[at_col], a_send, a_recv, a_ss, a_rs).T
    with scope("send_z"):
        outer = p_buf[...].astype(F32).reshape(2 * HEAD, ch)
        state_out, grad_out = outer[:HEAD], outer[HEAD:]
        bd_out = by_head((grad_out * m).astype(BF16) for m in mf)
        w_sum = a_plane + nt(m_plane, bd_out)
        w2[...] = w_sum.reshape(w2.shape)
        z_send[...] = w_sum.astype(BF16).reshape(z_send.shape)
        for k in range(1, nz):
            to = lax.rem(z + k, nz)
            start(rcopy(z_send.at[to], z_recv.at[z], z_ss.at[k], z_rs.at[z], (to, y, x, c)))

    with scope("value_grad"):
        own_after = after[nx - 1]
        for i in range(nx - 1):
            own_after = jnp.where(at_line == i, after[i], own_after)
        state = state_in + before * state_out
        grad = g_all[at_line] + own_after * grad_out
        bd_state = by_head((state * m).astype(BF16) for m in mf)
        bd_grad = by_head((grad * m).astype(BF16) for m in mf)
        value_grad = (gv_own + nn(bd_grad, k_end)).astype(BF16)

    with scope("input_grad"):
        width = 512 if d_model % 512 == 0 else d_model
        turned = value_grad.T
        for j in range(d_model // width):
            cols = pl.ds(j * width, width)
            ig[:, :, cols] = nn(turned, w_v[:, cols]).astype(BF16).reshape(2, tok // 2, width)
        ig_copy = rcopy(ig.at[1 - c], ig_recv, ig_ss, ig_rs, (z, y, x, 1 - c))
        ig_copy.start()

    with scope("query_forget"):
        g_query = growth * (gq_own + tn(bd_state, go))
        g_key = shrink * gk_own + remain * tn(bd_grad, v)
        gq_out[...] = (g_query * (q_sig * (1.0 + q * (1.0 - q_sig)))).astype(BF16)
        ends = grad * (total * state + update)
        ends_high = ends.astype(BF16)
        ends_low = (ends - ends_high.astype(F32)).astype(BF16)
        tall_ones = jnp.ones((HEAD, tok), BF16)
        boundary = tn(ends_high, tall_ones) + tn(ends_low, tall_ones)
        flow = query * g_query - k_rate * g_key
        flow_high = flow.astype(BF16)
        flow_low = (flow - flow_high.astype(F32)).astype(BF16)
        g_decay = nn(flow_high, lower_ones) + nn(flow_low, lower_ones) + boundary
        gf_out[...] = ((g_decay / (1.0 - k_rate) - g_key) * k_rate * f_sig).astype(BF16)

    with scope("input_sum"):
        ig_copy.wait_recv()
        gx_out[...] = (ig[c].astype(F32) + ig_recv[...].astype(F32)).astype(BF16)

    with scope("wait_z"):
        w_last = w2[z]
        for k in range(1, nz):
            frm = lax.rem(z + k, nz)
            rcopy(z_send.at[0], z_recv.at[frm], z_ss.at[k], z_rs.at[frm], (frm, y, x, c)).wait_recv()
            w_last = w_last + z_recv[frm].astype(F32)
        gw_out[...] = w_last

    with scope("drain"):
        for copy in sends:
            copy.wait_send()
        ig_copy.wait_send()
        for k in range(1, pln):
            to = lax.rem(me + k, pln)

            @pl.when(back == 0)
            def _():
                state_sends(k, to).wait_send()

            @pl.when((back == 1) & (c == 0))
            def _():
                line_sends(k, to).wait_send()

            @pl.when((back == 1) & (c == 1))
            def _():
                grad_sends(k, to).wait_send()

        @pl.when(c == 0)
        def _():
            for k in range(1, nx):
                reach_sends(k).wait_send()

        for k in range(1, nz):

            @pl.when(z_order + k < nz)
            def _():
                for copy in z_sends(k):
                    copy.wait_send()


def write_out(*refs):
    copies = [pltpu.make_async_copy(refs[k], refs[4 + k], refs[8].at[k]) for k in range(4)]
    for copy in copies:
        copy.start()
    for copy in copies:
        copy.wait()


def on_device(nz, ny, nx, block_input, value_weight, query_pre, forget_pre, lower_bound, out_grad):
    tok, d_model = block_input.shape
    ch = value_weight.shape[1]
    pln = ny * nx
    piece = 2 * HEAD // pln
    rows = d_model // (nz * pln)
    vm, dma = pltpu.VMEM, pltpu.SemaphoreType.DMA
    scratch = [
        vm((tok, d_model), BF16), vm((ch, d_model), BF16),
        vm((ch, tok), BF16), vm((ch, tok), BF16), vm((ch, tok), BF16), vm((1, ch), F32),
        vm((pln, piece, ch), BF16), vm((1, ch), F32),
        vm((pln, piece, ch), BF16), vm((pln, 1, ch), F32),
        vm((pln, piece, ch), BF16), vm((pln // 2, piece, ch), BF16), vm((pln // 2, nx, piece, ch), BF16),
        vm((pln // 2, piece, ch), BF16),
        vm((piece, ch), BF16), vm((1, ch), F32),
        vm((nz, piece, ch), BF16), vm((nz, 1, ch), F32),
        vm((piece, ch), BF16), vm((pln, piece, ch), BF16),
        vm((nx, ny, nz, rows, tok), BF16), vm((nx, ny, nz, rows, tok), BF16),
        vm((HEAD, ch), BF16), vm((nx, HEAD, ch), BF16),
        vm((ch, tok), BF16), vm((nx, ch, tok), BF16),
        vm((ch, tok), BF16), vm((nx, ch, tok), BF16),
        vm((nx, HEAD, ch), F32),
        vm((2, tok // 2, d_model), BF16), vm((tok // 2, d_model), BF16),
        vm((ny, ch, nz * rows), BF16), vm((ny, ch, nz * rows), BF16),
        vm((ny, ch, nz * rows), F32), vm((ny, ch, nz * rows), BF16), vm((ny, ch, nz * rows), BF16),
        vm((nz, rows, ch), F32), vm((nz, rows, ch), BF16), vm((nz, rows, ch), BF16),
        dma((6,)),
        dma((pln,)), dma((pln,)), dma((pln,)), dma((pln,)), dma((pln,)), dma((pln,)),
        dma((nz,)), dma((nz,)), dma((nz,)), dma((nz,)),
        dma((pln,)), dma((pln,)),
        *(dma((nx,)) for _ in range(8)),
        *(dma((ny,)) for _ in range(4)),
        dma((nz,)), dma((nz,)),
        dma, dma,
    ]
    hbm, near = pl.BlockSpec(memory_space=pl.ANY), pl.BlockSpec(memory_space=pltpu.VMEM)
    results = pl.pallas_call(
        functools.partial(kernel, nz, ny, nx),
        out_shape=(
            vm((ch, tok), BF16),
            vm((ch, tok), BF16),
            vm((tok // 2, d_model), BF16),
            vm((rows, ch), F32),
        ),
        in_specs=[hbm] * 6,
        out_specs=(near,) * 4,
        scratch_shapes=scratch,
        compiler_params=pltpu.CompilerParams(collective_id=0, has_side_effects=True),
    )(block_input, value_weight.T, query_pre.T, forget_pre.T, out_grad.T, lower_bound.reshape(1, ch))
    g_query, g_forget, g_input, g_weight = pl.pallas_call(
        write_out,
        out_shape=tuple(jax.ShapeDtypeStruct(a.shape, a.dtype) for a in results),
        in_specs=[near] * 4,
        out_specs=(hbm,) * 4,
        scratch_shapes=[dma((4,))],
    )(*(pltpu.with_memory_space_constraint(a, pltpu.VMEM) for a in results))
    return g_query.T, g_forget.T, g_input, g_weight


def on_mesh(devices):
    nz, ny, nx = devices.shape[:3]
    split = Mesh(devices, SP_TP)
    in_specs = (P(SP, None), P(None, "tp"), P(SP, "tp"), P(SP, "tp"), P("tp"), P(SP, "tp"))
    out_specs = (P(SP, "tp"), P(SP, "tp"), P(SP_TP, None), P(SP, "tp"))
    return jax.shard_map(
        functools.partial(on_device, nz, ny, nx), mesh=split, in_specs=in_specs, out_specs=out_specs, check_vma=False
    )


def solution(mesh):
    return on_mesh(mesh.devices.reshape(8, 4, 4, mesh.shape["tp"]))
```

```python
import functools

import jax
import jax.numpy as jnp
from jax import lax
from jax.experimental import pallas as pl
from jax.experimental.pallas import tpu as pltpu
from jax.sharding import Mesh
from jax.sharding import PartitionSpec as P

HEAD = 64
SP = ("sp_0", "sp_1", "sp_2")
SP_TP = ("sp_0", "sp_1", "sp_2", "tp")
F32, BF16 = jnp.float32, jnp.bfloat16
LOGICAL = pl.DeviceIdType.MESH


def nn(a, b):
    return lax.dot_general(a, b, (((1,), (0,)), ((), ())), preferred_element_type=F32)


def nt(a, b):
    return lax.dot_general(a, b, (((1,), (1,)), ((), ())), preferred_element_type=F32)


def tn(a, b):
    return lax.dot_general(a, b, (((0,), (0,)), ((), ())), preferred_element_type=F32)


def rcopy(src, dst, send, recv, device):
    return pltpu.make_async_remote_copy(
        src_ref=src, dst_ref=dst, send_sem=send, recv_sem=recv, device_id=device, device_id_type=LOGICAL
    )


def kernel(
    nz, ny, nx,
    x_hbm, w_hbm, q_hbm, f_hbm, go_hbm, lb_hbm,
    gq_out, gf_out, gx_out, gw_out,
    x_v, w_v, q_v, f_v, go_v, lb_v,
    s_send, e_send, s_buf, e_buf, l_send, q_state, q_grad, q_line, t_send, ft_send, t_buf, ft_buf, o_send, p_buf,
    xt, xtl, r_send, rl, k_send, kl, own_send, ownl, g_all, ig, ig_recv,
    m_send, m_recv, aacc, a_send, a_recv, w2, z_send, z_recv,
    lsem, s_ss, s_rs, e_ss, e_rs, ea_ss, ea_rs, q_ss, q_rs, t_ss, t_rs, ft_ss, ft_rs, p_ss, p_rs,
    xt_ss, xt_rs, r_ss, r_rs, k_ss, k_rs, own_ss, own_rs,
    m_ss, m_rs, a_ss, a_rs, z_ss, z_rs, ig_ss, ig_rs,
):
    pln = ny * nx
    tok, d_model = x_v.shape
    ch = w_v.shape[0]
    heads = ch // HEAD
    z, y, x, c = (lax.axis_index(a) for a in SP_TP)
    me = y * nx + x
    back = lax.rem(me, 2)
    at_line, at_col = x * (1 - c) + y * c, y * (1 - c) + x * c

    def line(i):
        return (z, y * (1 - c) + i * c, i * (1 - c) + x * c, c)

    def column(i):
        return (z, i * (1 - c) + y * c, x * (1 - c) + i * c, c)

    def spot(g, i):
        return lax.rem(i, nx) * ny + i // nx if g else i

    def owner(i):
        return (z, i // nx, lax.rem(i, nx), 1)

    def piece_of(i):
        return i // 2 + lax.rem(i, 2) * (pln // 2)

    def plane(i):
        return (z, i // nx, lax.rem(i, nx), c)

    def head_of(a, h):
        return a[HEAD * h : HEAD * (h + 1)]

    def by_head(parts):
        return jnp.concatenate(list(parts), axis=0)

    scope = jax.named_scope
    with scope("loads_barrier"):
        barrier = pltpu.get_barrier_semaphore()

        def greet(device):
            pl.semaphore_signal(barrier, inc=1, device_id=device, device_id_type=LOGICAL)

        for k in range(1, nz):
            greet((lax.rem(z + k, nz), y, x, c))
        for k in range(1, pln):
            to = lax.rem(me + k, pln)
            greet((z, to // nx, lax.rem(to, nx), 1 - c))

            @pl.when((c == 1) | (to // nx == y) | (lax.rem(to, nx) == x))
            def _():
                greet(plane(to))

        greet((z, y, x, 1 - c))
        loads = [
            pltpu.make_async_copy(src, dst, lsem.at[k])
            for k, (src, dst) in enumerate(
                ((f_hbm, f_v), (q_hbm, q_v), (go_hbm, go_v), (x_hbm, x_v), (w_hbm, w_v), (lb_hbm, lb_v))
            )
        ]
        for copy in loads:
            copy.start()

    lane = lax.broadcasted_iota(jnp.int32, (1, ch), 1)
    mf = [jnp.where((lane >= HEAD * h) & (lane < HEAD * (h + 1)), 1.0, 0.0).astype(F32) for h in range(heads)]
    row = lax.broadcasted_iota(jnp.int32, (tok, tok), 0)
    col = lax.broadcasted_iota(jnp.int32, (tok, tok), 1)
    lower, upper = row >= col, col >= row
    lower_ones = jnp.where(lower, 1.0, 0.0).astype(BF16)
    upper_ones = jnp.where(upper, 1.0, 0.0).astype(BF16)

    def folded(full):
        out = full[:HEAD] * mf[0]
        for h in range(1, heads):
            out = out + head_of(full, h) * mf[h]
        return out

    with scope("gates"):
        loads[5].wait()
        gap = jnp.broadcast_to(1.0 - lb_v[...], (tok, ch)).T
        loads[0].wait()
        f = f_v[...].astype(F32)
        f_neg = 1.0 / (1.0 + jnp.exp(f))
        f_sig = 1.0 / (1.0 + jnp.exp(-f))
        k_rate = gap * f_neg
        logs = jnp.log1p(-k_rate)
        high = logs.astype(BF16)
        low = (logs - high.astype(F32)).astype(BF16)
        cum = nn(high, upper_ones) + nn(low, upper_ones)
        row_ones = jnp.ones((8, tok), BF16)
        total = jnp.exp((nt(row_ones, high) + nt(row_ones, low))[:1])
        closing = cum[:, tok - 1 : tok]
        growth = jnp.exp(cum)
        shrink = jnp.exp(-cum)
        remain = jnp.exp(closing - cum)
        e_send[...] = total
        k_dec = (k_rate * shrink).astype(BF16)
        k_end = (k_rate * remain).astype(BF16)
        loads[1].wait()
        q = q_v[...].astype(F32)
        q_sig = 1.0 / (1.0 + jnp.exp(-q))
        query = q * q_sig
        q_dec = (query * growth).astype(BF16)
        loads[2].wait()
        go = go_v[...]
        reach = folded(nt(go, q_dec))
    with scope("values"):
        loads[3].wait()
        loads[4].wait()
        v = nt(w_v[...], x_v[...]).astype(BF16)
        update = folded(nt(v, k_end))
        s_send[...] = jnp.concatenate([update, reach], axis=0).reshape(s_send.shape).astype(BF16)
        r_send[...] = reach.astype(BF16)
        k_send[...] = k_end

    with scope("turn"):
        rows = d_model // (nz * ny * nx)
        per = tok // rows
        for b in range(d_model // tok):
            turned = x_v[:, tok * b : tok * (b + 1)].T
            for g in range(per):
                at = b * per + g
                zz, yy, xx = at // pln, (at // nx) % ny, at % nx
                group, into = xx * (1 - c) + yy * c, yy * (1 - c) + xx * c
                xt[group, into, zz] = turned[rows * g : rows * (g + 1)]

    with scope("barrier_wait"):
        pl.semaphore_wait(barrier, pln + nz - 1 + c * (pln - 1) + (1 - c) * (nx + ny - 2))

    sends = []

    def start(copy):
        copy.start()
        sends.append(copy)

    def to_line(source, target, send_sem, recv_sem):
        for k in range(1, nx):
            start(rcopy(source, target.at[at_line], send_sem.at[k], recv_sem.at[at_line], line(lax.rem(at_line + k, nx))))

    def from_line(source, target, send_sem, recv_sem):
        for k in range(1, nx):
            frm = lax.rem(at_line + k, nx)
            rcopy(source, target.at[frm], send_sem.at[k], recv_sem.at[frm], line(frm)).wait_recv()

    def to_column(source, target, send_sem, recv_sem):
        for k in range(1, ny):
            to = lax.rem(at_col + k, ny)
            start(rcopy(source.at[to], target.at[at_col], send_sem.at[k], recv_sem.at[at_col], column(to)))

    def from_column(own, source, target, send_sem, recv_sem):
        out = own[...].astype(F32)
        for k in range(1, ny):
            frm = lax.rem(at_col + k, ny)
            rcopy(source.at[0], target.at[frm], send_sem.at[k], recv_sem.at[frm], column(frm)).wait_recv()
            out = out + target[frm].astype(F32)
        return out

    def reach_sends(k):
        to = lax.rem(at_line + k, nx)
        return rcopy(r_send, rl.at[at_line], r_ss.at[k], r_rs.at[at_line], line(to))

    def piece_sends(k):
        to = lax.rem(me + k, pln)
        return (
            rcopy(e_send, e_buf.at[c, me], e_ss.at[k], e_rs.at[c, me], owner(to)),
            rcopy(s_send.at[piece_of(to)], s_buf.at[c, me], s_ss.at[k], s_rs.at[c, me], owner(to)),
        )

    with scope("send1"):
        for k in range(1, pln):
            for copy in piece_sends(k):
                start(copy)

        @pl.when(c == 0)
        def _():
            for copy in piece_sends(0):
                copy.start()

        @pl.when(c == 1)
        def _():
            s_buf[1, me] = s_send[piece_of(me)]
            e_buf[1, me] = e_send[...]

        for k in range(1, nx):
            to = lax.rem(at_line + k, nx)
            start(rcopy(xt.at[to], xtl.at[at_line], xt_ss.at[k], xt_rs.at[at_line], line(to)))
        to_line(k_send, kl, k_ss, k_rs)

        @pl.when(c == 0)
        def _():
            for k in range(1, nx):
                reach_sends(k).start()

        xtl[at_line] = xt[at_line]
        kl[at_line] = k_end
        rl[at_line] = r_send[...]

    with scope("pairs_value"):
        mixing = [jnp.where(lower, tn(head_of(q_dec, h), head_of(k_dec, h)), 0.0).astype(BF16) for h in range(heads)]
        gv_own = by_head(nn(head_of(go, h), mixing[h]) for h in range(heads))
        own_send[...] = gv_own.astype(BF16)
        ownl[at_line] = own_send[...]
        to_line(own_send, ownl, own_ss, own_rs)

    z_order = z + back * (nz - 1 - 2 * z)

    def z_sends(k):
        at = z_order + k
        to = at + back * (nz - 1 - 2 * at)
        return (
            rcopy(ft_send, ft_buf.at[z], ft_ss.at[k], ft_rs.at[z], (to, y, x, 1)),
            rcopy(t_send, t_buf.at[z], t_ss.at[k], t_rs.at[z], (to, y, x, 1)),
        )

    def carry_send(g, k, backward):
        to = lax.rem(me + k, pln)
        sems = (q_ss.at[g, k], q_rs.at[me], (z, to // nx, lax.rem(to, nx), g))
        if not backward:
            return rcopy(l_send.at[g, spot(g, to)], q_state.at[me // 2], *sems)
        if g == 0:
            return rcopy(l_send.at[0, to // nx * nx + nx - 1], q_line.at[me // 2], *sems)
        return rcopy(l_send.at[1, pl.ds(lax.rem(to, nx) * ny, ny)], q_grad.at[me // 2], *sems)

    targets = [(0, k) for k in range(pln)] + [(1, k) for k in range(1, pln)]
    e_all = rcopy(e_buf.at[0], e_buf.at[0], ea_ss, ea_rs, (z, y, x, 1 - c))

    @pl.when(c == 1)
    def _():
        with scope("wait1"):
            for g, k in targets:
                frm = lax.rem(me + k, pln)
                device = (z, frm // nx, lax.rem(frm, nx), g)
                rcopy(e_send, e_buf.at[g, frm], e_ss.at[k], e_rs.at[g, frm], device).wait_recv()
                rcopy(s_send.at[0], s_buf.at[g, frm], s_ss.at[k], s_rs.at[g, frm], device).wait_recv()
        with scope("scan1"):
            for g in (0, 1):
                held = jnp.zeros(t_send.shape[1:], F32)
                factor = jnp.ones((1, ch), F32)
                for o in range(pln):
                    it = o + back * (pln - 1 - 2 * o)
                    l_send[g, spot(g, it)] = held.astype(BF16)
                    decay = e_buf[g, it]
                    held = decay * held + s_buf[g, it].astype(F32)
                    factor = decay * factor
                t_send[g] = held.astype(BF16)
                ft_send[g] = factor
        with scope("send2"):
            for k in range(1, nz):

                @pl.when(z_order + k < nz)
                def _():
                    for copy in z_sends(k):
                        copy.start()

            for backward in (0, 1):

                @pl.when(back == backward)
                def _():
                    for g, k in targets:
                        carry_send(g, k, backward).start()

            e_all.start()

            @pl.when(back == 0)
            def _():
                q_state[me // 2] = l_send[1, spot(1, me)]

            @pl.when(back == 1)
            def _():
                q_grad[me // 2] = l_send[1, pl.ds(x * ny, ny)]

    with scope("pairs_query"):
        pairing = [jnp.where(upper, tn(head_of(v, h), head_of(go, h)), 0.0).astype(BF16) for h in range(heads)]
        gq_own = by_head(nn(head_of(k_dec, h), pairing[h]) for h in range(heads))
        gk_own = by_head(nt(head_of(q_dec, h), pairing[h]) for h in range(heads))

    with scope("decays"):
        @pl.when(c == 0)
        def _():
            e_all.wait_recv()

        decays = e_buf[c]
        before, after = jnp.ones((1, ch), F32), [jnp.ones((1, ch), F32)] * nx
        ids = [line(i)[1] * nx + line(i)[2] for i in range(nx)]
        for i in range(pln):
            before = before * jnp.where(i < me, decays[i], 1.0)
            after = [a * jnp.where(i > n, decays[i], 1.0) for a, n in zip(after, ids)]

    with scope("wait_line"):
        for k in range(1, nx):
            frm = lax.rem(at_line + k, nx)
            rcopy(xt.at[0], xtl.at[frm], xt_ss.at[k], xt_rs.at[frm], line(frm)).wait_recv()
        from_line(k_send, kl, k_ss, k_rs)
    def pairs(parts):
        return [jnp.concatenate(parts[i : i + 2], axis=1) for i in range(0, nx, 2)]

    def to_chunks(ref, total):
        for i in range(ny):
            ref[i] = total[:, i * nz * rows : (i + 1) * nz * rows].astype(ref.dtype)

    with scope("line_m"):
        turned_of = pairs([xtl[i].reshape(d_model // nx, tok) for i in range(nx)])
        tall_after = jnp.concatenate(after + [jnp.ones((8 - nx, ch), F32)], axis=0).T
        scaled = pairs([(kl[i].astype(F32) * tall_after[:, i : i + 1]).astype(BF16) for i in range(nx)])
        m_sum = nt(scaled[0], turned_of[0])
        for a, b in zip(scaled[1:], turned_of[1:]):
            m_sum = m_sum + nt(a, b)
        to_chunks(m_send, m_sum)

    def arriving(o, carried):
        frm = o + back * (nz - 1 - 2 * o)
        rcopy(ft_send, ft_buf.at[frm], ft_ss.at[0], ft_rs.at[frm], (frm, y, x, 1)).wait_recv()
        rcopy(t_send, t_buf.at[frm], t_ss.at[0], t_rs.at[frm], (frm, y, x, 1)).wait_recv()
        return ft_buf[frm] * carried + t_buf[frm].astype(F32)

    mine = piece_of(me)

    def plane_send(g, k):
        to = lax.rem(me + k, pln)
        device = (z, to // nx, lax.rem(to, nx), g)
        return rcopy(o_send.at[g], p_buf.at[mine], p_ss.at[g, k], p_rs.at[mine], device)

    @pl.when(c == 1)
    def _():
        with scope("wait2"):
            carried = lax.fori_loop(0, z_order, arriving, jnp.zeros(t_send.shape, F32))
        with scope("send3"):
            o_send[...] = carried.astype(BF16)
            for g, k in targets:
                plane_send(g, k).start()
            p_buf[mine] = o_send[1]

    with scope("send_m"):
        to_column(m_send, m_recv, m_ss, m_rs)

    with scope("wait_1b"):
        for j in range(pln // 2):

            @pl.when((me != 2 * j) | (c == 0))
            def _():
                rcopy(l_send.at[0, 0], q_state.at[j], q_ss.at[0, 0], q_rs.at[2 * j], owner(2 * j)).wait_recv()

            @pl.when(c == 0)
            def _():
                rcopy(
                    l_send.at[0, 0], q_line.at[j], q_ss.at[0, 0], q_rs.at[2 * j + 1], owner(2 * j + 1)
                ).wait_recv()

            @pl.when((me != 2 * j + 1) & (c == 1))
            def _():
                rcopy(
                    l_send.at[0, pl.ds(0, ny)], q_grad.at[j], q_ss.at[0, 0], q_rs.at[2 * j + 1], owner(2 * j + 1)
                ).wait_recv()

        @pl.when(c == 0)
        def _():
            from_line(r_send, rl, r_ss, r_rs)

    with scope("wait_own"):
        from_line(own_send, ownl, own_ss, own_rs)
    with scope("line_a"):
        state_in = q_state[...].astype(F32).reshape(HEAD, ch)

        @pl.when(c == 0)
        def _():
            grad_at = q_line[...].astype(F32).reshape(HEAD, ch)
            g_all[nx - 1] = grad_at
            for i in range(nx - 2, -1, -1):
                grad_at = e_buf[0, y * nx + i + 1] * grad_at + rl[i + 1].astype(F32)
                g_all[i] = grad_at

        @pl.when(c == 1)
        def _():
            for i in range(nx):
                g_all[i] = q_grad[:, i].astype(F32).reshape(HEAD, ch)

        parts = []
        for i in range(nx):
            grad_at = g_all[i]
            bd_in = by_head((grad_at * m).astype(BF16) for m in mf)
            parts.append((ownl[i].astype(F32) + nn(bd_in, kl[i])).astype(BF16))
        parts = pairs(parts)
        a_sum = nt(parts[0], turned_of[0])
        for a, b in zip(parts[1:], turned_of[1:]):
            a_sum = a_sum + nt(a, b)
        to_chunks(aacc, a_sum)
        to_chunks(a_send, a_sum)
        to_column(a_send, a_recv, a_ss, a_rs)

    with scope("wait_m"):
        m_plane = from_column(m_send.at[at_col], m_send, m_recv, m_ss, m_rs).T.astype(BF16)
    with scope("wait3"):
        for k in range(1, pln):
            frm = lax.rem(me + k, pln)
            part = piece_of(frm)
            rcopy(o_send.at[0], p_buf.at[part], p_ss.at[0, k], p_rs.at[part], owner(frm)).wait_recv()

        @pl.when(c == 0)
        def _():
            rcopy(o_send.at[0], p_buf.at[mine], p_ss.at[0, 0], p_rs.at[mine], owner(me)).wait_recv()
    with scope("wait_a"):
        a_plane = from_column(aacc.at[at_col], a_send, a_recv, a_ss, a_rs).T
    with scope("send_z"):
        outer = p_buf[...].astype(F32).reshape(2 * HEAD, ch)
        state_out, grad_out = outer[:HEAD], outer[HEAD:]
        bd_out = by_head((grad_out * m).astype(BF16) for m in mf)
        w_sum = a_plane + nt(m_plane, bd_out)
        w2[...] = w_sum.reshape(w2.shape)
        z_send[...] = w_sum.astype(BF16).reshape(z_send.shape)
        for k in range(1, nz):
            to = lax.rem(z + k, nz)
            start(rcopy(z_send.at[to], z_recv.at[z], z_ss.at[k], z_rs.at[z], (to, y, x, c)))

    with scope("value_grad"):
        own_after = after[nx - 1]
        for i in range(nx - 1):
            own_after = jnp.where(at_line == i, after[i], own_after)
        state = state_in + before * state_out
        grad = g_all[at_line] + own_after * grad_out
        bd_state = by_head((state * m).astype(BF16) for m in mf)
        bd_grad = by_head((grad * m).astype(BF16) for m in mf)
        value_grad = (gv_own + nn(bd_grad, k_end)).astype(BF16)

    with scope("input_grad"):
        width = 512 if d_model % 512 == 0 else d_model
        turned = value_grad.T
        for j in range(d_model // width):
            cols = pl.ds(j * width, width)
            ig[:, :, cols] = nn(turned, w_v[:, cols]).astype(BF16).reshape(2, tok // 2, width)
        ig_copy = rcopy(ig.at[1 - c], ig_recv, ig_ss, ig_rs, (z, y, x, 1 - c))
        ig_copy.start()

    with scope("query_forget"):
        g_query = growth * (gq_own + tn(bd_state, go))
        g_key = shrink * gk_own + remain * tn(bd_grad, v)
        gq_out[...] = (g_query * (q_sig * (1.0 + q * (1.0 - q_sig)))).astype(BF16)
        ends = grad * (total * state + update)
        ends_high = ends.astype(BF16)
        ends_low = (ends - ends_high.astype(F32)).astype(BF16)
        tall_ones = jnp.ones((HEAD, tok), BF16)
        boundary = tn(ends_high, tall_ones) + tn(ends_low, tall_ones)
        flow = query * g_query - k_rate * g_key
        flow_high = flow.astype(BF16)
        flow_low = (flow - flow_high.astype(F32)).astype(BF16)
        g_decay = nn(flow_high, lower_ones) + nn(flow_low, lower_ones) + boundary
        gf_out[...] = ((g_decay / (1.0 - k_rate) - g_key) * k_rate * f_sig).astype(BF16)

    with scope("input_sum"):
        ig_copy.wait_recv()
        gx_out[...] = (ig[c].astype(F32) + ig_recv[...].astype(F32)).astype(BF16)

    with scope("drain"):
        for copy in sends[: 1 - nz]:
            copy.wait_send()
        ig_copy.wait_send()

        @pl.when(c == 0)
        def _():
            for copy in piece_sends(0):
                copy.wait_send()
            for k in range(1, nx):
                reach_sends(k).wait_send()

        @pl.when(c == 1)
        def _():
            for k in range(1, nz):

                @pl.when(z_order + k < nz)
                def _():
                    for copy in z_sends(k):
                        copy.wait_send()

            for backward in (0, 1):

                @pl.when(back == backward)
                def _():
                    for g, k in targets:
                        carry_send(g, k, backward).wait_send()

            e_all.wait_send()
            for g, k in targets:
                plane_send(g, k).wait_send()

    with scope("wait_z"):
        w_last = w2[z]
        for k in range(1, nz):
            frm = lax.rem(z + k, nz)
            rcopy(z_send.at[0], z_recv.at[frm], z_ss.at[k], z_rs.at[frm], (frm, y, x, c)).wait_recv()
            w_last = w_last + z_recv[frm].astype(F32)
        gw_out[...] = w_last
        for copy in sends[1 - nz :]:
            copy.wait_send()


def write_out(*refs):
    copies = [pltpu.make_async_copy(refs[k], refs[4 + k], refs[8].at[k]) for k in range(4)]
    for copy in copies:
        copy.start()
    for copy in copies:
        copy.wait()


def on_device(nz, ny, nx, block_input, value_weight, query_pre, forget_pre, lower_bound, out_grad):
    tok, d_model = block_input.shape
    ch = value_weight.shape[1]
    pln = ny * nx
    piece = 2 * HEAD // pln
    rows = d_model // (nz * pln)
    vm, dma = pltpu.VMEM, pltpu.SemaphoreType.DMA
    scratch = [
        vm((tok, d_model), BF16), vm((ch, d_model), BF16),
        vm((ch, tok), BF16), vm((ch, tok), BF16), vm((ch, tok), BF16), vm((1, ch), F32),
        vm((pln, piece, ch), BF16), vm((1, ch), F32),
        vm((2, pln, piece, ch), BF16), vm((2, pln, 1, ch), F32),
        vm((2, pln, piece, ch), BF16), vm((pln // 2, piece, ch), BF16), vm((pln // 2, nx, piece, ch), BF16),
        vm((pln // 2, piece, ch), BF16),
        vm((2, piece, ch), BF16), vm((2, 1, ch), F32),
        vm((nz, 2, piece, ch), BF16), vm((nz, 2, 1, ch), F32),
        vm((2, piece, ch), BF16), vm((pln, piece, ch), BF16),
        vm((nx, ny, nz, rows, tok), BF16), vm((nx, ny, nz, rows, tok), BF16),
        vm((HEAD, ch), BF16), vm((nx, HEAD, ch), BF16),
        vm((ch, tok), BF16), vm((nx, ch, tok), BF16),
        vm((ch, tok), BF16), vm((nx, ch, tok), BF16),
        vm((nx, HEAD, ch), F32),
        vm((2, tok // 2, d_model), BF16), vm((tok // 2, d_model), BF16),
        vm((ny, ch, nz * rows), BF16), vm((ny, ch, nz * rows), BF16),
        vm((ny, ch, nz * rows), F32), vm((ny, ch, nz * rows), BF16), vm((ny, ch, nz * rows), BF16),
        vm((nz, rows, ch), F32), vm((nz, rows, ch), BF16), vm((nz, rows, ch), BF16),
        dma((6,)),
        dma((pln,)), dma((2, pln)), dma((pln,)), dma((2, pln)), dma, dma, dma((2, pln)), dma((pln,)),
        dma((nz,)), dma((nz,)), dma((nz,)), dma((nz,)),
        dma((2, pln)), dma((pln,)),
        *(dma((nx,)) for _ in range(8)),
        *(dma((ny,)) for _ in range(4)),
        dma((nz,)), dma((nz,)),
        dma, dma,
    ]
    hbm, near = pl.BlockSpec(memory_space=pl.ANY), pl.BlockSpec(memory_space=pltpu.VMEM)
    results = pl.pallas_call(
        functools.partial(kernel, nz, ny, nx),
        out_shape=(
            vm((ch, tok), BF16),
            vm((ch, tok), BF16),
            vm((tok // 2, d_model), BF16),
            vm((rows, ch), F32),
        ),
        in_specs=[hbm] * 6,
        out_specs=(near,) * 4,
        scratch_shapes=scratch,
        compiler_params=pltpu.CompilerParams(collective_id=0, has_side_effects=True),
    )(block_input, value_weight.T, query_pre.T, forget_pre.T, out_grad.T, lower_bound.reshape(1, ch))
    g_query, g_forget, g_input, g_weight = pl.pallas_call(
        write_out,
        out_shape=tuple(jax.ShapeDtypeStruct(a.shape, a.dtype) for a in results),
        in_specs=[near] * 4,
        out_specs=(hbm,) * 4,
        scratch_shapes=[dma((4,))],
    )(*(pltpu.with_memory_space_constraint(a, pltpu.VMEM) for a in results))
    return g_query.T, g_forget.T, g_input, g_weight


def on_mesh(devices):
    nz, ny, nx = devices.shape[:3]
    split = Mesh(devices, SP_TP)
    in_specs = (P(SP, None), P(None, "tp"), P(SP, "tp"), P(SP, "tp"), P("tp"), P(SP, "tp"))
    out_specs = (P(SP, "tp"), P(SP, "tp"), P(SP_TP, None), P(SP, "tp"))
    return jax.shard_map(
        functools.partial(on_device, nz, ny, nx), mesh=split, in_specs=in_specs, out_specs=out_specs, check_vma=False
    )


def solution(mesh):
    return on_mesh(mesh.devices.reshape(8, 4, 4, mesh.shape["tp"]))
```

```python
import functools

import jax
import jax.numpy as jnp
from jax import lax
from jax.experimental import pallas as pl
from jax.experimental.pallas import tpu as pltpu
from jax.sharding import Mesh
from jax.sharding import PartitionSpec as P

HEAD = 64
SP = ("sp_0", "sp_1", "sp_2")
SP_TP = ("sp_0", "sp_1", "sp_2", "tp")
F32, BF16 = jnp.float32, jnp.bfloat16
LOGICAL = pl.DeviceIdType.MESH


def nn(a, b):
    return lax.dot_general(a, b, (((1,), (0,)), ((), ())), preferred_element_type=F32)


def nt(a, b):
    return lax.dot_general(a, b, (((1,), (1,)), ((), ())), preferred_element_type=F32)


def tn(a, b):
    return lax.dot_general(a, b, (((0,), (0,)), ((), ())), preferred_element_type=F32)


def rcopy(src, dst, send, recv, device):
    return pltpu.make_async_remote_copy(
        src_ref=src, dst_ref=dst, send_sem=send, recv_sem=recv, device_id=device, device_id_type=LOGICAL
    )


def kernel(
    nz, ny, nx,
    x_hbm, w_hbm, q_hbm, f_hbm, go_hbm, lb_hbm,
    gq_out, gf_out, gx_out, gw_out,
    x_v, w_v, q_v, f_v, go_v, lb_v, wide, thin,
    s_send, e_send, s_buf, e_buf, l_send, q_state, q_grad, q_line, t_send, ft_send, t_buf, ft_buf, o_send, p_buf,
    xt, xtl, r_send, rl, k_send, kl, own_send, ownl, g_all, ig, ig_recv,
    m_send, m_recv, aacc, a_send, a_recv, w2, z_send, z_recv,
    lsem, s_ss, s_rs, e_ss, e_rs, ea_ss, ea_rs, q_ss, q_rs, t_ss, t_rs, ft_ss, ft_rs, p_ss, p_rs,
    xt_ss, xt_rs, r_ss, r_rs, k_ss, k_rs, own_ss, own_rs,
    m_ss, m_rs, a_ss, a_rs, z_ss, z_rs, ig_ss, ig_rs,
):
    pln = ny * nx
    tok, d_model = x_v.shape
    ch = w_v.shape[0]
    heads = ch // HEAD
    z, y, x, c = (lax.axis_index(a) for a in SP_TP)
    me = y * nx + x
    back = lax.rem(me, 2)
    at_line, at_col = x * (1 - c) + y * c, y * (1 - c) + x * c

    def line(i):
        return (z, y * (1 - c) + i * c, i * (1 - c) + x * c, c)

    def column(i):
        return (z, i * (1 - c) + y * c, x * (1 - c) + i * c, c)

    def spot(g, i):
        return lax.rem(i, nx) * ny + i // nx if g else i

    def owner(i):
        return (z, i // nx, lax.rem(i, nx), 1)

    def piece_of(i):
        return i // 2 + lax.rem(i, 2) * (pln // 2)

    def plane(i):
        return (z, i // nx, lax.rem(i, nx), c)

    def head_of(a, h):
        return a[HEAD * h : HEAD * (h + 1)]

    def by_head(parts):
        return jnp.concatenate(list(parts), axis=0)

    def arrived(ref, n, sem):
        part = ref.at[pl.ds(0, n)]
        rcopy(part, part, sem, sem, (z, y, x, 1 - c)).wait_recv()

    def left(ref, n, sem):
        part = ref.at[pl.ds(0, n)]
        rcopy(part, part, sem, sem, (z, y, x, 1 - c)).wait_send()

    scope = jax.named_scope
    with scope("loads_barrier"):
        barrier = pltpu.get_barrier_semaphore()

        def greet(device):
            pl.semaphore_signal(barrier, inc=1, device_id=device, device_id_type=LOGICAL)

        for k in range(1, nz):
            greet((lax.rem(z + k, nz), y, x, c))
        for k in range(1, pln):
            to = lax.rem(me + k, pln)
            greet((z, to // nx, lax.rem(to, nx), 1 - c))

            @pl.when((c == 1) | (to // nx == y) | (lax.rem(to, nx) == x))
            def _():
                greet(plane(to))

        greet((z, y, x, 1 - c))
        loads = [
            pltpu.make_async_copy(src, dst, lsem.at[k])
            for k, (src, dst) in enumerate(
                ((f_hbm, f_v), (q_hbm, q_v), (go_hbm, go_v), (x_hbm, x_v), (w_hbm, w_v), (lb_hbm, lb_v))
            )
        ]
        for copy in loads:
            copy.start()

    lane = lax.broadcasted_iota(jnp.int32, (1, ch), 1)
    mf = [jnp.where((lane >= HEAD * h) & (lane < HEAD * (h + 1)), 1.0, 0.0).astype(F32) for h in range(heads)]
    row = lax.broadcasted_iota(jnp.int32, (tok, tok), 0)
    col = lax.broadcasted_iota(jnp.int32, (tok, tok), 1)
    lower, upper = row >= col, col >= row
    lower_ones = jnp.where(lower, 1.0, 0.0).astype(BF16)
    upper_ones = jnp.where(upper, 1.0, 0.0).astype(BF16)

    def folded(full):
        out = full[:HEAD] * mf[0]
        for h in range(1, heads):
            out = out + head_of(full, h) * mf[h]
        return out

    with scope("gates"):
        loads[5].wait()
        gap = jnp.broadcast_to(1.0 - lb_v[...], (tok, ch)).T
        loads[0].wait()
        f = f_v[...].astype(F32)
        f_neg = 1.0 / (1.0 + jnp.exp(f))
        f_sig = 1.0 / (1.0 + jnp.exp(-f))
        k_rate = gap * f_neg
        logs = jnp.log1p(-k_rate)
        high = logs.astype(BF16)
        low = (logs - high.astype(F32)).astype(BF16)
        cum = nn(high, upper_ones) + nn(low, upper_ones)
        row_ones = jnp.ones((8, tok), BF16)
        total = jnp.exp((nt(row_ones, high) + nt(row_ones, low))[:1])
        closing = cum[:, tok - 1 : tok]
        growth = jnp.exp(cum)
        shrink = jnp.exp(-cum)
        remain = jnp.exp(closing - cum)
        e_send[...] = total
        k_dec = (k_rate * shrink).astype(BF16)
        k_end = (k_rate * remain).astype(BF16)
        loads[1].wait()
        q = q_v[...].astype(F32)
        q_sig = 1.0 / (1.0 + jnp.exp(-q))
        query = q * q_sig
        q_dec = (query * growth).astype(BF16)
        loads[2].wait()
        go = go_v[...]
        reach = folded(nt(go, q_dec))
    with scope("values"):
        loads[3].wait()
        loads[4].wait()
        v = nt(w_v[...], x_v[...]).astype(BF16)
        update = folded(nt(v, k_end))
        s_send[...] = jnp.concatenate([update, reach], axis=0).reshape(s_send.shape).astype(BF16)
        r_send[...] = reach.astype(BF16)
        k_send[...] = k_end

    with scope("turn"):
        rows = d_model // (nz * ny * nx)
        per = tok // rows
        for b in range(d_model // tok):
            turned = x_v[:, tok * b : tok * (b + 1)].T
            for g in range(per):
                at = b * per + g
                zz, yy, xx = at // pln, (at // nx) % ny, at % nx
                group, into = xx * (1 - c) + yy * c, yy * (1 - c) + xx * c
                xt[group, into, zz] = turned[rows * g : rows * (g + 1)]

    with scope("barrier_wait"):
        pl.semaphore_wait(barrier, pln + nz - 1 + c * (pln - 1) + (1 - c) * (nx + ny - 2))

    def to_line(source, target, send_sem, recv_sem):
        for k in range(1, nx):
            rcopy(source, target.at[at_line], send_sem, recv_sem, line(lax.rem(at_line + k, nx))).start()

    def to_column(source, target, send_sem, recv_sem):
        for k in range(1, ny):
            to = lax.rem(at_col + k, ny)
            rcopy(source.at[to], target.at[at_col], send_sem, recv_sem, column(to)).start()

    def from_column(own, target, recv_sem):
        arrived(target, ny - 1, recv_sem)
        out = own[...].astype(F32)
        for k in range(1, ny):
            out = out + target[lax.rem(at_col + k, ny)].astype(F32)
        return out

    def piece_sends(k):
        to = lax.rem(me + k, pln)
        return (
            rcopy(e_send, e_buf.at[c * pln + me], e_ss, e_rs, owner(to)),
            rcopy(s_send.at[piece_of(to)], s_buf.at[c * pln + me], s_ss, s_rs, owner(to)),
        )

    with scope("send1"):
        for k in range(1, pln):
            for copy in piece_sends(k):
                copy.start()

        @pl.when(c == 0)
        def _():
            for copy in piece_sends(0):
                copy.start()

        @pl.when(c == 1)
        def _():
            s_buf[pln + me] = s_send[piece_of(me)]
            e_buf[pln + me] = e_send[...]

        for k in range(1, nx):
            to = lax.rem(at_line + k, nx)
            rcopy(xt.at[to], xtl.at[at_line], xt_ss, xt_rs, line(to)).start()
        to_line(k_send, kl, k_ss, k_rs)

        @pl.when(c == 0)
        def _():
            to_line(r_send, rl, r_ss, r_rs)

        xtl[at_line] = xt[at_line]
        kl[at_line] = k_end
        rl[at_line] = r_send[...]

    with scope("pairs_value"):
        mixing = [jnp.where(lower, tn(head_of(q_dec, h), head_of(k_dec, h)), 0.0).astype(BF16) for h in range(heads)]
        gv_own = by_head(nn(head_of(go, h), mixing[h]) for h in range(heads))
        own_send[...] = gv_own.astype(BF16)
        ownl[at_line] = own_send[...]
        to_line(own_send, ownl, own_ss, own_rs)

    z_order = z + back * (nz - 1 - 2 * z)

    def z_sends(k):
        at = z_order + k
        to = at + back * (nz - 1 - 2 * at)
        return (
            rcopy(ft_send, ft_buf.at[z], ft_ss, ft_rs, (to, y, x, 1)),
            rcopy(t_send, t_buf.at[z], t_ss, t_rs, (to, y, x, 1)),
        )

    def carry_send(g, k, backward):
        to = lax.rem(me + k, pln)
        device = (z, to // nx, lax.rem(to, nx), g)
        if not backward:
            return rcopy(l_send.at[g * pln + spot(g, to)], q_state.at[me // 2], q_ss.at[g], q_rs.at[0], device)
        if g == 0:
            return rcopy(l_send.at[to // nx * nx + nx - 1], q_line.at[me // 2], q_ss.at[0], q_rs.at[1], device)
        first = pln + lax.rem(to, nx) * ny
        return rcopy(l_send.at[pl.ds(first, ny)], q_grad.at[pl.ds(me // 2 * ny, ny)], q_ss.at[1], q_rs.at[1], device)

    targets = [(0, k) for k in range(pln)] + [(1, k) for k in range(1, pln)]
    plane_decays = e_buf.at[pl.ds(0, pln)]
    e_all = rcopy(plane_decays, plane_decays, ea_ss, ea_rs, (z, y, x, 1 - c))

    @pl.when(c == 1)
    def _():
        with scope("wait1"):
            arrived(e_buf, 2 * pln - 1, e_rs)
            arrived(s_buf, 2 * pln - 1, s_rs)
        with scope("scan1"):
            for g in (0, 1):
                held = jnp.zeros(t_send.shape[1:], F32)
                factor = jnp.ones((1, ch), F32)
                for o in range(pln):
                    it = o + back * (pln - 1 - 2 * o)
                    l_send[g * pln + spot(g, it)] = held.astype(BF16)
                    decay = e_buf[g * pln + it]
                    held = decay * held + s_buf[g * pln + it].astype(F32)
                    factor = decay * factor
                t_send[g] = held.astype(BF16)
                ft_send[g] = factor
        with scope("send2"):
            for k in range(1, nz):

                @pl.when(z_order + k < nz)
                def _():
                    for copy in z_sends(k):
                        copy.start()

            for backward in (0, 1):

                @pl.when(back == backward)
                def _():
                    for g, k in targets:
                        carry_send(g, k, backward).start()

            e_all.start()

            @pl.when(back == 0)
            def _():
                q_state[me // 2] = l_send[pln + spot(1, me)]

            @pl.when(back == 1)
            def _():
                q_grad[pl.ds(me // 2 * ny, ny)] = l_send[pl.ds(pln + x * ny, ny)]

    with scope("pairs_query"):
        pairing = [jnp.where(upper, tn(head_of(v, h), head_of(go, h)), 0.0).astype(BF16) for h in range(heads)]
        gq_own = by_head(nn(head_of(k_dec, h), pairing[h]) for h in range(heads))
        gk_own = by_head(nt(head_of(q_dec, h), pairing[h]) for h in range(heads))

    with scope("decays"):
        @pl.when(c == 0)
        def _():
            e_all.wait_recv()

        decays = e_buf[pl.ds(c * pln, pln)]
        before, after = jnp.ones((1, ch), F32), [jnp.ones((1, ch), F32)] * nx
        ids = [line(i)[1] * nx + line(i)[2] for i in range(nx)]
        for i in range(pln):
            before = before * jnp.where(i < me, decays[i], 1.0)
            after = [a * jnp.where(i > n, decays[i], 1.0) for a, n in zip(after, ids)]

    with scope("wait_line"):
        arrived(xtl, nx - 1, xt_rs)
        arrived(kl, nx - 1, k_rs)

    def pairs(parts):
        return [jnp.concatenate(parts[i : i + 2], axis=1) for i in range(0, nx, 2)]

    def to_chunks(ref, total):
        for i in range(ny):
            ref[i] = total[:, i * nz * rows : (i + 1) * nz * rows].astype(ref.dtype)

    with scope("line_m"):
        turned_of = pairs([xtl[i].reshape(d_model // nx, tok) for i in range(nx)])
        tall_after = jnp.concatenate(after + [jnp.ones((8 - nx, ch), F32)], axis=0).T
        scaled = pairs([(kl[i].astype(F32) * tall_after[:, i : i + 1]).astype(BF16) for i in range(nx)])
        m_sum = nt(scaled[0], turned_of[0])
        for a, b in zip(scaled[1:], turned_of[1:]):
            m_sum = m_sum + nt(a, b)
        to_chunks(m_send, m_sum)

    def arriving(o, carried):
        frm = o + back * (nz - 1 - 2 * o)
        return ft_buf[frm] * carried + t_buf[frm].astype(F32)

    mine = piece_of(me)

    def plane_send(g, k):
        to = lax.rem(me + k, pln)
        device = (z, to // nx, lax.rem(to, nx), g)
        return rcopy(o_send.at[g], p_buf.at[mine], p_ss, p_rs, device)

    @pl.when(c == 1)
    def _():
        with scope("wait2"):
            for n in range(1, nz):

                @pl.when(z_order == n)
                def _():
                    arrived(ft_buf, n, ft_rs)
                    arrived(t_buf, n, t_rs)

            carried = lax.fori_loop(0, z_order, arriving, jnp.zeros(t_send.shape, F32))
        with scope("send3"):
            o_send[...] = carried.astype(BF16)
            for g, k in targets:
                plane_send(g, k).start()
            p_buf[mine] = o_send[1]

    with scope("send_m"):
        to_column(m_send, m_recv, m_ss, m_rs)

    some = pln // 2
    with scope("wait_1b"):

        @pl.when(c == 0)
        def _():
            arrived(q_state, some, q_rs.at[0])
            arrived(q_line, some, q_rs.at[1])
            arrived(rl, nx - 1, r_rs)

        @pl.when((c == 1) & (back == 0))
        def _():
            arrived(q_state, some - 1, q_rs.at[0])
            arrived(q_grad, some * ny, q_rs.at[1])

        @pl.when((c == 1) & (back == 1))
        def _():
            arrived(q_state, some, q_rs.at[0])
            arrived(q_grad, (some - 1) * ny, q_rs.at[1])

    with scope("wait_own"):
        arrived(ownl, nx - 1, own_rs)
    with scope("line_a"):
        state_in = q_state[...].astype(F32).reshape(HEAD, ch)

        @pl.when(c == 0)
        def _():
            grad_at = q_line[...].astype(F32).reshape(HEAD, ch)
            g_all[nx - 1] = grad_at
            for i in range(nx - 2, -1, -1):
                grad_at = e_buf[y * nx + i + 1] * grad_at + rl[i + 1].astype(F32)
                g_all[i] = grad_at

        @pl.when(c == 1)
        def _():
            for i in range(nx):
                part = [q_grad[j * ny + i].astype(F32) for j in range(some)]
                g_all[i] = jnp.concatenate(part, axis=0)

        parts = []
        for i in range(nx):
            grad_at = g_all[i]
            bd_in = by_head((grad_at * m).astype(BF16) for m in mf)
            parts.append((ownl[i].astype(F32) + nn(bd_in, kl[i])).astype(BF16))
        parts = pairs(parts)
        a_sum = nt(parts[0], turned_of[0])
        for a, b in zip(parts[1:], turned_of[1:]):
            a_sum = a_sum + nt(a, b)
        to_chunks(aacc, a_sum)
        to_chunks(a_send, a_sum)
        to_column(a_send, a_recv, a_ss, a_rs)

    with scope("wait_m"):
        m_plane = from_column(m_send.at[at_col], m_recv, m_rs).T.astype(BF16)
    with scope("wait3"):
        for core in (0, 1):

            @pl.when(c == core)
            def _():
                arrived(p_buf, pln - core, p_rs)

    with scope("wait_a"):
        a_plane = from_column(aacc.at[at_col], a_recv, a_rs).T
    with scope("send_z"):
        outer = p_buf[...].astype(F32).reshape(2 * HEAD, ch)
        state_out, grad_out = outer[:HEAD], outer[HEAD:]
        bd_out = by_head((grad_out * m).astype(BF16) for m in mf)
        w_sum = a_plane + nt(m_plane, bd_out)
        w2[...] = w_sum.reshape(w2.shape)
        z_send[...] = w_sum.astype(BF16).reshape(z_send.shape)
        for k in range(1, nz):
            to = lax.rem(z + k, nz)
            rcopy(z_send.at[to], z_recv.at[z], z_ss, z_rs, (to, y, x, c)).start()

    with scope("value_grad"):
        own_after = after[nx - 1]
        for i in range(nx - 1):
            own_after = jnp.where(at_line == i, after[i], own_after)
        state = state_in + before * state_out
        grad = g_all[at_line] + own_after * grad_out
        bd_state = by_head((state * m).astype(BF16) for m in mf)
        bd_grad = by_head((grad * m).astype(BF16) for m in mf)
        value_grad = (gv_own + nn(bd_grad, k_end)).astype(BF16)

    with scope("input_grad"):
        width = 512 if d_model % 512 == 0 else d_model
        turned = value_grad.T
        for j in range(d_model // width):
            cols = pl.ds(j * width, width)
            ig[:, :, cols] = nn(turned, w_v[:, cols]).astype(BF16).reshape(2, tok // 2, width)
        ig_copy = rcopy(ig.at[1 - c], ig_recv, ig_ss, ig_rs, (z, y, x, 1 - c))
        ig_copy.start()

    with scope("query_forget"):
        g_query = growth * (gq_own + tn(bd_state, go))
        g_key = shrink * gk_own + remain * tn(bd_grad, v)
        gq_out[...] = (g_query * (q_sig * (1.0 + q * (1.0 - q_sig)))).astype(BF16)
        ends = grad * (total * state + update)
        ends_high = ends.astype(BF16)
        ends_low = (ends - ends_high.astype(F32)).astype(BF16)
        tall_ones = jnp.ones((HEAD, tok), BF16)
        boundary = tn(ends_high, tall_ones) + tn(ends_low, tall_ones)
        flow = query * g_query - k_rate * g_key
        flow_high = flow.astype(BF16)
        flow_low = (flow - flow_high.astype(F32)).astype(BF16)
        g_decay = nn(flow_high, lower_ones) + nn(flow_low, lower_ones) + boundary
        gf_out[...] = ((g_decay / (1.0 - k_rate) - g_key) * k_rate * f_sig).astype(BF16)

    with scope("input_sum"):
        ig_copy.wait_recv()
        gx_out[...] = (ig[c].astype(F32) + ig_recv[...].astype(F32)).astype(BF16)

    with scope("drain"):
        left(xt, nx - 1, xt_ss)
        left(kl, nx - 1, k_ss)
        left(ownl, nx - 1, own_ss)
        left(m_send, ny - 1, m_ss)
        left(a_send, ny - 1, a_ss)
        ig_copy.wait_send()

        @pl.when(c == 0)
        def _():
            left(thin, pln, e_ss)
            left(s_send, pln, s_ss)
            left(rl, nx - 1, r_ss)

        @pl.when(c == 1)
        def _():
            left(thin, pln - 1, e_ss)
            left(s_send, pln - 1, s_ss)
            for n in range(1, nz):

                @pl.when(nz - 1 - z_order == n)
                def _():
                    left(ft_buf, n, ft_ss)
                    left(t_buf, n, t_ss)

            left(wide, pln, q_ss.at[0])
            for backward in (0, 1):

                @pl.when(back == backward)
                def _():
                    left(wide, (pln - 1) * (ny if backward else 1), q_ss.at[1])

            e_all.wait_send()
            left(wide, 2 * pln - 1, p_ss)

    with scope("wait_z"):
        arrived(z_recv, nz - 1, z_rs)
        w_last = w2[z]
        for k in range(1, nz):
            w_last = w_last + z_recv[lax.rem(z + k, nz)].astype(F32)
        gw_out[...] = w_last
        left(z_send, nz - 1, z_ss)


def write_out(*refs):
    copies = [pltpu.make_async_copy(refs[k], refs[4 + k], refs[8].at[k]) for k in range(4)]
    for copy in copies:
        copy.start()
    for copy in copies:
        copy.wait()


def on_device(nz, ny, nx, block_input, value_weight, query_pre, forget_pre, lower_bound, out_grad):
    tok, d_model = block_input.shape
    ch = value_weight.shape[1]
    pln = ny * nx
    piece = 2 * HEAD // pln
    rows = d_model // (nz * pln)
    vm, dma = pltpu.VMEM, pltpu.SemaphoreType.DMA
    scratch = [
        vm((tok, d_model), BF16), vm((ch, d_model), BF16),
        vm((ch, tok), BF16), vm((ch, tok), BF16), vm((ch, tok), BF16), vm((1, ch), F32),
        vm((pln * ny, piece, ch), BF16), vm((pln, 1, ch), F32),
        vm((pln, piece, ch), BF16), vm((1, ch), F32),
        vm((2 * pln, piece, ch), BF16), vm((2 * pln, 1, ch), F32),
        vm((2 * pln, piece, ch), BF16), vm((pln // 2, piece, ch), BF16), vm((pln // 2 * ny, piece, ch), BF16),
        vm((pln // 2, piece, ch), BF16),
        vm((2, piece, ch), BF16), vm((2, 1, ch), F32),
        vm((nz, 2, piece, ch), BF16), vm((nz, 2, 1, ch), F32),
        vm((2, piece, ch), BF16), vm((pln, piece, ch), BF16),
        vm((nx, ny, nz, rows, tok), BF16), vm((nx, ny, nz, rows, tok), BF16),
        vm((HEAD, ch), BF16), vm((nx, HEAD, ch), BF16),
        vm((ch, tok), BF16), vm((nx, ch, tok), BF16),
        vm((ch, tok), BF16), vm((nx, ch, tok), BF16),
        vm((nx, HEAD, ch), F32),
        vm((2, tok // 2, d_model), BF16), vm((tok // 2, d_model), BF16),
        vm((ny, ch, nz * rows), BF16), vm((ny, ch, nz * rows), BF16),
        vm((ny, ch, nz * rows), F32), vm((ny, ch, nz * rows), BF16), vm((ny, ch, nz * rows), BF16),
        vm((nz, rows, ch), F32), vm((nz, rows, ch), BF16), vm((nz, rows, ch), BF16),
        dma((6,)),
        *(dma for _ in range(6)), dma((2,)), dma((2,)),
        *(dma for _ in range(4 + 2 + 8 + 4 + 2 + 2)),
    ]
    hbm, near = pl.BlockSpec(memory_space=pl.ANY), pl.BlockSpec(memory_space=pltpu.VMEM)
    results = pl.pallas_call(
        functools.partial(kernel, nz, ny, nx),
        out_shape=(
            vm((ch, tok), BF16),
            vm((ch, tok), BF16),
            vm((tok // 2, d_model), BF16),
            vm((rows, ch), F32),
        ),
        in_specs=[hbm] * 6,
        out_specs=(near,) * 4,
        scratch_shapes=scratch,
        compiler_params=pltpu.CompilerParams(collective_id=0, has_side_effects=True),
    )(block_input, value_weight.T, query_pre.T, forget_pre.T, out_grad.T, lower_bound.reshape(1, ch))
    g_query, g_forget, g_input, g_weight = pl.pallas_call(
        write_out,
        out_shape=tuple(jax.ShapeDtypeStruct(a.shape, a.dtype) for a in results),
        in_specs=[near] * 4,
        out_specs=(hbm,) * 4,
        scratch_shapes=[dma((4,))],
    )(*(pltpu.with_memory_space_constraint(a, pltpu.VMEM) for a in results))
    return g_query.T, g_forget.T, g_input, g_weight


def on_mesh(devices):
    nz, ny, nx = devices.shape[:3]
    split = Mesh(devices, SP_TP)
    in_specs = (P(SP, None), P(None, "tp"), P(SP, "tp"), P(SP, "tp"), P("tp"), P(SP, "tp"))
    out_specs = (P(SP, "tp"), P(SP, "tp"), P(SP_TP, None), P(SP, "tp"))
    return jax.shard_map(
        functools.partial(on_device, nz, ny, nx), mesh=split, in_specs=in_specs, out_specs=out_specs, check_vma=False
    )


def solution(mesh):
    return on_mesh(mesh.devices.reshape(8, 4, 4, mesh.shape["tp"]))
```

```python
import functools

import jax
import jax.numpy as jnp
from jax import lax
from jax.experimental import pallas as pl
from jax.experimental.pallas import tpu as pltpu
from jax.sharding import Mesh
from jax.sharding import PartitionSpec as P

HEAD = 64
SP = ("sp_0", "sp_1", "sp_2")
SP_TP = ("sp_0", "sp_1", "sp_2", "tp")
F32, BF16 = jnp.float32, jnp.bfloat16
LOGICAL = pl.DeviceIdType.MESH


def nn(a, b):
    return lax.dot_general(a, b, (((1,), (0,)), ((), ())), preferred_element_type=F32)


def nt(a, b):
    return lax.dot_general(a, b, (((1,), (1,)), ((), ())), preferred_element_type=F32)


def tn(a, b):
    return lax.dot_general(a, b, (((0,), (0,)), ((), ())), preferred_element_type=F32)


def rcopy(src, dst, send, recv, device):
    return pltpu.make_async_remote_copy(
        src_ref=src, dst_ref=dst, send_sem=send, recv_sem=recv, device_id=device, device_id_type=LOGICAL
    )


def kernel(
    nz, ny, nx,
    x_hbm, w_hbm, q_hbm, f_hbm, go_hbm, lb_hbm,
    gq_out, gf_out, gx_out, gw_out,
    x_v, w_v, q_v, f_v, go_v, lb_v, wide, thin,
    s_send, e_send, s_buf, e_buf, l_send, q_state, q_grad, q_line, t_send, ft_send, t_buf, ft_buf, o_send, p_buf,
    xt, xtl, r_send, rl, k_send, kl, own_send, ownl, g_all, ig, ig_recv,
    m_send, m_recv, aacc, a_send, a_recv, w2, z_send, z_recv,
    lsem, s_ss, s_rs, e_ss, e_rs, ea_ss, ea_rs, q_ss, q_rs, t_ss, t_rs, ft_ss, ft_rs, p_ss, p_rs,
    xt_ss, xt_rs, r_ss, r_rs, k_ss, k_rs, own_ss, own_rs,
    m_ss, m_rs, a_ss, a_rs, z_ss, z_rs, ig_ss, ig_rs,
):
    pln = ny * nx
    tok, d_model = x_v.shape
    ch = w_v.shape[0]
    heads = ch // HEAD
    z, y, x, c = (lax.axis_index(a) for a in SP_TP)
    me = y * nx + x
    back = lax.rem(me, 2)
    zs, ys, xs = ([lax.rem(at + d, n) for d in range(n)] for at, n in ((z, nz), (y, ny), (x, nx)))
    across = lambda d, n: min(d, n - d)
    steps = [(dy, dx) for dy in range(ny) for dx in range(nx) if dy or dx]
    steps.sort(key=lambda t: -across(t[0], ny) - across(t[1], nx))
    others = [(ys[dy], xs[dx]) for dy, dx in steps]
    everyone = others + [(y, x)]
    z_steps = sorted(range(1, nz), key=lambda d: -across(d, nz))

    at_line, at_col = x * (1 - c) + y * c, y * (1 - c) + x * c
    lines = [xs[d] * (1 - c) + ys[d] * c for d in range(nx)]
    columns = [ys[d] * (1 - c) + xs[d] * c for d in range(ny)]

    def line(i):
        return (z, y * (1 - c) + i * c, i * (1 - c) + x * c, c)

    def column(i):
        return (z, i * (1 - c) + y * c, x * (1 - c) + i * c, c)

    def spot(g, i):
        return lax.rem(i, nx) * ny + lax.div(i, nx) if g else i

    def piece_of(ty, tx):
        return ty * (nx // 2) + lax.div(tx, 2) + lax.rem(tx, 2) * (pln // 2)

    def head_of(a, h):
        return a[HEAD * h : HEAD * (h + 1)]

    def by_head(parts):
        return jnp.concatenate(list(parts), axis=0)

    def arrived(ref, n, sem):
        part = ref.at[pl.ds(0, n)]
        rcopy(part, part, sem, sem, (z, y, x, 1 - c)).wait_recv()

    def left(ref, n, sem):
        part = ref.at[pl.ds(0, n)]
        rcopy(part, part, sem, sem, (z, y, x, 1 - c)).wait_send()

    scope = jax.named_scope
    with scope("loads_barrier"):
        loads = [
            pltpu.make_async_copy(src, dst, lsem.at[k])
            for k, (src, dst) in enumerate(
                ((f_hbm, f_v), (q_hbm, q_v), (go_hbm, go_v), (x_hbm, x_v), (w_hbm, w_v), (lb_hbm, lb_v))
            )
        ]
        for k in (0, 5, 1, 2, 3, 4):
            loads[k].start()
        barrier = pltpu.get_barrier_semaphore()

        def greet(device):
            pl.semaphore_signal(barrier, inc=1, device_id=device, device_id_type=LOGICAL)

        for ty, tx in others:
            greet((z, ty, tx, 1 - c))
        for d in z_steps:
            greet((zs[d], y, x, c))

        @pl.when(c == 1)
        def _():
            for ty, tx in others:
                greet((z, ty, tx, 1))

        @pl.when(c == 0)
        def _():
            for tx in xs[1:]:
                greet((z, y, tx, 0))
            for ty in ys[1:]:
                greet((z, ty, x, 0))

        greet((z, y, x, 1 - c))

    lane = lax.broadcasted_iota(jnp.int32, (1, ch), 1)
    mf = [jnp.where((lane >= HEAD * h) & (lane < HEAD * (h + 1)), 1.0, 0.0).astype(F32) for h in range(heads)]
    row = lax.broadcasted_iota(jnp.int32, (tok, tok), 0)
    col = lax.broadcasted_iota(jnp.int32, (tok, tok), 1)
    lower, upper = row >= col, col >= row
    lower_ones = jnp.where(lower, 1.0, 0.0).astype(BF16)
    upper_ones = jnp.where(upper, 1.0, 0.0).astype(BF16)

    def folded(full):
        out = full[:HEAD] * mf[0]
        for h in range(1, heads):
            out = out + head_of(full, h) * mf[h]
        return out

    with scope("gates"):
        loads[5].wait()
        gap = jnp.broadcast_to(1.0 - lb_v[...], (tok, ch)).T
        loads[0].wait()
        f = f_v[...].astype(F32)
        f_neg = 1.0 / (1.0 + jnp.exp(f))
        k_rate = gap * f_neg
        logs = jnp.log1p(-k_rate)
        high = logs.astype(BF16)
        low = (logs - high.astype(F32)).astype(BF16)
        cum = nn(high, upper_ones) + nn(low, upper_ones)
        row_ones = jnp.ones((8, tok), BF16)
        total = jnp.exp((nt(row_ones, high) + nt(row_ones, low))[:1])
        closing = cum[:, tok - 1 : tok]
        growth = jnp.exp(cum)
        remain = jnp.exp(closing - cum)
        e_send[...] = total
        k_end = (k_rate * remain).astype(BF16)
        loads[1].wait()
        q = q_v[...].astype(F32)
        q_sig = 1.0 / (1.0 + jnp.exp(-q))
        query = q * q_sig
        q_dec = (query * growth).astype(BF16)
        loads[2].wait()
        go = go_v[...]
        reach = folded(nt(go, q_dec))
    with scope("values"):
        loads[3].wait()
        loads[4].wait()
        v = nt(w_v[...], x_v[...]).astype(BF16)
        update = folded(nt(v, k_end))
        s_send[...] = jnp.concatenate([update, reach], axis=0).reshape(s_send.shape).astype(BF16)
        r_send[...] = reach.astype(BF16)
        k_send[...] = k_end

    with scope("barrier_wait"):
        pl.semaphore_wait(barrier, pln + nz - 1 + c * (pln - 1) + (1 - c) * (nx + ny - 2))

    def to_line(source, target, send_sem, recv_sem):
        for k in range(1, nx):
            rcopy(source, target.at[at_line], send_sem, recv_sem, line(lines[k])).start()

    def to_column(source, target, send_sem, recv_sem):
        for k in range(1, ny):
            to = columns[k]
            rcopy(source.at[to], target.at[at_col], send_sem, recv_sem, column(to)).start()

    def from_column(own, target, recv_sem):
        arrived(target, ny - 1, recv_sem)
        out = own[...].astype(F32)
        for k in range(1, ny):
            out = out + target[columns[k]].astype(F32)
        return out

    def piece_sends(ty, tx):
        to = (z, ty, tx, 1)
        return (
            rcopy(e_send, e_buf.at[c * pln + me], e_ss, e_rs, to),
            rcopy(s_send.at[piece_of(ty, tx)], s_buf.at[c * pln + me], s_ss, s_rs, to),
        )

    mine = piece_of(y, x)
    with scope("send1"):
        for ty, tx in others:
            for copy in piece_sends(ty, tx):
                copy.start()

        @pl.when(c == 0)
        def _():
            for copy in piece_sends(y, x):
                copy.start()

        @pl.when(c == 1)
        def _():
            s_buf[pln + me] = s_send[mine]
            e_buf[pln + me] = e_send[...]

        to_line(k_send, kl, k_ss, k_rs)
        kl[at_line] = k_end
        rl[at_line] = r_send[...]

    rows = d_model // (nz * ny * nx)
    with scope("turn"):
        per = tok // rows
        for b in range(d_model // tok):
            turned = x_v[:, tok * b : tok * (b + 1)].T
            for g in range(per):
                at = b * per + g
                zz, yy, xx = at // pln, (at // nx) % ny, at % nx
                group, into = xx * (1 - c) + yy * c, yy * (1 - c) + xx * c
                xt[group, into, zz] = turned[rows * g : rows * (g + 1)]

        for k in range(1, nx):
            to = lines[k]
            rcopy(xt.at[to], xtl.at[at_line], xt_ss, xt_rs, line(to)).start()

        @pl.when(c == 0)
        def _():
            to_line(r_send, rl, r_ss, r_rs)

        xtl[at_line] = xt[at_line]

    with scope("pairs_value"):
        shrink = jnp.exp(-cum)
        k_dec = (k_rate * shrink).astype(BF16)
        mixing = [jnp.where(lower, tn(head_of(q_dec, h), head_of(k_dec, h)), 0.0).astype(BF16) for h in range(heads)]
        gv_own = by_head(nn(head_of(go, h), mixing[h]) for h in range(heads))
        own_send[...] = gv_own.astype(BF16)
        ownl[at_line] = own_send[...]
        to_line(own_send, ownl, own_ss, own_rs)

    z_order = z + back * (nz - 1 - 2 * z)

    def z_sends(k):
        at = z_order + k
        to = at + back * (nz - 1 - 2 * at)
        return (
            rcopy(ft_send, ft_buf.at[z], ft_ss, ft_rs, (to, y, x, 1)),
            rcopy(t_send, t_buf.at[z], t_ss, t_rs, (to, y, x, 1)),
        )

    def carry_send(g, ty, tx, backward):
        device = (z, ty, tx, g)
        if not backward:
            at = pln + tx * ny + ty if g else ty * nx + tx
            return rcopy(l_send.at[at], q_state.at[me // 2], q_ss.at[g], q_rs.at[0], device)
        if g == 0:
            return rcopy(l_send.at[ty * nx + nx - 1], q_line.at[me // 2], q_ss.at[0], q_rs.at[1], device)
        rows_of = pl.ds(pln + tx * ny, ny)
        return rcopy(l_send.at[rows_of], q_grad.at[pl.ds(me // 2 * ny, ny)], q_ss.at[1], q_rs.at[1], device)

    targets = [(0, *t) for t in everyone] + [(1, *t) for t in others]
    plane_decays = e_buf.at[pl.ds(0, pln)]
    e_all = rcopy(plane_decays, plane_decays, ea_ss, ea_rs, (z, y, x, 1 - c))

    @pl.when(c == 1)
    def _():
        with scope("wait1"):
            arrived(e_buf, 2 * pln - 1, e_rs)
            arrived(s_buf, 2 * pln - 1, s_rs)
        with scope("scan1"):
            for g in (0, 1):
                held = jnp.zeros(t_send.shape[1:], F32)
                factor = jnp.ones((1, ch), F32)
                for o in range(pln):
                    it = o + back * (pln - 1 - 2 * o)
                    l_send[g * pln + spot(g, it)] = held.astype(BF16)
                    decay = e_buf[g * pln + it]
                    held = decay * held + s_buf[g * pln + it].astype(F32)
                    factor = decay * factor
                t_send[g] = held.astype(BF16)
                ft_send[g] = factor
        with scope("send2"):
            for k in range(1, nz):

                @pl.when(z_order + k < nz)
                def _():
                    for copy in z_sends(k):
                        copy.start()

            for backward in (0, 1):

                @pl.when(back == backward)
                def _():
                    for target in targets:
                        carry_send(*target, backward).start()

            e_all.start()

            @pl.when(back == 0)
            def _():
                q_state[me // 2] = l_send[pln + x * ny + y]

            @pl.when(back == 1)
            def _():
                q_grad[pl.ds(me // 2 * ny, ny)] = l_send[pl.ds(pln + x * ny, ny)]

    with scope("pairs_query"):
        pairing = [jnp.where(upper, tn(head_of(v, h), head_of(go, h)), 0.0).astype(BF16) for h in range(heads)]
        gq_own = by_head(nn(head_of(k_dec, h), pairing[h]) for h in range(heads))
        gk_own = by_head(nt(head_of(q_dec, h), pairing[h]) for h in range(heads))

    with scope("decays"):
        @pl.when(c == 0)
        def _():
            e_all.wait_recv()

        decays = e_buf[pl.ds(c * pln, pln)]
        before, after = jnp.ones((1, ch), F32), [jnp.ones((1, ch), F32)] * nx
        ids = [line(i)[1] * nx + line(i)[2] for i in range(nx)]
        for i in range(pln):
            before = before * jnp.where(i < me, decays[i], 1.0)
            after = [a * jnp.where(i > n, decays[i], 1.0) for a, n in zip(after, ids)]

    with scope("wait_line"):
        arrived(xtl, nx - 1, xt_rs)
        arrived(kl, nx - 1, k_rs)

    def pairs(parts):
        return [jnp.concatenate(parts[i : i + 2], axis=1) for i in range(0, nx, 2)]

    def to_chunks(ref, total):
        for i in range(ny):
            ref[i] = total[:, i * nz * rows : (i + 1) * nz * rows].astype(ref.dtype)

    with scope("line_m"):
        turned_of = pairs([xtl[i].reshape(d_model // nx, tok) for i in range(nx)])
        tall_after = jnp.concatenate(after + [jnp.ones((8 - nx, ch), F32)], axis=0).T
        scaled = pairs([(kl[i].astype(F32) * tall_after[:, i : i + 1]).astype(BF16) for i in range(nx)])
        m_sum = nt(scaled[0], turned_of[0])
        for a, b in zip(scaled[1:], turned_of[1:]):
            m_sum = m_sum + nt(a, b)
        to_chunks(m_send, m_sum)

    def arriving(o, carried):
        frm = o + back * (nz - 1 - 2 * o)
        return ft_buf[frm] * carried + t_buf[frm].astype(F32)

    def plane_send(g, ty, tx):
        return rcopy(o_send.at[g], p_buf.at[mine], p_ss, p_rs, (z, ty, tx, g))

    @pl.when(c == 1)
    def _():
        with scope("wait2"):
            for n in range(1, nz):

                @pl.when(z_order == n)
                def _():
                    arrived(ft_buf, n, ft_rs)
                    arrived(t_buf, n, t_rs)

            carried = lax.fori_loop(0, z_order, arriving, jnp.zeros(t_send.shape, F32))
        with scope("send3"):
            o_send[...] = carried.astype(BF16)
            for target in targets:
                plane_send(*target).start()
            p_buf[mine] = o_send[1]

    with scope("send_m"):
        to_column(m_send, m_recv, m_ss, m_rs)

    some = pln // 2
    with scope("wait_1b"):

        @pl.when(c == 0)
        def _():
            arrived(q_state, some, q_rs.at[0])
            arrived(q_line, some, q_rs.at[1])
            arrived(rl, nx - 1, r_rs)

        @pl.when((c == 1) & (back == 0))
        def _():
            arrived(q_state, some - 1, q_rs.at[0])
            arrived(q_grad, some * ny, q_rs.at[1])

        @pl.when((c == 1) & (back == 1))
        def _():
            arrived(q_state, some, q_rs.at[0])
            arrived(q_grad, (some - 1) * ny, q_rs.at[1])

    with scope("wait_own"):
        arrived(ownl, nx - 1, own_rs)
    with scope("line_a"):
        state_in = q_state[...].astype(F32).reshape(HEAD, ch)

        @pl.when(c == 0)
        def _():
            grad_at = q_line[...].astype(F32).reshape(HEAD, ch)
            g_all[nx - 1] = grad_at
            for i in range(nx - 2, -1, -1):
                grad_at = e_buf[y * nx + i + 1] * grad_at + rl[i + 1].astype(F32)
                g_all[i] = grad_at

        @pl.when(c == 1)
        def _():
            for i in range(nx):
                part = [q_grad[j * ny + i].astype(F32) for j in range(some)]
                g_all[i] = jnp.concatenate(part, axis=0)

        parts = []
        for i in range(nx):
            grad_at = g_all[i]
            bd_in = by_head((grad_at * m).astype(BF16) for m in mf)
            parts.append((ownl[i].astype(F32) + nn(bd_in, kl[i])).astype(BF16))
        parts = pairs(parts)
        a_sum = nt(parts[0], turned_of[0])
        for a, b in zip(parts[1:], turned_of[1:]):
            a_sum = a_sum + nt(a, b)
        to_chunks(aacc, a_sum)
        to_chunks(a_send, a_sum)
        to_column(a_send, a_recv, a_ss, a_rs)

    with scope("wait_m"):
        m_plane = from_column(m_send.at[at_col], m_recv, m_rs).T.astype(BF16)
    with scope("wait3"):
        for core in (0, 1):

            @pl.when(c == core)
            def _():
                arrived(p_buf, pln - core, p_rs)

    with scope("wait_a"):
        a_plane = from_column(aacc.at[at_col], a_recv, a_rs).T
    with scope("send_z"):
        outer = p_buf[...].astype(F32).reshape(2 * HEAD, ch)
        state_out, grad_out = outer[:HEAD], outer[HEAD:]
        bd_out = by_head((grad_out * m).astype(BF16) for m in mf)
        w_sum = a_plane + nt(m_plane, bd_out)
        w2[...] = w_sum.reshape(w2.shape)
        z_send[...] = w_sum.astype(BF16).reshape(z_send.shape)
        for d in z_steps:
            rcopy(z_send.at[zs[d]], z_recv.at[z], z_ss, z_rs, (zs[d], y, x, c)).start()

    with scope("value_grad"):
        own_after = after[nx - 1]
        for i in range(nx - 1):
            own_after = jnp.where(at_line == i, after[i], own_after)
        state = state_in + before * state_out
        grad = g_all[at_line] + own_after * grad_out
        bd_state = by_head((state * m).astype(BF16) for m in mf)
        bd_grad = by_head((grad * m).astype(BF16) for m in mf)
        value_grad = (gv_own + nn(bd_grad, k_end)).astype(BF16)

    with scope("input_grad"):
        width = 512 if d_model % 512 == 0 else d_model
        turned = value_grad.T
        for j in range(d_model // width):
            cols = pl.ds(j * width, width)
            ig[:, :, cols] = nn(turned, w_v[:, cols]).astype(BF16).reshape(2, tok // 2, width)
        ig_copy = rcopy(ig.at[1 - c], ig_recv, ig_ss, ig_rs, (z, y, x, 1 - c))
        ig_copy.start()

    with scope("query_forget"):
        g_query = growth * (gq_own + tn(bd_state, go))
        g_key = shrink * gk_own + remain * tn(bd_grad, v)
        gq_out[...] = (g_query * (q_sig * (1.0 + q * (1.0 - q_sig)))).astype(BF16)
        ends = grad * (total * state + update)
        ends_high = ends.astype(BF16)
        ends_low = (ends - ends_high.astype(F32)).astype(BF16)
        tall_ones = jnp.ones((HEAD, tok), BF16)
        boundary = tn(ends_high, tall_ones) + tn(ends_low, tall_ones)
        flow = query * g_query - k_rate * g_key
        flow_high = flow.astype(BF16)
        flow_low = (flow - flow_high.astype(F32)).astype(BF16)
        g_decay = nn(flow_high, lower_ones) + nn(flow_low, lower_ones) + boundary
        gf_out[...] = ((g_decay / (1.0 - k_rate) - g_key) * k_rate * (1.0 / (1.0 + jnp.exp(-f)))).astype(BF16)

    with scope("input_sum"):
        ig_copy.wait_recv()
        gx_out[...] = (ig[c].astype(F32) + ig_recv[...].astype(F32)).astype(BF16)

    with scope("drain"):
        left(xt, nx - 1, xt_ss)
        left(kl, nx - 1, k_ss)
        left(ownl, nx - 1, own_ss)
        left(m_send, ny - 1, m_ss)
        left(a_send, ny - 1, a_ss)
        ig_copy.wait_send()

        @pl.when(c == 0)
        def _():
            left(thin, pln, e_ss)
            left(s_send, pln, s_ss)
            left(rl, nx - 1, r_ss)

        @pl.when(c == 1)
        def _():
            left(thin, pln - 1, e_ss)
            left(s_send, pln - 1, s_ss)
            for n in range(1, nz):

                @pl.when(nz - 1 - z_order == n)
                def _():
                    left(ft_buf, n, ft_ss)
                    left(t_buf, n, t_ss)

            left(wide, pln, q_ss.at[0])
            for backward in (0, 1):

                @pl.when(back == backward)
                def _():
                    left(wide, (pln - 1) * (ny if backward else 1), q_ss.at[1])

            e_all.wait_send()
            left(wide, 2 * pln - 1, p_ss)

    with scope("wait_z"):
        arrived(z_recv, nz - 1, z_rs)
        w_last = w2[z]
        for k in range(1, nz):
            w_last = w_last + z_recv[zs[k]].astype(F32)
        gw_out[...] = w_last
        left(z_send, nz - 1, z_ss)


def write_out(*refs):
    copies = [pltpu.make_async_copy(refs[k], refs[4 + k], refs[8].at[k]) for k in range(4)]
    for copy in copies:
        copy.start()
    for copy in copies:
        copy.wait()


def on_device(nz, ny, nx, block_input, value_weight, query_pre, forget_pre, lower_bound, out_grad):
    tok, d_model = block_input.shape
    ch = value_weight.shape[1]
    pln = ny * nx
    piece = 2 * HEAD // pln
    rows = d_model // (nz * pln)
    vm, dma = pltpu.VMEM, pltpu.SemaphoreType.DMA
    scratch = [
        vm((tok, d_model), BF16), vm((ch, d_model), BF16),
        vm((ch, tok), BF16), vm((ch, tok), BF16), vm((ch, tok), BF16), vm((1, ch), F32),
        vm((pln * ny, piece, ch), BF16), vm((pln, 1, ch), F32),
        vm((pln, piece, ch), BF16), vm((1, ch), F32),
        vm((2 * pln, piece, ch), BF16), vm((2 * pln, 1, ch), F32),
        vm((2 * pln, piece, ch), BF16), vm((pln // 2, piece, ch), BF16), vm((pln // 2 * ny, piece, ch), BF16),
        vm((pln // 2, piece, ch), BF16),
        vm((2, piece, ch), BF16), vm((2, 1, ch), F32),
        vm((nz, 2, piece, ch), BF16), vm((nz, 2, 1, ch), F32),
        vm((2, piece, ch), BF16), vm((pln, piece, ch), BF16),
        vm((nx, ny, nz, rows, tok), BF16), vm((nx, ny, nz, rows, tok), BF16),
        vm((HEAD, ch), BF16), vm((nx, HEAD, ch), BF16),
        vm((ch, tok), BF16), vm((nx, ch, tok), BF16),
        vm((ch, tok), BF16), vm((nx, ch, tok), BF16),
        vm((nx, HEAD, ch), F32),
        vm((2, tok // 2, d_model), BF16), vm((tok // 2, d_model), BF16),
        vm((ny, ch, nz * rows), BF16), vm((ny, ch, nz * rows), BF16),
        vm((ny, ch, nz * rows), F32), vm((ny, ch, nz * rows), BF16), vm((ny, ch, nz * rows), BF16),
        vm((nz, rows, ch), F32), vm((nz, rows, ch), BF16), vm((nz, rows, ch), BF16),
        dma((6,)),
        *(dma for _ in range(6)), dma((2,)), dma((2,)),
        *(dma for _ in range(4 + 2 + 8 + 4 + 2 + 2)),
    ]
    hbm, near = pl.BlockSpec(memory_space=pl.ANY), pl.BlockSpec(memory_space=pltpu.VMEM)
    results = pl.pallas_call(
        functools.partial(kernel, nz, ny, nx),
        out_shape=(
            vm((ch, tok), BF16),
            vm((ch, tok), BF16),
            vm((tok // 2, d_model), BF16),
            vm((rows, ch), F32),
        ),
        in_specs=[hbm] * 6,
        out_specs=(near,) * 4,
        scratch_shapes=scratch,
        compiler_params=pltpu.CompilerParams(collective_id=0, has_side_effects=True),
    )(block_input, value_weight.T, query_pre.T, forget_pre.T, out_grad.T, lower_bound.reshape(1, ch))
    g_query, g_forget, g_input, g_weight = pl.pallas_call(
        write_out,
        out_shape=tuple(jax.ShapeDtypeStruct(a.shape, a.dtype) for a in results),
        in_specs=[near] * 4,
        out_specs=(hbm,) * 4,
        scratch_shapes=[dma((4,))],
    )(*(pltpu.with_memory_space_constraint(a, pltpu.VMEM) for a in results))
    return g_query.T, g_forget.T, g_input, g_weight


def on_mesh(devices):
    nz, ny, nx = devices.shape[:3]
    split = Mesh(devices, SP_TP)
    in_specs = (P(SP, None), P(None, "tp"), P(SP, "tp"), P(SP, "tp"), P("tp"), P(SP, "tp"))
    out_specs = (P(SP, "tp"), P(SP, "tp"), P(SP_TP, None), P(SP, "tp"))
    return jax.shard_map(
        functools.partial(on_device, nz, ny, nx), mesh=split, in_specs=in_specs, out_specs=out_specs, check_vma=False
    )


def solution(mesh):
    return on_mesh(mesh.devices.reshape(8, 4, 4, mesh.shape["tp"]))
```

```python
import functools

import jax
import jax.numpy as jnp
from jax import lax
from jax.experimental import pallas as pl
from jax.experimental.pallas import tpu as pltpu
from jax.sharding import Mesh
from jax.sharding import PartitionSpec as P

HEAD = 64
SP = ("sp_0", "sp_1", "sp_2")
SP_TP = ("sp_0", "sp_1", "sp_2", "tp")
F32, BF16 = jnp.float32, jnp.bfloat16
LOGICAL = pl.DeviceIdType.MESH


def nn(a, b):
    return lax.dot_general(a, b, (((1,), (0,)), ((), ())), preferred_element_type=F32)


def nt(a, b):
    return lax.dot_general(a, b, (((1,), (1,)), ((), ())), preferred_element_type=F32)


def tn(a, b):
    return lax.dot_general(a, b, (((0,), (0,)), ((), ())), preferred_element_type=F32)


def rcopy(src, dst, send, recv, device):
    return pltpu.make_async_remote_copy(
        src_ref=src, dst_ref=dst, send_sem=send, recv_sem=recv, device_id=device, device_id_type=LOGICAL
    )


def kernel(
    nz, ny, nx,
    x_hbm, w_hbm, q_hbm, f_hbm, go_hbm, lb_hbm,
    gq_out, gf_out, gx_out, gw_out,
    x_v, w_v, q_v, f_v, go_v, lb_v, wide, thin,
    s_send, e_send, s_buf, e_buf, l_send, q_state, q_grad, q_line, t_send, ft_send, t_buf, ft_buf, o_send, p_buf, p_both, outer,
    xt, xtl, r_send, rl, k_send, kl, own_send, ownl, g_all, ig, ig_recv,
    m_send, m_recv, aacc, a_send, a_recv, w2, z_send, z_recv,
    lsem, s_ss, s_rs, e_ss, e_rs, ea_ss, ea_rs, q_ss, q_rs, t_ss, t_rs, ft_ss, ft_rs, p_ss, p_rs,
    xt_ss, xt_rs, r_ss, r_rs, k_ss, k_rs, own_ss, own_rs,
    m_ss, m_rs, a_ss, a_rs, z_ss, z_rs, ig_ss, ig_rs,
):
    pln = ny * nx
    tok, d_model = x_v.shape
    ch = w_v.shape[0]
    heads = ch // HEAD
    z, y, x, c = (lax.axis_index(a) for a in SP_TP)
    me = y * nx + x
    back = lax.rem(me, 2)
    zs, ys, xs = ([lax.rem(at + d, n) for d in range(n)] for at, n in ((z, nz), (y, ny), (x, nx)))
    across = lambda d, n: min(d, n - d)
    steps = [(dy, dx) for dy in range(ny) for dx in range(nx) if dy or dx]
    steps.sort(key=lambda t: -across(t[0], ny) - across(t[1], nx))
    others = [(ys[dy], xs[dx]) for dy, dx in steps]
    everyone = others + [(y, x)]
    z_steps = sorted(range(1, nz), key=lambda d: -across(d, nz))

    at_line, at_col = x * (1 - c) + y * c, y * (1 - c) + x * c
    lines = [xs[d] * (1 - c) + ys[d] * c for d in range(nx)]
    columns = [ys[d] * (1 - c) + xs[d] * c for d in range(ny)]

    def line(i):
        return (z, y * (1 - c) + i * c, i * (1 - c) + x * c, c)

    def column(i):
        return (z, i * (1 - c) + y * c, x * (1 - c) + i * c, c)

    def spot(g, i):
        return lax.rem(i, nx) * ny + lax.div(i, nx) if g else i

    def piece_of(ty, tx):
        return ty * (nx // 2) + lax.div(tx, 2) + lax.rem(tx, 2) * (pln // 2)

    def head_of(a, h):
        return a[HEAD * h : HEAD * (h + 1)]

    def by_head(parts):
        return jnp.concatenate(list(parts), axis=0)

    def arrived(ref, n, sem):
        part = ref.at[pl.ds(0, n)]
        rcopy(part, part, sem, sem, (z, y, x, 1 - c)).wait_recv()

    def left(ref, n, sem):
        part = ref.at[pl.ds(0, n)]
        rcopy(part, part, sem, sem, (z, y, x, 1 - c)).wait_send()

    scope = jax.named_scope
    with scope("loads_barrier"):
        loads = [
            pltpu.make_async_copy(src, dst, lsem.at[k])
            for k, (src, dst) in enumerate(
                ((f_hbm, f_v), (q_hbm, q_v), (go_hbm, go_v), (x_hbm, x_v), (w_hbm, w_v), (lb_hbm, lb_v))
            )
        ]
        for k in (0, 5, 1, 2, 3, 4):
            loads[k].start()
        barrier = pltpu.get_barrier_semaphore()

        def greet(device):
            pl.semaphore_signal(barrier, inc=1, device_id=device, device_id_type=LOGICAL)

        for ty, tx in others:
            greet((z, ty, tx, 1 - c))
        for d in z_steps:
            greet((zs[d], y, x, 1))

        @pl.when(c == 1)
        def _():
            for d in z_steps:
                greet((zs[d], y, x, 0))
            for ty, tx in others:
                greet((z, ty, tx, 1))

        @pl.when(c == 0)
        def _():
            for tx in xs[1:]:
                greet((z, y, tx, 0))

        greet((z, y, x, 1 - c))

    lane = lax.broadcasted_iota(jnp.int32, (1, ch), 1)
    mf = [jnp.where((lane >= HEAD * h) & (lane < HEAD * (h + 1)), 1.0, 0.0).astype(F32) for h in range(heads)]
    row = lax.broadcasted_iota(jnp.int32, (tok, tok), 0)
    col = lax.broadcasted_iota(jnp.int32, (tok, tok), 1)
    lower, upper = row >= col, col >= row
    lower_ones = jnp.where(lower, 1.0, 0.0).astype(BF16)
    upper_ones = jnp.where(upper, 1.0, 0.0).astype(BF16)

    def folded(full):
        out = full[:HEAD] * mf[0]
        for h in range(1, heads):
            out = out + head_of(full, h) * mf[h]
        return out

    with scope("gates"):
        loads[5].wait()
        gap = jnp.broadcast_to(1.0 - lb_v[...], (tok, ch)).T
        loads[0].wait()
        f = f_v[...].astype(F32)
        f_neg = 1.0 / (1.0 + jnp.exp(f))
        k_rate = gap * f_neg
        logs = jnp.log1p(-k_rate)
        high = logs.astype(BF16)
        low = (logs - high.astype(F32)).astype(BF16)
        cum = nn(high, upper_ones) + nn(low, upper_ones)
        row_ones = jnp.ones((8, tok), BF16)
        total = jnp.exp((nt(row_ones, high) + nt(row_ones, low))[:1])
        closing = cum[:, tok - 1 : tok]
        growth = jnp.exp(cum)
        remain = jnp.exp(closing - cum)
        e_send[...] = total
        k_end = (k_rate * remain).astype(BF16)
        loads[1].wait()
        q = q_v[...].astype(F32)
        q_sig = 1.0 / (1.0 + jnp.exp(-q))
        query = q * q_sig
        q_dec = (query * growth).astype(BF16)
        loads[2].wait()
        go = go_v[...]
        reach = folded(nt(go, q_dec))
    with scope("values"):
        loads[3].wait()
        loads[4].wait()
        v = nt(w_v[...], x_v[...]).astype(BF16)
        update = folded(nt(v, k_end))
        s_send[...] = jnp.concatenate([update, reach], axis=0).reshape(s_send.shape).astype(BF16)
        r_send[...] = reach.astype(BF16)
        k_send[...] = k_end

    with scope("barrier_wait"):
        pl.semaphore_wait(barrier, pln + nz - 1 + c * (pln + nz - 2) + (1 - c) * (nx - 1))

    def to_line(source, target, send_sem, recv_sem):
        for k in range(1, nx):
            rcopy(source, target.at[at_line], send_sem, recv_sem, line(lines[k])).start()

    def to_column(source, target, send_sem, recv_sem):
        for k in range(1, ny):
            to = columns[k]
            device = (z, to * (1 - c) + y * c, x * (1 - c) + to * c, 1)
            rcopy(source.at[to], target.at[c * ny + at_col], send_sem, recv_sem.at[c], device).start()

        @pl.when(c == 0)
        def _():
            rcopy(source.at[y], target.at[y], send_sem, recv_sem.at[0], (z, y, x, 1)).start()

    def from_column(g, own, target, recv_sem):
        arrived(target, ny - g, recv_sem.at[g])
        if g == 0:
            out = target[0].astype(F32)
            for k in range(1, ny):
                out = out + target[k].astype(F32)
            return out.T
        out = own[...].astype(F32)
        for k in range(1, ny):
            out = out + target[ny + xs[k]].astype(F32)
        return out.T

    def piece_sends(ty, tx):
        to = (z, ty, tx, 1)
        return (
            rcopy(e_send, e_buf.at[c * pln + me], e_ss, e_rs, to),
            rcopy(s_send.at[piece_of(ty, tx)], s_buf.at[c * pln + me], s_ss, s_rs, to),
        )

    mine = piece_of(y, x)
    with scope("send1"):
        for ty, tx in others:
            for copy in piece_sends(ty, tx):
                copy.start()

        @pl.when(c == 0)
        def _():
            for copy in piece_sends(y, x):
                copy.start()

        @pl.when(c == 1)
        def _():
            s_buf[pln + me] = s_send[mine]
            e_buf[pln + me] = e_send[...]

        to_line(k_send, kl, k_ss, k_rs)
        kl[at_line] = k_end
        rl[at_line] = r_send[...]

    rows = d_model // (nz * ny * nx)
    with scope("turn"):
        per = tok // rows
        for b in range(d_model // tok):
            turned = x_v[:, tok * b : tok * (b + 1)].T
            for g in range(per):
                at = b * per + g
                zz, yy, xx = at // pln, (at // nx) % ny, at % nx
                group, into = xx * (1 - c) + yy * c, yy * (1 - c) + xx * c
                xt[group, into, zz] = turned[rows * g : rows * (g + 1)]

        for k in range(1, nx):
            to = lines[k]
            rcopy(xt.at[to], xtl.at[at_line], xt_ss, xt_rs, line(to)).start()

        @pl.when(c == 0)
        def _():
            to_line(r_send, rl, r_ss, r_rs)

        xtl[at_line] = xt[at_line]

    with scope("pairs_value"):
        shrink = jnp.exp(-cum)
        k_dec = (k_rate * shrink).astype(BF16)
        mixing = [jnp.where(lower, tn(head_of(q_dec, h), head_of(k_dec, h)), 0.0).astype(BF16) for h in range(heads)]
        gv_own = by_head(nn(head_of(go, h), mixing[h]) for h in range(heads))
        own_send[...] = gv_own.astype(BF16)
        ownl[at_line] = own_send[...]
        to_line(own_send, ownl, own_ss, own_rs)

    z_order = z + back * (nz - 1 - 2 * z)

    def z_sends(k):
        at = z_order + k
        to = at + back * (nz - 1 - 2 * at)
        return (
            rcopy(ft_send, ft_buf.at[z], ft_ss, ft_rs, (to, y, x, 1)),
            rcopy(t_send, t_buf.at[z], t_ss, t_rs, (to, y, x, 1)),
        )

    def carry_send(g, ty, tx, backward):
        device = (z, ty, tx, g)
        if not backward:
            at = pln + tx * ny + ty if g else ty * nx + tx
            return rcopy(l_send.at[at], q_state.at[me // 2], q_ss.at[g], q_rs.at[0], device)
        if g == 0:
            return rcopy(l_send.at[ty * nx + nx - 1], q_line.at[me // 2], q_ss.at[0], q_rs.at[1], device)
        rows_of = pl.ds(pln + tx * ny, ny)
        return rcopy(l_send.at[rows_of], q_grad.at[pl.ds(me // 2 * ny, ny)], q_ss.at[1], q_rs.at[1], device)

    targets = [(0, *t) for t in everyone] + [(1, *t) for t in others]
    plane_decays = e_buf.at[pl.ds(0, pln)]
    e_all = rcopy(plane_decays, plane_decays, ea_ss, ea_rs, (z, y, x, 1 - c))

    @pl.when(c == 1)
    def _():
        with scope("wait1"):
            arrived(e_buf, 2 * pln - 1, e_rs)
            arrived(s_buf, 2 * pln - 1, s_rs)
        with scope("scan1"):
            for g in (0, 1):
                held = jnp.zeros(t_send.shape[1:], F32)
                factor = jnp.ones((1, ch), F32)
                for o in range(pln):
                    it = o + back * (pln - 1 - 2 * o)
                    l_send[g * pln + spot(g, it)] = held.astype(BF16)
                    decay = e_buf[g * pln + it]
                    held = decay * held + s_buf[g * pln + it].astype(F32)
                    factor = decay * factor
                t_send[g] = held.astype(BF16)
                ft_send[g] = factor
        with scope("send2"):
            for k in range(1, nz):

                @pl.when(z_order + k < nz)
                def _():
                    for copy in z_sends(k):
                        copy.start()

            for backward in (0, 1):

                @pl.when(back == backward)
                def _():
                    for target in targets:
                        carry_send(*target, backward).start()

            e_all.start()

            @pl.when(back == 0)
            def _():
                q_state[me // 2] = l_send[pln + x * ny + y]

            @pl.when(back == 1)
            def _():
                q_grad[pl.ds(me // 2 * ny, ny)] = l_send[pl.ds(pln + x * ny, ny)]

    with scope("pairs_query"):
        pairing = [jnp.where(upper, tn(head_of(v, h), head_of(go, h)), 0.0).astype(BF16) for h in range(heads)]
        gq_own = by_head(nn(head_of(k_dec, h), pairing[h]) for h in range(heads))
        gk_own = by_head(nt(head_of(q_dec, h), pairing[h]) for h in range(heads))

    with scope("decays"):
        @pl.when(c == 0)
        def _():
            e_all.wait_recv()

        decays = e_buf[pl.ds(c * pln, pln)]
        before, after = jnp.ones((1, ch), F32), [jnp.ones((1, ch), F32)] * nx
        ids = [line(i)[1] * nx + line(i)[2] for i in range(nx)]
        for i in range(pln):
            before = before * jnp.where(i < me, decays[i], 1.0)
            after = [a * jnp.where(i > n, decays[i], 1.0) for a, n in zip(after, ids)]

    with scope("wait_line"):
        arrived(xtl, nx - 1, xt_rs)
        arrived(kl, nx - 1, k_rs)

    def pairs(parts):
        return [jnp.concatenate(parts[i : i + 2], axis=1) for i in range(0, nx, 2)]

    def to_chunks(ref, total):
        for i in range(ny):
            ref[i] = total[:, i * nz * rows : (i + 1) * nz * rows].astype(ref.dtype)

    with scope("line_m"):
        turned_of = pairs([xtl[i].reshape(d_model // nx, tok) for i in range(nx)])
        tall_after = jnp.concatenate(after + [jnp.ones((8 - nx, ch), F32)], axis=0).T
        scaled = pairs([(kl[i].astype(F32) * tall_after[:, i : i + 1]).astype(BF16) for i in range(nx)])
        m_sum = nt(scaled[0], turned_of[0])
        for a, b in zip(scaled[1:], turned_of[1:]):
            m_sum = m_sum + nt(a, b)
        to_chunks(m_send, m_sum)

    def arriving(o, carried):
        frm = o + back * (nz - 1 - 2 * o)
        return ft_buf[frm] * carried + t_buf[frm].astype(F32)

    def plane_send(g, ty, tx):
        if g:
            return rcopy(o_send, p_both.at[mine], p_ss, p_rs, (z, ty, tx, 1))
        return rcopy(o_send.at[0], p_buf.at[mine], p_ss, p_rs, (z, ty, tx, 0))

    @pl.when(c == 1)
    def _():
        with scope("wait2"):
            for n in range(1, nz):

                @pl.when(z_order == n)
                def _():
                    arrived(ft_buf, n, ft_rs)
                    arrived(t_buf, n, t_rs)

            carried = lax.fori_loop(0, z_order, arriving, jnp.zeros(t_send.shape, F32))
        with scope("send3"):
            o_send[...] = carried.astype(BF16)
            for target in targets:
                plane_send(*target).start()
            p_both[mine] = o_send[...]

    with scope("send_m"):
        to_column(m_send, m_recv, m_ss, m_rs)

    some = pln // 2
    with scope("wait_1b"):

        @pl.when(c == 0)
        def _():
            arrived(q_state, some, q_rs.at[0])
            arrived(q_line, some, q_rs.at[1])
            arrived(rl, nx - 1, r_rs)

        @pl.when((c == 1) & (back == 0))
        def _():
            arrived(q_state, some - 1, q_rs.at[0])
            arrived(q_grad, some * ny, q_rs.at[1])

        @pl.when((c == 1) & (back == 1))
        def _():
            arrived(q_state, some, q_rs.at[0])
            arrived(q_grad, (some - 1) * ny, q_rs.at[1])

    with scope("line_a"):
        state_in = q_state[...].astype(F32).reshape(HEAD, ch)

        @pl.when(c == 0)
        def _():
            grad_at = q_line[...].astype(F32).reshape(HEAD, ch)
            g_all[nx - 1] = grad_at
            for i in range(nx - 2, -1, -1):
                grad_at = e_buf[y * nx + i + 1] * grad_at + rl[i + 1].astype(F32)
                g_all[i] = grad_at

        @pl.when(c == 1)
        def _():
            for i in range(nx):
                part = [q_grad[j * ny + i].astype(F32) for j in range(some)]
                g_all[i] = jnp.concatenate(part, axis=0)

        parts = []
        for i in range(nx):
            grad_at = g_all[i]
            bd_in = by_head((grad_at * m).astype(BF16) for m in mf)
            parts.append(nn(bd_in, kl[i]))
    with scope("wait_own"):
        arrived(ownl, nx - 1, own_rs)
    with scope("line_a2"):
        parts = pairs([(ownl[i].astype(F32) + part).astype(BF16) for i, part in enumerate(parts)])
        a_sum = nt(parts[0], turned_of[0])
        for a, b in zip(parts[1:], turned_of[1:]):
            a_sum = a_sum + nt(a, b)
        to_chunks(aacc, a_sum)
        to_chunks(a_send, a_sum)
        to_column(a_send, a_recv, a_ss, a_rs)

    @pl.when(c == 1)
    def _():
        with scope("wait_m"):
            m_plane = [from_column(g, m_send.at[x], m_recv, m_rs).astype(BF16) for g in (0, 1)]
        with scope("wait3"):
            arrived(p_both, pln - 1, p_rs)
        for g in (0, 1):
            outer[g] = p_both[:, g].astype(F32).reshape(2 * HEAD, ch)
            bd_out = by_head((outer[g, HEAD:] * m).astype(BF16) for m in mf)
            with scope(f"wait_a{g}"):
                a_plane = from_column(g, aacc.at[x], a_recv, a_rs)
            with scope(f"send_z{g}"):
                w_sum = a_plane + nt(m_plane[g], bd_out)
                if g:
                    w2[...] = w_sum.reshape(w2.shape)
                z_send[pl.ds(g * nz, nz)] = w_sum.astype(BF16).reshape(nz, rows, ch)
                for d in z_steps if g else z_steps + [0]:
                    rcopy(z_send.at[g * nz + zs[d]], z_recv.at[z], z_ss, z_rs, (zs[d], y, x, g)).start()

    @pl.when(c == 0)
    def _():
        with scope("wait3"):
            arrived(p_buf, pln, p_rs)
        outer[0] = p_buf[...].astype(F32).reshape(2 * HEAD, ch)

    with scope("value_grad"):
        state_out, grad_out = outer[c, :HEAD], outer[c, HEAD:]
        own_after = after[nx - 1]
        for i in range(nx - 1):
            own_after = jnp.where(at_line == i, after[i], own_after)
        state = state_in + before * state_out
        grad = g_all[at_line] + own_after * grad_out
        bd_state = by_head((state * m).astype(BF16) for m in mf)
        bd_grad = by_head((grad * m).astype(BF16) for m in mf)
        value_grad = (gv_own + nn(bd_grad, k_end)).astype(BF16)

    with scope("input_grad"):
        width = 512 if d_model % 512 == 0 else d_model
        turned = value_grad.T
        for j in range(d_model // width):
            cols = pl.ds(j * width, width)
            ig[:, :, cols] = nn(turned, w_v[:, cols]).astype(BF16).reshape(2, tok // 2, width)
        ig_copy = rcopy(ig.at[1 - c], ig_recv, ig_ss, ig_rs, (z, y, x, 1 - c))
        ig_copy.start()

    with scope("query_forget"):
        g_query = growth * (gq_own + tn(bd_state, go))
        g_key = shrink * gk_own + remain * tn(bd_grad, v)
        gq_out[...] = (g_query * (q_sig * (1.0 + q * (1.0 - q_sig)))).astype(BF16)
        ends = grad * (total * state + update)
        ends_high = ends.astype(BF16)
        ends_low = (ends - ends_high.astype(F32)).astype(BF16)
        tall_ones = jnp.ones((HEAD, tok), BF16)
        boundary = tn(ends_high, tall_ones) + tn(ends_low, tall_ones)
        flow = query * g_query - k_rate * g_key
        flow_high = flow.astype(BF16)
        flow_low = (flow - flow_high.astype(F32)).astype(BF16)
        g_decay = nn(flow_high, lower_ones) + nn(flow_low, lower_ones) + boundary
        gf_out[...] = ((g_decay / (1.0 - k_rate) - g_key) * k_rate * (1.0 / (1.0 + jnp.exp(-f)))).astype(BF16)

    with scope("input_sum"):
        ig_copy.wait_recv()
        gx_out[...] = (ig[c].astype(F32) + ig_recv[...].astype(F32)).astype(BF16)

    with scope("drain"):
        left(xt, nx - 1, xt_ss)
        left(kl, nx - 1, k_ss)
        left(ownl, nx - 1, own_ss)
        ig_copy.wait_send()

        @pl.when(c == 0)
        def _():
            left(thin, pln, e_ss)
            left(s_send, pln, s_ss)
            left(rl, nx - 1, r_ss)
            left(m_send, ny, m_ss)
            left(a_send, ny, a_ss)

        @pl.when(c == 1)
        def _():
            left(m_send, ny - 1, m_ss)
            left(a_send, ny - 1, a_ss)
            left(thin, pln - 1, e_ss)
            left(s_send, pln - 1, s_ss)
            for n in range(1, nz):

                @pl.when(nz - 1 - z_order == n)
                def _():
                    left(ft_buf, n, ft_ss)
                    left(t_buf, n, t_ss)

            left(wide, pln, q_ss.at[0])
            for backward in (0, 1):

                @pl.when(back == backward)
                def _():
                    left(wide, (pln - 1) * (ny if backward else 1), q_ss.at[1])

            e_all.wait_send()
            left(wide, 3 * pln - 2, p_ss)

    with scope("wait_z"):

        @pl.when(c == 0)
        def _():
            arrived(z_recv, nz, z_rs)
            w_last = z_recv[0].astype(F32)
            for k in range(1, nz):
                w_last = w_last + z_recv[k].astype(F32)
            gw_out[...] = w_last

        @pl.when(c == 1)
        def _():
            arrived(z_recv, nz - 1, z_rs)
            w_last = w2[z]
            for k in range(1, nz):
                w_last = w_last + z_recv[zs[k]].astype(F32)
            gw_out[...] = w_last
            left(z_send, 2 * nz - 1, z_ss)


def write_out(*refs):
    copies = [pltpu.make_async_copy(refs[k], refs[4 + k], refs[8].at[k]) for k in range(4)]
    for copy in copies:
        copy.start()
    for copy in copies:
        copy.wait()


def on_device(nz, ny, nx, block_input, value_weight, query_pre, forget_pre, lower_bound, out_grad):
    tok, d_model = block_input.shape
    ch = value_weight.shape[1]
    pln = ny * nx
    piece = 2 * HEAD // pln
    rows = d_model // (nz * pln)
    vm, dma = pltpu.VMEM, pltpu.SemaphoreType.DMA
    scratch = [
        vm((tok, d_model), BF16), vm((ch, d_model), BF16),
        vm((ch, tok), BF16), vm((ch, tok), BF16), vm((ch, tok), BF16), vm((1, ch), F32),
        vm((pln * (ny + 1), piece, ch), BF16), vm((pln, 1, ch), F32),
        vm((pln, piece, ch), BF16), vm((1, ch), F32),
        vm((2 * pln, piece, ch), BF16), vm((2 * pln, 1, ch), F32),
        vm((2 * pln, piece, ch), BF16), vm((pln // 2, piece, ch), BF16), vm((pln // 2 * ny, piece, ch), BF16),
        vm((pln // 2, piece, ch), BF16),
        vm((2, piece, ch), BF16), vm((2, 1, ch), F32),
        vm((nz, 2, piece, ch), BF16), vm((nz, 2, 1, ch), F32),
        vm((2, piece, ch), BF16), vm((pln, piece, ch), BF16), vm((pln, 2, piece, ch), BF16),
        vm((2, 2 * HEAD, ch), F32),
        vm((nx, ny, nz, rows, tok), BF16), vm((nx, ny, nz, rows, tok), BF16),
        vm((HEAD, ch), BF16), vm((nx, HEAD, ch), BF16),
        vm((ch, tok), BF16), vm((nx, ch, tok), BF16),
        vm((ch, tok), BF16), vm((nx, ch, tok), BF16),
        vm((nx, HEAD, ch), F32),
        vm((2, tok // 2, d_model), BF16), vm((tok // 2, d_model), BF16),
        vm((ny, ch, nz * rows), BF16), vm((2 * ny, ch, nz * rows), BF16),
        vm((ny, ch, nz * rows), F32), vm((ny, ch, nz * rows), BF16), vm((2 * ny, ch, nz * rows), BF16),
        vm((nz, rows, ch), F32), vm((2 * nz, rows, ch), BF16), vm((nz, rows, ch), BF16),
        dma((6,)),
        *(dma for _ in range(6)), dma((2,)), dma((2,)),
        *(dma for _ in range(4 + 2 + 8)),
        dma, dma((2,)), dma, dma((2,)), dma, dma, dma, dma,
    ]
    hbm, near = pl.BlockSpec(memory_space=pl.ANY), pl.BlockSpec(memory_space=pltpu.VMEM)
    results = pl.pallas_call(
        functools.partial(kernel, nz, ny, nx),
        out_shape=(
            vm((ch, tok), BF16),
            vm((ch, tok), BF16),
            vm((tok // 2, d_model), BF16),
            vm((rows, ch), F32),
        ),
        in_specs=[hbm] * 6,
        out_specs=(near,) * 4,
        scratch_shapes=scratch,
        compiler_params=pltpu.CompilerParams(collective_id=0, has_side_effects=True),
    )(block_input, value_weight.T, query_pre.T, forget_pre.T, out_grad.T, lower_bound.reshape(1, ch))
    g_query, g_forget, g_input, g_weight = pl.pallas_call(
        write_out,
        out_shape=tuple(jax.ShapeDtypeStruct(a.shape, a.dtype) for a in results),
        in_specs=[near] * 4,
        out_specs=(hbm,) * 4,
        scratch_shapes=[dma((4,))],
    )(*(pltpu.with_memory_space_constraint(a, pltpu.VMEM) for a in results))
    return g_query.T, g_forget.T, g_input, g_weight


def on_mesh(devices):
    nz, ny, nx = devices.shape[:3]
    split = Mesh(devices, SP_TP)
    in_specs = (P(SP, None), P(None, "tp"), P(SP, "tp"), P(SP, "tp"), P("tp"), P(SP, "tp"))
    out_specs = (P(SP, "tp"), P(SP, "tp"), P(SP_TP, None), P(SP, "tp"))
    return jax.shard_map(
        functools.partial(on_device, nz, ny, nx), mesh=split, in_specs=in_specs, out_specs=out_specs, check_vma=False
    )


def solution(mesh):
    return on_mesh(mesh.devices.reshape(8, 4, 4, mesh.shape["tp"]))
```

```python
import functools

import jax
import jax.numpy as jnp
from jax import lax
from jax.experimental import pallas as pl
from jax.experimental.pallas import tpu as pltpu
from jax.sharding import Mesh
from jax.sharding import PartitionSpec as P

HEAD = 64
SP = ("sp_0", "sp_1", "sp_2")
SP_TP = ("sp_0", "sp_1", "sp_2", "tp")
F32, BF16 = jnp.float32, jnp.bfloat16
LOGICAL = pl.DeviceIdType.MESH


def nn(a, b):
    return lax.dot_general(a, b, (((1,), (0,)), ((), ())), preferred_element_type=F32)


def nt(a, b):
    return lax.dot_general(a, b, (((1,), (1,)), ((), ())), preferred_element_type=F32)


def tn(a, b):
    return lax.dot_general(a, b, (((0,), (0,)), ((), ())), preferred_element_type=F32)


def rcopy(src, dst, send, recv, device):
    return pltpu.make_async_remote_copy(
        src_ref=src, dst_ref=dst, send_sem=send, recv_sem=recv, device_id=device, device_id_type=LOGICAL
    )


def kernel(
    nz, ny, nx,
    x_hbm, w_hbm, q_hbm, f_hbm, go_hbm, lb_hbm,
    gq_out, gf_out, gx_out, gw_out,
    x_v, w_v, q_v, f_v, go_v, lb_v, wide, thin,
    s_send, e_send, s_buf, e_buf, l_send, q_state, q_grad, q_line, t_send, ft_send, t_buf, ft_buf, o_send, p_buf, p_both, outer,
    xt, xtl, r_send, rl, k_send, kl, own_send, ownl, g_all, ig, ig_recv,
    m_send, m_recv, aacc, a_send, a_recv, w2, z_send, z_recv,
    lsem, s_ss, s_rs, e_ss, e_rs, ea_ss, ea_rs, q_ss, q_rs, t_ss, t_rs, ft_ss, ft_rs, p_ss, p_rs,
    xt_ss, xt_rs, r_ss, r_rs, k_ss, k_rs, own_ss, own_rs,
    m_ss, m_rs, a_ss, a_rs, z_ss, z_rs, ig_ss, ig_rs,
):
    pln = ny * nx
    tok, d_model = x_v.shape
    ch = w_v.shape[0]
    heads = ch // HEAD
    z, y, x, c = (lax.axis_index(a) for a in SP_TP)
    me = y * nx + x
    back = lax.rem(x + y, 2)
    zs, ys, xs = ([lax.rem(at + d, n) for d in range(n)] for at, n in ((z, nz), (y, ny), (x, nx)))
    across = lambda d, n: min(d, n - d)
    steps = [(dy, dx) for dy in range(ny) for dx in range(nx) if dy or dx]
    steps.sort(key=lambda t: -across(t[0], ny) - across(t[1], nx))
    others = [(ys[dy], xs[dx]) for dy, dx in steps]
    everyone = others + [(y, x)]
    z_steps = sorted(range(1, nz), key=lambda d: -across(d, nz))
    far_first = sorted(range(1, nx), key=lambda d: -across(d, nx))

    at_line, at_col = x * (1 - c) + y * c, y * (1 - c) + x * c
    lines = [xs[d] * (1 - c) + ys[d] * c for d in range(nx)]
    columns = [ys[d] * (1 - c) + xs[d] * c for d in range(ny)]

    def line(i):
        return (z, y * (1 - c) + i * c, i * (1 - c) + x * c, c)

    def column(i):
        return (z, i * (1 - c) + y * c, x * (1 - c) + i * c, c)

    def spot(g, i):
        return lax.rem(i, nx) * ny + lax.div(i, nx) if g else i

    def piece_of(ty, tx):
        return ty * (nx // 2) + lax.div(tx, 2) + lax.rem(tx + ty, 2) * (pln // 2)

    def head_of(a, h):
        return a[HEAD * h : HEAD * (h + 1)]

    def by_head(parts):
        return jnp.concatenate(list(parts), axis=0)

    def arrived(ref, n, sem):
        part = ref.at[pl.ds(0, n)]
        rcopy(part, part, sem, sem, (z, y, x, 1 - c)).wait_recv()

    def left(ref, n, sem):
        part = ref.at[pl.ds(0, n)]
        rcopy(part, part, sem, sem, (z, y, x, 1 - c)).wait_send()

    scope = jax.named_scope
    with scope("loads_barrier"):
        loads = [
            pltpu.make_async_copy(src, dst, lsem.at[k])
            for k, (src, dst) in enumerate(
                ((f_hbm, f_v), (q_hbm, q_v), (go_hbm, go_v), (x_hbm, x_v), (w_hbm, w_v), (lb_hbm, lb_v))
            )
        ]
        for k in (0, 5, 1, 2, 3, 4):
            loads[k].start()
        barrier = pltpu.get_barrier_semaphore()

        def greet(device):
            pl.semaphore_signal(barrier, inc=1, device_id=device, device_id_type=LOGICAL)

        for ty, tx in others:
            greet((z, ty, tx, 1 - c))
        for d in z_steps:
            greet((zs[d], y, x, 1))

        @pl.when(c == 1)
        def _():
            for d in z_steps:
                greet((zs[d], y, x, 0))
            for ty, tx in others:
                greet((z, ty, tx, 1))

        @pl.when(c == 0)
        def _():
            for tx in xs[1:]:
                greet((z, y, tx, 0))

        greet((z, y, x, 1 - c))

    lane = lax.broadcasted_iota(jnp.int32, (1, ch), 1)
    mf = [jnp.where((lane >= HEAD * h) & (lane < HEAD * (h + 1)), 1.0, 0.0).astype(F32) for h in range(heads)]
    row = lax.broadcasted_iota(jnp.int32, (tok, tok), 0)
    col = lax.broadcasted_iota(jnp.int32, (tok, tok), 1)
    lower, upper = row >= col, col >= row
    lower_ones = jnp.where(lower, 1.0, 0.0).astype(BF16)
    upper_ones = jnp.where(upper, 1.0, 0.0).astype(BF16)

    def folded(full):
        out = full[:HEAD] * mf[0]
        for h in range(1, heads):
            out = out + head_of(full, h) * mf[h]
        return out

    with scope("gates"):
        loads[5].wait()
        gap = jnp.broadcast_to(1.0 - lb_v[...], (tok, ch)).T
        loads[0].wait()
        f = f_v[...].astype(F32)
        f_neg = 1.0 / (1.0 + jnp.exp(f))
        k_rate = gap * f_neg
        logs = jnp.log1p(-k_rate)
        high = logs.astype(BF16)
        low = (logs - high.astype(F32)).astype(BF16)
        cum = nn(high, upper_ones) + nn(low, upper_ones)
        row_ones = jnp.ones((8, tok), BF16)
        total = jnp.exp((nt(row_ones, high) + nt(row_ones, low))[:1])
        closing = cum[:, tok - 1 : tok]
        growth = jnp.exp(cum)
        remain = jnp.exp(closing - cum)
        e_send[...] = total
        k_end = (k_rate * remain).astype(BF16)
        loads[1].wait()
        q = q_v[...].astype(F32)
        q_sig = 1.0 / (1.0 + jnp.exp(-q))
        query = q * q_sig
        q_dec = (query * growth).astype(BF16)
        loads[2].wait()
        go = go_v[...]
        reach = folded(nt(go, q_dec))
    with scope("values"):
        loads[3].wait()
        loads[4].wait()
        v = nt(w_v[...], x_v[...]).astype(BF16)
        update = folded(nt(v, k_end))
        s_send[...] = jnp.concatenate([update, reach], axis=0).reshape(s_send.shape).astype(BF16)
        r_send[...] = reach.astype(BF16)
        k_send[...] = k_end

    with scope("barrier_wait"):
        pl.semaphore_wait(barrier, pln + nz - 1 + c * (pln + nz - 2) + (1 - c) * (nx - 1))

    def to_line(source, target, send_sem, recv_sem):
        for k in far_first:
            rcopy(source, target.at[at_line], send_sem, recv_sem, line(lines[k])).start()

    def to_column(source, target, send_sem, recv_sem):
        for k in far_first:
            to = columns[k]
            device = (z, to * (1 - c) + y * c, x * (1 - c) + to * c, 1)
            rcopy(source.at[to], target.at[c * ny + at_col], send_sem, recv_sem.at[c], device).start()

        @pl.when(c == 0)
        def _():
            rcopy(source.at[y], target.at[y], send_sem, recv_sem.at[0], (z, y, x, 1)).start()

    def from_column(g, own, target, recv_sem):
        arrived(target, ny - g, recv_sem.at[g])
        if g == 0:
            out = target[0].astype(F32)
            for k in range(1, ny):
                out = out + target[k].astype(F32)
            return out.T
        out = own[...].astype(F32)
        for k in range(1, ny):
            out = out + target[ny + xs[k]].astype(F32)
        return out.T

    def piece_sends(ty, tx):
        to = (z, ty, tx, 1)
        return (
            rcopy(e_send, e_buf.at[c * pln + me], e_ss, e_rs, to),
            rcopy(s_send.at[piece_of(ty, tx)], s_buf.at[c * pln + me], s_ss, s_rs, to),
        )

    mine = piece_of(y, x)
    with scope("send1"):
        for ty, tx in others:
            for copy in piece_sends(ty, tx):
                copy.start()

        @pl.when(c == 0)
        def _():
            for copy in piece_sends(y, x):
                copy.start()

        @pl.when(c == 1)
        def _():
            s_buf[pln + me] = s_send[mine]
            e_buf[pln + me] = e_send[...]

        to_line(k_send, kl, k_ss, k_rs)
        kl[at_line] = k_end
        rl[at_line] = r_send[...]

    rows = d_model // (nz * ny * nx)
    with scope("turn"):
        per = tok // rows
        for b in range(d_model // tok):
            turned = x_v[:, tok * b : tok * (b + 1)].T
            for g in range(per):
                at = b * per + g
                zz, yy, xx = at // pln, (at // nx) % ny, at % nx
                group, into = xx * (1 - c) + yy * c, yy * (1 - c) + xx * c
                xt[group, into, zz] = turned[rows * g : rows * (g + 1)]

        for k in far_first:
            to = lines[k]
            rcopy(xt.at[to], xtl.at[at_line], xt_ss, xt_rs, line(to)).start()

        @pl.when(c == 0)
        def _():
            to_line(r_send, rl, r_ss, r_rs)

        xtl[at_line] = xt[at_line]

    with scope("pairs_value"):
        shrink = jnp.exp(-cum)
        k_dec = (k_rate * shrink).astype(BF16)
        mixing = [jnp.where(lower, tn(head_of(q_dec, h), head_of(k_dec, h)), 0.0).astype(BF16) for h in range(heads)]
        gv_own = by_head(nn(head_of(go, h), mixing[h]) for h in range(heads))
        own_send[...] = gv_own.astype(BF16)
        ownl[at_line] = own_send[...]

        @pl.when(c == 0)
        def _():
            to_line(own_send, ownl, own_ss, own_rs)


    z_order = z + back * (nz - 1 - 2 * z)

    def z_sends(k):
        at = z_order + k
        to = at + back * (nz - 1 - 2 * at)
        return (
            rcopy(ft_send, ft_buf.at[z], ft_ss, ft_rs, (to, y, x, 1)),
            rcopy(t_send, t_buf.at[z], t_ss, t_rs, (to, y, x, 1)),
        )

    def carry_send(g, ty, tx, backward):
        device = (z, ty, tx, g)
        if not backward:
            at = pln + tx * ny + ty if g else ty * nx + tx
            return rcopy(l_send.at[at], q_state.at[me // 2], q_ss.at[g], q_rs.at[0], device)
        if g == 0:
            return rcopy(l_send.at[ty * nx + nx - 1], q_line.at[me // 2], q_ss.at[0], q_rs.at[1], device)
        rows_of = pl.ds(pln + tx * ny, ny)
        return rcopy(l_send.at[rows_of], q_grad.at[pl.ds(me // 2 * ny, ny)], q_ss.at[1], q_rs.at[1], device)

    targets = [(0, *t) for t in everyone] + [(1, *t) for t in others]
    plane_decays = e_buf.at[pl.ds(0, pln)]
    e_all = rcopy(plane_decays, plane_decays, ea_ss, ea_rs, (z, y, x, 1 - c))

    @pl.when(c == 1)
    def _():
        with scope("wait1"):
            arrived(e_buf, 2 * pln - 1, e_rs)
            arrived(s_buf, 2 * pln - 1, s_rs)
        with scope("scan1"):
            for g in (0, 1):
                held = jnp.zeros(t_send.shape[1:], F32)
                factor = jnp.ones((1, ch), F32)
                for o in range(pln):
                    it = o + back * (pln - 1 - 2 * o)
                    l_send[g * pln + spot(g, it)] = held.astype(BF16)
                    decay = e_buf[g * pln + it]
                    held = decay * held + s_buf[g * pln + it].astype(F32)
                    factor = decay * factor
                t_send[g] = held.astype(BF16)
                ft_send[g] = factor
        with scope("send2"):
            for k in range(1, nz):

                @pl.when(z_order + k < nz)
                def _():
                    for copy in z_sends(k):
                        copy.start()

            @pl.when(back == 1)
            def _():
                for target in targets:
                    carry_send(*target, 1).start()
                q_grad[pl.ds(me // 2 * ny, ny)] = l_send[pl.ds(pln + x * ny, ny)]

            to_line(own_send, ownl, own_ss, own_rs)
            e_all.start()

    with scope("pairs_query"):
        pairing = [jnp.where(upper, tn(head_of(v, h), head_of(go, h)), 0.0).astype(BF16) for h in range(heads)]
        gq_own = by_head(nn(head_of(k_dec, h), pairing[h]) for h in range(heads))
        gk_own = by_head(nt(head_of(q_dec, h), pairing[h]) for h in range(heads))

    with scope("decays"):
        @pl.when(c == 0)
        def _():
            e_all.wait_recv()

        decays = e_buf[pl.ds(c * pln, pln)]
        before, after = jnp.ones((1, ch), F32), [jnp.ones((1, ch), F32)] * nx
        ids = [line(i)[1] * nx + line(i)[2] for i in range(nx)]
        for i in range(pln):
            before = before * jnp.where(i < me, decays[i], 1.0)
            after = [a * jnp.where(i > n, decays[i], 1.0) for a, n in zip(after, ids)]

    with scope("wait_line"):
        arrived(xtl, nx - 1, xt_rs)
        arrived(kl, nx - 1, k_rs)

    def pairs(parts):
        return [jnp.concatenate(parts[i : i + 2], axis=1) for i in range(0, nx, 2)]

    def to_chunks(ref, total):
        for i in range(ny):
            ref[i] = total[:, i * nz * rows : (i + 1) * nz * rows].astype(ref.dtype)

    with scope("line_m"):
        turned_of = pairs([xtl[i].reshape(d_model // nx, tok) for i in range(nx)])
        tall_after = jnp.concatenate(after + [jnp.ones((8 - nx, ch), F32)], axis=0).T
        scaled = pairs([(kl[i].astype(F32) * tall_after[:, i : i + 1]).astype(BF16) for i in range(nx)])
        m_sum = nt(scaled[0], turned_of[0])
        for a, b in zip(scaled[1:], turned_of[1:]):
            m_sum = m_sum + nt(a, b)
        to_chunks(m_send, m_sum)
        to_column(m_send, m_recv, m_ss, m_rs)

    def arriving(o, carried):
        frm = o + back * (nz - 1 - 2 * o)
        return ft_buf[frm] * carried + t_buf[frm].astype(F32)

    def plane_send(g, ty, tx):
        if g:
            return rcopy(o_send, p_both.at[mine], p_ss, p_rs, (z, ty, tx, 1))
        return rcopy(o_send.at[0], p_buf.at[mine], p_ss, p_rs, (z, ty, tx, 0))

    @pl.when(c == 1)
    def _():
        with scope("wait2"):
            for n in range(1, nz):

                @pl.when(z_order == n)
                def _():
                    arrived(ft_buf, n, ft_rs)
                    arrived(t_buf, n, t_rs)

            carried = lax.fori_loop(0, z_order, arriving, jnp.zeros(t_send.shape, F32))
        with scope("send3"):
            o_send[...] = carried.astype(BF16)
            for target in targets[pln:] + targets[:pln]:
                plane_send(*target).start()
            p_both[mine] = o_send[...]

            @pl.when(back == 0)
            def _():
                for target in targets:
                    carry_send(*target, 0).start()
                q_state[me // 2] = l_send[pln + x * ny + y]


    some = pln // 2
    with scope("wait_1b"):

        @pl.when(c == 0)
        def _():
            arrived(q_line, some, q_rs.at[1])
            arrived(rl, nx - 1, r_rs)

        for odd in (0, 1):

            @pl.when((c == 1) & (back == odd))
            def _():
                arrived(q_grad, (some - odd) * ny, q_rs.at[1])

    with scope("line_a"):

        @pl.when(c == 0)
        def _():
            grad_at = q_line[...].astype(F32).reshape(HEAD, ch)
            g_all[nx - 1] = grad_at
            for i in range(nx - 2, -1, -1):
                grad_at = e_buf[y * nx + i + 1] * grad_at + rl[i + 1].astype(F32)
                g_all[i] = grad_at

        @pl.when(c == 1)
        def _():
            for i in range(nx):
                part = [q_grad[j * ny + i].astype(F32) for j in range(some)]
                g_all[i] = jnp.concatenate(part, axis=0)

        parts = []
        for i in range(nx):
            grad_at = g_all[i]
            bd_in = by_head((grad_at * m).astype(BF16) for m in mf)
            parts.append(nn(bd_in, kl[i]))
    with scope("wait_own"):
        arrived(ownl, nx - 1, own_rs)
    with scope("line_a2"):
        parts = pairs([(ownl[i].astype(F32) + part).astype(BF16) for i, part in enumerate(parts)])
        a_sum = nt(parts[0], turned_of[0])
        for a, b in zip(parts[1:], turned_of[1:]):
            a_sum = a_sum + nt(a, b)
        to_chunks(aacc, a_sum)
        to_chunks(a_send, a_sum)
        to_column(a_send, a_recv, a_ss, a_rs)

    @pl.when(c == 1)
    def _():
        with scope("wait_m1"):
            m_plane = from_column(1, m_send.at[x], m_recv, m_rs).astype(BF16)
        with scope("wait3"):
            arrived(p_both, pln - 1, p_rs)
        for g in (1, 0):
            outer[g] = p_both[:, g].astype(F32).reshape(2 * HEAD, ch)
            bd_out = by_head((outer[g, HEAD:] * m).astype(BF16) for m in mf)
            with scope(f"wait_a{g}"):
                if g == 0:
                    m_plane = from_column(0, None, m_recv, m_rs).astype(BF16)
                w_sum = nt(m_plane, bd_out)
                w_sum = w_sum + from_column(g, aacc.at[x], a_recv, a_rs)
            with scope(f"send_z{g}"):
                if g:
                    w2[...] = w_sum.reshape(w2.shape)
                z_send[pl.ds(g * nz, nz)] = w_sum.astype(BF16).reshape(nz, rows, ch)
                for d in z_steps if g else z_steps + [0]:
                    rcopy(z_send.at[g * nz + zs[d]], z_recv.at[z], z_ss, z_rs, (zs[d], y, x, g)).start()

    @pl.when(c == 0)
    def _():
        with scope("wait3"):
            arrived(p_buf, pln, p_rs)
        outer[0] = p_buf[...].astype(F32).reshape(2 * HEAD, ch)

    with scope("value_grad"):
        for even in (0, 1):

            @pl.when((1 - back) * c == even)
            def _():
                arrived(q_state, some - even, q_rs.at[0])

        state_in = q_state[...].astype(F32).reshape(HEAD, ch)
        state_out, grad_out = outer[c, :HEAD], outer[c, HEAD:]
        own_after = after[nx - 1]
        for i in range(nx - 1):
            own_after = jnp.where(at_line == i, after[i], own_after)
        state = state_in + before * state_out
        grad = g_all[at_line] + own_after * grad_out
        bd_state = by_head((state * m).astype(BF16) for m in mf)
        bd_grad = by_head((grad * m).astype(BF16) for m in mf)
        value_grad = (gv_own + nn(bd_grad, k_end)).astype(BF16)

    with scope("input_grad"):
        width = 512 if d_model % 512 == 0 else d_model
        turned = value_grad.T
        for j in range(d_model // width):
            cols = pl.ds(j * width, width)
            ig[:, :, cols] = nn(turned, w_v[:, cols]).astype(BF16).reshape(2, tok // 2, width)
        ig_copy = rcopy(ig.at[1 - c], ig_recv, ig_ss, ig_rs, (z, y, x, 1 - c))
        ig_copy.start()

    with scope("query_forget"):
        g_query = growth * (gq_own + tn(bd_state, go))
        g_key = shrink * gk_own + remain * tn(bd_grad, v)
        gq_out[...] = (g_query * (q_sig * (1.0 + q * (1.0 - q_sig)))).astype(BF16)
        ends = grad * (total * state + update)
        ends_high = ends.astype(BF16)
        ends_low = (ends - ends_high.astype(F32)).astype(BF16)
        tall_ones = jnp.ones((HEAD, tok), BF16)
        boundary = tn(ends_high, tall_ones) + tn(ends_low, tall_ones)
        flow = query * g_query - k_rate * g_key
        flow_high = flow.astype(BF16)
        flow_low = (flow - flow_high.astype(F32)).astype(BF16)
        g_decay = nn(flow_high, lower_ones) + nn(flow_low, lower_ones) + boundary
        gf_out[...] = ((g_decay / (1.0 - k_rate) - g_key) * k_rate * (1.0 / (1.0 + jnp.exp(-f)))).astype(BF16)

    with scope("input_sum"):
        ig_copy.wait_recv()
        gx_out[...] = (ig[c].astype(F32) + ig_recv[...].astype(F32)).astype(BF16)

    with scope("drain"):
        left(xt, nx - 1, xt_ss)
        left(kl, nx - 1, k_ss)
        left(ownl, nx - 1, own_ss)
        ig_copy.wait_send()

        @pl.when(c == 0)
        def _():
            left(thin, pln, e_ss)
            left(s_send, pln, s_ss)
            left(rl, nx - 1, r_ss)
            left(m_send, ny, m_ss)
            left(a_send, ny, a_ss)

        @pl.when(c == 1)
        def _():
            left(m_send, ny - 1, m_ss)
            left(a_send, ny - 1, a_ss)
            left(thin, pln - 1, e_ss)
            left(s_send, pln - 1, s_ss)
            for n in range(1, nz):

                @pl.when(nz - 1 - z_order == n)
                def _():
                    left(ft_buf, n, ft_ss)
                    left(t_buf, n, t_ss)

            left(wide, pln, q_ss.at[0])
            for backward in (0, 1):

                @pl.when(back == backward)
                def _():
                    left(wide, (pln - 1) * (ny if backward else 1), q_ss.at[1])

            e_all.wait_send()
            left(wide, 3 * pln - 2, p_ss)

    with scope("wait_z"):

        @pl.when(c == 0)
        def _():
            arrived(z_recv, nz, z_rs)
            w_last = z_recv[0].astype(F32)
            for k in range(1, nz):
                w_last = w_last + z_recv[k].astype(F32)
            gw_out[...] = w_last

        @pl.when(c == 1)
        def _():
            arrived(z_recv, nz - 1, z_rs)
            w_last = w2[z]
            for k in range(1, nz):
                w_last = w_last + z_recv[zs[k]].astype(F32)
            gw_out[...] = w_last
            left(z_send, 2 * nz - 1, z_ss)


def write_out(*refs):
    copies = [pltpu.make_async_copy(refs[k], refs[4 + k], refs[8].at[k]) for k in range(4)]
    for copy in copies:
        copy.start()
    for copy in copies:
        copy.wait()


def on_device(nz, ny, nx, block_input, value_weight, query_pre, forget_pre, lower_bound, out_grad):
    tok, d_model = block_input.shape
    ch = value_weight.shape[1]
    pln = ny * nx
    piece = 2 * HEAD // pln
    rows = d_model // (nz * pln)
    vm, dma = pltpu.VMEM, pltpu.SemaphoreType.DMA
    scratch = [
        vm((tok, d_model), BF16), vm((ch, d_model), BF16),
        vm((ch, tok), BF16), vm((ch, tok), BF16), vm((ch, tok), BF16), vm((1, ch), F32),
        vm((pln * (ny + 1), piece, ch), BF16), vm((pln, 1, ch), F32),
        vm((pln, piece, ch), BF16), vm((1, ch), F32),
        vm((2 * pln, piece, ch), BF16), vm((2 * pln, 1, ch), F32),
        vm((2 * pln, piece, ch), BF16), vm((pln // 2, piece, ch), BF16), vm((pln // 2 * ny, piece, ch), BF16),
        vm((pln // 2, piece, ch), BF16),
        vm((2, piece, ch), BF16), vm((2, 1, ch), F32),
        vm((nz, 2, piece, ch), BF16), vm((nz, 2, 1, ch), F32),
        vm((2, piece, ch), BF16), vm((pln, piece, ch), BF16), vm((pln, 2, piece, ch), BF16),
        vm((2, 2 * HEAD, ch), F32),
        vm((nx, ny, nz, rows, tok), BF16), vm((nx, ny, nz, rows, tok), BF16),
        vm((HEAD, ch), BF16), vm((nx, HEAD, ch), BF16),
        vm((ch, tok), BF16), vm((nx, ch, tok), BF16),
        vm((ch, tok), BF16), vm((nx, ch, tok), BF16),
        vm((nx, HEAD, ch), F32),
        vm((2, tok // 2, d_model), BF16), vm((tok // 2, d_model), BF16),
        vm((ny, ch, nz * rows), BF16), vm((2 * ny, ch, nz * rows), BF16),
        vm((ny, ch, nz * rows), F32), vm((ny, ch, nz * rows), BF16), vm((2 * ny, ch, nz * rows), BF16),
        vm((nz, rows, ch), F32), vm((2 * nz, rows, ch), BF16), vm((nz, rows, ch), BF16),
        dma((6,)),
        *(dma for _ in range(6)), dma((2,)), dma((2,)),
        *(dma for _ in range(4 + 2 + 8)),
        dma, dma((2,)), dma, dma((2,)), dma, dma, dma, dma,
    ]
    hbm, near = pl.BlockSpec(memory_space=pl.ANY), pl.BlockSpec(memory_space=pltpu.VMEM)
    results = pl.pallas_call(
        functools.partial(kernel, nz, ny, nx),
        out_shape=(
            vm((ch, tok), BF16),
            vm((ch, tok), BF16),
            vm((tok // 2, d_model), BF16),
            vm((rows, ch), F32),
        ),
        in_specs=[hbm] * 6,
        out_specs=(near,) * 4,
        scratch_shapes=scratch,
        compiler_params=pltpu.CompilerParams(collective_id=0, has_side_effects=True),
    )(block_input, value_weight.T, query_pre.T, forget_pre.T, out_grad.T, lower_bound.reshape(1, ch))
    g_query, g_forget, g_input, g_weight = pl.pallas_call(
        write_out,
        out_shape=tuple(jax.ShapeDtypeStruct(a.shape, a.dtype) for a in results),
        in_specs=[near] * 4,
        out_specs=(hbm,) * 4,
        scratch_shapes=[dma((4,))],
    )(*(pltpu.with_memory_space_constraint(a, pltpu.VMEM) for a in results))
    return g_query.T, g_forget.T, g_input, g_weight


def on_mesh(devices):
    nz, ny, nx = devices.shape[:3]
    split = Mesh(devices, SP_TP)
    in_specs = (P(SP, None), P(None, "tp"), P(SP, "tp"), P(SP, "tp"), P("tp"), P(SP, "tp"))
    out_specs = (P(SP, "tp"), P(SP, "tp"), P(SP_TP, None), P(SP, "tp"))
    return jax.shard_map(
        functools.partial(on_device, nz, ny, nx), mesh=split, in_specs=in_specs, out_specs=out_specs, check_vma=False
    )


def solution(mesh):
    return on_mesh(mesh.devices.reshape(8, 4, 4, mesh.shape["tp"]))
```

```python
import functools

import jax
import jax.numpy as jnp
from jax import lax
from jax.experimental import pallas as pl
from jax.experimental.pallas import tpu as pltpu
from jax.sharding import Mesh
from jax.sharding import PartitionSpec as P

HEAD = 64
SP = ("sp_0", "sp_1", "sp_2")
SP_TP = ("sp_0", "sp_1", "sp_2", "tp")
F32, BF16 = jnp.float32, jnp.bfloat16
LOGICAL = pl.DeviceIdType.MESH


def nn(a, b):
    return lax.dot_general(a, b, (((1,), (0,)), ((), ())), preferred_element_type=F32)


def nt(a, b):
    return lax.dot_general(a, b, (((1,), (1,)), ((), ())), preferred_element_type=F32)


def tn(a, b):
    return lax.dot_general(a, b, (((0,), (0,)), ((), ())), preferred_element_type=F32)


def rcopy(src, dst, send, recv, device):
    return pltpu.make_async_remote_copy(
        src_ref=src, dst_ref=dst, send_sem=send, recv_sem=recv, device_id=device, device_id_type=LOGICAL
    )


def kernel(
    nz, ny, nx,
    x_hbm, w_hbm, q_hbm, f_hbm, go_hbm, lb_hbm,
    gq_out, gf_out, gx_out, gw_out,
    x_v, w_v, q_v, f_v, go_v, lb_v, wide, thin, broad,
    s_send, e_send, s_buf, e_buf, l_send, lg_send, q_grad, q_line, t_send, ft_send, t_buf, ft_buf, held_out, o_send, p_buf, p_both, outer, st_send, st_buf,
    xt, xtl, r_send, rl, k_send, kl, own_send, ownl, g_all, ig, ig_recv,
    m_send, m_recv, aacc, a_send, a_recv, w2, z_send, z_recv,
    lsem, s_ss, s_rs, e_ss, e_rs, ea_ss, ea_rs, q_ss, q_rs, t_ss, t_rs, ft_ss, ft_rs, p_ss, p_rs, st_ss, st_rs,
    xt_ss, xt_rs, r_ss, r_rs, k_ss, k_rs, own_ss, own_rs,
    m_ss, m_rs, a_ss, a_rs, z_ss, z_rs, ig_ss, ig_rs,
):
    pln = ny * nx
    tok, d_model = x_v.shape
    ch = w_v.shape[0]
    heads = ch // HEAD
    z, y, x, c = (lax.axis_index(a) for a in SP_TP)
    me = y * nx + x
    back = lax.rem(x + y, 2)
    zs, ys, xs = ([lax.rem(at + d, n) for d in range(n)] for at, n in ((z, nz), (y, ny), (x, nx)))
    across = lambda d, n: min(d, n - d)
    steps = [(dy, dx) for dy in range(ny) for dx in range(nx) if dy or dx]
    steps.sort(key=lambda t: -across(t[0], ny) - across(t[1], nx))
    others = [(ys[dy], xs[dx]) for dy, dx in steps]
    everyone = others + [(y, x)]
    z_steps = sorted(range(1, nz), key=lambda d: -across(d, nz))
    far_first = sorted(range(1, nx), key=lambda d: -across(d, nx))

    at_line, at_col = x * (1 - c) + y * c, y * (1 - c) + x * c
    lines = [xs[d] * (1 - c) + ys[d] * c for d in range(nx)]
    columns = [ys[d] * (1 - c) + xs[d] * c for d in range(ny)]

    def line(i):
        return (z, y * (1 - c) + i * c, i * (1 - c) + x * c, c)

    def column(i):
        return (z, i * (1 - c) + y * c, x * (1 - c) + i * c, c)

    def piece_of(ty, tx):
        return ty * (nx // 2) + lax.div(tx, 2) + lax.rem(tx + ty, 2) * (pln // 2)

    def head_of(a, h):
        return a[HEAD * h : HEAD * (h + 1)]

    def by_head(parts):
        return jnp.concatenate(list(parts), axis=0)

    def arrived(ref, n, sem):
        part = ref.at[pl.ds(0, n)]
        rcopy(part, part, sem, sem, (z, y, x, 1 - c)).wait_recv()

    def left(ref, n, sem):
        part = ref.at[pl.ds(0, n)]
        rcopy(part, part, sem, sem, (z, y, x, 1 - c)).wait_send()

    scope = jax.named_scope
    with scope("loads_barrier"):
        loads = [
            pltpu.make_async_copy(src, dst, lsem.at[k])
            for k, (src, dst) in enumerate(
                ((f_hbm, f_v), (q_hbm, q_v), (go_hbm, go_v), (x_hbm, x_v), (w_hbm, w_v), (lb_hbm, lb_v))
            )
        ]
        for k in (0, 5, 1, 2, 3, 4):
            loads[k].start()
        barrier = pltpu.get_barrier_semaphore()

        def greet(device):
            pl.semaphore_signal(barrier, inc=1, device_id=device, device_id_type=LOGICAL)

        for ty, tx in others:
            greet((z, ty, tx, 1))
        for d in z_steps:
            greet((zs[d], y, x, 1))

        @pl.when(c == 1)
        def _():
            for ty, tx in others:
                greet((z, ty, tx, 0))
            for d in z_steps:
                greet((zs[d], y, x, 0))

        @pl.when(c == 0)
        def _():
            for tx in xs[1:]:
                greet((z, y, tx, 0))

        greet((z, y, x, 1 - c))

    lane = lax.broadcasted_iota(jnp.int32, (1, ch), 1)
    mf = [jnp.where((lane >= HEAD * h) & (lane < HEAD * (h + 1)), 1.0, 0.0).astype(F32) for h in range(heads)]
    row = lax.broadcasted_iota(jnp.int32, (tok, tok), 0)
    col = lax.broadcasted_iota(jnp.int32, (tok, tok), 1)
    lower, upper = row >= col, col >= row
    lower_ones = jnp.where(lower, 1.0, 0.0).astype(BF16)
    upper_ones = jnp.where(upper, 1.0, 0.0).astype(BF16)

    def folded(full):
        out = full[:HEAD] * mf[0]
        for h in range(1, heads):
            out = out + head_of(full, h) * mf[h]
        return out

    with scope("gates"):
        loads[5].wait()
        gap = jnp.broadcast_to(1.0 - lb_v[...], (tok, ch)).T
        loads[0].wait()
        f = f_v[...].astype(F32)
        f_neg = 1.0 / (1.0 + jnp.exp(f))
        k_rate = gap * f_neg
        logs = jnp.log1p(-k_rate)
        high = logs.astype(BF16)
        low = (logs - high.astype(F32)).astype(BF16)
        cum = nn(high, upper_ones) + nn(low, upper_ones)
        row_ones = jnp.ones((8, tok), BF16)
        total = jnp.exp((nt(row_ones, high) + nt(row_ones, low))[:1])
        closing = cum[:, tok - 1 : tok]
        growth = jnp.exp(cum)
        remain = jnp.exp(closing - cum)
        e_send[...] = total
        k_end = (k_rate * remain).astype(BF16)
        loads[1].wait()
        q = q_v[...].astype(F32)
        q_sig = 1.0 / (1.0 + jnp.exp(-q))
        query = q * q_sig
        q_dec = (query * growth).astype(BF16)
        loads[2].wait()
        go = go_v[...]
        reach = folded(nt(go, q_dec))
    with scope("values"):
        loads[3].wait()
        loads[4].wait()
        v = nt(w_v[...], x_v[...]).astype(BF16)
        update = folded(nt(v, k_end))
        s_send[...] = jnp.concatenate([update, reach], axis=0).reshape(s_send.shape).astype(BF16)
        r_send[...] = reach.astype(BF16)
        k_send[...] = k_end

    with scope("barrier_wait"):
        pl.semaphore_wait(barrier, pln + nz - 1 + c * (pln + nz - 2) + (1 - c) * (nx - 1))

    def to_line(source, target, send_sem, recv_sem):
        for k in far_first:
            rcopy(source, target.at[at_line], send_sem, recv_sem, line(lines[k])).start()

    def column_send(source, target, send_sem, recv_sem, to):
        device = (z, to * (1 - c) + y * c, x * (1 - c) + to * c, 1)
        return rcopy(source.at[to], target.at[c * ny + at_col], send_sem, recv_sem.at[c], device)

    def to_column(source, target, send_sem, recv_sem):
        for k in far_first:
            column_send(source, target, send_sem, recv_sem, columns[k]).start()

        @pl.when(c == 0)
        def _():
            rcopy(source.at[y], target.at[y], send_sem, recv_sem.at[0], (z, y, x, 1)).start()

    def from_column(g, own, target, recv_sem):
        arrived(target, ny - g, recv_sem.at[g])
        if g == 0:
            out = target[0].astype(F32)
            for k in range(1, ny):
                out = out + target[k].astype(F32)
            return out.T
        out = own[...].astype(F32)
        for k in range(1, ny):
            out = out + target[ny + xs[k]].astype(F32)
        return out.T

    def piece_sends(ty, tx):
        to = (z, ty, tx, 1)
        return (
            rcopy(e_send, e_buf.at[c * pln + me], e_ss, e_rs, to),
            rcopy(s_send.at[piece_of(ty, tx)], s_buf.at[c * pln + me], s_ss, s_rs, to),
        )

    mine = piece_of(y, x)
    with scope("send1"):
        for parity in (0, 1):

            @pl.when(back == parity)
            def _():
                for want in (1 - parity, parity):
                    for (dy, dx), target in zip(steps, others):
                        if (dy + dx) % 2 == want:
                            for copy in piece_sends(*target):
                                copy.start()

        @pl.when(c == 0)
        def _():
            for copy in piece_sends(y, x):
                copy.start()

        @pl.when(c == 1)
        def _():
            s_buf[pln + me] = s_send[mine]
            e_buf[pln + me] = e_send[...]

        to_line(k_send, kl, k_ss, k_rs)
        kl[at_line] = k_end
        rl[at_line] = r_send[...]

    rows = d_model // (nz * ny * nx)
    with scope("turn"):
        per = tok // rows
        for b in range(d_model // tok):
            turned = x_v[:, tok * b : tok * (b + 1)].T
            for g in range(per):
                at = b * per + g
                zz, yy, xx = at // pln, (at // nx) % ny, at % nx
                group, into = xx * (1 - c) + yy * c, yy * (1 - c) + xx * c
                xt[group, into, zz] = turned[rows * g : rows * (g + 1)]

        for k in far_first:
            to = lines[k]
            rcopy(xt.at[to], xtl.at[at_line], xt_ss, xt_rs, line(to)).start()

        @pl.when(c == 0)
        def _():
            to_line(r_send, rl, r_ss, r_rs)

        xtl[at_line] = xt[at_line]

    with scope("pairs_value"):
        shrink = jnp.exp(-cum)
        k_dec = (k_rate * shrink).astype(BF16)
        mixing = [jnp.where(lower, tn(head_of(q_dec, h), head_of(k_dec, h)), 0.0).astype(BF16) for h in range(heads)]
        gv_own = by_head(nn(head_of(go, h), mixing[h]) for h in range(heads))
        own_send[...] = gv_own.astype(BF16)
        ownl[at_line] = own_send[...]

        @pl.when(c == 0)
        def _():
            to_line(own_send, ownl, own_ss, own_rs)


    z_order = z + back * (nz - 1 - 2 * z)

    def z_sends(k):
        at = z_order + k
        to = at + back * (nz - 1 - 2 * at)
        return (
            rcopy(ft_send, ft_buf.at[z], ft_ss, ft_rs, (to, y, x, 1)),
            rcopy(t_send, t_buf.at[z], t_ss, t_rs, (to, y, x, 1)),
        )

    def carry_send(g, ty, tx):
        device = (z, ty, tx, g)
        if g == 0:
            return rcopy(l_send.at[ty * nx + nx - 1], q_line.at[me // 2], q_ss.at[0], q_rs, device)
        return rcopy(lg_send.at[tx], q_grad.at[me // 2], q_ss.at[1], q_rs, device)

    targets = [(0, *t) for t in everyone] + [(1, *t) for t in others]
    plane_decays = e_buf.at[pl.ds(0, pln)]
    e_all = rcopy(plane_decays, plane_decays, ea_ss, ea_rs, (z, y, x, 1 - c))

    @pl.when(c == 1)
    def _():
        with scope("wait1"):
            arrived(e_buf, 2 * pln - 1, e_rs)
            arrived(s_buf, 2 * pln - 1, s_rs)
        with scope("scan1"):
            for parity in (0, 1):

                @pl.when(back == parity)
                def _():
                    for g in (0, 1):
                        held = jnp.zeros(t_send.shape[1:], F32)
                        factor = jnp.ones((1, ch), F32)
                        for it in range(pln - 1, -1, -1) if parity else range(pln):
                            if g and parity:
                                lg_send[it % nx, :, ch * (it // nx) : ch * (it // nx + 1)] = held.astype(BF16)
                            else:
                                l_send[g * pln + it] = held.astype(BF16)
                            decay = e_buf[g * pln + it]
                            held = decay * held + s_buf[g * pln + it].astype(F32)
                            factor = decay * factor
                        t_send[g] = held.astype(BF16)
                        ft_send[g] = factor

        with scope("send2"):
            for k in range(1, nz):

                @pl.when(z_order + k < nz)
                def _():
                    for copy in z_sends(k):
                        copy.start()

            @pl.when(back == 1)
            def _():
                for target in targets:
                    carry_send(*target).start()
                q_grad[me // 2] = lg_send[x]

            to_line(own_send, ownl, own_ss, own_rs)
            e_all.start()

    with scope("pairs_query"):
        pairing = [jnp.where(upper, tn(head_of(v, h), head_of(go, h)), 0.0).astype(BF16) for h in range(heads)]
        gq_own = by_head(nn(head_of(k_dec, h), pairing[h]) for h in range(heads))
        gk_own = by_head(nt(head_of(q_dec, h), pairing[h]) for h in range(heads))

    with scope("decays"):
        @pl.when(c == 0)
        def _():
            e_all.wait_recv()

        decays = e_buf[pl.ds(c * pln, pln)]
        after = [jnp.ones((1, ch), F32)] * nx
        ids = [line(i)[1] * nx + line(i)[2] for i in range(nx)]
        for i in range(pln):
            after = [a * jnp.where(i > n, decays[i], 1.0) for a, n in zip(after, ids)]

    with scope("wait_line"):
        arrived(xtl, nx - 1, xt_rs)
        arrived(kl, nx - 1, k_rs)

    def pairs(parts):
        return [jnp.concatenate(parts[i : i + 2], axis=1) for i in range(0, nx, 2)]

    def to_chunks(ref, total):
        for i in range(ny):
            ref[i] = total[:, i * nz * rows : (i + 1) * nz * rows].astype(ref.dtype)

    with scope("line_m"):
        turned_of = pairs([xtl[i].reshape(d_model // nx, tok) for i in range(nx)])
        tall_after = jnp.concatenate(after + [jnp.ones((8 - nx, ch), F32)], axis=0).T
        scaled = pairs([(kl[i].astype(F32) * tall_after[:, i : i + 1]).astype(BF16) for i in range(nx)])
        m_sum = nt(scaled[0], turned_of[0])
        for a, b in zip(scaled[1:], turned_of[1:]):
            m_sum = m_sum + nt(a, b)
        to_chunks(m_send, m_sum)
        to_column(m_send, m_recv, m_ss, m_rs)

    def arriving(o, carried):
        frm = o + back * (nz - 1 - 2 * o)
        return ft_buf[frm] * carried + t_buf[frm].astype(F32)

    def plane_send(g, ty, tx):
        if g:
            return rcopy(o_send, p_both.at[me // 2], p_ss, p_rs, (z, ty, tx, 1))
        return rcopy(o_send.at[0], p_buf.at[me // 2], p_ss, p_rs, (z, ty, tx, 0))

    def state_send(g, ty, tx):
        return rcopy(st_send.at[g * pln + ty * nx + tx], st_buf.at[me // 2], st_ss, st_rs, (z, ty, tx, g))

    @pl.when(c == 1)
    def _():
        with scope("wait2"):
            for n in range(1, nz):

                @pl.when(z_order == n)
                def _():
                    arrived(ft_buf, n, ft_rs)
                    arrived(t_buf, n, t_rs)

            carried = lax.fori_loop(0, z_order, arriving, jnp.zeros(t_send.shape, F32))
        with scope("send3"):
            held_out[...] = carried
            o_send[...] = carried.astype(BF16)

            @pl.when(back == 1)
            def _():
                for target in targets[pln:] + targets[:pln]:
                    plane_send(*target).start()
                p_both[me // 2] = o_send[...]

    some = pln // 2
    with scope("wait_1b"):

        @pl.when(c == 0)
        def _():
            arrived(q_line, some, q_rs)
            arrived(rl, nx - 1, r_rs)

        for odd in (0, 1):

            @pl.when((c == 1) & (back == odd))
            def _():
                arrived(q_grad, some - odd, q_rs)

    with scope("line_a"):

        @pl.when(c == 0)
        def _():
            grad_at = q_line[...].astype(F32).reshape(HEAD, ch)
            g_all[nx - 1] = grad_at
            for i in range(nx - 2, -1, -1):
                grad_at = e_buf[y * nx + i + 1] * grad_at + rl[i + 1].astype(F32)
                g_all[i] = grad_at

        @pl.when(c == 1)
        def _():
            for i in range(nx):
                g_all[i] = q_grad[:, :, ch * i : ch * (i + 1)].astype(F32).reshape(HEAD, ch)

        parts = []
        for i in range(nx):
            grad_at = g_all[i]
            bd_in = by_head((grad_at * m).astype(BF16) for m in mf)
            parts.append(nn(bd_in, kl[i]))
    with scope("wait_own"):
        arrived(ownl, nx - 1, own_rs)
    with scope("line_a2"):
        parts = pairs([(ownl[i].astype(F32) + part).astype(BF16) for i, part in enumerate(parts)])
        def chunk_of(to):
            pieces = pairs([xtl[i, to].reshape(nz * rows, tok) for i in range(nx)])
            chunk = nt(parts[0], pieces[0])
            for a, b in zip(parts[1:], pieces[1:]):
                chunk = chunk + nt(a, b)
            return chunk

        for ks in (far_first[:1], far_first[1:] + [0]):
            chunks = [chunk_of(columns[k]) for k in ks]
            for k, chunk in zip(ks, chunks):
                a_send[columns[k]] = chunk.astype(BF16)
                if not k:
                    aacc[...] = chunk
            for k in ks:
                if k:
                    column_send(a_send, a_recv, a_ss, a_rs, columns[k]).start()

        @pl.when(c == 0)
        def _():
            rcopy(a_send.at[y], a_recv.at[y], a_ss, a_rs.at[0], (z, y, x, 1)).start()

    @pl.when((c == 1) & (back == 0))
    def _():
        with scope("states"):
            for g in (0, 1):
                start = held_out[g]
                for i in range(pln):
                    st_send[g * pln + i] = (l_send[g * pln + i].astype(F32) + start).astype(BF16)
                    start = e_buf[g * pln + i] * start
            for target in targets:
                state_send(*target).start()
            st_buf[me // 2] = st_send[pln + me]

    @pl.when(c == 1)
    def _():
        with scope("wait_m1"):
            m_plane = from_column(1, m_send.at[x], m_recv, m_rs).astype(BF16)
        with scope("wait3"):
            for odd in (0, 1):

                @pl.when(back == odd)
                def _():
                    arrived(p_both, some - odd, p_rs)

        for g in (1, 0):
            outer[g] = p_both[:, g].astype(F32).reshape(HEAD, ch)
            bd_out = by_head((outer[g] * m).astype(BF16) for m in mf)
            with scope(f"wait_a{g}"):
                if g == 0:
                    m_plane = from_column(0, None, m_recv, m_rs).astype(BF16)
                w_sum = nt(m_plane, bd_out)
                w_sum = w_sum + from_column(g, aacc, a_recv, a_rs)
            with scope(f"send_z{g}"):
                if g:
                    w2[...] = w_sum.reshape(w2.shape)
                z_send[pl.ds(g * nz, nz)] = w_sum.astype(BF16).reshape(nz, rows, ch)
                for d in z_steps if g else z_steps + [0]:
                    rcopy(z_send.at[g * nz + zs[d]], z_recv.at[z], z_ss, z_rs, (zs[d], y, x, g)).start()

    @pl.when(c == 0)
    def _():
        with scope("wait3"):
            arrived(p_buf, some, p_rs)
        outer[0] = p_buf[...].astype(F32).reshape(HEAD, ch)

    with scope("value_grad"):
        own_after = after[nx - 1]
        for i in range(nx - 1):
            own_after = jnp.where(at_line == i, after[i], own_after)
        grad = g_all[at_line] + own_after * outer[c]
        bd_grad = by_head((grad * m).astype(BF16) for m in mf)
        value_grad = (gv_own + nn(bd_grad, k_end)).astype(BF16)

    with scope("input_grad"):
        width = 512 if d_model % 512 == 0 else d_model
        turned = value_grad.T
        for j in range(d_model // width):
            cols = pl.ds(j * width, width)
            ig[:, :, cols] = nn(turned, w_v[:, cols]).astype(BF16).reshape(2, tok // 2, width)
        ig_copy = rcopy(ig.at[1 - c], ig_recv, ig_ss, ig_rs, (z, y, x, 1 - c))
        ig_copy.start()

    with scope("query_forget"):
        for even in (0, 1):

            @pl.when((1 - back) * c == even)
            def _():
                arrived(st_buf, some - even, st_rs)

        state = st_buf[...].astype(F32).reshape(HEAD, ch)
        bd_state = by_head((state * m).astype(BF16) for m in mf)
        g_query = growth * (gq_own + tn(bd_state, go))
        g_key = shrink * gk_own + remain * tn(bd_grad, v)
        gq_out[...] = (g_query * (q_sig * (1.0 + q * (1.0 - q_sig)))).astype(BF16)
        ends = grad * (total * state + update)
        ends_high = ends.astype(BF16)
        ends_low = (ends - ends_high.astype(F32)).astype(BF16)
        tall_ones = jnp.ones((HEAD, tok), BF16)
        boundary = tn(ends_high, tall_ones) + tn(ends_low, tall_ones)
        flow = query * g_query - k_rate * g_key
        flow_high = flow.astype(BF16)
        flow_low = (flow - flow_high.astype(F32)).astype(BF16)
        g_decay = nn(flow_high, lower_ones) + nn(flow_low, lower_ones) + boundary
        gf_out[...] = ((g_decay / (1.0 - k_rate) - g_key) * k_rate * (1.0 / (1.0 + jnp.exp(-f)))).astype(BF16)

    with scope("input_sum"):
        ig_copy.wait_recv()
        gx_out[...] = (ig[c].astype(F32) + ig_recv[...].astype(F32)).astype(BF16)

    with scope("drain"):
        left(xt, nx - 1, xt_ss)
        left(kl, nx - 1, k_ss)
        left(ownl, nx - 1, own_ss)
        ig_copy.wait_send()

        @pl.when(c == 0)
        def _():
            left(thin, pln, e_ss)
            left(s_send, pln, s_ss)
            left(rl, nx - 1, r_ss)
            left(m_send, ny, m_ss)
            left(a_send, ny, a_ss)

        @pl.when(c == 1)
        def _():
            left(m_send, ny - 1, m_ss)
            left(a_send, ny - 1, a_ss)
            left(thin, pln - 1, e_ss)
            left(s_send, pln - 1, s_ss)
            for n in range(1, nz):

                @pl.when(nz - 1 - z_order == n)
                def _():
                    left(ft_buf, n, ft_ss)
                    left(t_buf, n, t_ss)

            e_all.wait_send()

            @pl.when(back == 1)
            def _():
                left(wide, pln, q_ss.at[0])
                left(broad, pln - 1, q_ss.at[1])
                left(wide, 3 * pln - 2, p_ss)

            @pl.when(back == 0)
            def _():
                left(st_send, 2 * pln - 1, st_ss)

    with scope("wait_z"):

        @pl.when(c == 0)
        def _():
            arrived(z_recv, nz, z_rs)
            w_last = z_recv[0].astype(F32)
            for k in range(1, nz):
                w_last = w_last + z_recv[k].astype(F32)
            gw_out[...] = w_last

        @pl.when(c == 1)
        def _():
            arrived(z_recv, nz - 1, z_rs)
            w_last = w2[z]
            for k in range(1, nz):
                w_last = w_last + z_recv[zs[k]].astype(F32)
            gw_out[...] = w_last
            left(z_send, 2 * nz - 1, z_ss)


def write_out(*refs):
    copies = [pltpu.make_async_copy(refs[k], refs[4 + k], refs[8].at[k]) for k in range(4)]
    for copy in copies:
        copy.start()
    for copy in copies:
        copy.wait()


def on_device(nz, ny, nx, block_input, value_weight, query_pre, forget_pre, lower_bound, out_grad):
    tok, d_model = block_input.shape
    ch = value_weight.shape[1]
    pln = ny * nx
    piece = 2 * HEAD // pln
    rows = d_model // (nz * pln)
    vm, dma = pltpu.VMEM, pltpu.SemaphoreType.DMA
    scratch = [
        vm((tok, d_model), BF16), vm((ch, d_model), BF16),
        vm((ch, tok), BF16), vm((ch, tok), BF16), vm((ch, tok), BF16), vm((1, ch), F32),
        vm((pln * (ny + 1), piece, ch), BF16), vm((pln, 1, ch), F32),
        vm((pln, piece, ny * ch), BF16),
        vm((pln, piece, ch), BF16), vm((1, ch), F32),
        vm((2 * pln, piece, ch), BF16), vm((2 * pln, 1, ch), F32),
        vm((2 * pln, piece, ch), BF16), vm((nx, piece, ny * ch), BF16),
        vm((pln // 2, piece, ny * ch), BF16), vm((pln // 2, piece, ch), BF16),
        vm((2, piece, ch), BF16), vm((2, 1, ch), F32),
        vm((nz, 2, piece, ch), BF16), vm((nz, 2, 1, ch), F32),
        vm((2, piece, ch), F32), vm((2, piece, ch), BF16),
        vm((pln // 2, piece, ch), BF16), vm((pln // 2, 2, piece, ch), BF16),
        vm((2, HEAD, ch), F32), vm((2 * pln, piece, ch), BF16), vm((pln // 2, piece, ch), BF16),
        vm((nx, ny, nz, rows, tok), BF16), vm((nx, ny, nz, rows, tok), BF16),
        vm((HEAD, ch), BF16), vm((nx, HEAD, ch), BF16),
        vm((ch, tok), BF16), vm((nx, ch, tok), BF16),
        vm((ch, tok), BF16), vm((nx, ch, tok), BF16),
        vm((nx, HEAD, ch), F32),
        vm((2, tok // 2, d_model), BF16), vm((tok // 2, d_model), BF16),
        vm((ny, ch, nz * rows), BF16), vm((2 * ny, ch, nz * rows), BF16),
        vm((ch, nz * rows), F32), vm((ny, ch, nz * rows), BF16), vm((2 * ny, ch, nz * rows), BF16),
        vm((nz, rows, ch), F32), vm((2 * nz, rows, ch), BF16), vm((nz, rows, ch), BF16),
        dma((6,)),
        *(dma for _ in range(6)), dma((2,)), dma,
        *(dma for _ in range(4 + 2 + 2 + 8)),
        dma, dma((2,)), dma, dma((2,)), dma, dma, dma, dma,
    ]
    hbm, near = pl.BlockSpec(memory_space=pl.ANY), pl.BlockSpec(memory_space=pltpu.VMEM)
    results = pl.pallas_call(
        functools.partial(kernel, nz, ny, nx),
        out_shape=(
            vm((ch, tok), BF16),
            vm((ch, tok), BF16),
            vm((tok // 2, d_model), BF16),
            vm((rows, ch), F32),
        ),
        in_specs=[hbm] * 6,
        out_specs=(near,) * 4,
        scratch_shapes=scratch,
        compiler_params=pltpu.CompilerParams(collective_id=0, has_side_effects=True),
    )(block_input, value_weight.T, query_pre.T, forget_pre.T, out_grad.T, lower_bound.reshape(1, ch))
    g_query, g_forget, g_input, g_weight = pl.pallas_call(
        write_out,
        out_shape=tuple(jax.ShapeDtypeStruct(a.shape, a.dtype) for a in results),
        in_specs=[near] * 4,
        out_specs=(hbm,) * 4,
        scratch_shapes=[dma((4,))],
    )(*(pltpu.with_memory_space_constraint(a, pltpu.VMEM) for a in results))
    return g_query.T, g_forget.T, g_input, g_weight


def on_mesh(devices):
    nz, ny, nx = devices.shape[:3]
    split = Mesh(devices, SP_TP)
    in_specs = (P(SP, None), P(None, "tp"), P(SP, "tp"), P(SP, "tp"), P("tp"), P(SP, "tp"))
    out_specs = (P(SP, "tp"), P(SP, "tp"), P(SP_TP, None), P(SP, "tp"))
    return jax.shard_map(
        functools.partial(on_device, nz, ny, nx), mesh=split, in_specs=in_specs, out_specs=out_specs, check_vma=False
    )


def solution(mesh):
    return on_mesh(mesh.devices.reshape(8, 4, 4, mesh.shape["tp"]))
```

```python
import functools

import jax
import jax.numpy as jnp
from jax import lax
from jax.experimental import pallas as pl
from jax.experimental.pallas import tpu as pltpu
from jax.sharding import Mesh
from jax.sharding import PartitionSpec as P

HEAD = 64
SP = ("sp_0", "sp_1", "sp_2")
SP_TP = ("sp_0", "sp_1", "sp_2", "tp")
F32, BF16 = jnp.float32, jnp.bfloat16
LOGICAL = pl.DeviceIdType.MESH


def nn(a, b):
    return lax.dot_general(a, b, (((1,), (0,)), ((), ())), preferred_element_type=F32)


def nt(a, b):
    return lax.dot_general(a, b, (((1,), (1,)), ((), ())), preferred_element_type=F32)


def tn(a, b):
    return lax.dot_general(a, b, (((0,), (0,)), ((), ())), preferred_element_type=F32)


def rcopy(src, dst, send, recv, device):
    return pltpu.make_async_remote_copy(
        src_ref=src, dst_ref=dst, send_sem=send, recv_sem=recv, device_id=device, device_id_type=LOGICAL
    )


def kernel(
    nz, ny, nx,
    x_hbm, w_hbm, q_hbm, f_hbm, go_hbm, lb_hbm,
    gq_out, gf_out, gx_out, gw_out,
    x_v, w_v, q_v, f_v, go_v, lb_v, wide, thin, broad,
    s_send, e_send, s_buf, e_buf, l_send, lg_send, q_grad, q_line, t_send, ft_send, t_buf, ft_buf, held_out, o_send, p_buf, p_both, outer, st_send, st_buf,
    xt, xtl, r_send, rl, k_send, kl, own_send, ownl, g_all, ig, ig_recv,
    m_send, m_recv, aacc, a_send, a_recv, w2, z_send, z_recv,
    lsem, s_ss, s_rs, e_ss, e_rs, ea_ss, ea_rs, q_ss, q_rs, t_ss, t_rs, ft_ss, ft_rs, p_ss, p_rs, st_ss, st_rs,
    xt_ss, xt_rs, r_ss, r_rs, k_ss, k_rs, own_ss, own_rs,
    m_ss, m_rs, a_ss, a_rs, z_ss, z_rs, ig_ss, ig_rs,
):
    pln = ny * nx
    tok, d_model = x_v.shape
    ch = w_v.shape[0]
    heads = ch // HEAD
    z, y, x, c = (lax.axis_index(a) for a in SP_TP)
    me = y * nx + x
    back = lax.rem(x + y, 2)
    zs, ys, xs = ([lax.rem(at + d, n) for d in range(n)] for at, n in ((z, nz), (y, ny), (x, nx)))
    across = lambda d, n: min(d, n - d)
    steps = [(dy, dx) for dy in range(ny) for dx in range(nx) if dy or dx]
    steps.sort(key=lambda t: -across(t[0], ny) - across(t[1], nx))
    others = [(ys[dy], xs[dx]) for dy, dx in steps]
    everyone = others + [(y, x)]
    z_steps = sorted(range(1, nz), key=lambda d: -across(d, nz))
    far_first = sorted(range(1, nx), key=lambda d: -across(d, nx))

    at_line, at_col = x * (1 - c) + y * c, y * (1 - c) + x * c
    lines = [xs[d] * (1 - c) + ys[d] * c for d in range(nx)]
    columns = [ys[d] * (1 - c) + xs[d] * c for d in range(ny)]

    def line(i):
        return (z, y * (1 - c) + i * c, i * (1 - c) + x * c, c)

    def column(i):
        return (z, i * (1 - c) + y * c, x * (1 - c) + i * c, c)

    def piece_of(ty, tx):
        return ty * (nx // 2) + lax.div(tx, 2) + lax.rem(tx + ty, 2) * (pln // 2)

    def head_of(a, h):
        return a[HEAD * h : HEAD * (h + 1)]

    def by_head(parts):
        return jnp.concatenate(list(parts), axis=0)

    def arrived(ref, n, sem):
        part = ref.at[pl.ds(0, n)]
        rcopy(part, part, sem, sem, (z, y, x, 1 - c)).wait_recv()

    def left(ref, n, sem):
        part = ref.at[pl.ds(0, n)]
        rcopy(part, part, sem, sem, (z, y, x, 1 - c)).wait_send()

    scope = jax.named_scope
    with scope("loads_barrier"):
        loads = [
            pltpu.make_async_copy(src, dst, lsem.at[k])
            for k, (src, dst) in enumerate(
                ((f_hbm, f_v), (q_hbm, q_v), (go_hbm, go_v), (x_hbm, x_v), (w_hbm, w_v), (lb_hbm, lb_v))
            )
        ]
        for k in (0, 5, 1, 2, 3, 4):
            loads[k].start()
        barrier = pltpu.get_barrier_semaphore()

        def greet(device):
            pl.semaphore_signal(barrier, inc=1, device_id=device, device_id_type=LOGICAL)

        @pl.when(c == 1)
        def _():
            for ty, tx in others:
                greet((z, ty, tx, 1))
            for ty, tx in everyone:
                greet((z, ty, tx, 0))

        @pl.when(c == 0)
        def _():
            for tx in xs[1:]:
                greet((z, y, tx, 0))

        for d in z_steps:
            greet((zs[d], y, x, 1))

    lane = lax.broadcasted_iota(jnp.int32, (1, ch), 1)
    mf = [jnp.where((lane >= HEAD * h) & (lane < HEAD * (h + 1)), 1.0, 0.0).astype(F32) for h in range(heads)]
    row = lax.broadcasted_iota(jnp.int32, (tok, tok), 0)
    col = lax.broadcasted_iota(jnp.int32, (tok, tok), 1)
    lower, upper = row >= col, col >= row
    lower_ones = jnp.where(lower, 1.0, 0.0).astype(BF16)
    upper_ones = jnp.where(upper, 1.0, 0.0).astype(BF16)

    def folded(full):
        out = full[:HEAD] * mf[0]
        for h in range(1, heads):
            out = out + head_of(full, h) * mf[h]
        return out

    with scope("gates"):
        loads[5].wait()
        gap = jnp.broadcast_to(1.0 - lb_v[...], (tok, ch)).T
        loads[0].wait()
        f = f_v[...].astype(F32)
        f_neg = 1.0 / (1.0 + jnp.exp(f))
        k_rate = gap * f_neg
        logs = jnp.log1p(-k_rate)
        high = logs.astype(BF16)
        low = (logs - high.astype(F32)).astype(BF16)
        cum = nn(high, upper_ones) + nn(low, upper_ones)
        row_ones = jnp.ones((8, tok), BF16)
        total = jnp.exp((nt(row_ones, high) + nt(row_ones, low))[:1])
        closing = cum[:, tok - 1 : tok]
        growth = jnp.exp(cum)
        remain = jnp.exp(closing - cum)
        e_send[...] = total
        k_end = (k_rate * remain).astype(BF16)
        loads[1].wait()
        q = q_v[...].astype(F32)
        q_sig = 1.0 / (1.0 + jnp.exp(-q))
        query = q * q_sig
        q_dec = (query * growth).astype(BF16)
        loads[2].wait()
        go = go_v[...]
        reach = folded(nt(go, q_dec))
    with scope("values"):
        loads[3].wait()
        loads[4].wait()
        v = nt(w_v[...], x_v[...]).astype(BF16)
        update = folded(nt(v, k_end))
        s_send[...] = jnp.concatenate([update, reach], axis=0).reshape(s_send.shape).astype(BF16)
        r_send[...] = reach.astype(BF16)
        k_send[...] = k_end

    with scope("barrier_wait"):
        pl.semaphore_wait(barrier, c * (pln - 1 + 2 * (nz - 1)) + (1 - c) * (pln + nx - 1))

    def to_line(source, target, send_sem, recv_sem):
        for k in far_first:
            rcopy(source, target.at[at_line], send_sem, recv_sem, line(lines[k])).start()

    def column_send(source, target, send_sem, recv_sem, to):
        device = (z, to * (1 - c) + y * c, x * (1 - c) + to * c, 1)
        return rcopy(source.at[to], target.at[c * ny + at_col], send_sem, recv_sem.at[c], device)

    def to_column(source, target, send_sem, recv_sem):
        for k in far_first:
            column_send(source, target, send_sem, recv_sem, columns[k]).start()

        @pl.when(c == 0)
        def _():
            rcopy(source.at[y], target.at[y], send_sem, recv_sem.at[0], (z, y, x, 1)).start()

    def from_column(g, own, target, recv_sem):
        arrived(target, ny - g, recv_sem.at[g])
        if g == 0:
            out = target[0].astype(F32)
            for k in range(1, ny):
                out = out + target[k].astype(F32)
            return out.T
        out = own[...].astype(F32)
        for k in range(1, ny):
            out = out + target[ny + xs[k]].astype(F32)
        return out.T

    def piece_sends(ty, tx):
        to = (z, ty, tx, 1)
        return (
            rcopy(e_send, e_buf.at[c * pln + me], e_ss, e_rs, to),
            rcopy(s_send.at[piece_of(ty, tx)], s_buf.at[c * pln + me], s_ss, s_rs, to),
        )

    mine = piece_of(y, x)
    with scope("send1"):
        for parity in (0, 1):

            @pl.when(back == parity)
            def _():
                for want in (1 - parity, parity):
                    for (dy, dx), target in zip(steps, others):
                        if (dy + dx) % 2 == want:
                            for copy in piece_sends(*target):
                                copy.start()

        @pl.when(c == 0)
        def _():
            for copy in piece_sends(y, x):
                copy.start()

        @pl.when(c == 1)
        def _():
            s_buf[pln + me] = s_send[mine]
            e_buf[pln + me] = e_send[...]

        to_line(k_send, kl, k_ss, k_rs)
        kl[at_line] = k_end
        rl[at_line] = r_send[...]

    rows = d_model // (nz * ny * nx)
    with scope("turn"):
        per = tok // rows
        for b in range(d_model // tok):
            turned = x_v[:, tok * b : tok * (b + 1)].T
            for g in range(per):
                at = b * per + g
                zz, yy, xx = at // pln, (at // nx) % ny, at % nx
                group, into = xx * (1 - c) + yy * c, yy * (1 - c) + xx * c
                xt[group, into, zz] = turned[rows * g : rows * (g + 1)]

        for k in far_first:
            to = lines[k]
            rcopy(xt.at[to], xtl.at[at_line], xt_ss, xt_rs, line(to)).start()

        @pl.when(c == 0)
        def _():
            to_line(r_send, rl, r_ss, r_rs)

        xtl[at_line] = xt[at_line]

    with scope("pairs_value"):
        shrink = jnp.exp(-cum)
        k_dec = (k_rate * shrink).astype(BF16)
        mixing = [jnp.where(lower, tn(head_of(q_dec, h), head_of(k_dec, h)), 0.0).astype(BF16) for h in range(heads)]
        gv_own = by_head(nn(head_of(go, h), mixing[h]) for h in range(heads))
        own_send[...] = gv_own.astype(BF16)
        ownl[at_line] = own_send[...]

        @pl.when(c == 0)
        def _():
            to_line(own_send, ownl, own_ss, own_rs)


    z_order = z + back * (nz - 1 - 2 * z)

    def z_sends(k):
        at = z_order + k
        to = at + back * (nz - 1 - 2 * at)
        return (
            rcopy(ft_send, ft_buf.at[z], ft_ss, ft_rs, (to, y, x, 1)),
            rcopy(t_send, t_buf.at[z], t_ss, t_rs, (to, y, x, 1)),
        )

    def carry_send(g, ty, tx):
        device = (z, ty, tx, g)
        if g == 0:
            return rcopy(l_send.at[ty * nx + nx - 1], q_line.at[me // 2], q_ss.at[0], q_rs, device)
        return rcopy(lg_send.at[tx], q_grad.at[me // 2], q_ss.at[1], q_rs, device)

    targets = [(0, *t) for t in everyone] + [(1, *t) for t in others]
    plane_decays = e_buf.at[pl.ds(0, pln)]
    e_all = rcopy(plane_decays, plane_decays, ea_ss, ea_rs, (z, y, x, 1 - c))

    @pl.when(c == 1)
    def _():
        with scope("wait1"):
            arrived(e_buf, 2 * pln - 1, e_rs)
            arrived(s_buf, 2 * pln - 1, s_rs)
        with scope("scan1"):
            for parity in (0, 1):

                @pl.when(back == parity)
                def _():
                    for g in (0, 1):
                        held = jnp.zeros(t_send.shape[1:], F32)
                        factor = jnp.ones((1, ch), F32)
                        for it in range(pln - 1, -1, -1) if parity else range(pln):
                            if g and parity:
                                lg_send[it % nx, :, ch * (it // nx) : ch * (it // nx + 1)] = held.astype(BF16)
                            else:
                                l_send[g * pln + it] = held.astype(BF16)
                            decay = e_buf[g * pln + it]
                            held = decay * held + s_buf[g * pln + it].astype(F32)
                            factor = decay * factor
                        t_send[g] = held.astype(BF16)
                        ft_send[g] = factor

        with scope("send2"):
            for k in range(1, nz):

                @pl.when(z_order + k < nz)
                def _():
                    for copy in z_sends(k):
                        copy.start()

            @pl.when(back == 1)
            def _():
                for target in targets:
                    carry_send(*target).start()
                q_grad[me // 2] = lg_send[x]

            to_line(own_send, ownl, own_ss, own_rs)
            e_all.start()

    with scope("pairs_query"):
        pairing = [jnp.where(upper, tn(head_of(v, h), head_of(go, h)), 0.0).astype(BF16) for h in range(heads)]
        gq_own = by_head(nn(head_of(k_dec, h), pairing[h]) for h in range(heads))
        gk_own = by_head(nt(head_of(q_dec, h), pairing[h]) for h in range(heads))

    with scope("decays"):
        @pl.when(c == 0)
        def _():
            e_all.wait_recv()

        decays = e_buf[pl.ds(c * pln, pln)]
        after = [jnp.ones((1, ch), F32)] * nx
        ids = [line(i)[1] * nx + line(i)[2] for i in range(nx)]
        for i in range(pln):
            after = [a * jnp.where(i > n, decays[i], 1.0) for a, n in zip(after, ids)]

    with scope("wait_line"):
        arrived(xtl, nx - 1, xt_rs)
        arrived(kl, nx - 1, k_rs)

    def pairs(parts):
        return [jnp.concatenate(parts[i : i + 2], axis=1) for i in range(0, nx, 2)]

    def to_chunks(ref, total):
        for i in range(ny):
            ref[i] = total[:, i * nz * rows : (i + 1) * nz * rows].astype(ref.dtype)

    with scope("line_m"):
        turned_of = pairs([xtl[i].reshape(d_model // nx, tok) for i in range(nx)])
        tall_after = jnp.concatenate(after + [jnp.ones((8 - nx, ch), F32)], axis=0).T
        scaled = pairs([(kl[i].astype(F32) * tall_after[:, i : i + 1]).astype(BF16) for i in range(nx)])
        m_sum = nt(scaled[0], turned_of[0])
        for a, b in zip(scaled[1:], turned_of[1:]):
            m_sum = m_sum + nt(a, b)
        to_chunks(m_send, m_sum)
        to_column(m_send, m_recv, m_ss, m_rs)

    def arriving(o, carried):
        frm = o + back * (nz - 1 - 2 * o)
        return ft_buf[frm] * carried + t_buf[frm].astype(F32)

    def plane_send(g, ty, tx):
        if g:
            return rcopy(o_send, p_both.at[me // 2], p_ss, p_rs, (z, ty, tx, 1))
        return rcopy(o_send.at[0], p_buf.at[me // 2], p_ss, p_rs, (z, ty, tx, 0))

    def state_send(g, ty, tx):
        return rcopy(st_send.at[g * pln + ty * nx + tx], st_buf.at[me // 2], st_ss, st_rs, (z, ty, tx, g))

    @pl.when(c == 1)
    def _():
        with scope("wait2"):
            for n in range(1, nz):

                @pl.when(z_order == n)
                def _():
                    arrived(ft_buf, n, ft_rs)
                    arrived(t_buf, n, t_rs)

            carried = lax.fori_loop(0, z_order, arriving, jnp.zeros(t_send.shape, F32))
        with scope("send3"):
            held_out[...] = carried
            o_send[...] = carried.astype(BF16)

            @pl.when(back == 1)
            def _():
                for target in targets[pln:] + targets[:pln]:
                    plane_send(*target).start()
                p_both[me // 2] = o_send[...]

    some = pln // 2
    with scope("wait_1b"):

        @pl.when(c == 0)
        def _():
            arrived(q_line, some, q_rs)
            arrived(rl, nx - 1, r_rs)

        for odd in (0, 1):

            @pl.when((c == 1) & (back == odd))
            def _():
                arrived(q_grad, some - odd, q_rs)

    with scope("line_a"):

        @pl.when(c == 0)
        def _():
            grad_at = q_line[...].astype(F32).reshape(HEAD, ch)
            g_all[nx - 1] = grad_at
            for i in range(nx - 2, -1, -1):
                grad_at = e_buf[y * nx + i + 1] * grad_at + rl[i + 1].astype(F32)
                g_all[i] = grad_at

        @pl.when(c == 1)
        def _():
            for i in range(nx):
                g_all[i] = q_grad[:, :, ch * i : ch * (i + 1)].astype(F32).reshape(HEAD, ch)

        parts = []
        for i in range(nx):
            grad_at = g_all[i]
            bd_in = by_head((grad_at * m).astype(BF16) for m in mf)
            parts.append(nn(bd_in, kl[i]))
    with scope("wait_own"):
        arrived(ownl, nx - 1, own_rs)
    with scope("line_a2"):
        parts = pairs([(ownl[i].astype(F32) + part).astype(BF16) for i, part in enumerate(parts)])
        def chunk_of(to):
            pieces = pairs([xtl[i, to].reshape(nz * rows, tok) for i in range(nx)])
            chunk = nt(parts[0], pieces[0])
            for a, b in zip(parts[1:], pieces[1:]):
                chunk = chunk + nt(a, b)
            return chunk

        for ks in (far_first[:1], far_first[1:] + [0]):
            chunks = [chunk_of(columns[k]) for k in ks]
            for k, chunk in zip(ks, chunks):
                a_send[columns[k]] = chunk.astype(BF16)
                if not k:
                    aacc[...] = chunk
            for k in ks:
                if k:
                    column_send(a_send, a_recv, a_ss, a_rs, columns[k]).start()

        @pl.when(c == 0)
        def _():
            rcopy(a_send.at[y], a_recv.at[y], a_ss, a_rs.at[0], (z, y, x, 1)).start()

    @pl.when((c == 1) & (back == 0))
    def _():
        with scope("states"):
            for g in (0, 1):
                start = held_out[g]
                for i in range(pln):
                    st_send[g * pln + i] = (l_send[g * pln + i].astype(F32) + start).astype(BF16)
                    start = e_buf[g * pln + i] * start
            for target in targets:
                state_send(*target).start()
            st_buf[me // 2] = st_send[pln + me]

    @pl.when(c == 1)
    def _():
        with scope("wait_m1"):
            m_plane = from_column(1, m_send.at[x], m_recv, m_rs).astype(BF16)
        with scope("wait3"):
            for odd in (0, 1):

                @pl.when(back == odd)
                def _():
                    arrived(p_both, some - odd, p_rs)

        for g in (1, 0):
            outer[g] = p_both[:, g].astype(F32).reshape(HEAD, ch)
            bd_out = by_head((outer[g] * m).astype(BF16) for m in mf)
            with scope(f"wait_a{g}"):
                if g == 0:
                    m_plane = from_column(0, None, m_recv, m_rs).astype(BF16)
                w_sum = nt(m_plane, bd_out)
                w_sum = w_sum + from_column(g, aacc, a_recv, a_rs)
            with scope(f"send_z{g}"):
                if g:
                    w2[...] = w_sum.reshape(w2.shape)
                z_send[pl.ds(g * nz, nz)] = w_sum.astype(BF16).reshape(nz, rows, ch)
                for d in z_steps if g else z_steps + [0]:
                    rcopy(z_send.at[g * nz + zs[d]], z_recv.at[z], z_ss, z_rs, (zs[d], y, x, g)).start()

    @pl.when(c == 0)
    def _():
        with scope("wait3"):
            arrived(p_buf, some, p_rs)
        outer[0] = p_buf[...].astype(F32).reshape(HEAD, ch)

    with scope("value_grad"):
        own_after = after[nx - 1]
        for i in range(nx - 1):
            own_after = jnp.where(at_line == i, after[i], own_after)
        grad = g_all[at_line] + own_after * outer[c]
        bd_grad = by_head((grad * m).astype(BF16) for m in mf)
        value_grad = (gv_own + nn(bd_grad, k_end)).astype(BF16)

    with scope("input_grad"):
        width = 512 if d_model % 512 == 0 else d_model
        turned = value_grad.T
        for j in range(d_model // width):
            cols = pl.ds(j * width, width)
            ig[:, :, cols] = nn(turned, w_v[:, cols]).astype(BF16).reshape(2, tok // 2, width)
        ig_copy = rcopy(ig.at[1 - c], ig_recv, ig_ss, ig_rs, (z, y, x, 1 - c))
        ig_copy.start()

    with scope("query_forget"):
        for even in (0, 1):

            @pl.when((1 - back) * c == even)
            def _():
                arrived(st_buf, some - even, st_rs)

        state = st_buf[...].astype(F32).reshape(HEAD, ch)
        bd_state = by_head((state * m).astype(BF16) for m in mf)
        g_query = growth * (gq_own + tn(bd_state, go))
        g_key = shrink * gk_own + remain * tn(bd_grad, v)
        gq_out[...] = (g_query * (q_sig * (1.0 + q * (1.0 - q_sig)))).astype(BF16)
        ends = grad * (total * state + update)
        ends_high = ends.astype(BF16)
        ends_low = (ends - ends_high.astype(F32)).astype(BF16)
        tall_ones = jnp.ones((HEAD, tok), BF16)
        boundary = tn(ends_high, tall_ones) + tn(ends_low, tall_ones)
        flow = query * g_query - k_rate * g_key
        flow_high = flow.astype(BF16)
        flow_low = (flow - flow_high.astype(F32)).astype(BF16)
        g_decay = nn(flow_high, lower_ones) + nn(flow_low, lower_ones) + boundary
        gf_out[...] = ((g_decay / (1.0 - k_rate) - g_key) * k_rate * (1.0 / (1.0 + jnp.exp(-f)))).astype(BF16)

    with scope("input_sum"):
        ig_copy.wait_recv()
        gx_out[...] = (ig[c].astype(F32) + ig_recv[...].astype(F32)).astype(BF16)

    with scope("drain"):
        left(xt, nx - 1, xt_ss)
        left(kl, nx - 1, k_ss)
        left(ownl, nx - 1, own_ss)
        ig_copy.wait_send()

        @pl.when(c == 0)
        def _():
            left(thin, pln, e_ss)
            left(s_send, pln, s_ss)
            left(rl, nx - 1, r_ss)
            left(m_send, ny, m_ss)
            left(a_send, ny, a_ss)

        @pl.when(c == 1)
        def _():
            left(m_send, ny - 1, m_ss)
            left(a_send, ny - 1, a_ss)
            left(thin, pln - 1, e_ss)
            left(s_send, pln - 1, s_ss)
            for n in range(1, nz):

                @pl.when(nz - 1 - z_order == n)
                def _():
                    left(ft_buf, n, ft_ss)
                    left(t_buf, n, t_ss)

            e_all.wait_send()

            @pl.when(back == 1)
            def _():
                left(wide, pln, q_ss.at[0])
                left(broad, pln - 1, q_ss.at[1])
                left(wide, 3 * pln - 2, p_ss)

            @pl.when(back == 0)
            def _():
                left(st_send, 2 * pln - 1, st_ss)

    with scope("wait_z"):

        @pl.when(c == 0)
        def _():
            arrived(z_recv, nz, z_rs)
            w_last = z_recv[0].astype(F32)
            for k in range(1, nz):
                w_last = w_last + z_recv[k].astype(F32)
            gw_out[...] = w_last

        @pl.when(c == 1)
        def _():
            arrived(z_recv, nz - 1, z_rs)
            w_last = w2[z]
            for k in range(1, nz):
                w_last = w_last + z_recv[zs[k]].astype(F32)
            gw_out[...] = w_last
            left(z_send, 2 * nz - 1, z_ss)


def write_out(*refs):
    copies = [pltpu.make_async_copy(refs[k], refs[4 + k], refs[8].at[k]) for k in range(4)]
    for copy in copies:
        copy.start()
    for copy in copies:
        copy.wait()


def on_device(nz, ny, nx, block_input, value_weight, query_pre, forget_pre, lower_bound, out_grad):
    tok, d_model = block_input.shape
    ch = value_weight.shape[1]
    pln = ny * nx
    piece = 2 * HEAD // pln
    rows = d_model // (nz * pln)
    vm, dma = pltpu.VMEM, pltpu.SemaphoreType.DMA
    scratch = [
        vm((tok, d_model), BF16), vm((ch, d_model), BF16),
        vm((ch, tok), BF16), vm((ch, tok), BF16), vm((ch, tok), BF16), vm((1, ch), F32),
        vm((pln * (ny + 1), piece, ch), BF16), vm((pln, 1, ch), F32),
        vm((pln, piece, ny * ch), BF16),
        vm((pln, piece, ch), BF16), vm((1, ch), F32),
        vm((2 * pln, piece, ch), BF16), vm((2 * pln, 1, ch), F32),
        vm((2 * pln, piece, ch), BF16), vm((nx, piece, ny * ch), BF16),
        vm((pln // 2, piece, ny * ch), BF16), vm((pln // 2, piece, ch), BF16),
        vm((2, piece, ch), BF16), vm((2, 1, ch), F32),
        vm((nz, 2, piece, ch), BF16), vm((nz, 2, 1, ch), F32),
        vm((2, piece, ch), F32), vm((2, piece, ch), BF16),
        vm((pln // 2, piece, ch), BF16), vm((pln // 2, 2, piece, ch), BF16),
        vm((2, HEAD, ch), F32), vm((2 * pln, piece, ch), BF16), vm((pln // 2, piece, ch), BF16),
        vm((nx, ny, nz, rows, tok), BF16), vm((nx, ny, nz, rows, tok), BF16),
        vm((HEAD, ch), BF16), vm((nx, HEAD, ch), BF16),
        vm((ch, tok), BF16), vm((nx, ch, tok), BF16),
        vm((ch, tok), BF16), vm((nx, ch, tok), BF16),
        vm((nx, HEAD, ch), F32),
        vm((2, tok // 2, d_model), BF16), vm((tok // 2, d_model), BF16),
        vm((ny, ch, nz * rows), BF16), vm((2 * ny, ch, nz * rows), BF16),
        vm((ch, nz * rows), F32), vm((ny, ch, nz * rows), BF16), vm((2 * ny, ch, nz * rows), BF16),
        vm((nz, rows, ch), F32), vm((2 * nz, rows, ch), BF16), vm((nz, rows, ch), BF16),
        dma((6,)),
        *(dma for _ in range(6)), dma((2,)), dma,
        *(dma for _ in range(4 + 2 + 2 + 8)),
        dma, dma((2,)), dma, dma((2,)), dma, dma, dma, dma,
    ]
    hbm, near = pl.BlockSpec(memory_space=pl.ANY), pl.BlockSpec(memory_space=pltpu.VMEM)
    results = pl.pallas_call(
        functools.partial(kernel, nz, ny, nx),
        out_shape=(
            vm((ch, tok), BF16),
            vm((ch, tok), BF16),
            vm((tok // 2, d_model), BF16),
            vm((rows, ch), F32),
        ),
        in_specs=[hbm] * 6,
        out_specs=(near,) * 4,
        scratch_shapes=scratch,
        compiler_params=pltpu.CompilerParams(collective_id=0, has_side_effects=True),
    )(block_input, value_weight.T, query_pre.T, forget_pre.T, out_grad.T, lower_bound.reshape(1, ch))
    g_query, g_forget, g_input, g_weight = pl.pallas_call(
        write_out,
        out_shape=tuple(jax.ShapeDtypeStruct(a.shape, a.dtype) for a in results),
        in_specs=[near] * 4,
        out_specs=(hbm,) * 4,
        scratch_shapes=[dma((4,))],
    )(*(pltpu.with_memory_space_constraint(a, pltpu.VMEM) for a in results))
    return g_query.T, g_forget.T, g_input, g_weight


def on_mesh(devices):
    nz, ny, nx = devices.shape[:3]
    split = Mesh(devices, SP_TP)
    in_specs = (P(SP, None), P(None, "tp"), P(SP, "tp"), P(SP, "tp"), P("tp"), P(SP, "tp"))
    out_specs = (P(SP, "tp"), P(SP, "tp"), P(SP_TP, None), P(SP, "tp"))
    return jax.shard_map(
        functools.partial(on_device, nz, ny, nx), mesh=split, in_specs=in_specs, out_specs=out_specs, check_vma=False
    )


def solution(mesh):
    return on_mesh(mesh.devices.reshape(8, 4, 4, mesh.shape["tp"]))
```

```python
import functools

import jax
import jax.numpy as jnp
from jax import lax
from jax.experimental import pallas as pl
from jax.experimental.pallas import tpu as pltpu
from jax.sharding import Mesh
from jax.sharding import PartitionSpec as P

HEAD = 64
SP = ("sp_0", "sp_1", "sp_2")
SP_TP = ("sp_0", "sp_1", "sp_2", "tp")
F32, BF16 = jnp.float32, jnp.bfloat16
LOGICAL = pl.DeviceIdType.MESH


def nn(a, b):
    return lax.dot_general(a, b, (((1,), (0,)), ((), ())), preferred_element_type=F32)


def nt(a, b):
    return lax.dot_general(a, b, (((1,), (1,)), ((), ())), preferred_element_type=F32)


def tn(a, b):
    return lax.dot_general(a, b, (((0,), (0,)), ((), ())), preferred_element_type=F32)


def rcopy(src, dst, send, recv, device):
    return pltpu.make_async_remote_copy(
        src_ref=src, dst_ref=dst, send_sem=send, recv_sem=recv, device_id=device, device_id_type=LOGICAL
    )


def kernel(
    nz, ny, nx,
    x_hbm, w_hbm, q_hbm, f_hbm, go_hbm, lb_hbm,
    gq_out, gf_out, gx_out, gw_out,
    x_v, w_v, q_v, f_v, go_v, lb_v, wide, thin, broad,
    s_send, e_send, s_buf, e_buf, l_send, lg_send, q_grad, q_line, t_send, ft_send, t_buf, ft_buf, held_out, o_send, p_buf, p_both, outer, st_send, st_buf,
    xt, xtl, r_send, rl, k_send, kl, own_send, ownl, g_all, ig, ig_recv,
    m_send, m_recv, aacc, a_send, a_recv, w2, z_send, z_recv,
    lsem, s_ss, s_rs, e_ss, e_rs, ea_ss, ea_rs, q_ss, q_rs, t_ss, t_rs, ft_ss, ft_rs, p_ss, p_rs, st_ss, st_rs,
    xt_ss, xt_rs, r_ss, r_rs, k_ss, k_rs, own_ss, own_rs,
    m_ss, m_rs, a_ss, a_rs, z_ss, z_rs, ig_ss, ig_rs,
):
    pln = ny * nx
    tok, d_model = x_v.shape
    ch = w_v.shape[0]
    heads = ch // HEAD
    z, y, x, c = (lax.axis_index(a) for a in SP_TP)
    me = y * nx + x
    back = lax.rem(x + y, 2)
    zs, ys, xs = ([lax.rem(at + d, n) for d in range(n)] for at, n in ((z, nz), (y, ny), (x, nx)))
    across = lambda d, n: min(d, n - d)
    steps = [(dy, dx) for dy in range(ny) for dx in range(nx) if dy or dx]
    steps.sort(key=lambda t: -across(t[0], ny) - across(t[1], nx))
    others = [(ys[dy], xs[dx]) for dy, dx in steps]
    everyone = others + [(y, x)]
    z_steps = sorted(range(1, nz), key=lambda d: -across(d, nz))
    far_first = sorted(range(1, nx), key=lambda d: -across(d, nx))

    at_line, at_col = x * (1 - c) + y * c, y * (1 - c) + x * c
    lines = [xs[d] * (1 - c) + ys[d] * c for d in range(nx)]
    columns = [ys[d] * (1 - c) + xs[d] * c for d in range(ny)]

    def line(i):
        return (z, y * (1 - c) + i * c, i * (1 - c) + x * c, c)

    def column(i):
        return (z, i * (1 - c) + y * c, x * (1 - c) + i * c, c)

    def piece_of(ty, tx):
        return ty * (nx // 2) + lax.div(tx, 2) + lax.rem(tx + ty, 2) * (pln // 2)

    def head_of(a, h):
        return a[HEAD * h : HEAD * (h + 1)]

    def by_head(parts):
        return jnp.concatenate(list(parts), axis=0)

    def arrived(ref, n, sem):
        part = ref.at[pl.ds(0, n)]
        rcopy(part, part, sem, sem, (z, y, x, 1 - c)).wait_recv()

    def left(ref, n, sem):
        part = ref.at[pl.ds(0, n)]
        rcopy(part, part, sem, sem, (z, y, x, 1 - c)).wait_send()

    scope = jax.named_scope
    with scope("loads_barrier"):
        loads = [
            pltpu.make_async_copy(src, dst, lsem.at[k])
            for k, (src, dst) in enumerate(
                ((f_hbm, f_v), (q_hbm, q_v), (go_hbm, go_v), (x_hbm, x_v), (w_hbm, w_v), (lb_hbm, lb_v))
            )
        ]
        for k in (0, 5, 1, 2, 3, 4):
            loads[k].start()
        barrier = pltpu.get_barrier_semaphore()

        def greet(device):
            pl.semaphore_signal(barrier, inc=1, device_id=device, device_id_type=LOGICAL)

        @pl.when(c == 1)
        def _():
            for ty, tx in others:
                greet((z, ty, tx, 1))
            for ty, tx in everyone:
                greet((z, ty, tx, 0))

        @pl.when(c == 0)
        def _():
            for tx in xs[1:]:
                greet((z, y, tx, 0))

        for d in z_steps:
            greet((zs[d], y, x, 1))

    lane = lax.broadcasted_iota(jnp.int32, (1, ch), 1)
    mf = [jnp.where((lane >= HEAD * h) & (lane < HEAD * (h + 1)), 1.0, 0.0).astype(F32) for h in range(heads)]
    row = lax.broadcasted_iota(jnp.int32, (tok, tok), 0)
    col = lax.broadcasted_iota(jnp.int32, (tok, tok), 1)
    lower, upper = row >= col, col >= row
    lower_ones = jnp.where(lower, 1.0, 0.0).astype(BF16)
    upper_ones = jnp.where(upper, 1.0, 0.0).astype(BF16)

    def folded(full):
        out = full[:HEAD] * mf[0]
        for h in range(1, heads):
            out = out + head_of(full, h) * mf[h]
        return out

    with scope("gates"):
        loads[5].wait()
        gap = jnp.broadcast_to(1.0 - lb_v[...], (tok, ch)).T
        loads[0].wait()
        f = f_v[...].astype(F32)
        f_neg = 1.0 / (1.0 + jnp.exp(f))
        k_rate = gap * f_neg
        logs = jnp.log1p(-k_rate)
        high = logs.astype(BF16)
        low = (logs - high.astype(F32)).astype(BF16)
        cum = nn(high, upper_ones) + nn(low, upper_ones)
        row_ones = jnp.ones((8, tok), BF16)
        total = jnp.exp((nt(row_ones, high) + nt(row_ones, low))[:1])
        closing = cum[:, tok - 1 : tok]
        growth = jnp.exp(cum)
        remain = jnp.exp(closing - cum)
        e_send[...] = total
        k_end = (k_rate * remain).astype(BF16)
        loads[1].wait()
        q = q_v[...].astype(F32)
        q_sig = 1.0 / (1.0 + jnp.exp(-q))
        query = q * q_sig
        q_dec = (query * growth).astype(BF16)
        loads[2].wait()
        go = go_v[...]
        reach = folded(nt(go, q_dec))
    with scope("values"):
        loads[3].wait()
        loads[4].wait()
        v = nt(w_v[...], x_v[...]).astype(BF16)
        update = folded(nt(v, k_end))
        s_send[...] = jnp.concatenate([update, reach], axis=0).reshape(s_send.shape).astype(BF16)
        narrow, low_half = 2 * HEAD, HEAD // 2
        rest = jnp.concatenate([reach[:low_half, narrow:], reach[low_half:, narrow:]], axis=1)
        r_send[...] = jnp.concatenate([reach[:, :narrow], rest], axis=0).astype(BF16)
        k_send[...] = k_end

    with scope("barrier_wait"):
        pl.semaphore_wait(barrier, c * (pln - 1 + 2 * (nz - 1)) + (1 - c) * (pln + nx - 1))

    def to_line(source, target, send_sem, recv_sem):
        for k in far_first:
            rcopy(source, target.at[at_line], send_sem, recv_sem, line(lines[k])).start()

    def column_send(source, target, send_sem, recv_sem, to):
        device = (z, to * (1 - c) + y * c, x * (1 - c) + to * c, 1)
        return rcopy(source.at[to], target.at[c * ny + at_col], send_sem, recv_sem.at[c], device)

    def to_column(source, target, send_sem, recv_sem):
        for k in far_first:
            column_send(source, target, send_sem, recv_sem, columns[k]).start()

        @pl.when(c == 0)
        def _():
            rcopy(source.at[y], target.at[y], send_sem, recv_sem.at[0], (z, y, x, 1)).start()

    def from_column(g, own, target, recv_sem):
        arrived(target, ny - g, recv_sem.at[g])
        if g == 0:
            out = target[0].astype(F32)
            for k in range(1, ny):
                out = out + target[k].astype(F32)
            return out.T
        out = own[...].astype(F32)
        for k in range(1, ny):
            out = out + target[ny + xs[k]].astype(F32)
        return out.T

    def piece_sends(ty, tx):
        to = (z, ty, tx, 1)
        return (
            rcopy(e_send, e_buf.at[c * pln + me], e_ss, e_rs, to),
            rcopy(s_send.at[piece_of(ty, tx)], s_buf.at[c * pln + me], s_ss, s_rs, to),
        )

    mine = piece_of(y, x)
    with scope("send1"):
        for parity in (0, 1):

            @pl.when(back == parity)
            def _():
                for want in (1 - parity, parity):
                    for (dy, dx), target in zip(steps, others):
                        if (dy + dx) % 2 == want:
                            for copy in piece_sends(*target):
                                copy.start()

        @pl.when(c == 0)
        def _():
            for copy in piece_sends(y, x):
                copy.start()

        @pl.when(c == 1)
        def _():
            s_buf[pln + me] = s_send[mine]
            e_buf[pln + me] = e_send[...]

        to_line(k_send, kl, k_ss, k_rs)
        kl[at_line] = k_end
        rl[at_line] = r_send[...]

    rows = d_model // (nz * ny * nx)
    with scope("turn"):
        per = tok // rows
        for b in range(d_model // tok):
            turned = x_v[:, tok * b : tok * (b + 1)].T
            for g in range(per):
                at = b * per + g
                zz, yy, xx = at // pln, (at // nx) % ny, at % nx
                group, into = xx * (1 - c) + yy * c, yy * (1 - c) + xx * c
                xt[group, into, zz] = turned[rows * g : rows * (g + 1)]

        for k in far_first:
            to = lines[k]
            rcopy(xt.at[to], xtl.at[at_line], xt_ss, xt_rs, line(to)).start()

        @pl.when(c == 0)
        def _():
            to_line(r_send, rl, r_ss, r_rs)

        xtl[at_line] = xt[at_line]

    with scope("pairs_value"):
        shrink = jnp.exp(-cum)
        k_dec = (k_rate * shrink).astype(BF16)
        mixing = [jnp.where(lower, tn(head_of(q_dec, h), head_of(k_dec, h)), 0.0).astype(BF16) for h in range(heads)]
        gv_own = by_head(nn(head_of(go, h), mixing[h]) for h in range(heads))
        own_send[...] = gv_own.astype(BF16)
        ownl[at_line] = own_send[...]

        @pl.when(c == 0)
        def _():
            to_line(own_send, ownl, own_ss, own_rs)


    z_order = z + back * (nz - 1 - 2 * z)

    def z_sends(k):
        at = z_order + k
        to = at + back * (nz - 1 - 2 * at)
        return (
            rcopy(ft_send, ft_buf.at[z], ft_ss, ft_rs, (to, y, x, 1)),
            rcopy(t_send, t_buf.at[z], t_ss, t_rs, (to, y, x, 1)),
        )

    def carry_send(g, ty, tx):
        device = (z, ty, tx, g)
        if g == 0:
            return rcopy(l_send.at[ty * nx + nx - 1], q_line.at[me // 2], q_ss.at[0], q_rs, device)
        return rcopy(lg_send.at[tx], q_grad.at[me // 2], q_ss.at[1], q_rs, device)

    targets = [(0, *t) for t in everyone] + [(1, *t) for t in others]
    plane_decays = e_buf.at[pl.ds(0, pln)]
    e_all = rcopy(plane_decays, plane_decays, ea_ss, ea_rs, (z, y, x, 1 - c))

    @pl.when(c == 1)
    def _():
        with scope("wait1"):
            arrived(e_buf, 2 * pln - 1, e_rs)
            arrived(s_buf, 2 * pln - 1, s_rs)
        with scope("scan1"):
            for parity in (0, 1):

                @pl.when(back == parity)
                def _():
                    for g in (0, 1):
                        held = jnp.zeros(t_send.shape[1:], F32)
                        factor = jnp.ones((1, ch), F32)
                        for it in range(pln - 1, -1, -1) if parity else range(pln):
                            if g and parity:
                                lg_send[it % nx, :, ch * (it // nx) : ch * (it // nx + 1)] = held.astype(BF16)
                            else:
                                l_send[g * pln + it] = held.astype(BF16)
                            decay = e_buf[g * pln + it]
                            held = decay * held + s_buf[g * pln + it].astype(F32)
                            factor = decay * factor
                        t_send[g] = held.astype(BF16)
                        ft_send[g] = factor

        with scope("send2"):
            for k in range(1, nz):

                @pl.when(z_order + k < nz)
                def _():
                    for copy in z_sends(k):
                        copy.start()

            @pl.when(back == 1)
            def _():
                for target in targets:
                    carry_send(*target).start()
                q_grad[me // 2] = lg_send[x]

            to_line(own_send, ownl, own_ss, own_rs)
            e_all.start()

    with scope("pairs_query"):
        pairing = [jnp.where(upper, tn(head_of(v, h), head_of(go, h)), 0.0).astype(BF16) for h in range(heads)]
        gq_own = by_head(nn(head_of(k_dec, h), pairing[h]) for h in range(heads))
        gk_own = by_head(nt(head_of(q_dec, h), pairing[h]) for h in range(heads))

    with scope("decays"):
        @pl.when(c == 0)
        def _():
            e_all.wait_recv()

        decays = e_buf[pl.ds(c * pln, pln)]
        after = [jnp.ones((1, ch), F32)] * nx
        ids = [line(i)[1] * nx + line(i)[2] for i in range(nx)]
        for i in range(pln):
            after = [a * jnp.where(i > n, decays[i], 1.0) for a, n in zip(after, ids)]

    with scope("wait_line"):
        arrived(xtl, nx - 1, xt_rs)
        arrived(kl, nx - 1, k_rs)

    def pairs(parts):
        return [jnp.concatenate(parts[i : i + 2], axis=1) for i in range(0, nx, 2)]

    def to_chunks(ref, total):
        for i in range(ny):
            ref[i] = total[:, i * nz * rows : (i + 1) * nz * rows].astype(ref.dtype)

    with scope("line_m"):
        turned_of = pairs([xtl[i].reshape(d_model // nx, tok) for i in range(nx)])
        tall_after = jnp.concatenate(after + [jnp.ones((8 - nx, ch), F32)], axis=0).T
        scaled = pairs([(kl[i].astype(F32) * tall_after[:, i : i + 1]).astype(BF16) for i in range(nx)])
        m_sum = nt(scaled[0], turned_of[0])
        for a, b in zip(scaled[1:], turned_of[1:]):
            m_sum = m_sum + nt(a, b)
        to_chunks(m_send, m_sum)
        to_column(m_send, m_recv, m_ss, m_rs)

    def arriving(o, carried):
        frm = o + back * (nz - 1 - 2 * o)
        return ft_buf[frm] * carried + t_buf[frm].astype(F32)

    def plane_send(g, ty, tx):
        if g:
            return rcopy(o_send, p_both.at[me // 2], p_ss, p_rs, (z, ty, tx, 1))
        return rcopy(o_send.at[0], p_buf.at[me // 2], p_ss, p_rs, (z, ty, tx, 0))

    def state_send(g, ty, tx):
        return rcopy(st_send.at[g * pln + ty * nx + tx], st_buf.at[me // 2], st_ss, st_rs, (z, ty, tx, g))

    @pl.when(c == 1)
    def _():
        with scope("wait2"):
            for n in range(1, nz):

                @pl.when(z_order == n)
                def _():
                    arrived(ft_buf, n, ft_rs)
                    arrived(t_buf, n, t_rs)

            carried = lax.fori_loop(0, z_order, arriving, jnp.zeros(t_send.shape, F32))
        with scope("send3"):
            held_out[...] = carried
            o_send[...] = carried.astype(BF16)

            @pl.when(back == 1)
            def _():
                for target in targets[pln:] + targets[:pln]:
                    plane_send(*target).start()
                p_both[me // 2] = o_send[...]

    some = pln // 2
    with scope("wait_1b"):

        @pl.when(c == 0)
        def _():
            arrived(q_line, some, q_rs)
            arrived(rl, nx - 1, r_rs)

        for odd in (0, 1):

            @pl.when((c == 1) & (back == odd))
            def _():
                arrived(q_grad, some - odd, q_rs)

    with scope("line_a"):

        @pl.when(c == 0)
        def _():
            grad_at = q_line[...].astype(F32).reshape(HEAD, ch)
            g_all[nx - 1] = grad_at
            for i in range(nx - 2, -1, -1):
                near_reach = rl[i + 1].astype(F32)
                rest = near_reach[HEAD:]
                rest = jnp.concatenate([rest[:, :HEAD], rest[:, HEAD:]], axis=0)
                near_reach = jnp.concatenate([near_reach[:HEAD], rest], axis=1)
                grad_at = e_buf[y * nx + i + 1] * grad_at + near_reach
                g_all[i] = grad_at

        @pl.when(c == 1)
        def _():
            for i in range(nx):
                g_all[i] = q_grad[:, :, ch * i : ch * (i + 1)].astype(F32).reshape(HEAD, ch)

        parts = []
        for i in range(nx):
            grad_at = g_all[i]
            bd_in = by_head((grad_at * m).astype(BF16) for m in mf)
            parts.append(nn(bd_in, kl[i]))
    with scope("wait_own"):
        arrived(ownl, nx - 1, own_rs)
    with scope("line_a2"):
        parts = pairs([(ownl[i].astype(F32) + part).astype(BF16) for i, part in enumerate(parts)])
        def chunk_of(to):
            pieces = pairs([xtl[i, to].reshape(nz * rows, tok) for i in range(nx)])
            chunk = nt(parts[0], pieces[0])
            for a, b in zip(parts[1:], pieces[1:]):
                chunk = chunk + nt(a, b)
            return chunk

        for ks in (far_first[:1], far_first[1:] + [0]):
            chunks = [chunk_of(columns[k]) for k in ks]
            for k, chunk in zip(ks, chunks):
                a_send[columns[k]] = chunk.astype(BF16)
                if not k:
                    aacc[...] = chunk
            for k in ks:
                if k:
                    column_send(a_send, a_recv, a_ss, a_rs, columns[k]).start()

        @pl.when(c == 0)
        def _():
            rcopy(a_send.at[y], a_recv.at[y], a_ss, a_rs.at[0], (z, y, x, 1)).start()

    @pl.when((c == 1) & (back == 0))
    def _():
        with scope("states"):
            for g in (0, 1):
                start = held_out[g]
                for i in range(pln):
                    st_send[g * pln + i] = (l_send[g * pln + i].astype(F32) + start).astype(BF16)
                    start = e_buf[g * pln + i] * start
            for target in targets:
                state_send(*target).start()
            st_buf[me // 2] = st_send[pln + me]

    @pl.when(c == 1)
    def _():
        with scope("wait_m1"):
            m_plane = [from_column(g, m_send.at[x], m_recv, m_rs).astype(BF16) for g in (0, 1)]
        with scope("wait3"):
            for odd in (0, 1):

                @pl.when(back == odd)
                def _():
                    arrived(p_both, some - odd, p_rs)

            from_plane = []
            for g in (0, 1):
                outer[g] = p_both[:, g].astype(F32).reshape(HEAD, ch)
                bd_out = by_head((outer[g] * m).astype(BF16) for m in mf)
                from_plane.append(nt(m_plane[g], bd_out))
        for g in (1, 0):
            with scope(f"wait_a{g}"):
                w_sum = from_plane[g] + from_column(g, aacc, a_recv, a_rs)
            with scope(f"send_z{g}"):
                if g:
                    w2[...] = w_sum.reshape(w2.shape)
                z_send[pl.ds(g * nz, nz)] = w_sum.astype(BF16).reshape(nz, rows, ch)
                for d in z_steps if g else z_steps + [0]:
                    rcopy(z_send.at[g * nz + zs[d]], z_recv.at[z], z_ss, z_rs, (zs[d], y, x, g)).start()

    @pl.when(c == 0)
    def _():
        with scope("wait3"):
            arrived(p_buf, some, p_rs)
        outer[0] = p_buf[...].astype(F32).reshape(HEAD, ch)

    with scope("value_grad"):
        own_after = after[nx - 1]
        for i in range(nx - 1):
            own_after = jnp.where(at_line == i, after[i], own_after)
        grad = g_all[at_line] + own_after * outer[c]
        bd_grad = by_head((grad * m).astype(BF16) for m in mf)
        value_grad = (gv_own + nn(bd_grad, k_end)).astype(BF16)

    with scope("input_grad"):
        width = 512 if d_model % 512 == 0 else d_model
        turned = value_grad.T
        for j in range(d_model // width):
            cols = pl.ds(j * width, width)
            ig[:, :, cols] = nn(turned, w_v[:, cols]).astype(BF16).reshape(2, tok // 2, width)
        ig_copy = rcopy(ig.at[1 - c], ig_recv, ig_ss, ig_rs, (z, y, x, 1 - c))
        ig_copy.start()

    with scope("query_forget"):
        for even in (0, 1):

            @pl.when((1 - back) * c == even)
            def _():
                arrived(st_buf, some - even, st_rs)

        state = st_buf[...].astype(F32).reshape(HEAD, ch)
        bd_state = by_head((state * m).astype(BF16) for m in mf)
        g_query = growth * (gq_own + tn(bd_state, go))
        g_key = shrink * gk_own + remain * tn(bd_grad, v)
        gq_out[...] = (g_query * (q_sig * (1.0 + q * (1.0 - q_sig)))).astype(BF16)
        ends = grad * (total * state + update)
        ends_high = ends.astype(BF16)
        ends_low = (ends - ends_high.astype(F32)).astype(BF16)
        tall_ones = jnp.ones((HEAD, tok), BF16)
        boundary = tn(ends_high, tall_ones) + tn(ends_low, tall_ones)
        flow = query * g_query - k_rate * g_key
        flow_high = flow.astype(BF16)
        flow_low = (flow - flow_high.astype(F32)).astype(BF16)
        g_decay = nn(flow_high, lower_ones) + nn(flow_low, lower_ones) + boundary
        gf_out[...] = ((g_decay / (1.0 - k_rate) - g_key) * k_rate * (1.0 / (1.0 + jnp.exp(-f)))).astype(BF16)

    with scope("input_sum"):
        ig_copy.wait_recv()
        gx_out[...] = (ig[c].astype(F32) + ig_recv[...].astype(F32)).astype(BF16)

    with scope("drain"):
        left(xt, nx - 1, xt_ss)
        left(kl, nx - 1, k_ss)
        left(ownl, nx - 1, own_ss)
        ig_copy.wait_send()

        @pl.when(c == 0)
        def _():
            left(thin, pln, e_ss)
            left(s_send, pln, s_ss)
            left(rl, nx - 1, r_ss)
            left(m_send, ny, m_ss)
            left(a_send, ny, a_ss)

        @pl.when(c == 1)
        def _():
            left(m_send, ny - 1, m_ss)
            left(a_send, ny - 1, a_ss)
            left(thin, pln - 1, e_ss)
            left(s_send, pln - 1, s_ss)
            for n in range(1, nz):

                @pl.when(nz - 1 - z_order == n)
                def _():
                    left(ft_buf, n, ft_ss)
                    left(t_buf, n, t_ss)

            e_all.wait_send()

            @pl.when(back == 1)
            def _():
                left(wide, pln, q_ss.at[0])
                left(broad, pln - 1, q_ss.at[1])
                left(wide, 3 * pln - 2, p_ss)

            @pl.when(back == 0)
            def _():
                left(st_send, 2 * pln - 1, st_ss)

    with scope("wait_z"):

        @pl.when(c == 0)
        def _():
            arrived(z_recv, nz, z_rs)
            w_last = z_recv[0].astype(F32)
            for k in range(1, nz):
                w_last = w_last + z_recv[k].astype(F32)
            gw_out[...] = w_last

        @pl.when(c == 1)
        def _():
            arrived(z_recv, nz - 1, z_rs)
            w_last = w2[z]
            for k in range(1, nz):
                w_last = w_last + z_recv[zs[k]].astype(F32)
            gw_out[...] = w_last
            left(z_send, 2 * nz - 1, z_ss)


def write_out(*refs):
    copies = [pltpu.make_async_copy(refs[k], refs[4 + k], refs[8].at[k]) for k in range(4)]
    for copy in copies:
        copy.start()
    for copy in copies:
        copy.wait()


def on_device(nz, ny, nx, block_input, value_weight, query_pre, forget_pre, lower_bound, out_grad):
    tok, d_model = block_input.shape
    ch = value_weight.shape[1]
    pln = ny * nx
    piece = 2 * HEAD // pln
    rows = d_model // (nz * pln)
    vm, dma = pltpu.VMEM, pltpu.SemaphoreType.DMA
    scratch = [
        vm((tok, d_model), BF16), vm((ch, d_model), BF16),
        vm((ch, tok), BF16), vm((ch, tok), BF16), vm((ch, tok), BF16), vm((1, ch), F32),
        vm((pln * (ny + 1), piece, ch), BF16), vm((pln, 1, ch), F32),
        vm((pln, piece, ny * ch), BF16),
        vm((pln, piece, ch), BF16), vm((1, ch), F32),
        vm((2 * pln, piece, ch), BF16), vm((2 * pln, 1, ch), F32),
        vm((2 * pln, piece, ch), BF16), vm((nx, piece, ny * ch), BF16),
        vm((pln // 2, piece, ny * ch), BF16), vm((pln // 2, piece, ch), BF16),
        vm((2, piece, ch), BF16), vm((2, 1, ch), F32),
        vm((nz, 2, piece, ch), BF16), vm((nz, 2, 1, ch), F32),
        vm((2, piece, ch), F32), vm((2, piece, ch), BF16),
        vm((pln // 2, piece, ch), BF16), vm((pln // 2, 2, piece, ch), BF16),
        vm((2, HEAD, ch), F32), vm((2 * pln, piece, ch), BF16), vm((pln // 2, piece, ch), BF16),
        vm((nx, ny, nz, rows, tok), BF16), vm((nx, ny, nz, rows, tok), BF16),
        vm((ch // 2, 2 * HEAD), BF16), vm((nx, ch // 2, 2 * HEAD), BF16),
        vm((ch, tok), BF16), vm((nx, ch, tok), BF16),
        vm((ch, tok), BF16), vm((nx, ch, tok), BF16),
        vm((nx, HEAD, ch), F32),
        vm((2, tok // 2, d_model), BF16), vm((tok // 2, d_model), BF16),
        vm((ny, ch, nz * rows), BF16), vm((2 * ny, ch, nz * rows), BF16),
        vm((ch, nz * rows), F32), vm((ny, ch, nz * rows), BF16), vm((2 * ny, ch, nz * rows), BF16),
        vm((nz, rows, ch), F32), vm((2 * nz, rows, ch), BF16), vm((nz, rows, ch), BF16),
        dma((6,)),
        *(dma for _ in range(6)), dma((2,)), dma,
        *(dma for _ in range(4 + 2 + 2 + 8)),
        dma, dma((2,)), dma, dma((2,)), dma, dma, dma, dma,
    ]
    hbm, near = pl.BlockSpec(memory_space=pl.ANY), pl.BlockSpec(memory_space=pltpu.VMEM)
    results = pl.pallas_call(
        functools.partial(kernel, nz, ny, nx),
        out_shape=(
            vm((ch, tok), BF16),
            vm((ch, tok), BF16),
            vm((tok // 2, d_model), BF16),
            vm((rows, ch), F32),
        ),
        in_specs=[hbm] * 6,
        out_specs=(near,) * 4,
        scratch_shapes=scratch,
        compiler_params=pltpu.CompilerParams(collective_id=0, has_side_effects=True),
    )(block_input, value_weight.T, query_pre.T, forget_pre.T, out_grad.T, lower_bound.reshape(1, ch))
    g_query, g_forget, g_input, g_weight = pl.pallas_call(
        write_out,
        out_shape=tuple(jax.ShapeDtypeStruct(a.shape, a.dtype) for a in results),
        in_specs=[near] * 4,
        out_specs=(hbm,) * 4,
        scratch_shapes=[dma((4,))],
    )(*(pltpu.with_memory_space_constraint(a, pltpu.VMEM) for a in results))
    return g_query.T, g_forget.T, g_input, g_weight


def on_mesh(devices):
    nz, ny, nx = devices.shape[:3]
    split = Mesh(devices, SP_TP)
    in_specs = (P(SP, None), P(None, "tp"), P(SP, "tp"), P(SP, "tp"), P("tp"), P(SP, "tp"))
    out_specs = (P(SP, "tp"), P(SP, "tp"), P(SP_TP, None), P(SP, "tp"))
    return jax.shard_map(
        functools.partial(on_device, nz, ny, nx), mesh=split, in_specs=in_specs, out_specs=out_specs, check_vma=False
    )


def solution(mesh):
    return on_mesh(mesh.devices.reshape(8, 4, 4, mesh.shape["tp"]))
```

```python
import functools

import jax
import jax.numpy as jnp
from jax import lax
from jax.experimental import pallas as pl
from jax.experimental.pallas import tpu as pltpu
from jax.sharding import Mesh
from jax.sharding import PartitionSpec as P

HEAD = 64
SP = ("sp_0", "sp_1", "sp_2")
SP_TP = ("sp_0", "sp_1", "sp_2", "tp")
F32, BF16 = jnp.float32, jnp.bfloat16
LOGICAL = pl.DeviceIdType.MESH


def nn(a, b):
    return lax.dot_general(a, b, (((1,), (0,)), ((), ())), preferred_element_type=F32)


def nt(a, b):
    return lax.dot_general(a, b, (((1,), (1,)), ((), ())), preferred_element_type=F32)


def tn(a, b):
    return lax.dot_general(a, b, (((0,), (0,)), ((), ())), preferred_element_type=F32)


def rcopy(src, dst, send, recv, device):
    return pltpu.make_async_remote_copy(
        src_ref=src, dst_ref=dst, send_sem=send, recv_sem=recv, device_id=device, device_id_type=LOGICAL
    )


def kernel(
    nz, ny, nx,
    x_hbm, w_hbm, q_hbm, f_hbm, go_hbm, lb_hbm,
    gq_out, gf_out, gx_out, gw_out,
    x_v, w_v, q_v, f_v, go_v, lb_v, wide, thin, broad,
    s_send, e_send, s_buf, e_buf, l_send, lg_send, q_grad, q_line, t_send, ft_send, t_buf, ft_buf, held_out, o_send, p_buf, p_both, outer, st_send, st_buf,
    xt, xtl, r_send, rl, k_send, kl, own_send, ownl, g_all, ig, ig_recv,
    m_send, m_recv, aacc, a_send, a_recv, w2, z_send, z_recv,
    lsem, s_ss, s_rs, e_ss, e_rs, ea_ss, ea_rs, q_ss, q_rs, t_ss, t_rs, ft_ss, ft_rs, p_ss, p_rs, st_ss, st_rs,
    xt_ss, xt_rs, r_ss, r_rs, k_ss, k_rs, own_ss, own_rs,
    m_ss, m_rs, a_ss, a_rs, z_ss, z_rs, ig_ss, ig_rs,
):
    pln = ny * nx
    tok, d_model = x_v.shape
    ch = w_v.shape[0]
    heads = ch // HEAD
    z, y, x, c = (lax.axis_index(a) for a in SP_TP)
    me = y * nx + x
    back = lax.rem(x + y, 2)
    zs, ys, xs = ([lax.rem(at + d, n) for d in range(n)] for at, n in ((z, nz), (y, ny), (x, nx)))
    across = lambda d, n: min(d, n - d)
    steps = [(dy, dx) for dy in range(ny) for dx in range(nx) if dy or dx]
    steps.sort(key=lambda t: -across(t[0], ny) - across(t[1], nx))
    others = [(ys[dy], xs[dx]) for dy, dx in steps]
    everyone = others + [(y, x)]
    z_steps = sorted(range(1, nz), key=lambda d: -across(d, nz))
    far_first = sorted(range(1, nx), key=lambda d: -across(d, nx))

    at_line, at_col = x * (1 - c) + y * c, y * (1 - c) + x * c
    lines = [xs[d] * (1 - c) + ys[d] * c for d in range(nx)]
    columns = [ys[d] * (1 - c) + xs[d] * c for d in range(ny)]

    def line(i):
        return (z, y * (1 - c) + i * c, i * (1 - c) + x * c, c)

    def column(i):
        return (z, i * (1 - c) + y * c, x * (1 - c) + i * c, c)

    def piece_of(ty, tx):
        return ty * (nx // 2) + lax.div(tx, 2) + lax.rem(tx + ty, 2) * (pln // 2)

    def head_of(a, h):
        return a[HEAD * h : HEAD * (h + 1)]

    def by_head(parts):
        return jnp.concatenate(list(parts), axis=0)

    def arrived(ref, n, sem):
        part = ref.at[pl.ds(0, n)]
        rcopy(part, part, sem, sem, (z, y, x, 1 - c)).wait_recv()

    def left(ref, n, sem):
        part = ref.at[pl.ds(0, n)]
        rcopy(part, part, sem, sem, (z, y, x, 1 - c)).wait_send()

    scope = jax.named_scope
    with scope("loads_barrier"):
        loads = [
            pltpu.make_async_copy(src, dst, lsem.at[k])
            for k, (src, dst) in enumerate(
                ((f_hbm, f_v), (q_hbm, q_v), (go_hbm, go_v), (x_hbm, x_v), (w_hbm, w_v), (lb_hbm, lb_v))
            )
        ]
        for k in (0, 5, 1, 2, 3, 4):
            loads[k].start()
        barrier = pltpu.get_barrier_semaphore()

        def greet(device):
            pl.semaphore_signal(barrier, inc=1, device_id=device, device_id_type=LOGICAL)

        @pl.when(c == 1)
        def _():
            for ty, tx in others:
                greet((z, ty, tx, 1))
            for ty, tx in everyone:
                greet((z, ty, tx, 0))

        @pl.when(c == 0)
        def _():
            for tx in xs[1:]:
                greet((z, y, tx, 0))

        for d in z_steps:
            greet((zs[d], y, x, 1))

    lane = lax.broadcasted_iota(jnp.int32, (1, ch), 1)
    mf = [jnp.where((lane >= HEAD * h) & (lane < HEAD * (h + 1)), 1.0, 0.0).astype(F32) for h in range(heads)]
    row = lax.broadcasted_iota(jnp.int32, (tok, tok), 0)
    col = lax.broadcasted_iota(jnp.int32, (tok, tok), 1)
    lower, upper = row >= col, col >= row
    lower_ones = jnp.where(lower, 1.0, 0.0).astype(BF16)
    upper_ones = jnp.where(upper, 1.0, 0.0).astype(BF16)

    mb = [m.astype(BF16) for m in mf]

    def block_diagonal(a):
        a = a.astype(BF16)
        return by_head(a * m for m in mb)

    def folded(full):
        out = full[:HEAD] * mf[0]
        for h in range(1, heads):
            out = out + head_of(full, h) * mf[h]
        return out

    with scope("gates"):
        loads[5].wait()
        gap = jnp.broadcast_to(1.0 - lb_v[...], (tok, ch)).T
        loads[0].wait()
        f = f_v[...].astype(F32)
        f_neg = 1.0 / (1.0 + jnp.exp(f))
        k_rate = gap * f_neg
        logs = jnp.log1p(-k_rate)
        high = logs.astype(BF16)
        low = (logs - high.astype(F32)).astype(BF16)
        cum = nn(high, upper_ones) + nn(low, upper_ones)
        row_ones = jnp.ones((8, tok), BF16)
        total = jnp.exp((nt(row_ones, high) + nt(row_ones, low))[:1])
        closing = cum[:, tok - 1 : tok]
        growth = jnp.exp(cum)
        remain = jnp.exp(closing - cum)
        e_send[...] = total
        k_end = (k_rate * remain).astype(BF16)
        loads[1].wait()
        q = q_v[...].astype(F32)
        q_sig = 1.0 / (1.0 + jnp.exp(-q))
        query = q * q_sig
        q_dec = (query * growth).astype(BF16)
        loads[2].wait()
        go = go_v[...]
        reach = folded(nt(go, q_dec))
    with scope("values"):
        loads[3].wait()
        loads[4].wait()
        v = nt(w_v[...], x_v[...]).astype(BF16)
        update = folded(nt(v, k_end))
        s_send[...] = jnp.concatenate([update, reach], axis=0).reshape(s_send.shape).astype(BF16)
        narrow, low_half = 2 * HEAD, HEAD // 2
        rest = jnp.concatenate([reach[:low_half, narrow:], reach[low_half:, narrow:]], axis=1)
        r_send[...] = jnp.concatenate([reach[:, :narrow], rest], axis=0).astype(BF16)
        k_send[...] = k_end

    with scope("barrier_wait"):
        pl.semaphore_wait(barrier, c * (pln - 1 + 2 * (nz - 1)) + (1 - c) * (pln + nx - 1))

    def to_line(source, target, send_sem, recv_sem):
        for k in far_first:
            rcopy(source, target.at[at_line], send_sem, recv_sem, line(lines[k])).start()

    def column_send(source, target, send_sem, recv_sem, to):
        device = (z, to * (1 - c) + y * c, x * (1 - c) + to * c, 1)
        return rcopy(source.at[to], target.at[c * ny + at_col], send_sem, recv_sem.at[c], device)

    def to_column(source, target, send_sem, recv_sem):
        for k in far_first:
            column_send(source, target, send_sem, recv_sem, columns[k]).start()

        @pl.when(c == 0)
        def _():
            rcopy(source.at[y], target.at[y], send_sem, recv_sem.at[0], (z, y, x, 1)).start()

    def from_column(g, own, target, recv_sem):
        arrived(target, ny - g, recv_sem.at[g])
        if g == 0:
            out = target[0].astype(F32)
            for k in range(1, ny):
                out = out + target[k].astype(F32)
            return out.T
        out = own[...].astype(F32)
        for k in range(1, ny):
            out = out + target[ny + xs[k]].astype(F32)
        return out.T

    def piece_sends(ty, tx):
        to = (z, ty, tx, 1)
        return (
            rcopy(e_send, e_buf.at[c * pln + me], e_ss, e_rs, to),
            rcopy(s_send.at[piece_of(ty, tx)], s_buf.at[c * pln + me], s_ss, s_rs, to),
        )

    mine = piece_of(y, x)
    with scope("send1"):
        for parity in (0, 1):

            @pl.when(back == parity)
            def _():
                for want in (1 - parity, parity):
                    for (dy, dx), target in zip(steps, others):
                        if (dy + dx) % 2 == want:
                            for copy in piece_sends(*target):
                                copy.start()

        @pl.when(c == 0)
        def _():
            for copy in piece_sends(y, x):
                copy.start()

        @pl.when(c == 1)
        def _():
            s_buf[pln + me] = s_send[mine]
            e_buf[pln + me] = e_send[...]

        to_line(k_send, kl, k_ss, k_rs)
        kl[at_line] = k_end
        rl[at_line] = r_send[...]

    rows = d_model // (nz * ny * nx)
    with scope("turn"):
        per = tok // rows
        for b in range(d_model // tok):
            turned = x_v[:, tok * b : tok * (b + 1)].T
            for g in range(per):
                at = b * per + g
                zz, yy, xx = at // pln, (at // nx) % ny, at % nx
                group, into = xx * (1 - c) + yy * c, yy * (1 - c) + xx * c
                xt[group, into, zz] = turned[rows * g : rows * (g + 1)]

        for k in far_first:
            to = lines[k]
            rcopy(xt.at[to], xtl.at[at_line], xt_ss, xt_rs, line(to)).start()

        @pl.when(c == 0)
        def _():
            to_line(r_send, rl, r_ss, r_rs)

        xtl[at_line] = xt[at_line]

    with scope("pairs_value"):
        shrink = jnp.exp(-cum)
        k_dec = (k_rate * shrink).astype(BF16)
        mixing = [jnp.where(lower, tn(head_of(q_dec, h), head_of(k_dec, h)), 0.0).astype(BF16) for h in range(heads)]
        gv_own = by_head(nn(head_of(go, h), mixing[h]) for h in range(heads))
        own_send[...] = gv_own.astype(BF16)
        ownl[at_line] = own_send[...]

        @pl.when(c == 0)
        def _():
            to_line(own_send, ownl, own_ss, own_rs)


    z_order = z + back * (nz - 1 - 2 * z)

    def z_sends(k):
        at = z_order + k
        to = at + back * (nz - 1 - 2 * at)
        return (
            rcopy(ft_send, ft_buf.at[z], ft_ss, ft_rs, (to, y, x, 1)),
            rcopy(t_send, t_buf.at[z], t_ss, t_rs, (to, y, x, 1)),
        )

    def carry_send(g, ty, tx):
        device = (z, ty, tx, g)
        if g == 0:
            return rcopy(l_send.at[ty * nx + nx - 1], q_line.at[me // 2], q_ss.at[0], q_rs, device)
        return rcopy(lg_send.at[tx], q_grad.at[me // 2], q_ss.at[1], q_rs, device)

    targets = [(0, *t) for t in everyone] + [(1, *t) for t in others]
    plane_decays = e_buf.at[pl.ds(0, pln)]
    e_all = rcopy(plane_decays, plane_decays, ea_ss, ea_rs, (z, y, x, 1 - c))

    @pl.when(c == 1)
    def _():
        with scope("wait1"):
            arrived(e_buf, 2 * pln - 1, e_rs)
            arrived(s_buf, 2 * pln - 1, s_rs)
        with scope("scan1"):
            for parity in (0, 1):

                @pl.when(back == parity)
                def _():
                    for g in (0, 1):
                        held = jnp.zeros(t_send.shape[1:], F32)
                        factor = jnp.ones((1, ch), F32)
                        for it in range(pln - 1, -1, -1) if parity else range(pln):
                            if g and parity:
                                lg_send[it % nx, :, ch * (it // nx) : ch * (it // nx + 1)] = held.astype(BF16)
                            else:
                                l_send[g * pln + it] = held.astype(BF16)
                            decay = e_buf[g * pln + it]
                            held = decay * held + s_buf[g * pln + it].astype(F32)
                            factor = decay * factor
                        t_send[g] = held.astype(BF16)
                        ft_send[g] = factor

        with scope("send2"):
            for k in range(1, nz):

                @pl.when(z_order + k < nz)
                def _():
                    for copy in z_sends(k):
                        copy.start()

            @pl.when(back == 1)
            def _():
                for target in targets:
                    carry_send(*target).start()
                q_grad[me // 2] = lg_send[x]

            to_line(own_send, ownl, own_ss, own_rs)
            e_all.start()

    with scope("pairs_query"):
        pairing = [jnp.where(upper, tn(head_of(v, h), head_of(go, h)), 0.0).astype(BF16) for h in range(heads)]
        gq_own = by_head(nn(head_of(k_dec, h), pairing[h]) for h in range(heads))
        gk_own = by_head(nt(head_of(q_dec, h), pairing[h]) for h in range(heads))

    with scope("decays"):
        @pl.when(c == 0)
        def _():
            e_all.wait_recv()

        decays = e_buf[pl.ds(c * pln, pln)]
        after = [jnp.ones((1, ch), F32)] * nx
        ids = [line(i)[1] * nx + line(i)[2] for i in range(nx)]
        for i in range(pln):
            after = [a * jnp.where(i > n, decays[i], 1.0) for a, n in zip(after, ids)]

    with scope("wait_line"):
        arrived(xtl, nx - 1, xt_rs)
        arrived(kl, nx - 1, k_rs)

    def pairs(parts):
        return [jnp.concatenate(parts[i : i + 2], axis=1) for i in range(0, nx, 2)]

    def to_chunks(ref, total):
        for i in range(ny):
            ref[i] = total[:, i * nz * rows : (i + 1) * nz * rows].astype(ref.dtype)

    with scope("line_m"):
        turned_of = pairs([xtl[i].reshape(d_model // nx, tok) for i in range(nx)])
        tall_after = jnp.concatenate(after + [jnp.ones((8 - nx, ch), F32)], axis=0).T
        scaled = pairs([(kl[i].astype(F32) * tall_after[:, i : i + 1]).astype(BF16) for i in range(nx)])
        m_sum = nt(scaled[0], turned_of[0])
        for a, b in zip(scaled[1:], turned_of[1:]):
            m_sum = m_sum + nt(a, b)
        to_chunks(m_send, m_sum)
        to_column(m_send, m_recv, m_ss, m_rs)

    def arriving(o, carried):
        frm = o + back * (nz - 1 - 2 * o)
        return ft_buf[frm] * carried + t_buf[frm].astype(F32)

    def plane_send(g, ty, tx):
        if g:
            return rcopy(o_send, p_both.at[me // 2], p_ss, p_rs, (z, ty, tx, 1))
        return rcopy(o_send.at[0], p_buf.at[me // 2], p_ss, p_rs, (z, ty, tx, 0))

    def state_send(g, ty, tx):
        return rcopy(st_send.at[g * pln + ty * nx + tx], st_buf.at[me // 2], st_ss, st_rs, (z, ty, tx, g))

    @pl.when(c == 1)
    def _():
        with scope("wait2"):
            for n in range(1, nz):

                @pl.when(z_order == n)
                def _():
                    arrived(ft_buf, n, ft_rs)
                    arrived(t_buf, n, t_rs)

            carried = lax.fori_loop(0, z_order, arriving, jnp.zeros(t_send.shape, F32))
        with scope("send3"):
            held_out[...] = carried
            o_send[...] = carried.astype(BF16)

            @pl.when(back == 1)
            def _():
                for target in targets[pln:] + targets[:pln]:
                    plane_send(*target).start()
                p_both[me // 2] = o_send[...]

    some = pln // 2
    with scope("wait_1b"):

        @pl.when(c == 0)
        def _():
            arrived(q_line, some, q_rs)
            arrived(rl, nx - 1, r_rs)

        for odd in (0, 1):

            @pl.when((c == 1) & (back == odd))
            def _():
                arrived(q_grad, some - odd, q_rs)

    with scope("line_a"):

        @pl.when(c == 0)
        def _():
            grad_at = q_line[...].astype(F32).reshape(HEAD, ch)
            g_all[nx - 1] = grad_at
            for i in range(nx - 2, -1, -1):
                near_reach = rl[i + 1].astype(F32)
                rest = near_reach[HEAD:]
                rest = jnp.concatenate([rest[:, :HEAD], rest[:, HEAD:]], axis=0)
                near_reach = jnp.concatenate([near_reach[:HEAD], rest], axis=1)
                grad_at = e_buf[y * nx + i + 1] * grad_at + near_reach
                g_all[i] = grad_at

        @pl.when(c == 1)
        def _():
            for i in range(nx):
                g_all[i] = q_grad[:, :, ch * i : ch * (i + 1)].astype(F32).reshape(HEAD, ch)

        parts = []
        for i in range(nx):
            grad_at = g_all[i]
            bd_in = block_diagonal(grad_at)
            parts.append(nn(bd_in, kl[i]))
    with scope("wait_own"):
        arrived(ownl, nx - 1, own_rs)
    with scope("line_a2"):
        parts = pairs([(ownl[i].astype(F32) + part).astype(BF16) for i, part in enumerate(parts)])
        def chunk_of(to):
            pieces = pairs([xtl[i, to].reshape(nz * rows, tok) for i in range(nx)])
            chunk = nt(parts[0], pieces[0])
            for a, b in zip(parts[1:], pieces[1:]):
                chunk = chunk + nt(a, b)
            return chunk

        for ks in (far_first[:1], far_first[1:] + [0]):
            chunks = [chunk_of(columns[k]) for k in ks]
            for k, chunk in zip(ks, chunks):
                a_send[columns[k]] = chunk.astype(BF16)
                if not k:
                    aacc[...] = chunk
            for k in ks:
                if k:
                    column_send(a_send, a_recv, a_ss, a_rs, columns[k]).start()

        @pl.when(c == 0)
        def _():
            rcopy(a_send.at[y], a_recv.at[y], a_ss, a_rs.at[0], (z, y, x, 1)).start()

    @pl.when((c == 1) & (back == 0))
    def _():
        with scope("states"):
            for g in (0, 1):
                start = held_out[g]
                for i in range(pln):
                    st_send[g * pln + i] = (l_send[g * pln + i].astype(F32) + start).astype(BF16)
                    start = e_buf[g * pln + i] * start
            for target in targets:
                state_send(*target).start()
            st_buf[me // 2] = st_send[pln + me]

    @pl.when(c == 1)
    def _():
        with scope("wait_m1"):
            m_plane = [from_column(g, m_send.at[x], m_recv, m_rs).astype(BF16) for g in (0, 1)]
        with scope("wait3"):
            for odd in (0, 1):

                @pl.when(back == odd)
                def _():
                    arrived(p_both, some - odd, p_rs)

            from_plane = []
            for g in (0, 1):
                outer[g] = p_both[:, g].astype(F32).reshape(HEAD, ch)
                bd_out = block_diagonal(outer[g])
                from_plane.append(nt(m_plane[g], bd_out))
        for g in (1, 0):
            with scope(f"wait_a{g}"):
                w_sum = from_plane[g] + from_column(g, aacc, a_recv, a_rs)
            with scope(f"send_z{g}"):
                wide_part = w_sum[:, : 2 * HEAD].reshape(nz, rows, 2 * HEAD)
                rest = w_sum[:, 2 * HEAD :].reshape(nz, 2, rows // 2, HEAD)
                rest = jnp.concatenate([rest[:, 0], rest[:, 1]], axis=2)
                packed = jnp.concatenate([wide_part, rest], axis=1)
                if g:
                    w2[...] = packed
                z_send[pl.ds(g * nz, nz)] = packed.astype(BF16)
                for d in z_steps if g else z_steps + [0]:
                    rcopy(z_send.at[g * nz + zs[d]], z_recv.at[z], z_ss, z_rs, (zs[d], y, x, g)).start()

    @pl.when(c == 0)
    def _():
        with scope("wait3"):
            arrived(p_buf, some, p_rs)
        outer[0] = p_buf[...].astype(F32).reshape(HEAD, ch)

    with scope("value_grad"):
        own_after = after[nx - 1]
        for i in range(nx - 1):
            own_after = jnp.where(at_line == i, after[i], own_after)
        grad = g_all[at_line] + own_after * outer[c]
        bd_grad = block_diagonal(grad)
        value_grad = (gv_own + nn(bd_grad, k_end)).astype(BF16)

    with scope("input_grad"):
        width = 512 if d_model % 512 == 0 else d_model
        turned = value_grad.T
        for j in range(d_model // width):
            cols = pl.ds(j * width, width)
            ig[:, :, cols] = nn(turned, w_v[:, cols]).astype(BF16).reshape(2, tok // 2, width)
        ig_copy = rcopy(ig.at[1 - c], ig_recv, ig_ss, ig_rs, (z, y, x, 1 - c))
        ig_copy.start()

    with scope("query_forget"):
        for even in (0, 1):

            @pl.when((1 - back) * c == even)
            def _():
                arrived(st_buf, some - even, st_rs)

        state = st_buf[...].astype(F32).reshape(HEAD, ch)
        bd_state = block_diagonal(state)
        g_query = growth * (gq_own + tn(bd_state, go))
        g_key = shrink * gk_own + remain * tn(bd_grad, v)
        gq_out[...] = (g_query * (q_sig * (1.0 + q * (1.0 - q_sig)))).astype(BF16)
        ends = grad * (total * state + update)
        ends_high = ends.astype(BF16)
        ends_low = (ends - ends_high.astype(F32)).astype(BF16)
        tall_ones = jnp.ones((HEAD, tok), BF16)
        boundary = tn(ends_high, tall_ones) + tn(ends_low, tall_ones)
        flow = query * g_query - k_rate * g_key
        flow_high = flow.astype(BF16)
        flow_low = (flow - flow_high.astype(F32)).astype(BF16)
        g_decay = nn(flow_high, lower_ones) + nn(flow_low, lower_ones) + boundary
        gf_out[...] = ((g_decay / (1.0 - k_rate) - g_key) * k_rate * (1.0 / (1.0 + jnp.exp(-f)))).astype(BF16)

    with scope("input_sum"):
        ig_copy.wait_recv()
        gx_out[...] = (ig[c].astype(F32) + ig_recv[...].astype(F32)).astype(BF16)

    with scope("drain"):
        left(xt, nx - 1, xt_ss)
        left(kl, nx - 1, k_ss)
        left(ownl, nx - 1, own_ss)
        ig_copy.wait_send()

        @pl.when(c == 0)
        def _():
            left(thin, pln, e_ss)
            left(s_send, pln, s_ss)
            left(rl, nx - 1, r_ss)
            left(m_send, ny, m_ss)
            left(a_send, ny, a_ss)

        @pl.when(c == 1)
        def _():
            left(m_send, ny - 1, m_ss)
            left(a_send, ny - 1, a_ss)
            left(thin, pln - 1, e_ss)
            left(s_send, pln - 1, s_ss)
            for n in range(1, nz):

                @pl.when(nz - 1 - z_order == n)
                def _():
                    left(ft_buf, n, ft_ss)
                    left(t_buf, n, t_ss)

            e_all.wait_send()

            @pl.when(back == 1)
            def _():
                left(wide, pln, q_ss.at[0])
                left(broad, pln - 1, q_ss.at[1])
                left(wide, 3 * pln - 2, p_ss)

            @pl.when(back == 0)
            def _():
                left(st_send, 2 * pln - 1, st_ss)

    def unpacked(total):
        gw_out[:, : 2 * HEAD] = total[:rows]
        gw_out[: rows // 2, 2 * HEAD :] = total[rows:, :HEAD]
        gw_out[rows // 2 :, 2 * HEAD :] = total[rows:, HEAD:]

    with scope("wait_z"):

        @pl.when(c == 0)
        def _():
            arrived(z_recv, nz, z_rs)
            w_last = z_recv[0].astype(F32)
            for k in range(1, nz):
                w_last = w_last + z_recv[k].astype(F32)
            unpacked(w_last)

        @pl.when(c == 1)
        def _():
            arrived(z_recv, nz - 1, z_rs)
            w_last = w2[z]
            for k in range(1, nz):
                w_last = w_last + z_recv[zs[k]].astype(F32)
            unpacked(w_last)
            left(z_send, 2 * nz - 1, z_ss)


def write_out(*refs):
    copies = [pltpu.make_async_copy(refs[k], refs[4 + k], refs[8].at[k]) for k in range(4)]
    for copy in copies:
        copy.start()
    for copy in copies:
        copy.wait()


def on_device(nz, ny, nx, block_input, value_weight, query_pre, forget_pre, lower_bound, out_grad):
    tok, d_model = block_input.shape
    ch = value_weight.shape[1]
    pln = ny * nx
    piece = 2 * HEAD // pln
    rows = d_model // (nz * pln)
    vm, dma = pltpu.VMEM, pltpu.SemaphoreType.DMA
    scratch = [
        vm((tok, d_model), BF16), vm((ch, d_model), BF16),
        vm((ch, tok), BF16), vm((ch, tok), BF16), vm((ch, tok), BF16), vm((1, ch), F32),
        vm((pln * (ny + 1), piece, ch), BF16), vm((pln, 1, ch), F32),
        vm((pln, piece, ny * ch), BF16),
        vm((pln, piece, ch), BF16), vm((1, ch), F32),
        vm((2 * pln, piece, ch), BF16), vm((2 * pln, 1, ch), F32),
        vm((2 * pln, piece, ch), BF16), vm((nx, piece, ny * ch), BF16),
        vm((pln // 2, piece, ny * ch), BF16), vm((pln // 2, piece, ch), BF16),
        vm((2, piece, ch), BF16), vm((2, 1, ch), F32),
        vm((nz, 2, piece, ch), BF16), vm((nz, 2, 1, ch), F32),
        vm((2, piece, ch), F32), vm((2, piece, ch), BF16),
        vm((pln // 2, piece, ch), BF16), vm((pln // 2, 2, piece, ch), BF16),
        vm((2, HEAD, ch), F32), vm((2 * pln, piece, ch), BF16), vm((pln // 2, piece, ch), BF16),
        vm((nx, ny, nz, rows, tok), BF16), vm((nx, ny, nz, rows, tok), BF16),
        vm((ch // 2, 2 * HEAD), BF16), vm((nx, ch // 2, 2 * HEAD), BF16),
        vm((ch, tok), BF16), vm((nx, ch, tok), BF16),
        vm((ch, tok), BF16), vm((nx, ch, tok), BF16),
        vm((nx, HEAD, ch), F32),
        vm((2, tok // 2, d_model), BF16), vm((tok // 2, d_model), BF16),
        vm((ny, ch, nz * rows), BF16), vm((2 * ny, ch, nz * rows), BF16),
        vm((ch, nz * rows), F32), vm((ny, ch, nz * rows), BF16), vm((2 * ny, ch, nz * rows), BF16),
        vm((nz, rows * 3 // 2, 2 * HEAD), F32),
        vm((2 * nz, rows * 3 // 2, 2 * HEAD), BF16), vm((nz, rows * 3 // 2, 2 * HEAD), BF16),
        dma((6,)),
        *(dma for _ in range(6)), dma((2,)), dma,
        *(dma for _ in range(4 + 2 + 2 + 8)),
        dma, dma((2,)), dma, dma((2,)), dma, dma, dma, dma,
    ]
    hbm, near = pl.BlockSpec(memory_space=pl.ANY), pl.BlockSpec(memory_space=pltpu.VMEM)
    results = pl.pallas_call(
        functools.partial(kernel, nz, ny, nx),
        out_shape=(
            vm((ch, tok), BF16),
            vm((ch, tok), BF16),
            vm((tok // 2, d_model), BF16),
            vm((rows, ch), F32),
        ),
        in_specs=[hbm] * 6,
        out_specs=(near,) * 4,
        scratch_shapes=scratch,
        compiler_params=pltpu.CompilerParams(collective_id=0, has_side_effects=True),
    )(block_input, value_weight.T, query_pre.T, forget_pre.T, out_grad.T, lower_bound.reshape(1, ch))
    g_query, g_forget, g_input, g_weight = pl.pallas_call(
        write_out,
        out_shape=tuple(jax.ShapeDtypeStruct(a.shape, a.dtype) for a in results),
        in_specs=[near] * 4,
        out_specs=(hbm,) * 4,
        scratch_shapes=[dma((4,))],
    )(*(pltpu.with_memory_space_constraint(a, pltpu.VMEM) for a in results))
    return g_query.T, g_forget.T, g_input, g_weight


def on_mesh(devices):
    nz, ny, nx = devices.shape[:3]
    split = Mesh(devices, SP_TP)
    in_specs = (P(SP, None), P(None, "tp"), P(SP, "tp"), P(SP, "tp"), P("tp"), P(SP, "tp"))
    out_specs = (P(SP, "tp"), P(SP, "tp"), P(SP_TP, None), P(SP, "tp"))
    return jax.shard_map(
        functools.partial(on_device, nz, ny, nx), mesh=split, in_specs=in_specs, out_specs=out_specs, check_vma=False
    )


def solution(mesh):
    return on_mesh(mesh.devices.reshape(8, 4, 4, mesh.shape["tp"]))
```

```python
import functools

import jax
import jax.numpy as jnp
from jax import lax
from jax.experimental import pallas as pl
from jax.experimental.pallas import tpu as pltpu
from jax.sharding import Mesh
from jax.sharding import PartitionSpec as P

HEAD = 64
SP = ("sp_0", "sp_1", "sp_2")
SP_TP = ("sp_0", "sp_1", "sp_2", "tp")
F32, BF16 = jnp.float32, jnp.bfloat16
LOGICAL = pl.DeviceIdType.MESH


def nn(a, b):
    return lax.dot_general(a, b, (((1,), (0,)), ((), ())), preferred_element_type=F32)


def nt(a, b):
    return lax.dot_general(a, b, (((1,), (1,)), ((), ())), preferred_element_type=F32)


def tn(a, b):
    return lax.dot_general(a, b, (((0,), (0,)), ((), ())), preferred_element_type=F32)


def rcopy(src, dst, send, recv, device):
    return pltpu.make_async_remote_copy(
        src_ref=src, dst_ref=dst, send_sem=send, recv_sem=recv, device_id=device, device_id_type=LOGICAL
    )


def kernel(
    nz, ny, nx,
    x_hbm, w_hbm, q_hbm, f_hbm, go_hbm, lb_hbm,
    gq_out, gf_out, gx_out, gw_out,
    x_v, w_v, q_v, f_v, go_v, lb_v, wide, thin, broad,
    s_send, e_send, s_buf, e_buf, l_send, lg_send, q_grad, q_line, t_send, ft_send, t_buf, ft_buf, held_out, o_send, p_buf, p_both, outer, st_send, st_buf,
    xt, xtl, r_send, rl, k_send, kl, own_send, ownl, g_all, ig, ig_recv,
    m_send, m_recv, aacc, a_send, a_recv, w2, z_send, z_recv,
    lsem, s_ss, s_rs, e_ss, e_rs, ea_ss, ea_rs, q_ss, q_rs, t_ss, t_rs, ft_ss, ft_rs, p_ss, p_rs, st_ss, st_rs,
    xt_ss, xt_rs, r_ss, r_rs, k_ss, k_rs, own_ss, own_rs,
    m_ss, m_rs, a_ss, a_rs, z_ss, z_rs, ig_ss, ig_rs,
):
    pln = ny * nx
    tok, d_model = x_v.shape
    ch = w_v.shape[0]
    heads = ch // HEAD
    z, y, x, c = (lax.axis_index(a) for a in SP_TP)
    me = y * nx + x
    back = lax.rem(x + y, 2)
    zs, ys, xs = ([lax.rem(at + d, n) for d in range(n)] for at, n in ((z, nz), (y, ny), (x, nx)))
    across = lambda d, n: min(d, n - d)
    steps = [(dy, dx) for dy in range(ny) for dx in range(nx) if dy or dx]
    steps.sort(key=lambda t: -across(t[0], ny) - across(t[1], nx))
    others = [(ys[dy], xs[dx]) for dy, dx in steps]
    everyone = others + [(y, x)]
    z_steps = sorted(range(1, nz), key=lambda d: -across(d, nz))
    far_first = sorted(range(1, nx), key=lambda d: -across(d, nx))

    at_line, at_col = x * (1 - c) + y * c, y * (1 - c) + x * c
    lines = [xs[d] * (1 - c) + ys[d] * c for d in range(nx)]
    columns = [ys[d] * (1 - c) + xs[d] * c for d in range(ny)]

    def line(i):
        return (z, y * (1 - c) + i * c, i * (1 - c) + x * c, c)

    def column(i):
        return (z, i * (1 - c) + y * c, x * (1 - c) + i * c, c)

    def piece_of(ty, tx):
        return ty * (nx // 2) + lax.div(tx, 2) + lax.rem(tx + ty, 2) * (pln // 2)

    def head_of(a, h):
        return a[HEAD * h : HEAD * (h + 1)]

    def by_head(parts):
        return jnp.concatenate(list(parts), axis=0)

    def arrived(ref, n, sem):
        part = ref.at[pl.ds(0, n)]
        rcopy(part, part, sem, sem, (z, y, x, 1 - c)).wait_recv()

    def left(ref, n, sem):
        part = ref.at[pl.ds(0, n)]
        rcopy(part, part, sem, sem, (z, y, x, 1 - c)).wait_send()

    scope = jax.named_scope
    with scope("loads_barrier"):
        loads = [
            pltpu.make_async_copy(src, dst, lsem.at[k])
            for k, (src, dst) in enumerate(
                ((f_hbm, f_v), (q_hbm, q_v), (go_hbm, go_v), (x_hbm, x_v), (w_hbm, w_v), (lb_hbm, lb_v))
            )
        ]
        for k in (0, 5, 1, 2, 3, 4):
            loads[k].start()
        barrier = pltpu.get_barrier_semaphore()

        def greet(device):
            pl.semaphore_signal(barrier, inc=1, device_id=device, device_id_type=LOGICAL)

        @pl.when(c == 1)
        def _():
            for ty, tx in others:
                greet((z, ty, tx, 1))
            for ty, tx in everyone:
                greet((z, ty, tx, 0))

        @pl.when(c == 0)
        def _():
            for tx in xs[1:]:
                greet((z, y, tx, 0))

        for d in z_steps:
            greet((zs[d], y, x, 1))

    lane = lax.broadcasted_iota(jnp.int32, (1, ch), 1)
    mf = [jnp.where((lane >= HEAD * h) & (lane < HEAD * (h + 1)), 1.0, 0.0).astype(F32) for h in range(heads)]
    row = lax.broadcasted_iota(jnp.int32, (tok, tok), 0)
    col = lax.broadcasted_iota(jnp.int32, (tok, tok), 1)
    lower, upper = row >= col, col >= row
    lower_ones = jnp.where(lower, 1.0, 0.0).astype(BF16)
    upper_ones = jnp.where(upper, 1.0, 0.0).astype(BF16)

    mb = [m.astype(BF16) for m in mf]

    def block_diagonal(a):
        a = a.astype(BF16)
        return by_head(a * m for m in mb)

    def folded(full):
        out = full[:HEAD] * mf[0]
        for h in range(1, heads):
            out = out + head_of(full, h) * mf[h]
        return out

    with scope("gates"):
        loads[5].wait()
        gap = jnp.broadcast_to(1.0 - lb_v[...], (tok, ch)).T
        loads[0].wait()
        f = f_v[...].astype(F32)
        f_neg = 1.0 / (1.0 + jnp.exp(f))
        k_rate = gap * f_neg
        logs = jnp.log1p(-k_rate)
        high = logs.astype(BF16)
        low = (logs - high.astype(F32)).astype(BF16)
        cum = nn(high, upper_ones) + nn(low, upper_ones)
        row_ones = jnp.ones((8, tok), BF16)
        total = jnp.exp((nt(row_ones, high) + nt(row_ones, low))[:1])
        closing = cum[:, tok - 1 : tok]
        growth = jnp.exp(cum)
        remain = jnp.exp(closing - cum)
        e_send[...] = total
        k_end = (k_rate * remain).astype(BF16)
        loads[1].wait()
        q = q_v[...].astype(F32)
        q_sig = 1.0 / (1.0 + jnp.exp(-q))
        query = q * q_sig
        q_dec = (query * growth).astype(BF16)
        loads[2].wait()
        go = go_v[...]
        reach = folded(nt(go, q_dec))
    with scope("values"):
        loads[3].wait()
        loads[4].wait()
        v = nt(w_v[...], x_v[...]).astype(BF16)
        update = folded(nt(v, k_end))
        s_send[...] = jnp.concatenate([update, reach], axis=0).reshape(s_send.shape).astype(BF16)
        narrow, low_half = 2 * HEAD, HEAD // 2
        rest = jnp.concatenate([reach[:low_half, narrow:], reach[low_half:, narrow:]], axis=1)
        r_send[...] = jnp.concatenate([reach[:, :narrow], rest], axis=0).astype(BF16)
        k_send[...] = k_end

    with scope("barrier_wait"):
        pl.semaphore_wait(barrier, c * (pln - 1 + 2 * (nz - 1)) + (1 - c) * (pln + nx - 1))

    def to_line(source, target, send_sem, recv_sem):
        for k in far_first:
            rcopy(source, target.at[at_line], send_sem, recv_sem, line(lines[k])).start()

    def column_send(source, target, send_sem, recv_sem, to):
        device = (z, to * (1 - c) + y * c, x * (1 - c) + to * c, 1)
        return rcopy(source.at[to], target.at[c * ny + at_col], send_sem, recv_sem.at[c], device)

    def to_column(source, target, send_sem, recv_sem):
        for k in far_first:
            column_send(source, target, send_sem, recv_sem, columns[k]).start()

        @pl.when(c == 0)
        def _():
            rcopy(source.at[y], target.at[y], send_sem, recv_sem.at[0], (z, y, x, 1)).start()

    def from_column(g, own, target, recv_sem):
        arrived(target, ny - g, recv_sem.at[g])
        if g == 0:
            out = target[0].astype(F32)
            for k in range(1, ny):
                out = out + target[k].astype(F32)
            return out.T
        out = own[...].astype(F32)
        for k in range(1, ny):
            out = out + target[ny + xs[k]].astype(F32)
        return out.T

    def piece_sends(ty, tx):
        to = (z, ty, tx, 1)
        return (
            rcopy(e_send, e_buf.at[c * pln + me], e_ss, e_rs, to),
            rcopy(s_send.at[piece_of(ty, tx)], s_buf.at[c * pln + me], s_ss, s_rs, to),
        )

    mine = piece_of(y, x)
    with scope("send1"):
        for parity in (0, 1):

            @pl.when(back == parity)
            def _():
                for want in (1 - parity, parity):
                    for (dy, dx), target in zip(steps, others):
                        if (dy + dx) % 2 == want:
                            for copy in piece_sends(*target):
                                copy.start()

        @pl.when(c == 0)
        def _():
            for copy in piece_sends(y, x):
                copy.start()

        @pl.when(c == 1)
        def _():
            s_buf[pln + me] = s_send[mine]
            e_buf[pln + me] = e_send[...]

        to_line(k_send, kl, k_ss, k_rs)
        kl[at_line] = k_end
        rl[at_line] = r_send[...]

    rows = d_model // (nz * ny * nx)
    with scope("turn"):
        per = tok // rows
        for b in range(d_model // tok):
            turned = x_v[:, tok * b : tok * (b + 1)].T
            for g in range(per):
                at = b * per + g
                zz, yy, xx = at // pln, (at // nx) % ny, at % nx
                group, into = xx * (1 - c) + yy * c, yy * (1 - c) + xx * c
                xt[group, into, zz] = turned[rows * g : rows * (g + 1)]

        for k in far_first:
            to = lines[k]
            rcopy(xt.at[to], xtl.at[at_line], xt_ss, xt_rs, line(to)).start()

        @pl.when(c == 0)
        def _():
            to_line(r_send, rl, r_ss, r_rs)

        xtl[at_line] = xt[at_line]

    with scope("pairs_value"):
        shrink = jnp.exp(-cum)
        k_dec = (k_rate * shrink).astype(BF16)
        mixing = [jnp.where(lower, tn(head_of(q_dec, h), head_of(k_dec, h)), 0.0).astype(BF16) for h in range(heads)]
        gv_own = by_head(nn(head_of(go, h), mixing[h]) for h in range(heads))
        own_send[...] = gv_own.astype(BF16)
        ownl[at_line] = own_send[...]

        @pl.when(c == 0)
        def _():
            to_line(own_send, ownl, own_ss, own_rs)


    z_order = z + back * (nz - 1 - 2 * z)

    def z_sends(k):
        at = z_order + k
        to = at + back * (nz - 1 - 2 * at)
        return (
            rcopy(ft_send, ft_buf.at[z], ft_ss, ft_rs, (to, y, x, 1)),
            rcopy(t_send, t_buf.at[z], t_ss, t_rs, (to, y, x, 1)),
        )

    def carry_send(g, ty, tx):
        device = (z, ty, tx, g)
        if g == 0:
            return rcopy(l_send.at[ty * nx + nx - 1], q_line.at[me // 2], q_ss.at[0], q_rs, device)
        return rcopy(lg_send.at[tx], q_grad.at[me // 2], q_ss.at[1], q_rs, device)

    targets = [(0, *t) for t in everyone] + [(1, *t) for t in others]
    plane_decays = e_buf.at[pl.ds(0, pln)]
    e_all = rcopy(plane_decays, plane_decays, ea_ss, ea_rs, (z, y, x, 1 - c))

    @pl.when(c == 1)
    def _():
        with scope("wait1"):
            arrived(e_buf, 2 * pln - 1, e_rs)
            arrived(s_buf, 2 * pln - 1, s_rs)
        with scope("scan1"):
            for parity in (0, 1):

                @pl.when(back == parity)
                def _():
                    for g in (0, 1):
                        held = jnp.zeros(t_send.shape[1:], F32)
                        factor = jnp.ones((1, ch), F32)
                        for it in range(pln - 1, -1, -1) if parity else range(pln):
                            if g and parity:
                                lg_send[it % nx, :, ch * (it // nx) : ch * (it // nx + 1)] = held.astype(BF16)
                            else:
                                l_send[g * pln + it] = held.astype(BF16)
                            decay = e_buf[g * pln + it]
                            held = decay * held + s_buf[g * pln + it].astype(F32)
                            factor = decay * factor
                        t_send[g] = held.astype(BF16)
                        ft_send[g] = factor

        with scope("send2"):
            for k in range(1, nz):

                @pl.when(z_order + k < nz)
                def _():
                    for copy in z_sends(k):
                        copy.start()

            @pl.when(back == 1)
            def _():
                for target in targets:
                    carry_send(*target).start()
                q_grad[me // 2] = lg_send[x]

            to_line(own_send, ownl, own_ss, own_rs)
            e_all.start()

    with scope("pairs_query"):
        pairing = [jnp.where(upper, tn(head_of(v, h), head_of(go, h)), 0.0).astype(BF16) for h in range(heads)]
        gq_own = by_head(nn(head_of(k_dec, h), pairing[h]) for h in range(heads))
        gk_own = by_head(nt(head_of(q_dec, h), pairing[h]) for h in range(heads))

    with scope("decays"):
        @pl.when(c == 0)
        def _():
            e_all.wait_recv()

        decays = e_buf[pl.ds(c * pln, pln)]
        after = [jnp.ones((1, ch), F32)] * nx
        ids = [line(i)[1] * nx + line(i)[2] for i in range(nx)]
        for i in range(pln):
            after = [a * jnp.where(i > n, decays[i], 1.0) for a, n in zip(after, ids)]

    with scope("wait_line"):
        arrived(xtl, nx - 1, xt_rs)
        arrived(kl, nx - 1, k_rs)

    def pairs(parts):
        return [jnp.concatenate(parts[i : i + 2], axis=1) for i in range(0, nx, 2)]

    def to_chunks(ref, total):
        for i in range(ny):
            ref[i] = total[:, i * nz * rows : (i + 1) * nz * rows].astype(ref.dtype)

    with scope("line_m"):
        turned_of = pairs([xtl[i].reshape(d_model // nx, tok) for i in range(nx)])
        tall_after = jnp.concatenate(after + [jnp.ones((8 - nx, ch), F32)], axis=0).T
        scaled = pairs([(kl[i].astype(F32) * tall_after[:, i : i + 1]).astype(BF16) for i in range(nx)])
        m_sum = nt(scaled[0], turned_of[0])
        for a, b in zip(scaled[1:], turned_of[1:]):
            m_sum = m_sum + nt(a, b)
        to_chunks(m_send, m_sum)
        to_column(m_send, m_recv, m_ss, m_rs)

    def arriving(o, carried):
        frm = o + back * (nz - 1 - 2 * o)
        return ft_buf[frm] * carried + t_buf[frm].astype(F32)

    def plane_send(g, ty, tx):
        if g:
            return rcopy(o_send, p_both.at[me // 2], p_ss, p_rs, (z, ty, tx, 1))
        return rcopy(o_send.at[0], p_buf.at[me // 2], p_ss, p_rs, (z, ty, tx, 0))

    def state_send(g, ty, tx):
        return rcopy(st_send.at[g * pln + ty * nx + tx], st_buf.at[me // 2], st_ss, st_rs, (z, ty, tx, g))

    @pl.when(c == 1)
    def _():
        with scope("wait2"):
            for n in range(1, nz):

                @pl.when(z_order == n)
                def _():
                    arrived(ft_buf, n, ft_rs)
                    arrived(t_buf, n, t_rs)

            carried = lax.fori_loop(0, z_order, arriving, jnp.zeros(t_send.shape, F32))
        with scope("send3"):
            held_out[...] = carried
            o_send[...] = carried.astype(BF16)

            @pl.when(back == 1)
            def _():
                for target in targets[pln:] + targets[:pln]:
                    plane_send(*target).start()
                p_both[me // 2] = o_send[...]

    some = pln // 2
    with scope("wait_1b"):

        @pl.when(c == 0)
        def _():
            arrived(q_line, some, q_rs)
            arrived(rl, nx - 1, r_rs)

        for odd in (0, 1):

            @pl.when((c == 1) & (back == odd))
            def _():
                arrived(q_grad, some - odd, q_rs)

    with scope("line_a"):

        @pl.when(c == 0)
        def _():
            grad_at = q_line[...].astype(F32).reshape(HEAD, ch)
            g_all[nx - 1] = grad_at
            for i in range(nx - 2, -1, -1):
                near_reach = rl[i + 1].astype(F32)
                rest = near_reach[HEAD:]
                rest = jnp.concatenate([rest[:, :HEAD], rest[:, HEAD:]], axis=0)
                near_reach = jnp.concatenate([near_reach[:HEAD], rest], axis=1)
                grad_at = e_buf[y * nx + i + 1] * grad_at + near_reach
                g_all[i] = grad_at

        @pl.when(c == 1)
        def _():
            for i in range(nx):
                g_all[i] = q_grad[:, :, ch * i : ch * (i + 1)].astype(F32).reshape(HEAD, ch)

        parts = []
        for i in range(nx):
            grad_at = g_all[i]
            bd_in = block_diagonal(grad_at)
            parts.append(nn(bd_in, kl[i]))
    with scope("wait_own"):
        arrived(ownl, nx - 1, own_rs)
    with scope("line_a2"):
        parts = pairs([(ownl[i].astype(F32) + part).astype(BF16) for i, part in enumerate(parts)])
        def chunk_of(to):
            pieces = pairs([xtl[i, to].reshape(nz * rows, tok) for i in range(nx)])
            chunk = nt(parts[0], pieces[0])
            for a, b in zip(parts[1:], pieces[1:]):
                chunk = chunk + nt(a, b)
            return chunk

        for ks in (far_first[:1], far_first[1:], [0]):
            chunks = [chunk_of(columns[k]) for k in ks]
            for k, chunk in zip(ks, chunks):
                a_send[columns[k]] = chunk.astype(BF16)
                if not k:
                    aacc[...] = chunk
            for k in ks:
                if k:
                    column_send(a_send, a_recv, a_ss, a_rs, columns[k]).start()

        @pl.when(c == 0)
        def _():
            rcopy(a_send.at[y], a_recv.at[y], a_ss, a_rs.at[0], (z, y, x, 1)).start()

    @pl.when((c == 1) & (back == 0))
    def _():
        with scope("states"):
            for g in (0, 1):
                start = held_out[g]
                for i in range(pln):
                    st_send[g * pln + i] = (l_send[g * pln + i].astype(F32) + start).astype(BF16)
                    start = e_buf[g * pln + i] * start
            for target in targets:
                state_send(*target).start()
            st_buf[me // 2] = st_send[pln + me]

    @pl.when(c == 1)
    def _():
        with scope("wait_m1"):
            m_plane = [from_column(g, m_send.at[x], m_recv, m_rs).astype(BF16) for g in (0, 1)]
        with scope("wait3"):
            for odd in (0, 1):

                @pl.when(back == odd)
                def _():
                    arrived(p_both, some - odd, p_rs)

            from_plane = []
            for g in (0, 1):
                outer[g] = p_both[:, g].astype(F32).reshape(HEAD, ch)
                bd_out = block_diagonal(outer[g])
                from_plane.append(nt(m_plane[g], bd_out))
        for g in (1, 0):
            with scope(f"wait_a{g}"):
                w_sum = from_plane[g] + from_column(g, aacc, a_recv, a_rs)
            with scope(f"send_z{g}"):
                wide_part = w_sum[:, : 2 * HEAD].reshape(nz, rows, 2 * HEAD)
                rest = w_sum[:, 2 * HEAD :].reshape(nz, 2, rows // 2, HEAD)
                rest = jnp.concatenate([rest[:, 0], rest[:, 1]], axis=2)
                packed = jnp.concatenate([wide_part, rest], axis=1)
                if g:
                    w2[...] = packed
                z_send[pl.ds(g * nz, nz)] = packed.astype(BF16)
                for d in z_steps if g else z_steps + [0]:
                    rcopy(z_send.at[g * nz + zs[d]], z_recv.at[z], z_ss, z_rs, (zs[d], y, x, g)).start()

    @pl.when(c == 0)
    def _():
        with scope("wait3"):
            arrived(p_buf, some, p_rs)
        outer[0] = p_buf[...].astype(F32).reshape(HEAD, ch)

    with scope("value_grad"):
        own_after = after[nx - 1]
        for i in range(nx - 1):
            own_after = jnp.where(at_line == i, after[i], own_after)
        grad = g_all[at_line] + own_after * outer[c]
        bd_grad = block_diagonal(grad)
        value_grad = (gv_own + nn(bd_grad, k_end)).astype(BF16)

    with scope("input_grad"):
        width = 512 if d_model % 512 == 0 else d_model
        turned = value_grad.T
        for j in range(d_model // width):
            cols = pl.ds(j * width, width)
            ig[:, :, cols] = nn(turned, w_v[:, cols]).astype(BF16).reshape(2, tok // 2, width)
        ig_copy = rcopy(ig.at[1 - c], ig_recv, ig_ss, ig_rs, (z, y, x, 1 - c))
        ig_copy.start()

    with scope("query_forget"):
        for even in (0, 1):

            @pl.when((1 - back) * c == even)
            def _():
                arrived(st_buf, some - even, st_rs)

        state = st_buf[...].astype(F32).reshape(HEAD, ch)
        bd_state = block_diagonal(state)
        g_query = growth * (gq_own + tn(bd_state, go))
        g_key = shrink * gk_own + remain * tn(bd_grad, v)
        gq_out[...] = (g_query * (q_sig * (1.0 + q * (1.0 - q_sig)))).astype(BF16)
        ends = grad * (total * state + update)
        ends_high = ends.astype(BF16)
        ends_low = (ends - ends_high.astype(F32)).astype(BF16)
        tall_ones = jnp.ones((HEAD, tok), BF16)
        boundary = tn(ends_high, tall_ones) + tn(ends_low, tall_ones)
        flow = query * g_query - k_rate * g_key
        flow_high = flow.astype(BF16)
        flow_low = (flow - flow_high.astype(F32)).astype(BF16)
        g_decay = nn(flow_high, lower_ones) + nn(flow_low, lower_ones) + boundary
        gf_out[...] = ((g_decay / (1.0 - k_rate) - g_key) * k_rate * (1.0 / (1.0 + jnp.exp(-f)))).astype(BF16)

    with scope("input_sum"):
        ig_copy.wait_recv()
        gx_out[...] = (ig[c].astype(F32) + ig_recv[...].astype(F32)).astype(BF16)

    with scope("drain"):
        left(xt, nx - 1, xt_ss)
        left(kl, nx - 1, k_ss)
        left(ownl, nx - 1, own_ss)
        ig_copy.wait_send()

        @pl.when(c == 0)
        def _():
            left(thin, pln, e_ss)
            left(s_send, pln, s_ss)
            left(rl, nx - 1, r_ss)
            left(m_send, ny, m_ss)
            left(a_send, ny, a_ss)

        @pl.when(c == 1)
        def _():
            left(m_send, ny - 1, m_ss)
            left(a_send, ny - 1, a_ss)
            left(thin, pln - 1, e_ss)
            left(s_send, pln - 1, s_ss)
            for n in range(1, nz):

                @pl.when(nz - 1 - z_order == n)
                def _():
                    left(ft_buf, n, ft_ss)
                    left(t_buf, n, t_ss)

            e_all.wait_send()

            @pl.when(back == 1)
            def _():
                left(wide, pln, q_ss.at[0])
                left(broad, pln - 1, q_ss.at[1])
                left(wide, 3 * pln - 2, p_ss)

            @pl.when(back == 0)
            def _():
                left(st_send, 2 * pln - 1, st_ss)

    def unpacked(total):
        gw_out[:, : 2 * HEAD] = total[:rows]
        gw_out[: rows // 2, 2 * HEAD :] = total[rows:, :HEAD]
        gw_out[rows // 2 :, 2 * HEAD :] = total[rows:, HEAD:]

    with scope("wait_z"):

        @pl.when(c == 0)
        def _():
            arrived(z_recv, nz, z_rs)
            w_last = z_recv[0].astype(F32)
            for k in range(1, nz):
                w_last = w_last + z_recv[k].astype(F32)
            unpacked(w_last)

        @pl.when(c == 1)
        def _():
            arrived(z_recv, nz - 1, z_rs)
            w_last = w2[z]
            for k in range(1, nz):
                w_last = w_last + z_recv[zs[k]].astype(F32)
            unpacked(w_last)
            left(z_send, 2 * nz - 1, z_ss)


def write_out(*refs):
    copies = [pltpu.make_async_copy(refs[k], refs[4 + k], refs[8].at[k]) for k in range(4)]
    for copy in copies:
        copy.start()
    for copy in copies:
        copy.wait()


def on_device(nz, ny, nx, block_input, value_weight, query_pre, forget_pre, lower_bound, out_grad):
    tok, d_model = block_input.shape
    ch = value_weight.shape[1]
    pln = ny * nx
    piece = 2 * HEAD // pln
    rows = d_model // (nz * pln)
    vm, dma = pltpu.VMEM, pltpu.SemaphoreType.DMA
    scratch = [
        vm((tok, d_model), BF16), vm((ch, d_model), BF16),
        vm((ch, tok), BF16), vm((ch, tok), BF16), vm((ch, tok), BF16), vm((1, ch), F32),
        vm((pln * (ny + 1), piece, ch), BF16), vm((pln, 1, ch), F32),
        vm((pln, piece, ny * ch), BF16),
        vm((pln, piece, ch), BF16), vm((1, ch), F32),
        vm((2 * pln, piece, ch), BF16), vm((2 * pln, 1, ch), F32),
        vm((2 * pln, piece, ch), BF16), vm((nx, piece, ny * ch), BF16),
        vm((pln // 2, piece, ny * ch), BF16), vm((pln // 2, piece, ch), BF16),
        vm((2, piece, ch), BF16), vm((2, 1, ch), F32),
        vm((nz, 2, piece, ch), BF16), vm((nz, 2, 1, ch), F32),
        vm((2, piece, ch), F32), vm((2, piece, ch), BF16),
        vm((pln // 2, piece, ch), BF16), vm((pln // 2, 2, piece, ch), BF16),
        vm((2, HEAD, ch), F32), vm((2 * pln, piece, ch), BF16), vm((pln // 2, piece, ch), BF16),
        vm((nx, ny, nz, rows, tok), BF16), vm((nx, ny, nz, rows, tok), BF16),
        vm((ch // 2, 2 * HEAD), BF16), vm((nx, ch // 2, 2 * HEAD), BF16),
        vm((ch, tok), BF16), vm((nx, ch, tok), BF16),
        vm((ch, tok), BF16), vm((nx, ch, tok), BF16),
        vm((nx, HEAD, ch), F32),
        vm((2, tok // 2, d_model), BF16), vm((tok // 2, d_model), BF16),
        vm((ny, ch, nz * rows), BF16), vm((2 * ny, ch, nz * rows), BF16),
        vm((ch, nz * rows), F32), vm((ny, ch, nz * rows), BF16), vm((2 * ny, ch, nz * rows), BF16),
        vm((nz, rows * 3 // 2, 2 * HEAD), F32),
        vm((2 * nz, rows * 3 // 2, 2 * HEAD), BF16), vm((nz, rows * 3 // 2, 2 * HEAD), BF16),
        dma((6,)),
        *(dma for _ in range(6)), dma((2,)), dma,
        *(dma for _ in range(4 + 2 + 2 + 8)),
        dma, dma((2,)), dma, dma((2,)), dma, dma, dma, dma,
    ]
    hbm, near = pl.BlockSpec(memory_space=pl.ANY), pl.BlockSpec(memory_space=pltpu.VMEM)
    results = pl.pallas_call(
        functools.partial(kernel, nz, ny, nx),
        out_shape=(
            vm((ch, tok), BF16),
            vm((ch, tok), BF16),
            vm((tok // 2, d_model), BF16),
            vm((rows, ch), F32),
        ),
        in_specs=[hbm] * 6,
        out_specs=(near,) * 4,
        scratch_shapes=scratch,
        compiler_params=pltpu.CompilerParams(collective_id=0, has_side_effects=True),
    )(block_input, value_weight.T, query_pre.T, forget_pre.T, out_grad.T, lower_bound.reshape(1, ch))
    g_query, g_forget, g_input, g_weight = pl.pallas_call(
        write_out,
        out_shape=tuple(jax.ShapeDtypeStruct(a.shape, a.dtype) for a in results),
        in_specs=[near] * 4,
        out_specs=(hbm,) * 4,
        scratch_shapes=[dma((4,))],
    )(*(pltpu.with_memory_space_constraint(a, pltpu.VMEM) for a in results))
    return g_query.T, g_forget.T, g_input, g_weight


def on_mesh(devices):
    nz, ny, nx = devices.shape[:3]
    split = Mesh(devices, SP_TP)
    in_specs = (P(SP, None), P(None, "tp"), P(SP, "tp"), P(SP, "tp"), P("tp"), P(SP, "tp"))
    out_specs = (P(SP, "tp"), P(SP, "tp"), P(SP_TP, None), P(SP, "tp"))
    return jax.shard_map(
        functools.partial(on_device, nz, ny, nx), mesh=split, in_specs=in_specs, out_specs=out_specs, check_vma=False
    )


def solution(mesh):
    return on_mesh(mesh.devices.reshape(8, 4, 4, mesh.shape["tp"]))
```

```python
import functools

import jax
import jax.numpy as jnp
from jax import lax
from jax.experimental import pallas as pl
from jax.experimental.pallas import tpu as pltpu
from jax.sharding import Mesh
from jax.sharding import PartitionSpec as P

HEAD = 64
SP = ("sp_0", "sp_1", "sp_2")
SP_TP = ("sp_0", "sp_1", "sp_2", "tp")
F32, BF16 = jnp.float32, jnp.bfloat16
LOGICAL = pl.DeviceIdType.MESH


def nn(a, b):
    return lax.dot_general(a, b, (((1,), (0,)), ((), ())), preferred_element_type=F32)


def nt(a, b):
    return lax.dot_general(a, b, (((1,), (1,)), ((), ())), preferred_element_type=F32)


def tn(a, b):
    return lax.dot_general(a, b, (((0,), (0,)), ((), ())), preferred_element_type=F32)


def rcopy(src, dst, send, recv, device):
    return pltpu.make_async_remote_copy(
        src_ref=src, dst_ref=dst, send_sem=send, recv_sem=recv, device_id=device, device_id_type=LOGICAL
    )


def kernel(
    nz, ny, nx,
    x_hbm, w_hbm, q_hbm, f_hbm, go_hbm, lb_hbm,
    gq_out, gf_out, gx_out, gw_out,
    x_v, w_v, q_v, f_v, go_v, lb_v, wide, thin, broad,
    s_send, e_send, s_buf, e_buf, l_send, lg_send, q_grad, q_line, t_send, ft_send, t_buf, ft_buf, held_out, o_send, p_buf, p_both, outer, st_send, st_buf,
    xt, xtl, r_send, rl, k_send, kl, own_send, ownl, g_all, ig, ig_recv,
    m_send, m_recv, aacc, a_send, a_recv, w2, z_send, z_recv,
    lsem, s_ss, s_rs, e_ss, e_rs, ea_ss, ea_rs, q_ss, q_rs, t_ss, t_rs, ft_ss, ft_rs, p_ss, p_rs, st_ss, st_rs,
    xt_ss, xt_rs, r_ss, r_rs, k_ss, k_rs, own_ss, own_rs,
    m_ss, m_rs, a_ss, a_rs, z_ss, z_rs, ig_ss, ig_rs,
):
    pln = ny * nx
    tok, d_model = x_v.shape
    ch = w_v.shape[0]
    heads = ch // HEAD
    z, y, x, c = (lax.axis_index(a) for a in SP_TP)
    me = y * nx + x
    back = lax.rem(x + y, 2)
    zs, ys, xs = ([lax.rem(at + d, n) for d in range(n)] for at, n in ((z, nz), (y, ny), (x, nx)))
    across = lambda d, n: min(d, n - d)
    steps = [(dy, dx) for dy in range(ny) for dx in range(nx) if dy or dx]
    steps.sort(key=lambda t: -across(t[0], ny) - across(t[1], nx))
    others = [(ys[dy], xs[dx]) for dy, dx in steps]
    everyone = others + [(y, x)]
    z_steps = sorted(range(1, nz), key=lambda d: -across(d, nz))
    far_first = sorted(range(1, nx), key=lambda d: -across(d, nx))

    at_line, at_col = x * (1 - c) + y * c, y * (1 - c) + x * c
    lines = [xs[d] * (1 - c) + ys[d] * c for d in range(nx)]
    columns = [ys[d] * (1 - c) + xs[d] * c for d in range(ny)]

    def line(i):
        return (z, y * (1 - c) + i * c, i * (1 - c) + x * c, c)

    def column(i):
        return (z, i * (1 - c) + y * c, x * (1 - c) + i * c, c)

    def piece_of(ty, tx):
        return ty * (nx // 2) + lax.div(tx, 2) + lax.rem(tx + ty, 2) * (pln // 2)

    def head_of(a, h):
        return a[HEAD * h : HEAD * (h + 1)]

    def by_head(parts):
        return jnp.concatenate(list(parts), axis=0)

    def arrived(ref, n, sem):
        part = ref.at[pl.ds(0, n)]
        rcopy(part, part, sem, sem, (z, y, x, 1 - c)).wait_recv()

    def left(ref, n, sem):
        part = ref.at[pl.ds(0, n)]
        rcopy(part, part, sem, sem, (z, y, x, 1 - c)).wait_send()

    scope = jax.named_scope
    with scope("loads_barrier"):
        loads = [
            pltpu.make_async_copy(src, dst, lsem.at[k])
            for k, (src, dst) in enumerate(
                ((f_hbm, f_v), (q_hbm, q_v), (go_hbm, go_v), (x_hbm, x_v), (w_hbm, w_v), (lb_hbm, lb_v))
            )
        ]
        for k in (0, 5, 1, 2, 3, 4):
            loads[k].start()
        barrier = pltpu.get_barrier_semaphore()

        def greet(device):
            pl.semaphore_signal(barrier, inc=1, device_id=device, device_id_type=LOGICAL)

        @pl.when(c == 1)
        def _():
            for ty, tx in others:
                greet((z, ty, tx, 1))

        for d in z_steps:
            greet((zs[d], y, x, 1))

        @pl.when(c == 1)
        def _():
            for ty, tx in everyone:
                greet((z, ty, tx, 0))

        @pl.when(c == 0)
        def _():
            for tx in xs[1:]:
                greet((z, y, tx, 0))

    lane = lax.broadcasted_iota(jnp.int32, (1, ch), 1)
    mf = [jnp.where((lane >= HEAD * h) & (lane < HEAD * (h + 1)), 1.0, 0.0).astype(F32) for h in range(heads)]
    row = lax.broadcasted_iota(jnp.int32, (tok, tok), 0)
    col = lax.broadcasted_iota(jnp.int32, (tok, tok), 1)
    lower, upper = row >= col, col >= row
    lower_ones = jnp.where(lower, 1.0, 0.0).astype(BF16)
    upper_ones = jnp.where(upper, 1.0, 0.0).astype(BF16)

    mb = [m.astype(BF16) for m in mf]

    def block_diagonal(a):
        a = a.astype(BF16)
        return by_head(a * m for m in mb)

    def folded(full):
        out = full[:HEAD] * mf[0]
        for h in range(1, heads):
            out = out + head_of(full, h) * mf[h]
        return out

    with scope("gates"):
        loads[5].wait()
        gap = jnp.broadcast_to(1.0 - lb_v[...], (tok, ch)).T
        loads[0].wait()
        f = f_v[...].astype(F32)
        f_neg = 1.0 / (1.0 + jnp.exp(f))
        k_rate = gap * f_neg
        logs = jnp.log1p(-k_rate)
        high = logs.astype(BF16)
        low = (logs - high.astype(F32)).astype(BF16)
        cum = nn(high, upper_ones) + nn(low, upper_ones)
        row_ones = jnp.ones((8, tok), BF16)
        total = jnp.exp((nt(row_ones, high) + nt(row_ones, low))[:1])
        closing = cum[:, tok - 1 : tok]
        growth = jnp.exp(cum)
        remain = jnp.exp(closing - cum)
        e_send[...] = total
        k_end = (k_rate * remain).astype(BF16)
        loads[1].wait()
        q = q_v[...].astype(F32)
        q_sig = 1.0 / (1.0 + jnp.exp(-q))
        query = q * q_sig
        q_dec = (query * growth).astype(BF16)
        loads[2].wait()
        go = go_v[...]
        reach = folded(nt(go, q_dec))
    with scope("values"):
        loads[3].wait()
        loads[4].wait()
        v = nt(w_v[...], x_v[...]).astype(BF16)
        update = folded(nt(v, k_end))
        s_send[...] = jnp.concatenate([update, reach], axis=0).reshape(s_send.shape).astype(BF16)
        narrow, low_half = 2 * HEAD, HEAD // 2
        rest = jnp.concatenate([reach[:low_half, narrow:], reach[low_half:, narrow:]], axis=1)
        r_send[...] = jnp.concatenate([reach[:, :narrow], rest], axis=0).astype(BF16)
        k_send[...] = k_end

    with scope("barrier_wait"):
        pl.semaphore_wait(barrier, c * (pln - 1 + 2 * (nz - 1)) + (1 - c) * (pln + nx - 1))

    def to_line(source, target, send_sem, recv_sem):
        for k in far_first:
            rcopy(source, target.at[at_line], send_sem, recv_sem, line(lines[k])).start()

    def column_send(source, target, send_sem, recv_sem, to):
        device = (z, to * (1 - c) + y * c, x * (1 - c) + to * c, 1)
        return rcopy(source.at[to], target.at[c * ny + at_col], send_sem, recv_sem.at[c], device)

    def to_column(source, target, send_sem, recv_sem):
        for k in far_first:
            column_send(source, target, send_sem, recv_sem, columns[k]).start()

        @pl.when(c == 0)
        def _():
            rcopy(source.at[y], target.at[y], send_sem, recv_sem.at[0], (z, y, x, 1)).start()

    def from_column(g, own, target, recv_sem):
        arrived(target, ny - g, recv_sem.at[g])
        if g == 0:
            out = target[0].astype(F32)
            for k in range(1, ny):
                out = out + target[k].astype(F32)
            return out.T
        out = own[...].astype(F32)
        for k in range(1, ny):
            out = out + target[ny + xs[k]].astype(F32)
        return out.T

    def piece_sends(ty, tx):
        to = (z, ty, tx, 1)
        return (
            rcopy(e_send, e_buf.at[c * pln + me], e_ss, e_rs, to),
            rcopy(s_send.at[piece_of(ty, tx)], s_buf.at[c * pln + me], s_ss, s_rs, to),
        )

    mine = piece_of(y, x)
    with scope("send1"):
        for parity in (0, 1):

            @pl.when(back == parity)
            def _():
                for want in (1 - parity, parity):
                    for (dy, dx), target in zip(steps, others):
                        if (dy + dx) % 2 == want:
                            for copy in piece_sends(*target):
                                copy.start()

        @pl.when(c == 0)
        def _():
            for copy in piece_sends(y, x):
                copy.start()

        @pl.when(c == 1)
        def _():
            s_buf[pln + me] = s_send[mine]
            e_buf[pln + me] = e_send[...]

        to_line(k_send, kl, k_ss, k_rs)
        kl[at_line] = k_end
        rl[at_line] = r_send[...]

    rows = d_model // (nz * ny * nx)
    with scope("turn"):
        per = tok // rows
        for b in range(d_model // tok):
            turned = x_v[:, tok * b : tok * (b + 1)].T
            for g in range(per):
                at = b * per + g
                zz, yy, xx = at // pln, (at // nx) % ny, at % nx
                group, into = xx * (1 - c) + yy * c, yy * (1 - c) + xx * c
                xt[group, into, zz] = turned[rows * g : rows * (g + 1)]

        for k in far_first:
            to = lines[k]
            rcopy(xt.at[to], xtl.at[at_line], xt_ss, xt_rs, line(to)).start()

        @pl.when(c == 0)
        def _():
            to_line(r_send, rl, r_ss, r_rs)

        xtl[at_line] = xt[at_line]

    with scope("pairs_value"):
        shrink = jnp.exp(-cum)
        k_dec = (k_rate * shrink).astype(BF16)
        mixing = [jnp.where(lower, tn(head_of(q_dec, h), head_of(k_dec, h)), 0.0).astype(BF16) for h in range(heads)]
        gv_own = by_head(nn(head_of(go, h), mixing[h]) for h in range(heads))
        own_send[...] = gv_own.astype(BF16)
        ownl[at_line] = own_send[...]

        @pl.when(c == 0)
        def _():
            to_line(own_send, ownl, own_ss, own_rs)


    z_order = z + back * (nz - 1 - 2 * z)

    def z_sends(k):
        at = z_order + k
        to = at + back * (nz - 1 - 2 * at)
        return (
            rcopy(ft_send, ft_buf.at[z], ft_ss, ft_rs, (to, y, x, 1)),
            rcopy(t_send, t_buf.at[z], t_ss, t_rs, (to, y, x, 1)),
        )

    def carry_send(g, ty, tx):
        device = (z, ty, tx, g)
        if g == 0:
            return rcopy(l_send.at[ty * nx + nx - 1], q_line.at[me // 2], q_ss.at[0], q_rs, device)
        return rcopy(lg_send.at[tx], q_grad.at[me // 2], q_ss.at[1], q_rs, device)

    targets = [(0, *t) for t in everyone] + [(1, *t) for t in others]
    plane_decays = e_buf.at[pl.ds(0, pln)]
    e_all = rcopy(plane_decays, plane_decays, ea_ss, ea_rs, (z, y, x, 1 - c))

    @pl.when(c == 1)
    def _():
        with scope("wait1"):
            arrived(e_buf, 2 * pln - 1, e_rs)
            arrived(s_buf, 2 * pln - 1, s_rs)
        with scope("scan1"):
            for parity in (0, 1):

                @pl.when(back == parity)
                def _():
                    for g in (0, 1):
                        held = jnp.zeros(t_send.shape[1:], F32)
                        factor = jnp.ones((1, ch), F32)
                        for it in range(pln - 1, -1, -1) if parity else range(pln):
                            if g and parity:
                                lg_send[it % nx, :, ch * (it // nx) : ch * (it // nx + 1)] = held.astype(BF16)
                            else:
                                l_send[g * pln + it] = held.astype(BF16)
                            decay = e_buf[g * pln + it]
                            held = decay * held + s_buf[g * pln + it].astype(F32)
                            factor = decay * factor
                        t_send[g] = held.astype(BF16)
                        ft_send[g] = factor

        with scope("send2"):
            for k in range(1, nz):

                @pl.when(z_order + k < nz)
                def _():
                    for copy in z_sends(k):
                        copy.start()

            @pl.when(back == 1)
            def _():
                for target in targets:
                    carry_send(*target).start()
                q_grad[me // 2] = lg_send[x]

            to_line(own_send, ownl, own_ss, own_rs)
            e_all.start()

    with scope("pairs_query"):
        pairing = [jnp.where(upper, tn(head_of(v, h), head_of(go, h)), 0.0).astype(BF16) for h in range(heads)]
        gq_own = by_head(nn(head_of(k_dec, h), pairing[h]) for h in range(heads))
        gk_own = by_head(nt(head_of(q_dec, h), pairing[h]) for h in range(heads))

    with scope("decays"):
        @pl.when(c == 0)
        def _():
            e_all.wait_recv()

        decays = e_buf[pl.ds(c * pln, pln)]
        after = [jnp.ones((1, ch), F32)] * nx
        ids = [line(i)[1] * nx + line(i)[2] for i in range(nx)]
        for i in range(pln):
            after = [a * jnp.where(i > n, decays[i], 1.0) for a, n in zip(after, ids)]

    with scope("wait_line"):
        arrived(xtl, nx - 1, xt_rs)
        arrived(kl, nx - 1, k_rs)

    def pairs(parts):
        return [jnp.concatenate(parts[i : i + 2], axis=1) for i in range(0, nx, 2)]

    def to_chunks(ref, total):
        for i in range(ny):
            ref[i] = total[:, i * nz * rows : (i + 1) * nz * rows].astype(ref.dtype)

    with scope("line_m"):
        turned_of = pairs([xtl[i].reshape(d_model // nx, tok) for i in range(nx)])
        tall_after = jnp.concatenate(after + [jnp.ones((8 - nx, ch), F32)], axis=0).T
        scaled = pairs([(kl[i].astype(F32) * tall_after[:, i : i + 1]).astype(BF16) for i in range(nx)])
        m_sum = nt(scaled[0], turned_of[0])
        for a, b in zip(scaled[1:], turned_of[1:]):
            m_sum = m_sum + nt(a, b)
        to_chunks(m_send, m_sum)
        to_column(m_send, m_recv, m_ss, m_rs)

    def arriving(o, carried):
        frm = o + back * (nz - 1 - 2 * o)
        return ft_buf[frm] * carried + t_buf[frm].astype(F32)

    def plane_send(g, ty, tx):
        if g:
            return rcopy(o_send, p_both.at[me // 2], p_ss, p_rs, (z, ty, tx, 1))
        return rcopy(o_send.at[0], p_buf.at[me // 2], p_ss, p_rs, (z, ty, tx, 0))

    def state_send(g, ty, tx):
        return rcopy(st_send.at[g * pln + ty * nx + tx], st_buf.at[me // 2], st_ss, st_rs, (z, ty, tx, g))

    @pl.when(c == 1)
    def _():
        with scope("wait2"):
            for n in range(1, nz):

                @pl.when(z_order == n)
                def _():
                    arrived(ft_buf, n, ft_rs)
                    arrived(t_buf, n, t_rs)

            carried = lax.fori_loop(0, z_order, arriving, jnp.zeros(t_send.shape, F32))
        with scope("send3"):
            held_out[...] = carried
            o_send[...] = carried.astype(BF16)

            @pl.when(back == 1)
            def _():
                for target in targets[pln:] + targets[:pln]:
                    plane_send(*target).start()
                p_both[me // 2] = o_send[...]

    some = pln // 2
    with scope("wait_1b"):

        @pl.when(c == 0)
        def _():
            arrived(q_line, some, q_rs)
            arrived(rl, nx - 1, r_rs)

        for odd in (0, 1):

            @pl.when((c == 1) & (back == odd))
            def _():
                arrived(q_grad, some - odd, q_rs)

    with scope("line_a"):

        @pl.when(c == 0)
        def _():
            grad_at = q_line[...].astype(F32).reshape(HEAD, ch)
            g_all[nx - 1] = grad_at
            for i in range(nx - 2, -1, -1):
                near_reach = rl[i + 1].astype(F32)
                rest = near_reach[HEAD:]
                rest = jnp.concatenate([rest[:, :HEAD], rest[:, HEAD:]], axis=0)
                near_reach = jnp.concatenate([near_reach[:HEAD], rest], axis=1)
                grad_at = e_buf[y * nx + i + 1] * grad_at + near_reach
                g_all[i] = grad_at

        @pl.when(c == 1)
        def _():
            for i in range(nx):
                g_all[i] = q_grad[:, :, ch * i : ch * (i + 1)].astype(F32).reshape(HEAD, ch)

        parts = []
        for i in range(nx):
            grad_at = g_all[i]
            bd_in = block_diagonal(grad_at)
            parts.append(nn(bd_in, kl[i]))
    with scope("wait_own"):
        arrived(ownl, nx - 1, own_rs)
    with scope("line_a2"):
        parts = pairs([(ownl[i].astype(F32) + part).astype(BF16) for i, part in enumerate(parts)])
        def chunk_of(to):
            pieces = pairs([xtl[i, to].reshape(nz * rows, tok) for i in range(nx)])
            chunk = nt(parts[0], pieces[0])
            for a, b in zip(parts[1:], pieces[1:]):
                chunk = chunk + nt(a, b)
            return chunk

        for ks in (far_first[:1], far_first[1:] + [0]):
            chunks = [chunk_of(columns[k]) for k in ks]
            for k, chunk in zip(ks, chunks):
                a_send[columns[k]] = chunk.astype(BF16)
                if not k:
                    aacc[...] = chunk
            for k in ks:
                if k:
                    column_send(a_send, a_recv, a_ss, a_rs, columns[k]).start()

        @pl.when(c == 0)
        def _():
            rcopy(a_send.at[y], a_recv.at[y], a_ss, a_rs.at[0], (z, y, x, 1)).start()

    @pl.when((c == 1) & (back == 0))
    def _():
        with scope("states"):
            for g in (0, 1):
                start = held_out[g]
                for i in range(pln):
                    st_send[g * pln + i] = (l_send[g * pln + i].astype(F32) + start).astype(BF16)
                    start = e_buf[g * pln + i] * start
            for target in targets:
                state_send(*target).start()
            st_buf[me // 2] = st_send[pln + me]

    @pl.when(c == 1)
    def _():
        with scope("wait_m1"):
            m_plane = [from_column(g, m_send.at[x], m_recv, m_rs).astype(BF16) for g in (0, 1)]
        with scope("wait3"):
            for odd in (0, 1):

                @pl.when(back == odd)
                def _():
                    arrived(p_both, some - odd, p_rs)

            from_plane = []
            for g in (0, 1):
                outer[g] = p_both[:, g].astype(F32).reshape(HEAD, ch)
                bd_out = block_diagonal(outer[g])
                from_plane.append(nt(m_plane[g], bd_out))
        for g in (1, 0):
            with scope(f"wait_a{g}"):
                w_sum = from_plane[g] + from_column(g, aacc, a_recv, a_rs)
            with scope(f"send_z{g}"):
                wide_part = w_sum[:, : 2 * HEAD].reshape(nz, rows, 2 * HEAD)
                rest = w_sum[:, 2 * HEAD :].reshape(nz, 2, rows // 2, HEAD)
                rest = jnp.concatenate([rest[:, 0], rest[:, 1]], axis=2)
                packed = jnp.concatenate([wide_part, rest], axis=1)
                if g:
                    w2[...] = packed
                z_send[pl.ds(g * nz, nz)] = packed.astype(BF16)
                for d in z_steps if g else z_steps + [0]:
                    rcopy(z_send.at[g * nz + zs[d]], z_recv.at[z], z_ss, z_rs, (zs[d], y, x, g)).start()

    @pl.when(c == 0)
    def _():
        with scope("wait3"):
            arrived(p_buf, some, p_rs)
        outer[0] = p_buf[...].astype(F32).reshape(HEAD, ch)

    with scope("value_grad"):
        own_after = after[nx - 1]
        for i in range(nx - 1):
            own_after = jnp.where(at_line == i, after[i], own_after)
        grad = g_all[at_line] + own_after * outer[c]
        bd_grad = block_diagonal(grad)
        value_grad = (gv_own + nn(bd_grad, k_end)).astype(BF16)

    with scope("input_grad"):
        width = 512 if d_model % 512 == 0 else d_model
        turned = value_grad.T
        for j in range(d_model // width):
            cols = pl.ds(j * width, width)
            ig[:, :, cols] = nn(turned, w_v[:, cols]).astype(BF16).reshape(2, tok // 2, width)
        ig_copy = rcopy(ig.at[1 - c], ig_recv, ig_ss, ig_rs, (z, y, x, 1 - c))
        ig_copy.start()

    with scope("query_forget"):
        for even in (0, 1):

            @pl.when((1 - back) * c == even)
            def _():
                arrived(st_buf, some - even, st_rs)

        state = st_buf[...].astype(F32).reshape(HEAD, ch)
        bd_state = block_diagonal(state)
        g_query = growth * (gq_own + tn(bd_state, go))
        g_key = shrink * gk_own + remain * tn(bd_grad, v)
        gq_out[...] = (g_query * (q_sig * (1.0 + q * (1.0 - q_sig)))).astype(BF16)
        ends = grad * (total * state + update)
        ends_high = ends.astype(BF16)
        ends_low = (ends - ends_high.astype(F32)).astype(BF16)
        tall_ones = jnp.ones((HEAD, tok), BF16)
        boundary = tn(ends_high, tall_ones) + tn(ends_low, tall_ones)
        flow = query * g_query - k_rate * g_key
        flow_high = flow.astype(BF16)
        flow_low = (flow - flow_high.astype(F32)).astype(BF16)
        g_decay = nn(flow_high, lower_ones) + nn(flow_low, lower_ones) + boundary
        gf_out[...] = ((g_decay / (1.0 - k_rate) - g_key) * k_rate * (1.0 / (1.0 + jnp.exp(-f)))).astype(BF16)

    with scope("input_sum"):
        ig_copy.wait_recv()
        gx_out[...] = (ig[c].astype(F32) + ig_recv[...].astype(F32)).astype(BF16)

    with scope("drain"):
        left(xt, nx - 1, xt_ss)
        left(kl, nx - 1, k_ss)
        left(ownl, nx - 1, own_ss)
        ig_copy.wait_send()

        @pl.when(c == 0)
        def _():
            left(thin, pln, e_ss)
            left(s_send, pln, s_ss)
            left(rl, nx - 1, r_ss)
            left(m_send, ny, m_ss)
            left(a_send, ny, a_ss)

        @pl.when(c == 1)
        def _():
            left(m_send, ny - 1, m_ss)
            left(a_send, ny - 1, a_ss)
            left(thin, pln - 1, e_ss)
            left(s_send, pln - 1, s_ss)
            for n in range(1, nz):

                @pl.when(nz - 1 - z_order == n)
                def _():
                    left(ft_buf, n, ft_ss)
                    left(t_buf, n, t_ss)

            e_all.wait_send()

            @pl.when(back == 1)
            def _():
                left(wide, pln, q_ss.at[0])
                left(broad, pln - 1, q_ss.at[1])
                left(wide, 3 * pln - 2, p_ss)

            @pl.when(back == 0)
            def _():
                left(st_send, 2 * pln - 1, st_ss)

    def unpacked(total):
        gw_out[:, : 2 * HEAD] = total[:rows]
        gw_out[: rows // 2, 2 * HEAD :] = total[rows:, :HEAD]
        gw_out[rows // 2 :, 2 * HEAD :] = total[rows:, HEAD:]

    with scope("wait_z"):

        @pl.when(c == 0)
        def _():
            arrived(z_recv, nz, z_rs)
            w_last = z_recv[0].astype(F32)
            for k in range(1, nz):
                w_last = w_last + z_recv[k].astype(F32)
            unpacked(w_last)

        @pl.when(c == 1)
        def _():
            arrived(z_recv, nz - 1, z_rs)
            w_last = w2[z]
            for k in range(1, nz):
                w_last = w_last + z_recv[zs[k]].astype(F32)
            unpacked(w_last)
            left(z_send, 2 * nz - 1, z_ss)


def write_out(*refs):
    copies = [pltpu.make_async_copy(refs[k], refs[4 + k], refs[8].at[k]) for k in range(4)]
    for copy in copies:
        copy.start()
    for copy in copies:
        copy.wait()


def on_device(nz, ny, nx, block_input, value_weight, query_pre, forget_pre, lower_bound, out_grad):
    tok, d_model = block_input.shape
    ch = value_weight.shape[1]
    pln = ny * nx
    piece = 2 * HEAD // pln
    rows = d_model // (nz * pln)
    vm, dma = pltpu.VMEM, pltpu.SemaphoreType.DMA
    scratch = [
        vm((tok, d_model), BF16), vm((ch, d_model), BF16),
        vm((ch, tok), BF16), vm((ch, tok), BF16), vm((ch, tok), BF16), vm((1, ch), F32),
        vm((pln * (ny + 1), piece, ch), BF16), vm((pln, 1, ch), F32),
        vm((pln, piece, ny * ch), BF16),
        vm((pln, piece, ch), BF16), vm((1, ch), F32),
        vm((2 * pln, piece, ch), BF16), vm((2 * pln, 1, ch), F32),
        vm((2 * pln, piece, ch), BF16), vm((nx, piece, ny * ch), BF16),
        vm((pln // 2, piece, ny * ch), BF16), vm((pln // 2, piece, ch), BF16),
        vm((2, piece, ch), BF16), vm((2, 1, ch), F32),
        vm((nz, 2, piece, ch), BF16), vm((nz, 2, 1, ch), F32),
        vm((2, piece, ch), F32), vm((2, piece, ch), BF16),
        vm((pln // 2, piece, ch), BF16), vm((pln // 2, 2, piece, ch), BF16),
        vm((2, HEAD, ch), F32), vm((2 * pln, piece, ch), BF16), vm((pln // 2, piece, ch), BF16),
        vm((nx, ny, nz, rows, tok), BF16), vm((nx, ny, nz, rows, tok), BF16),
        vm((ch // 2, 2 * HEAD), BF16), vm((nx, ch // 2, 2 * HEAD), BF16),
        vm((ch, tok), BF16), vm((nx, ch, tok), BF16),
        vm((ch, tok), BF16), vm((nx, ch, tok), BF16),
        vm((nx, HEAD, ch), F32),
        vm((2, tok // 2, d_model), BF16), vm((tok // 2, d_model), BF16),
        vm((ny, ch, nz * rows), BF16), vm((2 * ny, ch, nz * rows), BF16),
        vm((ch, nz * rows), F32), vm((ny, ch, nz * rows), BF16), vm((2 * ny, ch, nz * rows), BF16),
        vm((nz, rows * 3 // 2, 2 * HEAD), F32),
        vm((2 * nz, rows * 3 // 2, 2 * HEAD), BF16), vm((nz, rows * 3 // 2, 2 * HEAD), BF16),
        dma((6,)),
        *(dma for _ in range(6)), dma((2,)), dma,
        *(dma for _ in range(4 + 2 + 2 + 8)),
        dma, dma((2,)), dma, dma((2,)), dma, dma, dma, dma,
    ]
    hbm, near = pl.BlockSpec(memory_space=pl.ANY), pl.BlockSpec(memory_space=pltpu.VMEM)
    results = pl.pallas_call(
        functools.partial(kernel, nz, ny, nx),
        out_shape=(
            vm((ch, tok), BF16),
            vm((ch, tok), BF16),
            vm((tok // 2, d_model), BF16),
            vm((rows, ch), F32),
        ),
        in_specs=[hbm] * 6,
        out_specs=(near,) * 4,
        scratch_shapes=scratch,
        compiler_params=pltpu.CompilerParams(collective_id=0, has_side_effects=True),
    )(block_input, value_weight.T, query_pre.T, forget_pre.T, out_grad.T, lower_bound.reshape(1, ch))
    g_query, g_forget, g_input, g_weight = pl.pallas_call(
        write_out,
        out_shape=tuple(jax.ShapeDtypeStruct(a.shape, a.dtype) for a in results),
        in_specs=[near] * 4,
        out_specs=(hbm,) * 4,
        scratch_shapes=[dma((4,))],
    )(*(pltpu.with_memory_space_constraint(a, pltpu.VMEM) for a in results))
    return g_query.T, g_forget.T, g_input, g_weight


def on_mesh(devices):
    nz, ny, nx = devices.shape[:3]
    split = Mesh(devices, SP_TP)
    in_specs = (P(SP, None), P(None, "tp"), P(SP, "tp"), P(SP, "tp"), P("tp"), P(SP, "tp"))
    out_specs = (P(SP, "tp"), P(SP, "tp"), P(SP_TP, None), P(SP, "tp"))
    return jax.shard_map(
        functools.partial(on_device, nz, ny, nx), mesh=split, in_specs=in_specs, out_specs=out_specs, check_vma=False
    )


def solution(mesh):
    return on_mesh(mesh.devices.reshape(8, 4, 4, mesh.shape["tp"]))
```

```python
import functools

import jax
import jax.numpy as jnp
from jax import lax
from jax.experimental import pallas as pl
from jax.experimental.pallas import tpu as pltpu
from jax.sharding import Mesh
from jax.sharding import PartitionSpec as P

HEAD = 64
SP = ("sp_0", "sp_1", "sp_2")
SP_TP = ("sp_0", "sp_1", "sp_2", "tp")
F32, BF16 = jnp.float32, jnp.bfloat16
LOGICAL = pl.DeviceIdType.MESH


def nn(a, b):
    return lax.dot_general(a, b, (((1,), (0,)), ((), ())), preferred_element_type=F32)


def nt(a, b):
    return lax.dot_general(a, b, (((1,), (1,)), ((), ())), preferred_element_type=F32)


def tn(a, b):
    return lax.dot_general(a, b, (((0,), (0,)), ((), ())), preferred_element_type=F32)


def rcopy(src, dst, send, recv, device):
    return pltpu.make_async_remote_copy(
        src_ref=src, dst_ref=dst, send_sem=send, recv_sem=recv, device_id=device, device_id_type=LOGICAL
    )


def kernel(
    nz, ny, nx,
    x_hbm, w_hbm, q_hbm, f_hbm, go_hbm, lb_hbm,
    gq_out, gf_out, gx_out, gw_out,
    x_v, w_v, q_v, f_v, go_v, lb_v, wide, thin, broad,
    s_send, e_send, s_buf, e_buf, l_send, lg_send, q_grad, q_line, t_send, ft_send, t_buf, ft_buf, held_out, o_send, p_buf, p_both, outer, st_send, st_buf,
    xt, xtl, r_send, rl, k_send, kl, own_send, ownl, g_all, ig, ig_recv,
    m_send, m_recv, aacc, a_send, a_recv, w2, z_send, z_recv,
    lsem, s_ss, s_rs, e_ss, e_rs, ea_ss, ea_rs, q_ss, q_rs, t_ss, t_rs, ft_ss, ft_rs, p_ss, p_rs, st_ss, st_rs,
    xt_ss, xt_rs, r_ss, r_rs, k_ss, k_rs, own_ss, own_rs,
    m_ss, m_rs, a_ss, a_rs, z_ss, z_rs, ig_ss, ig_rs,
):
    pln = ny * nx
    tok, d_model = x_v.shape
    ch = w_v.shape[0]
    heads = ch // HEAD
    z, y, x, c = (lax.axis_index(a) for a in SP_TP)
    me = y * nx + x
    back = lax.rem(x + y, 2)
    zs, ys, xs = ([lax.rem(at + d, n) for d in range(n)] for at, n in ((z, nz), (y, ny), (x, nx)))
    across = lambda d, n: min(d, n - d)
    steps = [(dy, dx) for dy in range(ny) for dx in range(nx) if dy or dx]
    steps.sort(key=lambda t: -across(t[0], ny) - across(t[1], nx))
    others = [(ys[dy], xs[dx]) for dy, dx in steps]
    everyone = others + [(y, x)]
    z_steps = sorted(range(1, nz), key=lambda d: -across(d, nz))
    far_first = sorted(range(1, nx), key=lambda d: -across(d, nx))

    at_line, at_col = x * (1 - c) + y * c, y * (1 - c) + x * c
    lines = [xs[d] * (1 - c) + ys[d] * c for d in range(nx)]
    columns = [ys[d] * (1 - c) + xs[d] * c for d in range(ny)]

    def line(i):
        return (z, y * (1 - c) + i * c, i * (1 - c) + x * c, c)

    def column(i):
        return (z, i * (1 - c) + y * c, x * (1 - c) + i * c, c)

    def piece_of(ty, tx):
        return ty * (nx // 2) + lax.div(tx, 2) + lax.rem(tx + ty, 2) * (pln // 2)

    def head_of(a, h):
        return a[HEAD * h : HEAD * (h + 1)]

    def by_head(parts):
        return jnp.concatenate(list(parts), axis=0)

    def arrived(ref, n, sem):
        part = ref.at[pl.ds(0, n)]
        rcopy(part, part, sem, sem, (z, y, x, 1 - c)).wait_recv()

    def left(ref, n, sem):
        part = ref.at[pl.ds(0, n)]
        rcopy(part, part, sem, sem, (z, y, x, 1 - c)).wait_send()

    scope = jax.named_scope
    with scope("loads_barrier"):
        loads = [
            pltpu.make_async_copy(src, dst, lsem.at[k])
            for k, (src, dst) in enumerate(
                ((f_hbm, f_v), (q_hbm, q_v), (go_hbm, go_v), (x_hbm, x_v), (w_hbm, w_v), (lb_hbm, lb_v))
            )
        ]
        for k in (0, 5, 1, 2, 3, 4):
            loads[k].start()
        barrier = pltpu.get_barrier_semaphore()

        def greet(device):
            pl.semaphore_signal(barrier, inc=1, device_id=device, device_id_type=LOGICAL)

        @pl.when(c == 1)
        def _():
            for ty, tx in others:
                greet((z, ty, tx, 1))
            for ty, tx in everyone:
                greet((z, ty, tx, 0))

        @pl.when(c == 0)
        def _():
            for tx in xs[1:]:
                greet((z, y, tx, 0))

        for d in z_steps:
            greet((zs[d], y, x, 1))

    lane = lax.broadcasted_iota(jnp.int32, (1, ch), 1)
    mf = [jnp.where((lane >= HEAD * h) & (lane < HEAD * (h + 1)), 1.0, 0.0).astype(F32) for h in range(heads)]
    row = lax.broadcasted_iota(jnp.int32, (tok, tok), 0)
    col = lax.broadcasted_iota(jnp.int32, (tok, tok), 1)
    lower, upper = row >= col, col >= row
    lower_ones = jnp.where(lower, 1.0, 0.0).astype(BF16)
    upper_ones = jnp.where(upper, 1.0, 0.0).astype(BF16)

    mb = [m.astype(BF16) for m in mf]

    def block_diagonal(a):
        a = a.astype(BF16)
        return by_head(a * m for m in mb)

    def folded(full):
        out = full[:HEAD] * mf[0]
        for h in range(1, heads):
            out = out + head_of(full, h) * mf[h]
        return out

    with scope("gates"):
        loads[5].wait()
        gap = jnp.broadcast_to(1.0 - lb_v[...], (tok, ch)).T
        loads[0].wait()
        f = f_v[...].astype(F32)
        f_neg = 1.0 / (1.0 + jnp.exp(f))
        k_rate = gap * f_neg
        logs = jnp.log1p(-k_rate)
        high = logs.astype(BF16)
        low = (logs - high.astype(F32)).astype(BF16)
        cum = nn(high, upper_ones) + nn(low, upper_ones)
        row_ones = jnp.ones((8, tok), BF16)
        total = jnp.exp((nt(row_ones, high) + nt(row_ones, low))[:1])
        closing = cum[:, tok - 1 : tok]
        growth = jnp.exp(cum)
        remain = jnp.exp(closing - cum)
        e_send[...] = total
        k_end = (k_rate * remain).astype(BF16)
        loads[1].wait()
        q = q_v[...].astype(F32)
        q_sig = 1.0 / (1.0 + jnp.exp(-q))
        query = q * q_sig
        q_dec = (query * growth).astype(BF16)
        loads[2].wait()
        go = go_v[...]
        reach = folded(nt(go, q_dec))
    with scope("values"):
        loads[3].wait()
        loads[4].wait()
        v = nt(w_v[...], x_v[...]).astype(BF16)
        update = folded(nt(v, k_end))
        s_send[...] = jnp.concatenate([update, reach], axis=0).reshape(s_send.shape).astype(BF16)
        narrow, low_half = 2 * HEAD, HEAD // 2
        rest = jnp.concatenate([reach[:low_half, narrow:], reach[low_half:, narrow:]], axis=1)
        r_send[...] = jnp.concatenate([reach[:, :narrow], rest], axis=0).astype(BF16)
        k_send[...] = k_end

    with scope("barrier_wait"):
        pl.semaphore_wait(barrier, c * (pln - 1 + 2 * (nz - 1)) + (1 - c) * (pln + nx - 1))

    def to_line(source, target, send_sem, recv_sem):
        for k in far_first:
            rcopy(source, target.at[at_line], send_sem, recv_sem, line(lines[k])).start()

    def column_send(source, target, send_sem, recv_sem, to):
        device = (z, to * (1 - c) + y * c, x * (1 - c) + to * c, 1)
        return rcopy(source.at[to], target.at[c * ny + at_col], send_sem, recv_sem.at[c], device)

    def to_column(source, target, send_sem, recv_sem):
        for k in far_first:
            column_send(source, target, send_sem, recv_sem, columns[k]).start()

        @pl.when(c == 0)
        def _():
            rcopy(source.at[y], target.at[y], send_sem, recv_sem.at[0], (z, y, x, 1)).start()

    def from_column(g, own, target, recv_sem):
        arrived(target, ny - g, recv_sem.at[g])
        if g == 0:
            out = target[0].astype(F32)
            for k in range(1, ny):
                out = out + target[k].astype(F32)
            return out.T
        out = own[...].astype(F32)
        for k in range(1, ny):
            out = out + target[ny + xs[k]].astype(F32)
        return out.T

    def piece_sends(ty, tx):
        to = (z, ty, tx, 1)
        return (
            rcopy(e_send, e_buf.at[c * pln + me], e_ss, e_rs, to),
            rcopy(s_send.at[piece_of(ty, tx)], s_buf.at[c * pln + me], s_ss, s_rs, to),
        )

    mine = piece_of(y, x)
    with scope("send1"):
        for parity in (0, 1):

            @pl.when(back == parity)
            def _():
                for want in (1 - parity, parity):
                    for (dy, dx), target in zip(steps, others):
                        if (dy + dx) % 2 == want:
                            for copy in piece_sends(*target):
                                copy.start()

        @pl.when(c == 0)
        def _():
            for copy in piece_sends(y, x):
                copy.start()

        @pl.when(c == 1)
        def _():
            s_buf[pln + me] = s_send[mine]
            e_buf[pln + me] = e_send[...]

        to_line(k_send, kl, k_ss, k_rs)
        kl[at_line] = k_end
        rl[at_line] = r_send[...]

    rows = d_model // (nz * ny * nx)
    with scope("turn"):
        per = tok // rows
        for b in range(d_model // tok):
            turned = x_v[:, tok * b : tok * (b + 1)].T
            for g in range(per):
                at = b * per + g
                zz, yy, xx = at // pln, (at // nx) % ny, at % nx
                group, into = xx * (1 - c) + yy * c, yy * (1 - c) + xx * c
                xt[group, into, zz] = turned[rows * g : rows * (g + 1)]

        for k in far_first:
            to = lines[k]
            rcopy(xt.at[to], xtl.at[at_line], xt_ss, xt_rs, line(to)).start()

        @pl.when(c == 0)
        def _():
            to_line(r_send, rl, r_ss, r_rs)

        xtl[at_line] = xt[at_line]

    with scope("pairs_value"):
        shrink = jnp.exp(-cum)
        k_dec = (k_rate * shrink).astype(BF16)
        mixing = [jnp.where(lower, tn(head_of(q_dec, h), head_of(k_dec, h)), 0.0).astype(BF16) for h in range(heads)]
        gv_own = by_head(nn(head_of(go, h), mixing[h]) for h in range(heads))
        own_send[...] = gv_own.astype(BF16)
        ownl[at_line] = own_send[...]

        @pl.when(c == 0)
        def _():
            to_line(own_send, ownl, own_ss, own_rs)


    z_order = z + back * (nz - 1 - 2 * z)

    def z_sends(k):
        at = z_order + k
        to = at + back * (nz - 1 - 2 * at)
        return (
            rcopy(ft_send, ft_buf.at[z], ft_ss, ft_rs, (to, y, x, 1)),
            rcopy(t_send, t_buf.at[z], t_ss, t_rs, (to, y, x, 1)),
        )

    def carry_send(g, ty, tx):
        device = (z, ty, tx, g)
        if g == 0:
            return rcopy(l_send.at[ty * nx + nx - 1], q_line.at[me // 2], q_ss.at[0], q_rs, device)
        return rcopy(lg_send.at[tx], q_grad.at[me // 2], q_ss.at[1], q_rs, device)

    targets = [(0, *t) for t in everyone] + [(1, *t) for t in others]
    plane_decays = e_buf.at[pl.ds(0, pln)]
    e_all = rcopy(plane_decays, plane_decays, ea_ss, ea_rs, (z, y, x, 1 - c))

    @pl.when(c == 1)
    def _():
        with scope("wait1"):
            arrived(e_buf, 2 * pln - 1, e_rs)
            arrived(s_buf, 2 * pln - 1, s_rs)
        with scope("scan1"):
            for parity in (0, 1):

                @pl.when(back == parity)
                def _():
                    for g in (0, 1):
                        held = jnp.zeros(t_send.shape[1:], F32)
                        factor = jnp.ones((1, ch), F32)
                        for it in range(pln - 1, -1, -1) if parity else range(pln):
                            if g and parity:
                                lg_send[it % nx, :, ch * (it // nx) : ch * (it // nx + 1)] = held.astype(BF16)
                            else:
                                l_send[g * pln + it] = held.astype(BF16)
                            decay = e_buf[g * pln + it]
                            held = decay * held + s_buf[g * pln + it].astype(F32)
                            factor = decay * factor
                        t_send[g] = held.astype(BF16)
                        ft_send[g] = factor

        with scope("send2"):
            for k in range(1, nz):

                @pl.when(z_order + k < nz)
                def _():
                    for copy in z_sends(k):
                        copy.start()

            @pl.when(back == 1)
            def _():
                for target in targets[pln:] + targets[:pln]:
                    carry_send(*target).start()
                q_grad[me // 2] = lg_send[x]

            to_line(own_send, ownl, own_ss, own_rs)
            e_all.start()

    with scope("pairs_query"):
        pairing = [jnp.where(upper, tn(head_of(v, h), head_of(go, h)), 0.0).astype(BF16) for h in range(heads)]
        gq_own = by_head(nn(head_of(k_dec, h), pairing[h]) for h in range(heads))
        gk_own = by_head(nt(head_of(q_dec, h), pairing[h]) for h in range(heads))

    with scope("decays"):
        @pl.when(c == 0)
        def _():
            e_all.wait_recv()

        decays = e_buf[pl.ds(c * pln, pln)]
        after = [jnp.ones((1, ch), F32)] * nx
        ids = [line(i)[1] * nx + line(i)[2] for i in range(nx)]
        for i in range(pln):
            after = [a * jnp.where(i > n, decays[i], 1.0) for a, n in zip(after, ids)]

    with scope("wait_line"):
        arrived(xtl, nx - 1, xt_rs)
        arrived(kl, nx - 1, k_rs)

    def pairs(parts):
        return [jnp.concatenate(parts[i : i + 2], axis=1) for i in range(0, nx, 2)]

    def to_chunks(ref, total):
        for i in range(ny):
            ref[i] = total[:, i * nz * rows : (i + 1) * nz * rows].astype(ref.dtype)

    with scope("line_m"):
        turned_of = pairs([xtl[i].reshape(d_model // nx, tok) for i in range(nx)])
        tall_after = jnp.concatenate(after + [jnp.ones((8 - nx, ch), F32)], axis=0).T
        scaled = pairs([(kl[i].astype(F32) * tall_after[:, i : i + 1]).astype(BF16) for i in range(nx)])
        m_sum = nt(scaled[0], turned_of[0])
        for a, b in zip(scaled[1:], turned_of[1:]):
            m_sum = m_sum + nt(a, b)
        to_chunks(m_send, m_sum)
        to_column(m_send, m_recv, m_ss, m_rs)

    def arriving(o, carried):
        frm = o + back * (nz - 1 - 2 * o)
        return ft_buf[frm] * carried + t_buf[frm].astype(F32)

    def plane_send(g, ty, tx):
        if g:
            return rcopy(o_send, p_both.at[me // 2], p_ss, p_rs, (z, ty, tx, 1))
        return rcopy(o_send.at[0], p_buf.at[me // 2], p_ss, p_rs, (z, ty, tx, 0))

    def state_send(g, ty, tx):
        return rcopy(st_send.at[g * pln + ty * nx + tx], st_buf.at[me // 2], st_ss, st_rs, (z, ty, tx, g))

    @pl.when(c == 1)
    def _():
        with scope("wait2"):
            for n in range(1, nz):

                @pl.when(z_order == n)
                def _():
                    arrived(ft_buf, n, ft_rs)
                    arrived(t_buf, n, t_rs)

            carried = lax.fori_loop(0, z_order, arriving, jnp.zeros(t_send.shape, F32))
        with scope("send3"):
            held_out[...] = carried
            o_send[...] = carried.astype(BF16)

            @pl.when(back == 1)
            def _():
                for target in targets[pln:] + targets[:pln]:
                    plane_send(*target).start()
                p_both[me // 2] = o_send[...]

    some = pln // 2
    with scope("wait_1b"):

        @pl.when(c == 0)
        def _():
            arrived(q_line, some, q_rs)
            arrived(rl, nx - 1, r_rs)

        for odd in (0, 1):

            @pl.when((c == 1) & (back == odd))
            def _():
                arrived(q_grad, some - odd, q_rs)

    with scope("line_a"):

        @pl.when(c == 0)
        def _():
            grad_at = q_line[...].astype(F32).reshape(HEAD, ch)
            g_all[nx - 1] = grad_at
            for i in range(nx - 2, -1, -1):
                near_reach = rl[i + 1].astype(F32)
                rest = near_reach[HEAD:]
                rest = jnp.concatenate([rest[:, :HEAD], rest[:, HEAD:]], axis=0)
                near_reach = jnp.concatenate([near_reach[:HEAD], rest], axis=1)
                grad_at = e_buf[y * nx + i + 1] * grad_at + near_reach
                g_all[i] = grad_at

        @pl.when(c == 1)
        def _():
            for i in range(nx):
                g_all[i] = q_grad[:, :, ch * i : ch * (i + 1)].astype(F32).reshape(HEAD, ch)

        parts = []
        for i in range(nx):
            grad_at = g_all[i]
            bd_in = block_diagonal(grad_at)
            parts.append(nn(bd_in, kl[i]))
    with scope("wait_own"):
        arrived(ownl, nx - 1, own_rs)
    with scope("line_a2"):
        parts = pairs([(ownl[i].astype(F32) + part).astype(BF16) for i, part in enumerate(parts)])
        def chunk_of(to):
            pieces = pairs([xtl[i, to].reshape(nz * rows, tok) for i in range(nx)])
            chunk = nt(parts[0], pieces[0])
            for a, b in zip(parts[1:], pieces[1:]):
                chunk = chunk + nt(a, b)
            return chunk

        for ks in (far_first[:1], far_first[1:] + [0]):
            chunks = [chunk_of(columns[k]) for k in ks]
            for k, chunk in zip(ks, chunks):
                a_send[columns[k]] = chunk.astype(BF16)
                if not k:
                    aacc[...] = chunk
            for k in ks:
                if k:
                    column_send(a_send, a_recv, a_ss, a_rs, columns[k]).start()

        @pl.when(c == 0)
        def _():
            rcopy(a_send.at[y], a_recv.at[y], a_ss, a_rs.at[0], (z, y, x, 1)).start()

    @pl.when((c == 1) & (back == 0))
    def _():
        with scope("states"):
            for g in (0, 1):
                start = held_out[g]
                for i in range(pln):
                    st_send[g * pln + i] = (l_send[g * pln + i].astype(F32) + start).astype(BF16)
                    start = e_buf[g * pln + i] * start
            for target in targets:
                state_send(*target).start()
            st_buf[me // 2] = st_send[pln + me]

    @pl.when(c == 1)
    def _():
        with scope("wait_m1"):
            m_plane = [from_column(g, m_send.at[x], m_recv, m_rs).astype(BF16) for g in (0, 1)]
        with scope("wait3"):
            for odd in (0, 1):

                @pl.when(back == odd)
                def _():
                    arrived(p_both, some - odd, p_rs)

            from_plane = []
            for g in (0, 1):
                outer[g] = p_both[:, g].astype(F32).reshape(HEAD, ch)
                bd_out = block_diagonal(outer[g])
                from_plane.append(nt(m_plane[g], bd_out))
        for g in (1, 0):
            with scope(f"wait_a{g}"):
                w_sum = from_plane[g] + from_column(g, aacc, a_recv, a_rs)
            with scope(f"send_z{g}"):
                wide_part = w_sum[:, : 2 * HEAD].reshape(nz, rows, 2 * HEAD)
                rest = w_sum[:, 2 * HEAD :].reshape(nz, 2, rows // 2, HEAD)
                rest = jnp.concatenate([rest[:, 0], rest[:, 1]], axis=2)
                packed = jnp.concatenate([wide_part, rest], axis=1)
                if g:
                    w2[...] = packed
                z_send[pl.ds(g * nz, nz)] = packed.astype(BF16)
                for d in z_steps if g else z_steps + [0]:
                    rcopy(z_send.at[g * nz + zs[d]], z_recv.at[z], z_ss, z_rs, (zs[d], y, x, g)).start()

    @pl.when(c == 0)
    def _():
        with scope("wait3"):
            arrived(p_buf, some, p_rs)
        outer[0] = p_buf[...].astype(F32).reshape(HEAD, ch)

    with scope("value_grad"):
        own_after = after[nx - 1]
        for i in range(nx - 1):
            own_after = jnp.where(at_line == i, after[i], own_after)
        grad = g_all[at_line] + own_after * outer[c]
        bd_grad = block_diagonal(grad)
        value_grad = (gv_own + nn(bd_grad, k_end)).astype(BF16)

    with scope("input_grad"):
        width = 512 if d_model % 512 == 0 else d_model
        turned = value_grad.T
        for j in range(d_model // width):
            cols = pl.ds(j * width, width)
            ig[:, :, cols] = nn(turned, w_v[:, cols]).astype(BF16).reshape(2, tok // 2, width)
        ig_copy = rcopy(ig.at[1 - c], ig_recv, ig_ss, ig_rs, (z, y, x, 1 - c))
        ig_copy.start()

    with scope("query_forget"):
        for even in (0, 1):

            @pl.when((1 - back) * c == even)
            def _():
                arrived(st_buf, some - even, st_rs)

        state = st_buf[...].astype(F32).reshape(HEAD, ch)
        bd_state = block_diagonal(state)
        g_query = growth * (gq_own + tn(bd_state, go))
        g_key = shrink * gk_own + remain * tn(bd_grad, v)
        gq_out[...] = (g_query * (q_sig * (1.0 + q * (1.0 - q_sig)))).astype(BF16)
        ends = grad * (total * state + update)
        ends_high = ends.astype(BF16)
        ends_low = (ends - ends_high.astype(F32)).astype(BF16)
        tall_ones = jnp.ones((HEAD, tok), BF16)
        boundary = tn(ends_high, tall_ones) + tn(ends_low, tall_ones)
        flow = query * g_query - k_rate * g_key
        flow_high = flow.astype(BF16)
        flow_low = (flow - flow_high.astype(F32)).astype(BF16)
        g_decay = nn(flow_high, lower_ones) + nn(flow_low, lower_ones) + boundary
        gf_out[...] = ((g_decay / (1.0 - k_rate) - g_key) * k_rate * (1.0 / (1.0 + jnp.exp(-f)))).astype(BF16)

    with scope("input_sum"):
        ig_copy.wait_recv()
        gx_out[...] = (ig[c].astype(F32) + ig_recv[...].astype(F32)).astype(BF16)

    with scope("drain"):
        left(xt, nx - 1, xt_ss)
        left(kl, nx - 1, k_ss)
        left(ownl, nx - 1, own_ss)
        ig_copy.wait_send()

        @pl.when(c == 0)
        def _():
            left(thin, pln, e_ss)
            left(s_send, pln, s_ss)
            left(rl, nx - 1, r_ss)
            left(m_send, ny, m_ss)
            left(a_send, ny, a_ss)

        @pl.when(c == 1)
        def _():
            left(m_send, ny - 1, m_ss)
            left(a_send, ny - 1, a_ss)
            left(thin, pln - 1, e_ss)
            left(s_send, pln - 1, s_ss)
            for n in range(1, nz):

                @pl.when(nz - 1 - z_order == n)
                def _():
                    left(ft_buf, n, ft_ss)
                    left(t_buf, n, t_ss)

            e_all.wait_send()

            @pl.when(back == 1)
            def _():
                left(wide, pln, q_ss.at[0])
                left(broad, pln - 1, q_ss.at[1])
                left(wide, 3 * pln - 2, p_ss)

            @pl.when(back == 0)
            def _():
                left(st_send, 2 * pln - 1, st_ss)

    def unpacked(total):
        gw_out[:, : 2 * HEAD] = total[:rows]
        gw_out[: rows // 2, 2 * HEAD :] = total[rows:, :HEAD]
        gw_out[rows // 2 :, 2 * HEAD :] = total[rows:, HEAD:]

    with scope("wait_z"):

        @pl.when(c == 0)
        def _():
            arrived(z_recv, nz, z_rs)
            w_last = z_recv[0].astype(F32)
            for k in range(1, nz):
                w_last = w_last + z_recv[k].astype(F32)
            unpacked(w_last)

        @pl.when(c == 1)
        def _():
            arrived(z_recv, nz - 1, z_rs)
            w_last = w2[z]
            for k in range(1, nz):
                w_last = w_last + z_recv[zs[k]].astype(F32)
            unpacked(w_last)
            left(z_send, 2 * nz - 1, z_ss)


def write_out(*refs):
    copies = [pltpu.make_async_copy(refs[k], refs[4 + k], refs[8].at[k]) for k in range(4)]
    for copy in copies:
        copy.start()
    for copy in copies:
        copy.wait()


def on_device(nz, ny, nx, block_input, value_weight, query_pre, forget_pre, lower_bound, out_grad):
    tok, d_model = block_input.shape
    ch = value_weight.shape[1]
    pln = ny * nx
    piece = 2 * HEAD // pln
    rows = d_model // (nz * pln)
    vm, dma = pltpu.VMEM, pltpu.SemaphoreType.DMA
    scratch = [
        vm((tok, d_model), BF16), vm((ch, d_model), BF16),
        vm((ch, tok), BF16), vm((ch, tok), BF16), vm((ch, tok), BF16), vm((1, ch), F32),
        vm((pln * (ny + 1), piece, ch), BF16), vm((pln, 1, ch), F32),
        vm((pln, piece, ny * ch), BF16),
        vm((pln, piece, ch), BF16), vm((1, ch), F32),
        vm((2 * pln, piece, ch), BF16), vm((2 * pln, 1, ch), F32),
        vm((2 * pln, piece, ch), BF16), vm((nx, piece, ny * ch), BF16),
        vm((pln // 2, piece, ny * ch), BF16), vm((pln // 2, piece, ch), BF16),
        vm((2, piece, ch), BF16), vm((2, 1, ch), F32),
        vm((nz, 2, piece, ch), BF16), vm((nz, 2, 1, ch), F32),
        vm((2, piece, ch), F32), vm((2, piece, ch), BF16),
        vm((pln // 2, piece, ch), BF16), vm((pln // 2, 2, piece, ch), BF16),
        vm((2, HEAD, ch), F32), vm((2 * pln, piece, ch), BF16), vm((pln // 2, piece, ch), BF16),
        vm((nx, ny, nz, rows, tok), BF16), vm((nx, ny, nz, rows, tok), BF16),
        vm((ch // 2, 2 * HEAD), BF16), vm((nx, ch // 2, 2 * HEAD), BF16),
        vm((ch, tok), BF16), vm((nx, ch, tok), BF16),
        vm((ch, tok), BF16), vm((nx, ch, tok), BF16),
        vm((nx, HEAD, ch), F32),
        vm((2, tok // 2, d_model), BF16), vm((tok // 2, d_model), BF16),
        vm((ny, ch, nz * rows), BF16), vm((2 * ny, ch, nz * rows), BF16),
        vm((ch, nz * rows), F32), vm((ny, ch, nz * rows), BF16), vm((2 * ny, ch, nz * rows), BF16),
        vm((nz, rows * 3 // 2, 2 * HEAD), F32),
        vm((2 * nz, rows * 3 // 2, 2 * HEAD), BF16), vm((nz, rows * 3 // 2, 2 * HEAD), BF16),
        dma((6,)),
        *(dma for _ in range(6)), dma((2,)), dma,
        *(dma for _ in range(4 + 2 + 2 + 8)),
        dma, dma((2,)), dma, dma((2,)), dma, dma, dma, dma,
    ]
    hbm, near = pl.BlockSpec(memory_space=pl.ANY), pl.BlockSpec(memory_space=pltpu.VMEM)
    results = pl.pallas_call(
        functools.partial(kernel, nz, ny, nx),
        out_shape=(
            vm((ch, tok), BF16),
            vm((ch, tok), BF16),
            vm((tok // 2, d_model), BF16),
            vm((rows, ch), F32),
        ),
        in_specs=[hbm] * 6,
        out_specs=(near,) * 4,
        scratch_shapes=scratch,
        compiler_params=pltpu.CompilerParams(collective_id=0, has_side_effects=True),
    )(block_input, value_weight.T, query_pre.T, forget_pre.T, out_grad.T, lower_bound.reshape(1, ch))
    g_query, g_forget, g_input, g_weight = pl.pallas_call(
        write_out,
        out_shape=tuple(jax.ShapeDtypeStruct(a.shape, a.dtype) for a in results),
        in_specs=[near] * 4,
        out_specs=(hbm,) * 4,
        scratch_shapes=[dma((4,))],
    )(*(pltpu.with_memory_space_constraint(a, pltpu.VMEM) for a in results))
    return g_query.T, g_forget.T, g_input, g_weight


def on_mesh(devices):
    nz, ny, nx = devices.shape[:3]
    split = Mesh(devices, SP_TP)
    in_specs = (P(SP, None), P(None, "tp"), P(SP, "tp"), P(SP, "tp"), P("tp"), P(SP, "tp"))
    out_specs = (P(SP, "tp"), P(SP, "tp"), P(SP_TP, None), P(SP, "tp"))
    return jax.shard_map(
        functools.partial(on_device, nz, ny, nx), mesh=split, in_specs=in_specs, out_specs=out_specs, check_vma=False
    )


def solution(mesh):
    return on_mesh(mesh.devices.reshape(8, 4, 4, mesh.shape["tp"]))
```
